768 devices in a mesh: sp: 384 (over z, y, x), tp: 2 (over core).
Axes of the slice: x: 4, y: 8, z: 12, core: 2. Of those that a mesh axis runs over, the one named last changes fastest.
Arguments:
- queries: bfloat16 [98304, 512], P('sp', 'tp'), may hold values from -6 to 6
- keys: bfloat16 [98304, 512], P('sp', 'tp'), may hold values from -6 to 6
- values: bfloat16 [98304, 512], P('sp', 'tp'), may hold values from -6 to 6
- gains: float32 [2, 128], replicated, may hold values from 0.1 to 1.9
- bias_table: float32 [192, 4], P(None, 'tp'), may hold values from -6 to 270
- d_out: bfloat16 [98304, 512], P('sp', 'tp'), may hold values from -32 to 32
Outputs:
- d_queries: bfloat16 [98304, 512], P('sp', 'tp')
- d_keys: bfloat16 [98304, 512], P('sp', 'tp')
- d_values: bfloat16 [98304, 512], P('sp', 'tp')
- d_table: float32 [192, 4], P(None, 'tp')
- d_gains: float32 [2, 128], replicated
The draws below stay inside these ranges and needn't reach their ends.
All inputs are finite; a program needn't handle non-finite values.
Results may differ from the reference program's by a relative error of at most 0.008.
Values may be sent and summed in bfloat16 or wider, within the bound.
A program may use at most 32 MiB of HBM per device.

```python
import jax
import jax.numpy as jnp
from jax import lax

HEADS = 4
HEAD_DIM = 128
SEG = 64
LEFT = 4
MAX_REL = 128
TOKENS = 98304


def draw_bias_table(key, part):
    entries = MAX_REL + SEG
    rough = jnp.clip(jax.random.normal(key, (entries, HEADS), jnp.float32), -6.0, 6.0)
    return rough.astype(jnp.float32)


def draw_d_out(key, part):
    width = HEADS * HEAD_DIM
    position = jnp.arange(TOKENS).astype(jnp.float32)[:, None] / TOKENS
    spread = 10.0 ** (jax.random.uniform(jax.random.fold_in(key, 1), (TOKENS, 1), jnp.float32) - 1.0)
    base = jnp.clip(jax.random.normal(jax.random.fold_in(key, 2), (TOKENS, width), jnp.float32), -6.0, 6.0)
    rise = 3.0 ** position
    return (base * spread * rise).astype(jnp.bfloat16)


def shard_levels(own_key, dims, shards, smallest, high):
    gain = 1.0
    for axis_at, shards_of in shards:
        heights = jax.random.uniform(jax.random.fold_in(jax.random.fold_in(own_key, 6), axis_at), (shards_of,), jnp.float32, smallest / len(shards), high / len(shards))
        gain = gain * jnp.repeat(jnp.exp(heights), dims[axis_at] // shards_of).reshape((-1,) + (1,) * (len(dims) - 1 - axis_at))
    return gain


def centred(own_key, shape, scale, bound, cuts=(), held_as=jnp.bfloat16):
    values = scale * jax.random.normal(own_key, shape, jnp.float32)
    if cuts:
        values = values * shard_levels(own_key, shape, cuts, -0.22, 0.18)
    return jnp.clip(values, -bound, bound).astype(held_as)


def setup_inputs(seed: int = 0) -> dict:
    streams_of = jax.random.split(jax.random.key(seed), 7)
    return {
        "queries": centred(streams_of[0], (TOKENS, HEADS * HEAD_DIM), 1.0, 6.0, ((0, 384), (1, 2))),
        "keys": centred(streams_of[1], (TOKENS, HEADS * HEAD_DIM), 1.0, 6.0, ((0, 384), (1, 2))),
        "values": centred(streams_of[2], (TOKENS, HEADS * HEAD_DIM), 1.0, 6.0, ((0, 384), (1, 2))),
        "gains": jnp.clip(1.0 + 0.18 * jax.random.normal(streams_of[3], (2, HEAD_DIM), jnp.float32), 0.1, 1.9),
        "bias_table": draw_bias_table(jax.random.fold_in(streams_of[6], 71), 0),
        "d_out": draw_d_out(jax.random.fold_in(streams_of[6], 71), 0),
    }


EPSILON = 1e-06

def unit_rows(row_block):
    widened = row_block.astype(jnp.float32).reshape(row_block.shape[0], HEADS, HEAD_DIM)
    inv_rms = lax.rsqrt(lax.optimization_barrier(jnp.mean(widened * widened, axis=-1, keepdims=True)) + EPSILON)
    return (widened * inv_rms, inv_rms)

def rows_back(d_normed, row_block, gain_vec):
    unit_part, inv_rms = unit_rows(row_block)
    d_unit = d_normed * gain_vec
    d_rows = inv_rms * (d_unit - unit_part * lax.optimization_barrier(jnp.mean(d_unit * unit_part, axis=-1, keepdims=True)))
    return (d_rows.reshape(row_block.shape[0], -1).astype(jnp.bfloat16), lax.optimization_barrier(jnp.sum(d_normed * unit_part, axis=(0, 1))))

def lowered(array_in):
    return lax.optimization_barrier(array_in.astype(jnp.bfloat16)).astype(jnp.float32)

def reference(queries, keys, values, gains, bias_table, d_out):
    tail_rows = LEFT * SEG
    blocks = TOKENS // tail_rows
    factor = HEAD_DIM ** (-0.5)
    q_unit, _ = unit_rows(queries)
    q_norm = (q_unit * gains[0]).astype(jnp.bfloat16)
    k_unit, _ = unit_rows(keys)
    k_norm = (k_unit * gains[1]).astype(jnp.bfloat16)
    leading = jnp.zeros((tail_rows, HEADS, HEAD_DIM), jnp.bfloat16)
    k_all = jnp.concatenate([leading, k_norm])
    v_all = jnp.concatenate([leading, values.reshape(TOKENS, HEADS, HEAD_DIM)])
    q_blocks = q_norm.reshape(blocks, tail_rows, HEADS, HEAD_DIM)
    do_blocks = d_out.reshape(blocks, tail_rows, HEADS, HEAD_DIM)
    query_idx = jnp.arange(tail_rows, dtype=jnp.int32)[:, None]
    key_idx = jnp.arange(2 * tail_rows, dtype=jnp.int32)[None, :]
    rel_index = (jnp.clip(query_idx + tail_rows - key_idx, -(SEG - 1), MAX_REL) + SEG - 1).astype(jnp.int32)
    bias_tiles = jnp.transpose(bias_table[rel_index], (2, 0, 1))
    flat_index = rel_index.reshape(-1)

    def advance(state, entry):
        pend_k, pend_v, table_sum = state
        number, q_block, do_block = entry
        start = number * tail_rows
        k_ext = lax.dynamic_slice_in_dim(k_all, start, 2 * tail_rows, 0).astype(jnp.float32)
        v_ext = lax.dynamic_slice_in_dim(v_all, start, 2 * tail_rows, 0).astype(jnp.float32)
        query_seg = (start + query_idx) // SEG
        key_pos = start - tail_rows + key_idx
        key_seg = key_pos // SEG
        key_valid = (key_pos >= 0) & (key_seg >= query_seg - LEFT) & (key_seg <= query_seg)
        q_float = q_block.astype(jnp.float32)
        do_float = do_block.astype(jnp.float32)
        scores = jnp.einsum('ihd,jhd->hij', q_float, k_ext) * factor + bias_tiles
        scores = jnp.where(key_valid[None], scores, -jnp.inf)
        row_max = lax.optimization_barrier(jnp.max(scores, axis=-1, keepdims=True))
        log_total = row_max + jnp.log(lax.optimization_barrier(jnp.sum(jnp.exp(scores - row_max), axis=-1, keepdims=True)))
        prob = jnp.exp(scores - log_total)
        d_prob = jnp.einsum('ihd,jhd->hij', do_float, v_ext)
        row_delta = lax.optimization_barrier(jnp.sum(prob * d_prob, axis=-1, keepdims=True))
        d_score = prob * (d_prob - row_delta)
        prob_low = lowered(prob)
        d_low = lowered(d_score)
        grad_v = jnp.einsum('hij,ihd->jhd', prob_low, do_float)
        grad_k = jnp.einsum('hij,ihd->jhd', d_low, q_float) * factor
        grad_q = jnp.einsum('hij,jhd->ihd', d_low, k_ext) * factor
        table_part = jax.ops.segment_sum(jnp.transpose(d_score, (1, 2, 0)).reshape(-1, HEADS), flat_index, num_segments=MAX_REL + SEG)
        emitted = (pend_k + grad_k[:tail_rows], pend_v + grad_v[:tail_rows], grad_q)
        return ((grad_k[tail_rows:], grad_v[tail_rows:], table_sum + table_part), emitted)
    zero_rows = jnp.zeros((tail_rows, HEADS, HEAD_DIM), jnp.float32)
    initial = (zero_rows, zero_rows, jnp.zeros((MAX_REL + SEG, HEADS), jnp.float32))
    numbers = jnp.arange(blocks, dtype=jnp.int32)
    (last_k, last_v, d_table), (ys_k, ys_v, ys_q) = lax.scan(advance, initial, (numbers, q_blocks, do_blocks))
    d_kn = jnp.concatenate([ys_k[1:].reshape(-1, HEADS, HEAD_DIM), last_k])
    d_vn = jnp.concatenate([ys_v[1:].reshape(-1, HEADS, HEAD_DIM), last_v])
    d_qn = ys_q.reshape(TOKENS, HEADS, HEAD_DIM)
    d_queries, gain_q = rows_back(d_qn, queries, gains[0])
    d_keys, gain_k = rows_back(d_kn, keys, gains[1])
    d_values = d_vn.reshape(TOKENS, -1).astype(jnp.bfloat16)
    return (d_queries, d_keys, d_values, d_table, jnp.stack([gain_q, gain_k]))
```

```python
import functools

import jax
import jax.numpy as jnp
import numpy as np
from jax import lax
from jax.experimental import pallas as pl
from jax.experimental.pallas import tpu as pltpu
from jax.sharding import Mesh
from jax.sharding import PartitionSpec as P

HEAD_DIM = 128
SEG = 64
LEFT = 4
MAX_REL = 128
ENTRIES = MAX_REL + SEG
ROWS = LEFT * SEG
HEADS = 2
PAIR = 2 * SEG
AXES = ("sp_0", "sp_1", "sp_2", "tp")
SP = AXES[:3]

EPSILON = 1e-06
FACTOR = HEAD_DIM ** (-0.5)
LOG2E = 1.4426950408889634
MASKED = -1e30
F32, BF16 = jnp.float32, jnp.bfloat16


def dot(a, b, a_dim, b_dim):
    return lax.dot_general(a, b, (((a_dim,), (b_dim,)), ((), ())), preferred_element_type=F32)


def near(size, step=1):
    return sorted({step % size, -step % size} - {0})


def far_first(size):
    return sorted(range(1, size), key=lambda d: -min(d, size - d))


def unit(raw):
    wide = raw.astype(F32)
    inv_rms = lax.rsqrt(jnp.mean(wide * wide, axis=-1, keepdims=True) + EPSILON)
    return wide * inv_rms, inv_rms


def kernel(sizes, q_hbm, k_hbm, v_hbm, do_hbm, gains_hbm, table_hbm,
           dq_hbm, dk_hbm, dv_hbm, dtab_hbm, dgain_hbm,
           qx, kx, vx, dox, gains_v, table_v,
           qn, qu, qr, kn, ku, kr, bias_v, e_v, dp_v,
           dkx, dvx, dqx, d_v, back_out, back_in,
           dq_v, dk_v, dv_v, dtab_v, dgain_v, xbuf, ybuf, zbuf, fin,
           in_sem, halo_send, halo_recv, back_send, back_recv,
           x_send, x_recv, y_send, y_recv, z_send, z_recv, fin_send, fin_recv, out_sem,
           round1, round2, round3, row_sem):
    nz, ny, nx = sizes
    z, y, x, tp = (lax.axis_index(a) for a in AXES)
    place = (z * ny + y) * nx + x
    total = nz * ny * nx

    def at(number, core):
        return (number // (ny * nx), (number // nx) % ny, number % nx, core)

    after = at(lax.rem(place + 1, total), tp)
    before = at(lax.rem(place + total - 1, total), tp)

    def along(axis, offset, core=1):
        if axis == 0:
            return (lax.rem(z + offset, nz), y, x, core)
        if axis == 1:
            return (z, lax.rem(y + offset, ny), x, core)
        return (z, y, lax.rem(x + offset, nx), core)

    def signal(sem, target):
        pl.semaphore_signal(sem, inc=1, device_id=target, device_id_type=pl.DeviceIdType.MESH)

    def remote(src, dst, send, recv, target):
        return pltpu.make_async_remote_copy(
            src_ref=src, dst_ref=dst, send_sem=send, recv_sem=recv,
            device_id=target, device_id_type=pl.DeviceIdType.MESH)

    barrier = pltpu.get_barrier_semaphore()
    signal(barrier, before)
    signal(barrier, after)
    loads = []
    for n, (src, dst, first) in enumerate(((k_hbm, kx, ROWS), (v_hbm, vx, ROWS), (q_hbm, qx, 0), (do_hbm, dox, 0))):
        for h in range(HEADS):
            loads.append(pltpu.make_async_copy(
                src.at[:, h * HEAD_DIM:(h + 1) * HEAD_DIM], dst.at[h, first:first + ROWS], in_sem.at[2 * n + h]))
    loads.append(pltpu.make_async_copy(gains_hbm, gains_v, in_sem.at[8]))
    loads.append(pltpu.make_async_copy(table_hbm, table_v, in_sem.at[9]))
    for load in loads:
        load.start()

    close = [(a, o) for a, n in enumerate(sizes) for o in near(n)]

    @pl.when(tp == 1)
    def _():
        for a, o in close:
            signal(barrier, along(a, o))
        signal(barrier, (z, y, x, 0))
        pl.semaphore_wait(barrier, 3 + len(close))

    @pl.when(tp == 0)
    def _():
        signal(barrier, (z, y, x, 1))
        pl.semaphore_wait(barrier, 3)

    halo = {}
    for load in loads[:4]:
        load.wait()
    for h in range(HEADS):
        for half in (1, 0):
            for n, buf in enumerate((kx, vx)):
                slot = (h * 2 + half) * 2 + n
                copy = remote(
                    buf.at[h, ROWS + half * PAIR:ROWS + (half + 1) * PAIR],
                    buf.at[h, half * PAIR:(half + 1) * PAIR],
                    halo_send.at[slot], halo_recv.at[slot], after)
                copy.start()
                halo[h, half, n] = copy

    @pl.when(tp == 1)
    def _():
        for a, o in close:
            signal(round1, along(a, o))

    for load in loads[4:]:
        load.wait()

    gains = gains_v[...]
    gain_q, gain_k = gains[0:1, :], gains[1:2, :]

    def norm_keys(h, first, size):
        u, r = unit(kx[h, first:first + size])
        ku[h, first:first + size] = u
        kn[h, first:first + size] = (u * gain_k).astype(BF16)
        if first >= ROWS:
            kr[h, first - ROWS:first - ROWS + size] = jnp.broadcast_to(r, u.shape)

    for h in range(HEADS):
        u, r = unit(qx[h])
        qu[h] = u
        qr[h] = jnp.broadcast_to(r, u.shape)
        qn[h] = (u * gain_q).astype(BF16)
        norm_keys(h, ROWS, ROWS)

    key_at = lax.broadcasted_iota(jnp.int32, (PAIR, PAIR), 0)
    query_at = lax.broadcasted_iota(jnp.int32, (PAIR, PAIR), 1)
    past = query_at >= key_at
    early = query_at < SEG
    high = key_at >= SEG
    lane = lax.broadcasted_iota(jnp.int32, (1, PAIR), 1)
    table = table_v[...]
    low_part = table[:, :PAIR]
    high_part = jnp.concatenate([table[:, PAIR:], jnp.zeros((HEADS, 2 * PAIR - ENTRIES), F32)], axis=1)
    low_rolled = pltpu.roll(low_part, PAIR - SEG + 1, 1)
    high_rolled = pltpu.roll(high_part, PAIR - SEG + 1, 1)
    is_first = place == 0
    for h in range(HEADS):
        last = table[h:h + 1, ENTRIES - 1:ENTRIES]
        dist_low = low_rolled[h:h + 1]
        dist_row = jnp.where(lane <= SEG, dist_low, high_rolled[h:h + 1])
        ahead = pltpu.roll(jnp.broadcast_to(dist_low, (PAIR, PAIR)), 0, 1, stride=1, stride_axis=0)
        behind = pltpu.roll(jnp.broadcast_to(dist_row, (PAIR, PAIR)), 0, 1, stride=1, stride_axis=0)
        tile0 = jnp.where(jnp.logical_or(early, high), last, MASKED)
        tile1 = jnp.where(past, last, behind)
        tile2 = jnp.where(jnp.logical_and(early, high), MASKED, jnp.where(past, behind, ahead))
        tile0 = jnp.where(is_first, MASKED, tile0)
        for p in range(2):
            mid = jnp.where(is_first, MASKED, tile1) if p == 0 else tile1
            top = jnp.max(jnp.maximum(jnp.maximum(tile0, mid), tile2), axis=0, keepdims=True)
            for b, tile in enumerate((tile0, mid, tile2)):
                bias_v[h, p, b * PAIR:(b + 1) * PAIR] = (tile - top) * LOG2E

    sums = {(h, p): (jnp.zeros((1, PAIR), F32), jnp.zeros((1, PAIR), F32)) for h in range(HEADS) for p in range(2)}

    def block(h, p, b):
        first = (p + b) * PAIR
        own = slice(p * PAIR, (p + 1) * PAIR)
        s = dot(kn[h, first:first + PAIR], qn[h, own], 1, 1)
        e = jnp.exp2(s * (FACTOR * LOG2E) + bias_v[h, p, b * PAIR:(b + 1) * PAIR])
        dp = dot(vx[h, first:first + PAIR], dox[h, own], 1, 1)
        e_v[h, p, b * PAIR:(b + 1) * PAIR] = e
        dp_v[h, p, b * PAIR:(b + 1) * PAIR] = dp
        norm, weighted = sums[h, p]
        sums[h, p] = (norm + jnp.sum(e, axis=0, keepdims=True), weighted + jnp.sum(e * dp, axis=0, keepdims=True))

    gain_sums = [jnp.zeros((1, HEAD_DIM), F32), jnp.zeros((1, HEAD_DIM), F32)]

    def finish(h, p):
        norm, weighted = sums[h, p]
        inv = 1.0 / norm
        delta = weighted * inv
        own = slice(p * PAIR, (p + 1) * PAIR)
        keys = slice(p * PAIR, (p + 3) * PAIR)
        prob = e_v[h, p] * inv
        d_score = prob * (dp_v[h, p] - delta)
        prob_low = prob.astype(BF16)
        d_low = d_score.astype(BF16)
        dv = dot(prob_low, dox[h, own], 1, 0)
        dk = dot(d_low, qn[h, own], 1, 0)
        dq = dot(d_low, kn[h, keys], 0, 0)
        dqx[h, own] = dq
        gain_sums[0] = gain_sums[0] + jnp.sum(dq * qu[h, own], axis=0, keepdims=True)
        gain_sums[1] = gain_sums[1] + jnp.sum(dk * ku[h, keys], axis=0, keepdims=True)
        if p == 1:
            dkx[h, keys] = dk
            dvx[h, keys] = dv
            d_v[h] = d_score
        else:
            dkx[h, 0:PAIR] = dk[:PAIR]
            dvx[h, 0:PAIR] = dv[:PAIR]
            dkx[h, PAIR:3 * PAIR] = dkx[h, PAIR:3 * PAIR] + dk[PAIR:]
            dvx[h, PAIR:3 * PAIR] = dvx[h, PAIR:3 * PAIR] + dv[PAIR:]
            d_v[h] = d_v[h] + d_score

    table_rows = []
    sublane = lax.broadcasted_iota(jnp.int32, (8, PAIR), 0)

    def skewed_sum(tile):
        total = tile[:8]
        for first in range(8, PAIR, 8):
            total = total + pltpu.roll(tile[first:first + 8], PAIR - first, 1)
        for bit in (1, 2, 4):
            total = jnp.where((sublane & bit) == 0, total, pltpu.roll(total, PAIR - bit, 1))
        return jnp.sum(total, axis=0, keepdims=True)

    def fold_table(h):
        d0, d1, d2 = (d_v[h, b * PAIR:(b + 1) * PAIR] for b in range(3))
        mixed = jnp.where(past, d2, d1)
        ahead = jnp.where(past, 0.0, d2)
        rest = d0 + jnp.where(past, d1, 0.0)
        behind_row, ahead_row = skewed_sum(mixed), skewed_sum(ahead)
        rest_sum = jnp.sum(jnp.sum(rest, axis=0, keepdims=True), axis=1, keepdims=True)
        behind_row = pltpu.roll(behind_row, SEG - 1, 1)
        ahead_row = pltpu.roll(ahead_row, SEG - 1, 1)
        table_rows.append((
            jnp.where(lane < SEG - 1, ahead_row, behind_row),
            jnp.where(lane == SEG - 1, rest_sum, behind_row),
        ))

    for h in range(HEADS):
        block(h, 1, 1)
        block(h, 1, 2)
        block(h, 0, 2)

    @pl.when(tp == 1)
    def _():
        pl.semaphore_wait(round1, len(close))
        signal(row_sem, (z, y, x, 0))
        for a, n in enumerate(sizes[:2]):
            if n > 5:
                for o in near(n, 2):
                    signal(round2, along(a, o))

    for h in range(HEADS):
        for half in (1, 0):
            halo[h, half, 0].wait_recv()
            norm_keys(h, half * PAIR, PAIR)
            halo[h, half, 1].wait_recv()
            if half:
                block(h, 1, 0)
                block(h, 0, 1)
                finish(h, 1)
            else:
                block(h, 0, 0)
                finish(h, 0)
        fold_table(h)
        if h == 0:
            @pl.when(tp == 1)
            def _():
                count = sum(len(near(n, 2)) for n in sizes[:2] if n > 5)
                if count:
                    pl.semaphore_wait(round2, count)
                if nz > 9:
                    for o in near(nz, 2):
                        signal(round3, along(0, o))

    row = lax.broadcasted_iota(jnp.int32, (8, HEAD_DIM), 0)
    vec = jnp.zeros((8, HEAD_DIM), F32)
    second = jnp.where(lane < SEG, table_rows[0][1], pltpu.roll(table_rows[1][1], SEG, 1))
    for j, part in enumerate((table_rows[0][0], table_rows[1][0], second)):
        vec = jnp.where(row == 3 * tp + j, part, vec)
    for j in range(2):
        vec = jnp.where(row == 6 + j, gain_sums[j] * FACTOR, vec)
    mine = 2 * x + tp
    xbuf[mine] = vec

    def back_copies(h):
        return [
            remote(back_out.at[n, h], back_in.at[n, h], back_send.at[2 * n + h], back_recv.at[2 * n + h], before)
            for n in range(2)]

    def stage_back():
        for h in range(HEADS):
            back_out[0, h] = (dkx[h, :ROWS] * FACTOR).astype(BF16)
            back_out[1, h] = dvx[h, :ROWS].astype(BF16)

    def finish_queries():
        for h in range(HEADS):
            g = dqx[h] * FACTOR * gain_q
            u = qu[h]
            dq_v[:, h * HEAD_DIM:(h + 1) * HEAD_DIM] = (
                qr[h] * (g - u * jnp.mean(g * u, axis=-1, keepdims=True))).astype(BF16)

    dq_copy = pltpu.make_async_copy(dq_v, dq_hbm, out_sem.at[0])

    @pl.when(tp == 1)
    def _():
        if nz > 9:
            pl.semaphore_wait(round3, len(near(nz, 2)))
        sends = [
            remote(xbuf.at[mine], xbuf.at[mine], x_send.at[o], x_recv.at[mine], along(2, o)) for o in far_first(nx)]
        for copy in sends:
            copy.start()
        stage_back()
        for o in range(nx):
            for core in range(2):
                if o or not core:
                    slot = 2 * lax.rem(x + o, nx) + core
                    pltpu.make_async_copy(xbuf.at[slot], xbuf.at[slot], x_recv.at[slot]).wait()
        part = xbuf[0]
        for n in range(1, 2 * nx):
            part = part + xbuf[n]
        ybuf[y] = part
        moves = [remote(ybuf.at[y], ybuf.at[y], y_send.at[o], y_recv.at[y], along(1, o)) for o in far_first(ny)]
        for copy in moves:
            copy.start()
        sends += moves
        finish_queries()
        for o in range(1, ny):
            slot = lax.rem(y + o, ny)
            pltpu.make_async_copy(ybuf.at[slot], ybuf.at[slot], y_recv.at[slot]).wait()
        part = ybuf[0]
        for n in range(1, ny):
            part = part + ybuf[n]
        zbuf[z] = part
        moves = [remote(zbuf.at[z], zbuf.at[z], z_send.at[o], z_recv.at[z], along(0, o)) for o in far_first(nz)]
        for copy in moves:
            copy.start()
        sends += moves
        for h in range(HEADS):
            for copy in back_copies(h):
                copy.start()
        dq_copy.start()
        for copy in sends:
            copy.wait_send()

    @pl.when(tp == 0)
    def _():
        pl.semaphore_wait(row_sem, 1)
        sends = [
            remote(xbuf.at[mine], xbuf.at[mine], x_send.at[o], x_recv.at[mine], along(2, o))
            for o in [*far_first(nx), 0]]
        for copy in sends:
            copy.start()
        stage_back()
        finish_queries()
        for h in range(HEADS):
            for copy in back_copies(h):
                copy.start()
        dq_copy.start()
        for copy in sends:
            copy.wait_send()

    for copy in halo.values():
        copy.wait_send()
    out_copies = [dq_copy]
    for h in range(HEADS):
        back_k, back_v = back_copies(h)
        back_k.wait()
        back_v.wait()
        lanes = slice(h * HEAD_DIM, (h + 1) * HEAD_DIM)
        keep = jnp.where(place == total - 1, 0.0, 1.0)
        g = (dkx[h, ROWS:] * FACTOR + back_in[0, h].astype(F32) * keep) * gain_k
        u = ku[h, ROWS:]
        dk_v[:, lanes] = (kr[h] * (g - u * jnp.mean(g * u, axis=-1, keepdims=True))).astype(BF16)
        dv_v[:, lanes] = (dvx[h, ROWS:] + back_in[1, h].astype(F32) * keep).astype(BF16)
    for n, (src, dst) in enumerate(((dk_v, dk_hbm), (dv_v, dv_hbm))):
        copy = pltpu.make_async_copy(src, dst, out_sem.at[1 + n])
        copy.start()
        out_copies.append(copy)

    pass_on = remote(fin, fin, fin_send, fin_recv, (z, y, x, 0))

    @pl.when(tp == 1)
    def _():
        for o in range(1, nz):
            slot = lax.rem(z + o, nz)
            pltpu.make_async_copy(zbuf.at[slot], zbuf.at[slot], z_recv.at[slot]).wait()
        part = zbuf[0]
        for n in range(1, nz):
            part = part + zbuf[n]
        fin[...] = part
        pass_on.start()

    @pl.when(tp == 0)
    def _():
        pltpu.make_async_copy(fin, fin, fin_recv).wait()

    tail = fin[pl.ds(3 * tp + 2, 1), :]
    for j in range(HEADS):
        dtab_v[j:j + 1, :PAIR] = fin[pl.ds(3 * tp + j, 1), :]
        dtab_v[j:j + 1, PAIR:] = tail[:, j * SEG:(j + 1) * SEG]
    dgain_v[...] = fin[6:8, :]
    for n, (src, dst) in enumerate(((dtab_v, dtab_hbm), (dgain_v, dgain_hbm))):
        copy = pltpu.make_async_copy(src, dst, out_sem.at[3 + n])
        copy.start()
        out_copies.append(copy)

    @pl.when(tp == 1)
    def _():
        pass_on.wait_send()

    for copy in out_copies:
        copy.wait()


def local(sizes, queries, keys, values, gains, bias_table, d_out):
    nz, ny, nx = sizes
    width = HEADS * HEAD_DIM
    any_spec = pl.BlockSpec(memory_space=pl.ANY)
    tile = (HEADS, ROWS, HEAD_DIM)
    wide = (HEADS, 2 * ROWS, HEAD_DIM)
    pairs = (HEADS, 2, 3 * PAIR, PAIR)
    dma, regular = pltpu.SemaphoreType.DMA, pltpu.SemaphoreType.REGULAR
    vmem = pltpu.VMEM
    out = pl.pallas_call(
        functools.partial(kernel, sizes),
        out_shape=(
            jax.ShapeDtypeStruct((ROWS, width), BF16),
            jax.ShapeDtypeStruct((ROWS, width), BF16),
            jax.ShapeDtypeStruct((ROWS, width), BF16),
            jax.ShapeDtypeStruct((HEADS, ENTRIES), F32),
            jax.ShapeDtypeStruct((2, HEAD_DIM), F32),
        ),
        in_specs=[any_spec] * 6,
        out_specs=(any_spec,) * 5,
        scratch_shapes=[
            vmem(tile, BF16), vmem(wide, BF16), vmem(wide, BF16), vmem(tile, BF16),
            vmem((2, HEAD_DIM), F32), vmem((HEADS, ENTRIES), F32),
            vmem(tile, BF16), vmem(tile, F32), vmem(tile, F32),
            vmem(wide, BF16), vmem(wide, F32), vmem(tile, F32),
            vmem(pairs, F32), vmem(pairs, F32), vmem(pairs, F32),
            vmem(wide, F32), vmem(wide, F32), vmem(tile, F32), vmem((HEADS, 3 * PAIR, PAIR), F32),
            vmem((2, *tile), BF16), vmem((2, *tile), BF16),
            vmem((ROWS, width), BF16), vmem((ROWS, width), BF16), vmem((ROWS, width), BF16),
            vmem((HEADS, ENTRIES), F32), vmem((2, HEAD_DIM), F32),
            vmem((2 * nx, 8, HEAD_DIM), F32), vmem((ny, 8, HEAD_DIM), F32), vmem((nz, 8, HEAD_DIM), F32),
            vmem((8, HEAD_DIM), F32),
            dma((10,)), dma((8,)), dma((8,)), dma((4,)), dma((4,)),
            dma((nx,)), dma((2 * nx,)), dma((ny,)), dma((ny,)), dma((nz,)), dma((nz,)), dma, dma, dma((5,)),
            regular, regular, regular, regular,
        ],
        compiler_params=pltpu.CompilerParams(
            collective_id=0, has_side_effects=True, vmem_limit_bytes=56 * 1024 * 1024),
        name="segment_attention_grad",
    )(queries, keys, values, d_out, gains, bias_table.T)
    d_queries, d_keys, d_values, d_table, d_gains = out
    return d_queries, d_keys, d_values, d_table.T, d_gains


def solution(mesh):
    shape = (12, 8, 4)
    if mesh.shape["sp"] != int(np.prod(shape)):
        shape = mesh.small_shape
    split = Mesh(mesh.devices.reshape(*shape, mesh.shape["tp"]), AXES)
    placed = (P(SP, "tp"), P(SP, "tp"), P(SP, "tp"), P(), P(None, "tp"), P(SP, "tp"))
    return jax.shard_map(
        functools.partial(local, shape),
        mesh=split,
        in_specs=placed,
        out_specs=(P(SP, "tp"), P(SP, "tp"), P(SP, "tp"), P(None, "tp"), P()),
        check_vma=False,
    )
```

```python
import functools

import jax
import jax.numpy as jnp
import numpy as np
from jax import lax
from jax.experimental import pallas as pl
from jax.experimental.pallas import tpu as pltpu
from jax.sharding import Mesh
from jax.sharding import PartitionSpec as P

HEAD_DIM = 128
SEG = 64
LEFT = 4
MAX_REL = 128
ENTRIES = MAX_REL + SEG
ROWS = LEFT * SEG
HEADS = 2
PAIR = 2 * SEG
AXES = ("sp_0", "sp_1", "sp_2", "tp")
SP = AXES[:3]

EPSILON = 1e-06
FACTOR = HEAD_DIM ** (-0.5)
LOG2E = 1.4426950408889634
MASKED = -1e30
F32, BF16 = jnp.float32, jnp.bfloat16


def dot(a, b, a_dim, b_dim):
    return lax.dot_general(a, b, (((a_dim,), (b_dim,)), ((), ())), preferred_element_type=F32)


def near(size, step=1):
    return sorted({step % size, -step % size} - {0})


def far_first(size):
    return sorted(range(1, size), key=lambda d: -min(d, size - d))


def unit(raw):
    wide = raw.astype(F32)
    inv_rms = lax.rsqrt(jnp.mean(wide * wide, axis=-1, keepdims=True) + EPSILON)
    return wide * inv_rms, inv_rms


def kernel(sizes, q_hbm, k_hbm, v_hbm, do_hbm, gains_hbm, table_hbm,
           dq_v, dk_v, dv_v, dtab_v, dgain_v,
           qx, kx, vx, dox, gains_v, table_v,
           qn, qu, qr, kn, ku, kr, bias_v, e_v, dp_v,
           dkx, dvx, dqx, d_v, back_out, back_in,
           xbuf, ybuf, zbuf, fin,
           in_sem, halo_send, halo_recv, back_send, back_recv,
           x_send, x_recv, y_send, y_recv, z_send, z_recv, fin_send, fin_recv,
           round1, round2, round3, row_sem):
    nz, ny, nx = sizes
    z, y, x, tp = (lax.axis_index(a) for a in AXES)
    place = (z * ny + y) * nx + x
    total = nz * ny * nx

    def at(number, core):
        return (number // (ny * nx), (number // nx) % ny, number % nx, core)

    after = at(lax.rem(place + 1, total), tp)
    before = at(lax.rem(place + total - 1, total), tp)

    def along(axis, offset, core=1):
        if axis == 0:
            return (lax.rem(z + offset, nz), y, x, core)
        if axis == 1:
            return (z, lax.rem(y + offset, ny), x, core)
        return (z, y, lax.rem(x + offset, nx), core)

    def signal(sem, target):
        pl.semaphore_signal(sem, inc=1, device_id=target, device_id_type=pl.DeviceIdType.MESH)

    def remote(src, dst, send, recv, target):
        return pltpu.make_async_remote_copy(
            src_ref=src, dst_ref=dst, send_sem=send, recv_sem=recv,
            device_id=target, device_id_type=pl.DeviceIdType.MESH)

    barrier = pltpu.get_barrier_semaphore()
    signal(barrier, before)
    signal(barrier, after)
    loads = []
    for n, (src, dst, first) in enumerate(((k_hbm, kx, ROWS), (v_hbm, vx, ROWS), (q_hbm, qx, 0), (do_hbm, dox, 0))):
        for h in range(HEADS):
            loads.append(pltpu.make_async_copy(
                src.at[:, h * HEAD_DIM:(h + 1) * HEAD_DIM], dst.at[h, first:first + ROWS], in_sem.at[2 * n + h]))
    loads.append(pltpu.make_async_copy(gains_hbm, gains_v, in_sem.at[8]))
    loads.append(pltpu.make_async_copy(table_hbm, table_v, in_sem.at[9]))
    for load in loads:
        load.start()

    close = [(a, o) for a, n in enumerate(sizes) for o in near(n)]

    @pl.when(tp == 1)
    def _():
        for a, o in close:
            signal(barrier, along(a, o))
        signal(barrier, (z, y, x, 0))
        pl.semaphore_wait(barrier, 3 + len(close))

    @pl.when(tp == 0)
    def _():
        signal(barrier, (z, y, x, 1))
        pl.semaphore_wait(barrier, 3)

    halo = {}
    for load in loads[:4]:
        load.wait()
    for h in range(HEADS):
        for half in (1, 0):
            for n, buf in enumerate((kx, vx)):
                slot = (h * 2 + half) * 2 + n
                copy = remote(
                    buf.at[h, ROWS + half * PAIR:ROWS + (half + 1) * PAIR],
                    buf.at[h, half * PAIR:(half + 1) * PAIR],
                    halo_send.at[slot], halo_recv.at[slot], after)
                copy.start()
                halo[h, half, n] = copy

    @pl.when(tp == 1)
    def _():
        for a, o in close:
            signal(round1, along(a, o))

    for load in loads[4:]:
        load.wait()

    gains = gains_v[...]
    gain_q, gain_k = gains[0:1, :], gains[1:2, :]

    def norm_keys(h, first, size):
        u, r = unit(kx[h, first:first + size])
        ku[h, first:first + size] = u
        kn[h, first:first + size] = (u * gain_k).astype(BF16)
        if first >= ROWS:
            kr[h, first - ROWS:first - ROWS + size] = jnp.broadcast_to(r, u.shape)

    for h in range(HEADS):
        u, r = unit(qx[h])
        qu[h] = u
        qr[h] = jnp.broadcast_to(r, u.shape)
        qn[h] = (u * gain_q).astype(BF16)
        norm_keys(h, ROWS, ROWS)

    key_at = lax.broadcasted_iota(jnp.int32, (PAIR, PAIR), 0)
    query_at = lax.broadcasted_iota(jnp.int32, (PAIR, PAIR), 1)
    past = query_at >= key_at
    early = query_at < SEG
    high = key_at >= SEG
    lane = lax.broadcasted_iota(jnp.int32, (1, PAIR), 1)
    table = table_v[...]
    low_part = table[:, :PAIR]
    high_part = jnp.concatenate([table[:, PAIR:], jnp.zeros((HEADS, 2 * PAIR - ENTRIES), F32)], axis=1)
    low_rolled = pltpu.roll(low_part, PAIR - SEG + 1, 1)
    high_rolled = pltpu.roll(high_part, PAIR - SEG + 1, 1)
    is_first = place == 0
    for h in range(HEADS):
        last = table[h:h + 1, ENTRIES - 1:ENTRIES]
        dist_low = low_rolled[h:h + 1]
        dist_row = jnp.where(lane <= SEG, dist_low, high_rolled[h:h + 1])
        ahead = pltpu.roll(jnp.broadcast_to(dist_low, (PAIR, PAIR)), 0, 1, stride=1, stride_axis=0)
        behind = pltpu.roll(jnp.broadcast_to(dist_row, (PAIR, PAIR)), 0, 1, stride=1, stride_axis=0)
        tile0 = jnp.where(jnp.logical_or(early, high), last, MASKED)
        tile1 = jnp.where(past, last, behind)
        tile2 = jnp.where(jnp.logical_and(early, high), MASKED, jnp.where(past, behind, ahead))
        tile0 = jnp.where(is_first, MASKED, tile0)
        for p in range(2):
            mid = jnp.where(is_first, MASKED, tile1) if p == 0 else tile1
            top = jnp.max(jnp.maximum(jnp.maximum(tile0, mid), tile2), axis=0, keepdims=True)
            for b, tile in enumerate((tile0, mid, tile2)):
                bias_v[h, p, b * PAIR:(b + 1) * PAIR] = (tile - top) * LOG2E

    sums = {(h, p): (jnp.zeros((1, PAIR), F32), jnp.zeros((1, PAIR), F32)) for h in range(HEADS) for p in range(2)}

    def block(h, p, b):
        first = (p + b) * PAIR
        own = slice(p * PAIR, (p + 1) * PAIR)
        s = dot(kn[h, first:first + PAIR], qn[h, own], 1, 1)
        e = jnp.exp2(s * (FACTOR * LOG2E) + bias_v[h, p, b * PAIR:(b + 1) * PAIR])
        dp = dot(vx[h, first:first + PAIR], dox[h, own], 1, 1)
        e_v[h, p, b * PAIR:(b + 1) * PAIR] = e
        dp_v[h, p, b * PAIR:(b + 1) * PAIR] = dp
        norm, weighted = sums[h, p]
        sums[h, p] = (norm + jnp.sum(e, axis=0, keepdims=True), weighted + jnp.sum(e * dp, axis=0, keepdims=True))

    gain_sums = [jnp.zeros((1, HEAD_DIM), F32), jnp.zeros((1, HEAD_DIM), F32)]

    def finish(h, p):
        norm, weighted = sums[h, p]
        inv = 1.0 / norm
        delta = weighted * inv
        own = slice(p * PAIR, (p + 1) * PAIR)
        keys = slice(p * PAIR, (p + 3) * PAIR)
        prob = e_v[h, p] * inv
        d_score = prob * (dp_v[h, p] - delta)
        prob_low = prob.astype(BF16)
        d_low = d_score.astype(BF16)
        dv = dot(prob_low, dox[h, own], 1, 0)
        dk = dot(d_low, qn[h, own], 1, 0)
        dq = dot(d_low, kn[h, keys], 0, 0)
        dqx[h, own] = dq
        gain_sums[0] = gain_sums[0] + jnp.sum(dq * qu[h, own], axis=0, keepdims=True)
        gain_sums[1] = gain_sums[1] + jnp.sum(dk * ku[h, keys], axis=0, keepdims=True)
        if p == 1:
            dkx[h, keys] = dk
            dvx[h, keys] = dv
            d_v[h] = d_score
        else:
            dkx[h, 0:PAIR] = dk[:PAIR]
            dvx[h, 0:PAIR] = dv[:PAIR]
            dkx[h, PAIR:3 * PAIR] = dkx[h, PAIR:3 * PAIR] + dk[PAIR:]
            dvx[h, PAIR:3 * PAIR] = dvx[h, PAIR:3 * PAIR] + dv[PAIR:]
            d_v[h] = d_v[h] + d_score

    table_rows = []
    sublane = lax.broadcasted_iota(jnp.int32, (8, PAIR), 0)

    def skewed_sum(tile):
        total = tile[:8]
        for first in range(8, PAIR, 8):
            total = total + pltpu.roll(tile[first:first + 8], PAIR - first, 1)
        for bit in (1, 2, 4):
            total = jnp.where((sublane & bit) == 0, total, pltpu.roll(total, PAIR - bit, 1))
        return jnp.sum(total, axis=0, keepdims=True)

    def fold_table(h):
        d0, d1, d2 = (d_v[h, b * PAIR:(b + 1) * PAIR] for b in range(3))
        mixed = jnp.where(past, d2, d1)
        ahead = jnp.where(past, 0.0, d2)
        rest = d0 + jnp.where(past, d1, 0.0)
        behind_row, ahead_row = skewed_sum(mixed), skewed_sum(ahead)
        rest_sum = jnp.sum(jnp.sum(rest, axis=0, keepdims=True), axis=1, keepdims=True)
        behind_row = pltpu.roll(behind_row, SEG - 1, 1)
        ahead_row = pltpu.roll(ahead_row, SEG - 1, 1)
        table_rows.append((
            jnp.where(lane < SEG - 1, ahead_row, behind_row),
            jnp.where(lane == SEG - 1, rest_sum, behind_row),
        ))

    for h in range(HEADS):
        block(h, 1, 1)
        block(h, 1, 2)
        block(h, 0, 2)

    @pl.when(tp == 1)
    def _():
        pl.semaphore_wait(round1, len(close))
        signal(row_sem, (z, y, x, 0))
        for a, n in enumerate(sizes[:2]):
            if n > 5:
                for o in near(n, 2):
                    signal(round2, along(a, o))

    for h in range(HEADS):
        for half in (1, 0):
            halo[h, half, 0].wait_recv()
            norm_keys(h, half * PAIR, PAIR)
            halo[h, half, 1].wait_recv()
            if half:
                block(h, 1, 0)
                block(h, 0, 1)
                finish(h, 1)
            else:
                block(h, 0, 0)
                finish(h, 0)
        fold_table(h)
        if h == 0:
            @pl.when(tp == 1)
            def _():
                count = sum(len(near(n, 2)) for n in sizes[:2] if n > 5)
                if count:
                    pl.semaphore_wait(round2, count)
                if nz > 9:
                    for o in near(nz, 2):
                        signal(round3, along(0, o))

    row = lax.broadcasted_iota(jnp.int32, (8, HEAD_DIM), 0)
    vec = jnp.zeros((8, HEAD_DIM), F32)
    second = jnp.where(lane < SEG, table_rows[0][1], pltpu.roll(table_rows[1][1], SEG, 1))
    for j, part in enumerate((table_rows[0][0], table_rows[1][0], second)):
        vec = jnp.where(row == 3 * tp + j, part, vec)
    for j in range(2):
        vec = jnp.where(row == 6 + j, gain_sums[j] * FACTOR, vec)
    mine = 2 * x + tp
    xbuf[mine] = vec

    def back_copies(h):
        return [
            remote(back_out.at[n, h], back_in.at[n, h], back_send.at[2 * n + h], back_recv.at[2 * n + h], before)
            for n in range(2)]

    def stage_back():
        for h in range(HEADS):
            back_out[0, h] = (dkx[h, :ROWS] * FACTOR).astype(BF16)
            back_out[1, h] = dvx[h, :ROWS].astype(BF16)

    def finish_queries():
        for h in range(HEADS):
            g = dqx[h] * FACTOR * gain_q
            u = qu[h]
            dq_v[:, h * HEAD_DIM:(h + 1) * HEAD_DIM] = (
                qr[h] * (g - u * jnp.mean(g * u, axis=-1, keepdims=True))).astype(BF16)

    @pl.when(tp == 1)
    def _():
        if nz > 9:
            pl.semaphore_wait(round3, len(near(nz, 2)))
        sends = [
            remote(xbuf.at[mine], xbuf.at[mine], x_send.at[o], x_recv.at[mine], along(2, o)) for o in far_first(nx)]
        for copy in sends:
            copy.start()
        stage_back()
        for o in range(nx):
            for core in range(2):
                if o or not core:
                    slot = 2 * lax.rem(x + o, nx) + core
                    pltpu.make_async_copy(xbuf.at[slot], xbuf.at[slot], x_recv.at[slot]).wait()
        part = xbuf[0]
        for n in range(1, 2 * nx):
            part = part + xbuf[n]
        ybuf[y] = part
        moves = [remote(ybuf.at[y], ybuf.at[y], y_send.at[o], y_recv.at[y], along(1, o)) for o in far_first(ny)]
        for copy in moves:
            copy.start()
        sends += moves
        finish_queries()
        for o in range(1, ny):
            slot = lax.rem(y + o, ny)
            pltpu.make_async_copy(ybuf.at[slot], ybuf.at[slot], y_recv.at[slot]).wait()
        part = ybuf[0]
        for n in range(1, ny):
            part = part + ybuf[n]
        zbuf[z] = part
        moves = [remote(zbuf.at[z], zbuf.at[z], z_send.at[o], z_recv.at[z], along(0, o)) for o in far_first(nz)]
        for copy in moves:
            copy.start()
        sends += moves
        for h in range(HEADS):
            for copy in back_copies(h):
                copy.start()
        for copy in sends:
            copy.wait_send()

    @pl.when(tp == 0)
    def _():
        pl.semaphore_wait(row_sem, 1)
        sends = [
            remote(xbuf.at[mine], xbuf.at[mine], x_send.at[o], x_recv.at[mine], along(2, o))
            for o in [*far_first(nx), 0]]
        for copy in sends:
            copy.start()
        stage_back()
        finish_queries()
        for h in range(HEADS):
            for copy in back_copies(h):
                copy.start()
        for copy in sends:
            copy.wait_send()

    for copy in halo.values():
        copy.wait_send()
    for h in range(HEADS):
        back_k, back_v = back_copies(h)
        back_k.wait()
        back_v.wait()
        lanes = slice(h * HEAD_DIM, (h + 1) * HEAD_DIM)
        keep = jnp.where(place == total - 1, 0.0, 1.0)
        g = (dkx[h, ROWS:] * FACTOR + back_in[0, h].astype(F32) * keep) * gain_k
        u = ku[h, ROWS:]
        dk_v[:, lanes] = (kr[h] * (g - u * jnp.mean(g * u, axis=-1, keepdims=True))).astype(BF16)
        dv_v[:, lanes] = (dvx[h, ROWS:] + back_in[1, h].astype(F32) * keep).astype(BF16)
    pass_on = remote(fin, fin, fin_send, fin_recv, (z, y, x, 0))

    @pl.when(tp == 1)
    def _():
        for o in range(1, nz):
            slot = lax.rem(z + o, nz)
            pltpu.make_async_copy(zbuf.at[slot], zbuf.at[slot], z_recv.at[slot]).wait()
        part = zbuf[0]
        for n in range(1, nz):
            part = part + zbuf[n]
        fin[...] = part
        pass_on.start()

    @pl.when(tp == 0)
    def _():
        pltpu.make_async_copy(fin, fin, fin_recv).wait()

    tail = fin[pl.ds(3 * tp + 2, 1), :]
    for j in range(HEADS):
        dtab_v[j:j + 1, :PAIR] = fin[pl.ds(3 * tp + j, 1), :]
        dtab_v[j:j + 1, PAIR:] = tail[:, j * SEG:(j + 1) * SEG]
    dgain_v[...] = fin[6:8, :]
    @pl.when(tp == 1)
    def _():
        pass_on.wait_send()


def write_out(*refs):
    count = len(refs) // 2
    copies = [pltpu.make_async_copy(refs[n], refs[count + n], refs[-1].at[n]) for n in range(count)]
    for copy in copies:
        copy.start()
    for copy in copies:
        copy.wait()


def local(sizes, queries, keys, values, gains, bias_table, d_out):
    nz, ny, nx = sizes
    width = HEADS * HEAD_DIM
    hbm_spec = pl.BlockSpec(memory_space=pltpu.HBM)
    vmem_spec = pl.BlockSpec(memory_space=pltpu.VMEM)
    tile = (HEADS, ROWS, HEAD_DIM)
    wide = (HEADS, 2 * ROWS, HEAD_DIM)
    pairs = (HEADS, 2, 3 * PAIR, PAIR)
    dma, regular = pltpu.SemaphoreType.DMA, pltpu.SemaphoreType.REGULAR
    vmem = pltpu.VMEM
    outs = [((ROWS, width), BF16)] * 3 + [((HEADS, ENTRIES), F32), ((2, HEAD_DIM), F32)]
    out = pl.pallas_call(
        functools.partial(kernel, sizes),
        out_shape=tuple(vmem(*o) for o in outs),
        in_specs=[hbm_spec] * 6,
        out_specs=(vmem_spec,) * 5,
        scratch_shapes=[
            vmem(tile, BF16), vmem(wide, BF16), vmem(wide, BF16), vmem(tile, BF16),
            vmem((2, HEAD_DIM), F32), vmem((HEADS, ENTRIES), F32),
            vmem(tile, BF16), vmem(tile, F32), vmem(tile, F32),
            vmem(wide, BF16), vmem(wide, F32), vmem(tile, F32),
            vmem(pairs, F32), vmem(pairs, F32), vmem(pairs, F32),
            vmem(wide, F32), vmem(wide, F32), vmem(tile, F32), vmem((HEADS, 3 * PAIR, PAIR), F32),
            vmem((2, *tile), BF16), vmem((2, *tile), BF16),
            vmem((2 * nx, 8, HEAD_DIM), F32), vmem((ny, 8, HEAD_DIM), F32), vmem((nz, 8, HEAD_DIM), F32),
            vmem((8, HEAD_DIM), F32),
            dma((10,)), dma((8,)), dma((8,)), dma((4,)), dma((4,)),
            dma((nx,)), dma((2 * nx,)), dma((ny,)), dma((ny,)), dma((nz,)), dma((nz,)), dma, dma,
            regular, regular, regular, regular,
        ],
        compiler_params=pltpu.CompilerParams(
            collective_id=0, has_side_effects=True, vmem_limit_bytes=32 * 1024 * 1024),
        name="segment_attention_grad",
    )(*(pltpu.with_memory_space_constraint(a, pltpu.HBM) for a in (queries, keys, values, d_out, gains, bias_table.T)))
    d_queries, d_keys, d_values, d_table, d_gains = pl.pallas_call(
        write_out,
        out_shape=tuple(jax.ShapeDtypeStruct(*o) for o in outs),
        in_specs=[vmem_spec] * 5,
        out_specs=(hbm_spec,) * 5,
        scratch_shapes=[dma((5,))],
        name="write_out",
    )(*(pltpu.with_memory_space_constraint(o, pltpu.VMEM) for o in out))
    return d_queries, d_keys, d_values, d_table.T, d_gains


def solution(mesh):
    shape = (12, 8, 4)
    if mesh.shape["sp"] != int(np.prod(shape)):
        shape = mesh.small_shape
    split = Mesh(mesh.devices.reshape(*shape, mesh.shape["tp"]), AXES)
    placed = (P(SP, "tp"), P(SP, "tp"), P(SP, "tp"), P(), P(None, "tp"), P(SP, "tp"))
    return jax.shard_map(
        functools.partial(local, shape),
        mesh=split,
        in_specs=placed,
        out_specs=(P(SP, "tp"), P(SP, "tp"), P(SP, "tp"), P(None, "tp"), P()),
        check_vma=False,
    )
```

```python
import functools

import jax
import jax.numpy as jnp
import numpy as np
from jax import lax
from jax.experimental import pallas as pl
from jax.experimental.pallas import tpu as pltpu
from jax.sharding import Mesh
from jax.sharding import PartitionSpec as P

HEAD_DIM = 128
SEG = 64
LEFT = 4
MAX_REL = 128
ENTRIES = MAX_REL + SEG
ROWS = LEFT * SEG
HEADS = 2
PAIR = 2 * SEG
AXES = ("sp_0", "sp_1", "sp_2", "tp")
SP = AXES[:3]

EPSILON = 1e-06
FACTOR = HEAD_DIM ** (-0.5)
LOG2E = 1.4426950408889634
MASKED = -1e30
F32, BF16 = jnp.float32, jnp.bfloat16


def dot(a, b, a_dim, b_dim):
    return lax.dot_general(a, b, (((a_dim,), (b_dim,)), ((), ())), preferred_element_type=F32)


def near(size, step=1):
    return sorted({step % size, -step % size} - {0})


def far_first(size):
    return sorted(range(1, size), key=lambda d: -min(d, size - d))


def unit(raw):
    wide = raw.astype(F32)
    inv_rms = lax.rsqrt(jnp.mean(wide * wide, axis=-1, keepdims=True) + EPSILON)
    return wide * inv_rms, inv_rms


def kernel(sizes, q_hbm, k_hbm, v_hbm, do_hbm, gains_hbm, table_hbm,
           dq_v, dk_v, dv_v, dtab_v, dgain_v,
           qdx, kvx, gains_v, table_v,
           qn, qu, qr, kn, ku, kr, bias_v, e_v, dp_v,
           dkx, dvx, dqx, d_v, back_out, back_in,
           lines, zout, zbuf,
           load_sem, gains_sem, table_sem, halo_send, halo_recv, back_send, back_recv,
           xy_send, x_recv, y_recv, z_send, z_recv, round1, round2, round3, row_sem):
    nz, ny, nx = sizes
    z, y, x, tp = (lax.axis_index(a) for a in AXES)
    place = (z * ny + y) * nx + x
    total = nz * ny * nx

    def at(number, core):
        return (number // (ny * nx), (number // nx) % ny, number % nx, core)

    after = at(lax.rem(place + 1, total), tp)
    before = at(lax.rem(place + total - 1, total), tp)

    def along(axis, offset, core=1):
        if axis == 0:
            return (lax.rem(z + offset, nz), y, x, core)
        if axis == 1:
            return (z, lax.rem(y + offset, ny), x, core)
        return (z, y, lax.rem(x + offset, nx), core)

    def signal(sem, target):
        pl.semaphore_signal(sem, inc=1, device_id=target, device_id_type=pl.DeviceIdType.MESH)

    def remote(src, dst, send, recv, target):
        return pltpu.make_async_remote_copy(
            src_ref=src, dst_ref=dst, send_sem=send, recv_sem=recv,
            device_id=target, device_id_type=pl.DeviceIdType.MESH)

    barrier = pltpu.get_barrier_semaphore()
    signal(barrier, before)
    signal(barrier, after)
    for n, (src, dst, first) in enumerate(((k_hbm, kvx.at[0], ROWS), (v_hbm, kvx.at[1], ROWS), (q_hbm, qdx.at[0], 0), (do_hbm, qdx.at[1], 0))):
        for h in range(HEADS):
            pltpu.make_async_copy(
                src.at[:, h * HEAD_DIM:(h + 1) * HEAD_DIM], dst.at[h, first:first + ROWS], load_sem.at[n // 2]).start()
    small_loads = [pltpu.make_async_copy(gains_hbm, gains_v, gains_sem), pltpu.make_async_copy(table_hbm, table_v, table_sem)]
    for load in small_loads:
        load.start()

    def wait_bytes(ref, sem):
        pltpu.make_async_copy(ref, ref, sem).wait()

    close = [(a, o) for a, n in enumerate(sizes) for o in near(n)]

    @pl.when(tp == 1)
    def _():
        for a, o in close:
            signal(barrier, along(a, o))
        signal(barrier, (z, y, x, 0))
        pl.semaphore_wait(barrier, 3 + len(close))

    @pl.when(tp == 0)
    def _():
        signal(barrier, (z, y, x, 1))
        pl.semaphore_wait(barrier, 3)

    wait_bytes(kvx.at[:, :, ROWS:], load_sem.at[0])
    halo = {}
    for h in range(HEADS):
        for half in (1, 0):
            slot = h * 2 + half
            halo[h, half] = remote(
                kvx.at[:, h, ROWS + half * PAIR:ROWS + (half + 1) * PAIR],
                kvx.at[:, h, half * PAIR:(half + 1) * PAIR],
                halo_send, halo_recv.at[slot], after)
            halo[h, half].start()

    @pl.when(tp == 1)
    def _():
        for a, o in close:
            signal(round1, along(a, o))

    wait_bytes(qdx, load_sem.at[1])
    for load in small_loads:
        load.wait()

    gains = gains_v[...]
    gain_q, gain_k = gains[0:1, :], gains[1:2, :]

    def norm_keys(h, first, size):
        u, r = unit(kvx[0, h, first:first + size])
        ku[h, first:first + size] = u
        kn[h, first:first + size] = (u * gain_k).astype(BF16)
        if first >= ROWS:
            kr[h, first - ROWS:first - ROWS + size] = jnp.broadcast_to(r, u.shape)

    for h in range(HEADS):
        u, r = unit(qdx[0, h])
        qu[h] = u
        qr[h] = jnp.broadcast_to(r, u.shape)
        qn[h] = (u * gain_q).astype(BF16)
        norm_keys(h, ROWS, ROWS)

    key_at = lax.broadcasted_iota(jnp.int32, (PAIR, PAIR), 0)
    query_at = lax.broadcasted_iota(jnp.int32, (PAIR, PAIR), 1)
    past = query_at >= key_at
    early = query_at < SEG
    high = key_at >= SEG
    lane = lax.broadcasted_iota(jnp.int32, (1, PAIR), 1)
    table = table_v[...]
    low_part = table[:, :PAIR]
    high_part = jnp.concatenate([table[:, PAIR:], jnp.zeros((HEADS, 2 * PAIR - ENTRIES), F32)], axis=1)
    low_rolled = pltpu.roll(low_part, PAIR - SEG + 1, 1)
    high_rolled = pltpu.roll(high_part, PAIR - SEG + 1, 1)
    is_first = place == 0
    for h in range(HEADS):
        last = table[h:h + 1, ENTRIES - 1:ENTRIES]
        dist_low = low_rolled[h:h + 1]
        dist_row = jnp.where(lane <= SEG, dist_low, high_rolled[h:h + 1])
        ahead = pltpu.roll(jnp.broadcast_to(dist_low, (PAIR, PAIR)), 0, 1, stride=1, stride_axis=0)
        behind = pltpu.roll(jnp.broadcast_to(dist_row, (PAIR, PAIR)), 0, 1, stride=1, stride_axis=0)
        tile0 = jnp.where(jnp.logical_or(early, high), last, MASKED)
        tile1 = jnp.where(past, last, behind)
        tile2 = jnp.where(jnp.logical_and(early, high), MASKED, jnp.where(past, behind, ahead))
        tile0 = jnp.where(is_first, MASKED, tile0)
        for p in range(2):
            mid = jnp.where(is_first, MASKED, tile1) if p == 0 else tile1
            top = jnp.max(jnp.maximum(jnp.maximum(tile0, mid), tile2), axis=0, keepdims=True)
            for b, tile in enumerate((tile0, mid, tile2)):
                bias_v[h, p, b * PAIR:(b + 1) * PAIR] = (tile - top) * LOG2E

    sums = {(h, p): (jnp.zeros((1, PAIR), F32), jnp.zeros((1, PAIR), F32)) for h in range(HEADS) for p in range(2)}

    def block(h, p, b):
        first = (p + b) * PAIR
        own = slice(p * PAIR, (p + 1) * PAIR)
        s = dot(kn[h, first:first + PAIR], qn[h, own], 1, 1)
        e = jnp.exp2(s * (FACTOR * LOG2E) + bias_v[h, p, b * PAIR:(b + 1) * PAIR])
        dp = dot(kvx[1, h, first:first + PAIR], qdx[1, h, own], 1, 1)
        e_v[h, p, b * PAIR:(b + 1) * PAIR] = e
        dp_v[h, p, b * PAIR:(b + 1) * PAIR] = dp
        norm, weighted = sums[h, p]
        sums[h, p] = (norm + jnp.sum(e, axis=0, keepdims=True), weighted + jnp.sum(e * dp, axis=0, keepdims=True))

    gain_sums = [jnp.zeros((1, HEAD_DIM), F32), jnp.zeros((1, HEAD_DIM), F32)]

    def finish(h, p):
        norm, weighted = sums[h, p]
        inv = 1.0 / norm
        delta = weighted * inv
        own = slice(p * PAIR, (p + 1) * PAIR)
        keys = slice(p * PAIR, (p + 3) * PAIR)
        prob = e_v[h, p] * inv
        d_score = prob * (dp_v[h, p] - delta)
        prob_low = prob.astype(BF16)
        d_low = d_score.astype(BF16)
        dv = dot(prob_low, qdx[1, h, own], 1, 0)
        dk = dot(d_low, qn[h, own], 1, 0)
        dq = dot(d_low, kn[h, keys], 0, 0)
        dqx[h, own] = dq
        gain_sums[0] = gain_sums[0] + jnp.sum(dq * qu[h, own], axis=0, keepdims=True)
        gain_sums[1] = gain_sums[1] + jnp.sum(dk * ku[h, keys], axis=0, keepdims=True)
        if p == 1:
            dkx[h, keys] = dk
            dvx[h, keys] = dv
            d_v[h] = d_score
        else:
            dkx[h, 0:PAIR] = dk[:PAIR]
            dvx[h, 0:PAIR] = dv[:PAIR]
            dkx[h, PAIR:3 * PAIR] = dkx[h, PAIR:3 * PAIR] + dk[PAIR:]
            dvx[h, PAIR:3 * PAIR] = dvx[h, PAIR:3 * PAIR] + dv[PAIR:]
            d_v[h] = d_v[h] + d_score

    table_rows = []
    sublane = lax.broadcasted_iota(jnp.int32, (8, PAIR), 0)

    def skewed_sum(tile):
        total = tile[:8]
        for first in range(8, PAIR, 8):
            total = total + pltpu.roll(tile[first:first + 8], PAIR - first, 1)
        for bit in (1, 2, 4):
            total = jnp.where((sublane & bit) == 0, total, pltpu.roll(total, PAIR - bit, 1))
        return jnp.sum(total, axis=0, keepdims=True)

    def fold_table(h):
        d0, d1, d2 = (d_v[h, b * PAIR:(b + 1) * PAIR] for b in range(3))
        mixed = jnp.where(past, d2, d1)
        ahead = jnp.where(past, 0.0, d2)
        rest = d0 + jnp.where(past, d1, 0.0)
        behind_row, ahead_row = skewed_sum(mixed), skewed_sum(ahead)
        rest_sum = jnp.sum(jnp.sum(rest, axis=0, keepdims=True), axis=1, keepdims=True)
        behind_row = pltpu.roll(behind_row, SEG - 1, 1)
        ahead_row = pltpu.roll(ahead_row, SEG - 1, 1)
        table_rows.append((
            jnp.where(lane < SEG - 1, ahead_row, behind_row),
            jnp.where(lane == SEG - 1, rest_sum, behind_row),
        ))

    for h in range(HEADS):
        block(h, 1, 1)
        block(h, 1, 2)
        block(h, 0, 2)

    @pl.when(tp == 1)
    def _():
        pl.semaphore_wait(round1, len(close))
        signal(row_sem, (z, y, x, 0))
        for a, n in enumerate(sizes[:2]):
            if n > 5:
                for o in near(n, 2):
                    signal(round2, along(a, o))

    for h in range(HEADS):
        for half in (1, 0):
            halo[h, half].wait_recv()
            norm_keys(h, half * PAIR, PAIR)
            if half:
                block(h, 1, 0)
                block(h, 0, 1)
                finish(h, 1)
            else:
                block(h, 0, 0)
                finish(h, 0)
        fold_table(h)
        if h == 0:
            @pl.when(tp == 1)
            def _():
                count = sum(len(near(n, 2)) for n in sizes[:2] if n > 5)
                if count:
                    pl.semaphore_wait(round2, count)
                if nz > 9:
                    for o in near(nz, 3):
                        signal(round3, along(0, o))

    row = lax.broadcasted_iota(jnp.int32, (8, HEAD_DIM), 0)
    vec = jnp.zeros((8, HEAD_DIM), F32)
    second = jnp.where(lane < SEG, table_rows[0][1], pltpu.roll(table_rows[1][1], SEG, 1))
    for j, part in enumerate((table_rows[0][0], table_rows[1][0], second)):
        vec = jnp.where(row == 3 * tp + j, part, vec)
    for j in range(2):
        vec = jnp.where(row == 6 + j, gain_sums[j] * FACTOR, vec)
    mine = 2 * x + tp
    lines[mine] = vec

    backs = [
        remote(back_out.at[:, h], back_in.at[:, h], back_send, back_recv.at[h], before) for h in range(HEADS)]

    def stage_back():
        for h in range(HEADS):
            back_out[0, h] = (dkx[h, :ROWS] * FACTOR).astype(BF16)
            back_out[1, h] = dvx[h, :ROWS].astype(BF16)

    def finish_queries():
        for h in range(HEADS):
            g = dqx[h] * FACTOR * gain_q
            u = qu[h]
            dq_v[:, h * HEAD_DIM:(h + 1) * HEAD_DIM] = (
                qr[h] * (g - u * jnp.mean(g * u, axis=-1, keepdims=True))).astype(BF16)

    def line_sum(first, count):
        part = lines[first]
        for n in range(first + 1, first + count):
            part = part + lines[n]
        return part

    ys, zs = 2 * nx, 2 * nx + ny

    @pl.when(tp == 1)
    def _():
        if nz > 9:
            pl.semaphore_wait(round3, len(near(nz, 3)))
        for o in far_first(nx):
            remote(lines.at[mine], lines.at[mine], xy_send, x_recv, along(2, o)).start()
        stage_back()
        wait_bytes(lines.at[:2 * nx - 1], x_recv)
        lines[ys + y] = line_sum(0, 2 * nx)
        for o in far_first(ny):
            remote(lines.at[ys + y], lines.at[ys + y], xy_send, y_recv, along(1, o)).start()
        finish_queries()
        if ny > 1:
            wait_bytes(lines.at[:ny - 1], y_recv)
        part = line_sum(ys, ny)
        for core in range(2):
            zout[core, :3] = part[3 * core:3 * core + 3]
            zout[core, 3:] = part[6:]
        zbuf[z] = zout[1]
        for o in [*far_first(nz), 0]:
            for core in range(2 if o else 1):
                remote(zout.at[core], zbuf.at[z], z_send, z_recv, along(0, o, core)).start()
        for copy in backs:
            copy.start()

    @pl.when(tp == 0)
    def _():
        pl.semaphore_wait(row_sem, 1)
        for o in [*far_first(nx), 0]:
            remote(lines.at[mine], lines.at[mine], xy_send, x_recv, along(2, o)).start()
        stage_back()
        finish_queries()
        for copy in backs:
            copy.start()

    wait_bytes(kvx.at[:, :, ROWS:], halo_send)
    for h in range(HEADS):
        backs[h].wait_recv()
        lanes = slice(h * HEAD_DIM, (h + 1) * HEAD_DIM)
        keep = jnp.where(place == total - 1, 0.0, 1.0)
        g = (dkx[h, ROWS:] * FACTOR + back_in[0, h].astype(F32) * keep) * gain_k
        u = ku[h, ROWS:]
        dk_v[:, lanes] = (kr[h] * (g - u * jnp.mean(g * u, axis=-1, keepdims=True))).astype(BF16)
        dv_v[:, lanes] = (dvx[h, ROWS:] + back_in[1, h].astype(F32) * keep).astype(BF16)
    wait_bytes(back_out, back_send)

    @pl.when(tp == 1)
    def _():
        if nx + ny > 2:
            wait_bytes(lines.at[:nx + ny - 2], xy_send)
        wait_bytes(zbuf.at[:2 * nz - 1], z_send)
        if nz > 1:
            wait_bytes(zbuf.at[:nz - 1], z_recv)

    @pl.when(tp == 0)
    def _():
        wait_bytes(lines.at[:nx], xy_send)
        wait_bytes(zbuf.at[:nz], z_recv)

    result = zbuf[0]
    for n in range(1, nz):
        result = result + zbuf[n]
    for j in range(HEADS):
        dtab_v[j:j + 1, :PAIR] = result[j:j + 1]
        dtab_v[j:j + 1, PAIR:] = result[2:3, j * SEG:(j + 1) * SEG]
    dgain_v[...] = result[3:]


def write_out(*refs):
    count = len(refs) // 2
    copies = [pltpu.make_async_copy(refs[n], refs[count + n], refs[-1].at[n]) for n in range(count)]
    for copy in copies:
        copy.start()
    for copy in copies:
        copy.wait()


def local(sizes, queries, keys, values, gains, bias_table, d_out):
    nz, ny, nx = sizes
    width = HEADS * HEAD_DIM
    hbm_spec = pl.BlockSpec(memory_space=pltpu.HBM)
    vmem_spec = pl.BlockSpec(memory_space=pltpu.VMEM)
    tile = (HEADS, ROWS, HEAD_DIM)
    wide = (HEADS, 2 * ROWS, HEAD_DIM)
    pairs = (HEADS, 2, 3 * PAIR, PAIR)
    dma, regular = pltpu.SemaphoreType.DMA, pltpu.SemaphoreType.REGULAR
    vmem = pltpu.VMEM
    outs = [((ROWS, width), BF16)] * 3 + [((HEADS, ENTRIES), F32), ((2, HEAD_DIM), F32)]
    out = pl.pallas_call(
        functools.partial(kernel, sizes),
        out_shape=tuple(vmem(*o) for o in outs),
        in_specs=[hbm_spec] * 6,
        out_specs=(vmem_spec,) * 5,
        scratch_shapes=[
            vmem((2, *tile), BF16), vmem((2, *wide), BF16),
            vmem((2, HEAD_DIM), F32), vmem((HEADS, ENTRIES), F32),
            vmem(tile, BF16), vmem(tile, F32), vmem(tile, F32),
            vmem(wide, BF16), vmem(wide, F32), vmem(tile, F32),
            vmem(pairs, F32), vmem(pairs, F32), vmem(pairs, F32),
            vmem(wide, F32), vmem(wide, F32), vmem(tile, F32), vmem((HEADS, 3 * PAIR, PAIR), F32),
            vmem((2, *tile), BF16), vmem((2, *tile), BF16),
            vmem((2 * nx + ny, 8, HEAD_DIM), F32), vmem((2, 5, HEAD_DIM), F32), vmem((2 * nz, 5, HEAD_DIM), F32),
            dma((2,)), dma, dma, dma, dma((4,)), dma, dma((HEADS,)),
            dma, dma, dma, dma, dma, regular, regular, regular, regular,
        ],
        compiler_params=pltpu.CompilerParams(
            collective_id=0, has_side_effects=True, vmem_limit_bytes=32 * 1024 * 1024),
        name="segment_attention_grad",
    )(*(pltpu.with_memory_space_constraint(a, pltpu.HBM) for a in (queries, keys, values, d_out, gains, bias_table.T)))
    d_queries, d_keys, d_values, d_table, d_gains = pl.pallas_call(
        write_out,
        out_shape=tuple(jax.ShapeDtypeStruct(*o) for o in outs),
        in_specs=[vmem_spec] * 5,
        out_specs=(hbm_spec,) * 5,
        scratch_shapes=[dma((5,))],
        name="write_out",
    )(*(pltpu.with_memory_space_constraint(o, pltpu.VMEM) for o in out))
    return d_queries, d_keys, d_values, d_table.T, d_gains


def solution(mesh):
    shape = (12, 8, 4)
    if mesh.shape["sp"] != int(np.prod(shape)):
        shape = mesh.small_shape
    split = Mesh(mesh.devices.reshape(*shape, mesh.shape["tp"]), AXES)
    placed = (P(SP, "tp"), P(SP, "tp"), P(SP, "tp"), P(), P(None, "tp"), P(SP, "tp"))
    return jax.shard_map(
        functools.partial(local, shape),
        mesh=split,
        in_specs=placed,
        out_specs=(P(SP, "tp"), P(SP, "tp"), P(SP, "tp"), P(None, "tp"), P()),
        check_vma=False,
    )
```

```python
import functools

import jax
import jax.numpy as jnp
import numpy as np
from jax import lax
from jax.experimental import pallas as pl
from jax.experimental.pallas import tpu as pltpu
from jax.sharding import Mesh
from jax.sharding import PartitionSpec as P

HEAD_DIM = 128
SEG = 64
LEFT = 4
MAX_REL = 128
ENTRIES = MAX_REL + SEG
ROWS = LEFT * SEG
HEADS = 2
PAIR = 2 * SEG
BEFORE = 3 * SEG
AXES = ("sp_0", "sp_1", "sp_2", "tp")
SP = AXES[:3]

EPSILON = 1e-06
FACTOR = HEAD_DIM ** (-0.5)
LOG2E = 1.4426950408889634
MASKED = -1e30
F32, BF16 = jnp.float32, jnp.bfloat16


def dot(a, b, a_dim, b_dim):
    return lax.dot_general(a, b, (((a_dim,), (b_dim,)), ((), ())), preferred_element_type=F32)


def near(size, step=1):
    return sorted({step % size, -step % size} - {0})


def far_first(size):
    return sorted(range(1, size), key=lambda d: -min(d, size - d))


def unit(raw):
    wide = raw.astype(F32)
    inv_rms = lax.rsqrt(jnp.mean(wide * wide, axis=-1, keepdims=True) + EPSILON)
    return wide * inv_rms, inv_rms


def kernel(sizes, q_hbm, k_hbm, v_hbm, do_hbm, gains_hbm, table_hbm,
           dq_v, dk_v, dv_v, dtab_v, dgain_v,
           qdx, qd0, kvx, gains_v, table_v,
           qn, qu, qr, kn, ku, kr, bias_v, e_v, dp_v,
           dkx, dvx, dqx, d_v, extra_gains,
           to_before, from_after, to_after, from_before, dq_to_after, dq_from_before,
           lines, zout, zbuf,
           load_sem, gains_sem, table_sem, halo_send, left_recv, right_recv, back_send, after_recv, before_recv,
           xy_send, x_recv, y_recv, z_send, z_recv, round1, round2, round3, row_sem):
    nz, ny, nx = sizes
    z, y, x, tp = (lax.axis_index(a) for a in AXES)
    place = (z * ny + y) * nx + x
    total = nz * ny * nx
    is_first, is_last = place == 0, place == total - 1

    def at(number, core):
        return (number // (ny * nx), (number // nx) % ny, number % nx, core)

    after = at(jnp.minimum(place + 1, total - 1), tp)
    before = at(jnp.maximum(place - 1, 0), tp)

    def along(axis, offset, core=1):
        if axis == 0:
            return (lax.rem(z + offset, nz), y, x, core)
        if axis == 1:
            return (z, lax.rem(y + offset, ny), x, core)
        return (z, y, lax.rem(x + offset, nx), core)

    def signal(sem, target):
        pl.semaphore_signal(sem, inc=1, device_id=target, device_id_type=pl.DeviceIdType.MESH)

    def remote(src, dst, send, recv, target):
        return pltpu.make_async_remote_copy(
            src_ref=src, dst_ref=dst, send_sem=send, recv_sem=recv,
            device_id=target, device_id_type=pl.DeviceIdType.MESH)

    def wait_bytes(ref, sem):
        pltpu.make_async_copy(ref, ref, sem).wait()

    barrier = pltpu.get_barrier_semaphore()

    @pl.when(place > 0)
    def _():
        signal(barrier, before)

    @pl.when(place < total - 1)
    def _():
        signal(barrier, after)

    sides = jnp.where(is_first, 0, 1) + jnp.where(is_last, 0, 1)
    for n, (src, dst) in enumerate(((k_hbm, kvx.at[0]), (v_hbm, kvx.at[1]), (q_hbm, qdx.at[0]), (do_hbm, qdx.at[1]))):
        for h in range(HEADS):
            lanes = slice(h * HEAD_DIM, (h + 1) * HEAD_DIM)
            if n < 2:
                pltpu.make_async_copy(src.at[:, lanes], dst.at[h, BEFORE:BEFORE + ROWS], load_sem.at[0]).start()
            else:
                pltpu.make_async_copy(src.at[:SEG, lanes], qd0.at[n - 2, h], load_sem.at[0]).start()
                pltpu.make_async_copy(src.at[SEG:, lanes], dst.at[h, :BEFORE], load_sem.at[1]).start()
    small_loads = [pltpu.make_async_copy(gains_hbm, gains_v, gains_sem), pltpu.make_async_copy(table_hbm, table_v, table_sem)]
    for load in small_loads:
        load.start()

    close = [(a, o) for a, n in enumerate(sizes) for o in near(n)]

    @pl.when(tp == 1)
    def _():
        for a, o in close:
            signal(barrier, along(a, o))
        signal(barrier, (z, y, x, 0))
        pl.semaphore_wait(barrier, 1 + len(close) + sides)

    @pl.when(tp == 0)
    def _():
        signal(barrier, (z, y, x, 1))
        pl.semaphore_wait(barrier, 1 + sides)

    wait_bytes(kvx.at[:, :, :ROWS + SEG], load_sem.at[0])
    forth, back = {}, {}
    for h in range(HEADS):
        forth[h, 1] = remote(
            kvx.at[:, h, ROWS + PAIR:ROWS + BEFORE], kvx.at[:, h, PAIR:BEFORE],
            halo_send.at[0], left_recv.at[2 * h + 1], after)
        forth[h, 0] = remote(
            kvx.at[:, h, ROWS:ROWS + PAIR], kvx.at[:, h, :PAIR],
            halo_send.at[0], left_recv.at[2 * h], after)
        back[h] = [
            remote(kvx.at[:, h, BEFORE:ROWS], kvx.at[:, h, BEFORE + ROWS:], halo_send.at[1], right_recv.at[h], before),
            remote(qd0.at[:, h], qdx.at[:, h, BEFORE:], halo_send.at[1], right_recv.at[h], before)]

    @pl.when(place < total - 1)
    def _():
        for copy in forth.values():
            copy.start()

    @pl.when(place > 0)
    def _():
        for copies in back.values():
            for copy in copies:
                copy.start()

    @pl.when(tp == 1)
    def _():
        for a, o in close:
            signal(round1, along(a, o))

    wait_bytes(qdx.at[:, :, :BEFORE], load_sem.at[1])
    for load in small_loads:
        load.wait()

    @pl.when(is_first)
    def _():
        for h in range(HEADS):
            for n in range(2):
                kvx[n, h, :BEFORE] = kvx[n, h, BEFORE:2 * BEFORE]
                from_before[n, h] = jnp.zeros((SEG, HEAD_DIM), BF16)
        extra_gains[...] = jnp.zeros((2, HEAD_DIM), F32)

    @pl.when(is_last)
    def _():
        for h in range(HEADS):
            for n in range(2):
                kvx[n, h, BEFORE + ROWS:] = kvx[n, h, BEFORE:ROWS]
                from_after[n, h] = jnp.zeros((BEFORE, HEAD_DIM), BF16)
            qdx[0, h, BEFORE:] = qd0[0, h]
            qdx[1, h, BEFORE:] = jnp.zeros((SEG, HEAD_DIM), BF16)

    gains = gains_v[...]
    gain_q, gain_k = gains[0:1, :], gains[1:2, :]

    def norm_keys(h, first, size):
        u, r = unit(kvx[0, h, first:first + size])
        ku[h, first:first + size] = u
        kn[h, first:first + size] = (u * gain_k).astype(BF16)
        if size == ROWS:
            kr[h] = jnp.broadcast_to(r, u.shape)

    def norm_queries(h, first, size):
        u, r = unit(qdx[0, h, first:first + size])
        qu[h, first:first + size] = u
        qr[h, first:first + size] = jnp.broadcast_to(r, u.shape)
        qn[h, first:first + size] = (u * gain_q).astype(BF16)

    for h in range(HEADS):
        norm_queries(h, 0, BEFORE)
        norm_keys(h, BEFORE, ROWS)

    key_at = lax.broadcasted_iota(jnp.int32, (PAIR, PAIR), 0)
    query_at = lax.broadcasted_iota(jnp.int32, (PAIR, PAIR), 1)
    past = query_at >= key_at
    early = query_at < SEG
    high = key_at >= SEG
    lane = lax.broadcasted_iota(jnp.int32, (1, PAIR), 1)
    table = table_v[...]
    low_part = table[:, :PAIR]
    high_part = jnp.concatenate([table[:, PAIR:], jnp.zeros((HEADS, 2 * PAIR - ENTRIES), F32)], axis=1)
    low_rolled = pltpu.roll(low_part, PAIR - SEG + 1, 1)
    high_rolled = pltpu.roll(high_part, PAIR - SEG + 1, 1)
    for h in range(HEADS):
        last = table[h:h + 1, ENTRIES - 1:ENTRIES]
        dist_low = low_rolled[h:h + 1]
        dist_row = jnp.where(lane <= SEG, dist_low, high_rolled[h:h + 1])
        ahead = pltpu.roll(jnp.broadcast_to(dist_low, (PAIR, PAIR)), 0, 1, stride=1, stride_axis=0)
        behind = pltpu.roll(jnp.broadcast_to(dist_row, (PAIR, PAIR)), 0, 1, stride=1, stride_axis=0)
        tile0 = jnp.where(jnp.logical_or(early, high), last, MASKED)
        tile1 = jnp.where(past, last, behind)
        tile2 = jnp.where(jnp.logical_and(early, high), MASKED, jnp.where(past, behind, ahead))
        none, low = (jnp.where(is_first, MASKED, t) for t in (tile0, tile1))
        for p, tiles in enumerate((
                (none, jnp.where(high, tile1, low), tile2),
                (jnp.where(high, tile0, none), tile1, tile2))):
            top = jnp.max(jnp.maximum(jnp.maximum(tiles[0], tiles[1]), tiles[2]), axis=0, keepdims=True)
            for b, tile in enumerate(tiles):
                bias_v[h, p, b * PAIR:(b + 1) * PAIR] = (tile - top) * LOG2E

    sums = {(h, p): (jnp.zeros((1, PAIR), F32), jnp.zeros((1, PAIR), F32)) for h in range(HEADS) for p in range(2)}

    def block(h, p, b):
        first = (p + b) * PAIR
        own = slice(p * PAIR, (p + 1) * PAIR)
        s = dot(kn[h, first:first + PAIR], qn[h, own], 1, 1)
        e = jnp.exp2(s * (FACTOR * LOG2E) + bias_v[h, p, b * PAIR:(b + 1) * PAIR])
        dp = dot(kvx[1, h, first:first + PAIR], qdx[1, h, own], 1, 1)
        e_v[h, p, b * PAIR:(b + 1) * PAIR] = e
        dp_v[h, p, b * PAIR:(b + 1) * PAIR] = dp
        norm, weighted = sums[h, p]
        sums[h, p] = (norm + jnp.sum(e, axis=0, keepdims=True), weighted + jnp.sum(e * dp, axis=0, keepdims=True))

    gain_sums = [jnp.zeros((1, HEAD_DIM), F32), jnp.zeros((1, HEAD_DIM), F32)]

    def finish(h, p):
        norm, weighted = sums[h, p]
        inv = 1.0 / norm
        delta = weighted * inv
        own = slice(p * PAIR, (p + 1) * PAIR)
        keys = slice(p * PAIR, (p + 3) * PAIR)
        prob = e_v[h, p] * inv
        d_score = prob * (dp_v[h, p] - delta)
        prob_low = prob.astype(BF16)
        d_low = d_score.astype(BF16)
        dv = dot(prob_low, qdx[1, h, own], 1, 0)
        dk = dot(d_low, qn[h, own], 1, 0)
        dq = dot(d_low, kn[h, keys], 0, 0)
        dqx[h, own] = dq
        gain_sums[0] = gain_sums[0] + jnp.sum(dq * qu[h, own], axis=0, keepdims=True)
        gain_sums[1] = gain_sums[1] + jnp.sum(dk * ku[h, keys], axis=0, keepdims=True)
        if p == 1:
            dkx[h, keys] = dk
            dvx[h, keys] = dv
            d_v[h] = d_score
        else:
            dkx[h, 0:PAIR] = dk[:PAIR]
            dvx[h, 0:PAIR] = dv[:PAIR]
            dkx[h, PAIR:3 * PAIR] = dkx[h, PAIR:3 * PAIR] + dk[PAIR:]
            dvx[h, PAIR:3 * PAIR] = dvx[h, PAIR:3 * PAIR] + dv[PAIR:]
            d_v[h] = d_v[h] + d_score

    def query_rows(g, u, r):
        g = g * FACTOR * gain_q
        return (r * (g - u * jnp.mean(g * u, axis=-1, keepdims=True))).astype(BF16)

    def first_segment(h):
        u, r = unit(qd0[0, h])
        queries = (u * gain_q).astype(BF16)
        keys = kn[h, BEFORE:ROWS]
        bias = bias_v[h, 0, 2 * PAIR:2 * PAIR + SEG][:, :SEG]
        bias = bias - jnp.max(bias, axis=0, keepdims=True)
        e = jnp.exp2(dot(keys, queries, 1, 1) * (FACTOR * LOG2E) + bias)
        dp = dot(kvx[1, h, BEFORE:ROWS], qd0[1, h], 1, 1)
        inv = 1.0 / jnp.sum(e, axis=0, keepdims=True)
        delta = jnp.sum(e * dp, axis=0, keepdims=True) * inv
        prob = e * inv
        d_score = prob * (dp - delta)
        d_low = d_score.astype(BF16)
        dk = dot(d_low, queries, 1, 0)
        dq = dot(d_low, keys, 0, 0)
        from_before[0, h] = (dk * FACTOR).astype(BF16)
        from_before[1, h] = dot(prob.astype(BF16), qd0[1, h], 1, 0).astype(BF16)
        dq_from_before[:, h * HEAD_DIM:(h + 1) * HEAD_DIM] = query_rows(dq, u, r)
        at_tile = slice(2 * PAIR, 2 * PAIR + SEG)
        d_v[h, at_tile] = d_v[h, at_tile] + jnp.concatenate([d_score, jnp.zeros((SEG, SEG), F32)], axis=1)
        extra_gains[0:1] = extra_gains[0:1] + jnp.sum(dq * u, axis=0, keepdims=True)
        extra_gains[1:2] = extra_gains[1:2] + jnp.sum(dk * ku[h, BEFORE:ROWS], axis=0, keepdims=True)

    table_rows = []
    sublane = lax.broadcasted_iota(jnp.int32, (8, PAIR), 0)

    def skewed_sum(tile):
        total = pltpu.roll(tile[:8], SEG - 1, 1)
        for first in range(8, PAIR, 8):
            total = total + pltpu.roll(tile[first:first + 8], (SEG - 1 - first) % PAIR, 1)
        for bit in (1, 2, 4):
            total = jnp.where((sublane & bit) == 0, total, pltpu.roll(total, PAIR - bit, 1))
        return jnp.sum(total, axis=0, keepdims=True)

    def fold_table(h):
        d0, d1, d2 = (d_v[h, b * PAIR:(b + 1) * PAIR] for b in range(3))
        mixed = jnp.where(past, d2, d1)
        ahead = jnp.where(past, 0.0, d2)
        rest = d0 + jnp.where(past, d1, 0.0)
        behind_row, ahead_row = skewed_sum(mixed), skewed_sum(ahead)
        rest_sum = jnp.sum(jnp.sum(rest, axis=0, keepdims=True), axis=1, keepdims=True)
        table_rows.append((
            jnp.where(lane < SEG - 1, ahead_row, behind_row),
            jnp.where(lane == SEG - 1, rest_sum, behind_row),
        ))

    for h in range(HEADS):
        block(h, 0, 2)

    @pl.when(tp == 1)
    def _():
        pl.semaphore_wait(round1, len(close))
        signal(row_sem, (z, y, x, 0))
        for a, n in enumerate(sizes[:2]):
            if n > 5:
                for o in near(n, 2):
                    signal(round2, along(a, o))

    for h in range(HEADS):
        @pl.when(place < total - 1)
        def _(h=h):
            wait_bytes(kvx.at[:, h, :PAIR], right_recv.at[h])

        norm_keys(h, BEFORE + ROWS, SEG)
        norm_queries(h, BEFORE, SEG)
        block(h, 1, 1)
        block(h, 1, 2)

        @pl.when(place > 0)
        def _(h=h):
            forth[h, 1].wait_recv()

        norm_keys(h, PAIR, SEG)
        block(h, 1, 0)
        block(h, 0, 1)
        finish(h, 1)

        @pl.when(is_first)
        def _(h=h):
            first_segment(h)

        @pl.when(place > 0)
        def _(h=h):
            forth[h, 0].wait_recv()

        norm_keys(h, 0, PAIR)
        block(h, 0, 0)
        finish(h, 0)
        fold_table(h)
        if h == 0:
            @pl.when(tp == 1)
            def _():
                count = sum(len(near(n, 2)) for n in sizes[:2] if n > 5)
                if count:
                    pl.semaphore_wait(round2, count)
                if nz > 9:
                    for o in near(nz, 3):
                        signal(round3, along(0, o))

    row = lax.broadcasted_iota(jnp.int32, (8, HEAD_DIM), 0)
    vec = jnp.zeros((8, HEAD_DIM), F32)
    second = jnp.where(lane < SEG, table_rows[0][1], pltpu.roll(table_rows[1][1], SEG, 1))
    for j, part in enumerate((table_rows[0][0], table_rows[1][0], second)):
        vec = jnp.where(row == 3 * tp + j, part, vec)
    for j in range(2):
        part = gain_sums[j] + jnp.where(is_first, extra_gains[j:j + 1], 0.0)
        vec = jnp.where(row == 6 + j, part * FACTOR, vec)
    mine = 2 * x + tp
    lines[mine] = vec

    to_neighbours = [
        remote(to_before.at[:, h], from_after.at[:, h], back_send.at[0], after_recv.at[h], before) for h in range(HEADS)]
    to_next = [
        remote(to_after, from_before, back_send.at[1], before_recv, after),
        remote(dq_to_after, dq_from_before, back_send.at[1], before_recv, after)]

    def stage_results():
        for h in range(HEADS):
            lanes = slice(h * HEAD_DIM, (h + 1) * HEAD_DIM)
            to_before[0, h] = (dkx[h, :BEFORE] * FACTOR).astype(BF16)
            to_before[1, h] = dvx[h, :BEFORE].astype(BF16)
            to_after[0, h] = (dkx[h, BEFORE + ROWS:] * FACTOR).astype(BF16)
            to_after[1, h] = dvx[h, BEFORE + ROWS:].astype(BF16)
            rows = query_rows(dqx[h], qu[h], qr[h])
            dq_v[SEG:, lanes] = rows[:BEFORE]
            dq_to_after[:, lanes] = rows[BEFORE:]

    def send_results(when):
        @pl.when(jnp.logical_and(when, place > 0))
        def _():
            for copy in to_neighbours:
                copy.start()

        @pl.when(jnp.logical_and(when, place < total - 1))
        def _():
            for copy in to_next:
                copy.start()

    def line_sum(first, count):
        part = lines[first]
        for n in range(first + 1, first + count):
            part = part + lines[n]
        return part

    ys, zs = 2 * nx, 2 * nx + ny
    at_end = jnp.logical_or(x == 0, x == nx - 1)

    @pl.when(tp == 1)
    def _():
        if nz > 9:
            pl.semaphore_wait(round3, len(near(nz, 3)))
        for o in far_first(nx):
            remote(lines.at[mine], lines.at[mine], xy_send, x_recv, along(2, o)).start()
        stage_results()
        send_results(jnp.logical_not(at_end))
        wait_bytes(lines.at[:2 * nx - 1], x_recv)
        lines[ys + y] = line_sum(0, 2 * nx)
        for o in far_first(ny):
            remote(lines.at[ys + y], lines.at[ys + y], xy_send, y_recv, along(1, o)).start()
        send_results(at_end)
        if ny > 1:
            wait_bytes(lines.at[:ny - 1], y_recv)
        part = line_sum(ys, ny)
        for core in range(2):
            zout[core, :3] = part[3 * core:3 * core + 3]
            zout[core, 3:] = part[6:]
        zbuf[z] = zout[1]
        for o in [*far_first(nz), 0]:
            for core in range(2 if o else 1):
                remote(zout.at[core], zbuf.at[z], z_send, z_recv, along(0, o, core)).start()

    @pl.when(tp == 0)
    def _():
        pl.semaphore_wait(row_sem, 1)
        for o in [*far_first(nx), 0]:
            remote(lines.at[mine], lines.at[mine], xy_send, x_recv, along(2, o)).start()
        stage_results()
        send_results(place >= 0)

    @pl.when(place > 0)
    def _():
        wait_bytes(from_after.at[:, 0], before_recv)

    dq_v[:SEG] = dq_from_before[...]
    for h in range(HEADS):
        @pl.when(place < total - 1)
        def _(h=h):
            to_neighbours[h].wait_recv()

        lanes = slice(h * HEAD_DIM, (h + 1) * HEAD_DIM)
        sums_in = [
            jnp.concatenate([from_before[n, h].astype(F32), from_after[n, h].astype(F32)], axis=0) for n in range(2)]
        g = (dkx[h, BEFORE:BEFORE + ROWS] * FACTOR + sums_in[0]) * gain_k
        u = ku[h, BEFORE:BEFORE + ROWS]
        dk_v[:, lanes] = (kr[h] * (g - u * jnp.mean(g * u, axis=-1, keepdims=True))).astype(BF16)
        dv_v[:, lanes] = (dvx[h, BEFORE:BEFORE + ROWS] + sums_in[1]).astype(BF16)

    @pl.when(place < total - 1)
    def _():
        wait_bytes(kvx.at[:, :, :BEFORE], halo_send.at[0])
        wait_bytes(from_after.at[:, 0], back_send.at[1])

    @pl.when(place > 0)
    def _():
        wait_bytes(kvx.at[:, :, :PAIR], halo_send.at[1])
        wait_bytes(from_after, back_send.at[0])

    @pl.when(tp == 1)
    def _():
        if nx + ny > 2:
            wait_bytes(lines.at[:nx + ny - 2], xy_send)
        wait_bytes(zbuf.at[:2 * nz - 1], z_send)
        if nz > 1:
            wait_bytes(zbuf.at[:nz - 1], z_recv)

    @pl.when(tp == 0)
    def _():
        wait_bytes(lines.at[:nx], xy_send)
        wait_bytes(zbuf.at[:nz], z_recv)

    result = zbuf[0]
    for n in range(1, nz):
        result = result + zbuf[n]
    for j in range(HEADS):
        dtab_v[j:j + 1, :PAIR] = result[j:j + 1]
        dtab_v[j:j + 1, PAIR:] = result[2:3, j * SEG:(j + 1) * SEG]
    dgain_v[...] = result[3:]


def write_out(*refs):
    count = len(refs) // 2
    copies = [pltpu.make_async_copy(refs[n], refs[count + n], refs[-1].at[n]) for n in range(count)]
    for copy in copies:
        copy.start()
    for copy in copies:
        copy.wait()


def local(sizes, queries, keys, values, gains, bias_table, d_out):
    nz, ny, nx = sizes
    width = HEADS * HEAD_DIM
    hbm_spec = pl.BlockSpec(memory_space=pltpu.HBM)
    vmem_spec = pl.BlockSpec(memory_space=pltpu.VMEM)
    first = (HEADS, SEG, HEAD_DIM)
    tile = (HEADS, ROWS, HEAD_DIM)
    wide = (HEADS, 2 * ROWS, HEAD_DIM)
    pairs = (HEADS, 2, 3 * PAIR, PAIR)
    dma, regular = pltpu.SemaphoreType.DMA, pltpu.SemaphoreType.REGULAR
    vmem = pltpu.VMEM
    outs = [((ROWS, width), BF16)] * 3 + [((HEADS, ENTRIES), F32), ((2, HEAD_DIM), F32)]
    out = pl.pallas_call(
        functools.partial(kernel, sizes),
        out_shape=tuple(vmem(*o) for o in outs),
        in_specs=[hbm_spec] * 6,
        out_specs=(vmem_spec,) * 5,
        scratch_shapes=[
            vmem((2, *tile), BF16), vmem((2, *first), BF16), vmem((2, *wide), BF16),
            vmem((2, HEAD_DIM), F32), vmem((HEADS, ENTRIES), F32),
            vmem(tile, BF16), vmem(tile, F32), vmem(tile, F32),
            vmem(wide, BF16), vmem(wide, F32), vmem(tile, F32),
            vmem(pairs, F32), vmem(pairs, F32), vmem(pairs, F32),
            vmem(wide, F32), vmem(wide, F32), vmem(tile, F32), vmem((HEADS, 3 * PAIR, PAIR), F32), vmem((2, HEAD_DIM), F32),
            vmem((2, HEADS, BEFORE, HEAD_DIM), BF16), vmem((2, HEADS, BEFORE, HEAD_DIM), BF16),
            vmem((2, *first), BF16), vmem((2, *first), BF16), vmem((SEG, width), BF16), vmem((SEG, width), BF16),
            vmem((2 * nx + ny, 8, HEAD_DIM), F32), vmem((2, 5, HEAD_DIM), F32), vmem((2 * nz, 5, HEAD_DIM), F32),
            dma((2,)), dma, dma, dma((2,)), dma((4,)), dma((HEADS,)), dma((2,)), dma((HEADS,)), dma,
            dma, dma, dma, dma, dma, regular, regular, regular, regular,
        ],
        compiler_params=pltpu.CompilerParams(
            collective_id=0, has_side_effects=True, vmem_limit_bytes=32 * 1024 * 1024),
        name="segment_attention_grad",
    )(*(pltpu.with_memory_space_constraint(a, pltpu.HBM) for a in (queries, keys, values, d_out, gains, bias_table.T)))
    d_queries, d_keys, d_values, d_table, d_gains = pl.pallas_call(
        write_out,
        out_shape=tuple(jax.ShapeDtypeStruct(*o) for o in outs),
        in_specs=[vmem_spec] * 5,
        out_specs=(hbm_spec,) * 5,
        scratch_shapes=[dma((5,))],
        name="write_out",
    )(*(pltpu.with_memory_space_constraint(o, pltpu.VMEM) for o in out))
    return d_queries, d_keys, d_values, d_table.T, d_gains


def solution(mesh):
    shape = (12, 8, 4)
    if mesh.shape["sp"] != int(np.prod(shape)):
        shape = mesh.small_shape
    split = Mesh(mesh.devices.reshape(*shape, mesh.shape["tp"]), AXES)
    placed = (P(SP, "tp"), P(SP, "tp"), P(SP, "tp"), P(), P(None, "tp"), P(SP, "tp"))
    return jax.shard_map(
        functools.partial(local, shape),
        mesh=split,
        in_specs=placed,
        out_specs=(P(SP, "tp"), P(SP, "tp"), P(SP, "tp"), P(None, "tp"), P()),
        check_vma=False,
    )
```

```python
import functools

import jax
import jax.numpy as jnp
import numpy as np
from jax import lax
from jax.experimental import pallas as pl
from jax.experimental.pallas import tpu as pltpu
from jax.sharding import Mesh
from jax.sharding import PartitionSpec as P

HEAD_DIM = 128
SEG = 64
LEFT = 4
MAX_REL = 128
ENTRIES = MAX_REL + SEG
ROWS = LEFT * SEG
HEADS = 2
PAIR = 2 * SEG
BEFORE = 3 * SEG
AXES = ("sp_0", "sp_1", "sp_2", "tp")
SP = AXES[:3]

EPSILON = 1e-06
FACTOR = HEAD_DIM ** (-0.5)
LOG2E = 1.4426950408889634
MASKED = -1e30
F32, BF16 = jnp.float32, jnp.bfloat16


def dot(a, b, a_dim, b_dim):
    return lax.dot_general(a, b, (((a_dim,), (b_dim,)), ((), ())), preferred_element_type=F32)


def near(size, step=1):
    return sorted({step % size, -step % size} - {0})


def far_first(size):
    return sorted(range(1, size), key=lambda d: -min(d, size - d))


def unit(raw):
    wide = raw.astype(F32)
    inv_rms = lax.rsqrt(jnp.mean(wide * wide, axis=-1, keepdims=True) + EPSILON)
    return wide * inv_rms, inv_rms


def kernel(sizes, q_hbm, k_hbm, v_hbm, do_hbm, gains_hbm, table_hbm,
           dq_v, dk_v, dv_v, dtab_v, dgain_v,
           qdx, qd0, kvx, gains_v, table_v,
           qn, qu, qr, kn, ku, kr, bias_v, e_v, dp_v,
           dkx, dvx, dqx, d_v, prob_v, sum_v, gain_v, table_v2, extra_gains,
           to_before, from_after, to_after, from_before, dq_to_after, dq_from_before,
           lines, zout, zbuf,
           load_sem, gains_sem, table_sem, halo_send, left_recv, right_recv, back_send, after_recv, before_recv,
           xy_send, x_recv, y_recv, z_send, z_recv, round1, round2, round3, row_sem):
    nz, ny, nx = sizes
    z, y, x, tp = (lax.axis_index(a) for a in AXES)
    place = (z * ny + y) * nx + x
    total = nz * ny * nx
    is_first, is_last = place == 0, place == total - 1

    def at(number, core):
        return (number // (ny * nx), (number // nx) % ny, number % nx, core)

    after = at(jnp.minimum(place + 1, total - 1), tp)
    before = at(jnp.maximum(place - 1, 0), tp)

    def along(axis, offset, core=1):
        if axis == 0:
            return (lax.rem(z + offset, nz), y, x, core)
        if axis == 1:
            return (z, lax.rem(y + offset, ny), x, core)
        return (z, y, lax.rem(x + offset, nx), core)

    def signal(sem, target):
        pl.semaphore_signal(sem, inc=1, device_id=target, device_id_type=pl.DeviceIdType.MESH)

    def remote(src, dst, send, recv, target):
        return pltpu.make_async_remote_copy(
            src_ref=src, dst_ref=dst, send_sem=send, recv_sem=recv,
            device_id=target, device_id_type=pl.DeviceIdType.MESH)

    def wait_bytes(ref, sem):
        pltpu.make_async_copy(ref, ref, sem).wait()

    barrier = pltpu.get_barrier_semaphore()

    @pl.when(place > 0)
    def _():
        signal(barrier, before)

    @pl.when(place < total - 1)
    def _():
        signal(barrier, after)

    sides = jnp.where(is_first, 0, 1) + jnp.where(is_last, 0, 1)
    for n, (src, dst) in enumerate(((k_hbm, kvx.at[0]), (v_hbm, kvx.at[1]), (q_hbm, qdx.at[0]), (do_hbm, qdx.at[1]))):
        for h in range(HEADS):
            lanes = slice(h * HEAD_DIM, (h + 1) * HEAD_DIM)
            if n < 2:
                pltpu.make_async_copy(src.at[:, lanes], dst.at[h, BEFORE:BEFORE + ROWS], load_sem.at[0]).start()
            else:
                pltpu.make_async_copy(src.at[:SEG, lanes], qd0.at[n - 2, h], load_sem.at[0]).start()
                pltpu.make_async_copy(src.at[SEG:, lanes], dst.at[h, :BEFORE], load_sem.at[1]).start()
    small_loads = [pltpu.make_async_copy(gains_hbm, gains_v, gains_sem), pltpu.make_async_copy(table_hbm, table_v, table_sem)]
    for load in small_loads:
        load.start()

    close = [(a, o) for a, n in enumerate(sizes) for o in near(n)]

    @pl.when(tp == 1)
    def _():
        for a, o in close:
            signal(barrier, along(a, o))
        signal(barrier, (z, y, x, 0))
        pl.semaphore_wait(barrier, 1 + len(close) + sides)

    @pl.when(tp == 0)
    def _():
        signal(barrier, (z, y, x, 1))
        pl.semaphore_wait(barrier, 1 + sides)

    wait_bytes(kvx.at[:, :, :ROWS + SEG], load_sem.at[0])
    forth = [remote(
        kvx.at[:, :, ROWS + PAIR:ROWS + BEFORE], kvx.at[:, :, PAIR:BEFORE], halo_send.at[0], left_recv.at[HEADS], after)]
    back = {}
    for h in range(HEADS):
        forth.append(remote(
            kvx.at[:, h, ROWS:ROWS + PAIR], kvx.at[:, h, :PAIR], halo_send.at[0], left_recv.at[h], after))
        back[h] = [
            remote(kvx.at[:, h, BEFORE:ROWS], kvx.at[:, h, BEFORE + ROWS:], halo_send.at[1], right_recv.at[h], before),
            remote(qd0.at[:, h], qdx.at[:, h, BEFORE:], halo_send.at[1], right_recv.at[h], before)]

    @pl.when(place < total - 1)
    def _():
        for copy in forth:
            copy.start()

    @pl.when(place > 0)
    def _():
        for copies in back.values():
            for copy in copies:
                copy.start()

    @pl.when(tp == 1)
    def _():
        for a, o in close:
            signal(round1, along(a, o))

    wait_bytes(qdx.at[:, :, :BEFORE], load_sem.at[1])
    for load in small_loads:
        load.wait()

    @pl.when(is_first)
    def _():
        for h in range(HEADS):
            for n in range(2):
                kvx[n, h, :BEFORE] = kvx[n, h, BEFORE:2 * BEFORE]
                from_before[n, h] = jnp.zeros((SEG, HEAD_DIM), BF16)
        extra_gains[...] = jnp.zeros((2, HEAD_DIM), F32)

    @pl.when(is_last)
    def _():
        for h in range(HEADS):
            for n in range(2):
                kvx[n, h, BEFORE + ROWS:] = kvx[n, h, BEFORE:ROWS]
                from_after[n, h] = jnp.zeros((BEFORE, HEAD_DIM), BF16)
            qdx[0, h, BEFORE:] = qd0[0, h]
            qdx[1, h, BEFORE:] = jnp.zeros((SEG, HEAD_DIM), BF16)

    gains = gains_v[...]
    gain_q, gain_k = gains[0:1, :], gains[1:2, :]

    def norm_keys(h, first, size):
        u, r = unit(kvx[0, h, first:first + size])
        ku[h, first:first + size] = u
        kn[h, first:first + size] = (u * gain_k).astype(BF16)
        if size == ROWS:
            kr[h] = jnp.broadcast_to(r, u.shape)

    def norm_queries(h, first, size):
        u, r = unit(qdx[0, h, first:first + size])
        qu[h, first:first + size] = u
        qr[h, first:first + size] = jnp.broadcast_to(r, u.shape)
        qn[h, first:first + size] = (u * gain_q).astype(BF16)

    for h in range(HEADS):
        norm_queries(h, 0, BEFORE)
        norm_keys(h, BEFORE, ROWS)

    key_at = lax.broadcasted_iota(jnp.int32, (PAIR, PAIR), 0)
    query_at = lax.broadcasted_iota(jnp.int32, (PAIR, PAIR), 1)
    past = query_at >= key_at
    early = query_at < SEG
    high = key_at >= SEG
    lane = lax.broadcasted_iota(jnp.int32, (1, PAIR), 1)
    table = table_v[...]
    low_part = table[:, :PAIR]
    high_part = jnp.concatenate([table[:, PAIR:], jnp.zeros((HEADS, 2 * PAIR - ENTRIES), F32)], axis=1)
    low_rolled = pltpu.roll(low_part, PAIR - SEG + 1, 1)
    high_rolled = pltpu.roll(high_part, PAIR - SEG + 1, 1)
    for h in range(HEADS):
        last = table[h:h + 1, ENTRIES - 1:ENTRIES]
        dist_low = low_rolled[h:h + 1]
        dist_row = jnp.where(lane <= SEG, dist_low, high_rolled[h:h + 1])
        ahead = pltpu.roll(jnp.broadcast_to(dist_low, (PAIR, PAIR)), 0, 1, stride=1, stride_axis=0)
        behind = pltpu.roll(jnp.broadcast_to(dist_row, (PAIR, PAIR)), 0, 1, stride=1, stride_axis=0)
        tile0 = jnp.where(jnp.logical_or(early, high), last, MASKED)
        tile1 = jnp.where(past, last, behind)
        tile2 = jnp.where(jnp.logical_and(early, high), MASKED, jnp.where(past, behind, ahead))
        none, low = (jnp.where(is_first, MASKED, t) for t in (tile0, tile1))
        for p, tiles in enumerate((
                (none, jnp.where(high, tile1, low), tile2),
                (jnp.where(high, tile0, none), tile1, tile2))):
            top = jnp.max(jnp.maximum(jnp.maximum(tiles[0], tiles[1]), tiles[2]), axis=0, keepdims=True)
            for b, tile in enumerate(tiles):
                bias_v[h, p, b * PAIR:(b + 1) * PAIR] = (tile - top) * LOG2E

    def block(h, p, b):
        first = (p + b) * PAIR
        own = slice(p * PAIR, (p + 1) * PAIR)
        s = dot(kn[h, first:first + PAIR], qn[h, own], 1, 1)
        e = jnp.exp2(s * (FACTOR * LOG2E) + bias_v[h, p, b * PAIR:(b + 1) * PAIR])
        dp = dot(kvx[1, h, first:first + PAIR], qdx[1, h, own], 1, 1)
        e_v[h, p, b * PAIR:(b + 1) * PAIR] = e
        dp_v[h, p, b * PAIR:(b + 1) * PAIR] = dp
        sum_v[h, p, b] = jnp.sum(e, axis=0, keepdims=True)
        sum_v[h, p, 3 + b] = jnp.sum(e * dp, axis=0, keepdims=True)

    def finish(h, p, again):
        inv = 1.0 / (sum_v[h, p, 0] + sum_v[h, p, 1] + sum_v[h, p, 2])
        delta = (sum_v[h, p, 3] + sum_v[h, p, 4] + sum_v[h, p, 5]) * inv
        own = slice(p * PAIR, (p + 1) * PAIR)
        keys = slice(p * PAIR, (p + 3) * PAIR)
        prob = e_v[h, p] * inv
        d_score = prob * (dp_v[h, p] - delta)
        prob_low = prob.astype(BF16)
        d_low = d_score.astype(BF16)
        prob_v[h, p] = prob_low
        dk = dot(d_low, qn[h, own], 1, 0)
        dq = dot(d_low, kn[h, keys], 0, 0)
        dqx[h, own] = dq
        gain_v[h, p, 0] = jnp.sum(dq * qu[h, own], axis=0, keepdims=True)
        gain_v[h, p, 1] = jnp.sum(dk * ku[h, keys], axis=0, keepdims=True)
        if again:
            shared, alone = slice(PAIR, 3 * PAIR), slice(3 * p * PAIR, (3 * p + 1) * PAIR)
            ours = slice((1 - p) * PAIR, (3 - p) * PAIR)
            rest = slice(2 * p * PAIR, (2 * p + 1) * PAIR)
            dkx[h, alone] = dk[rest]
            dkx[h, shared] = dkx[h, shared] + dk[ours]
            return d_v[h] + d_score
        dkx[h, keys] = dk
        d_v[h] = d_score

    def query_rows(g, u, r):
        g = g * FACTOR * gain_q
        return (r * (g - u * jnp.mean(g * u, axis=-1, keepdims=True))).astype(BF16)

    def first_segment(h):
        u, r = unit(qd0[0, h])
        queries = (u * gain_q).astype(BF16)
        keys = kn[h, BEFORE:ROWS]
        bias = bias_v[h, 0, 2 * PAIR:2 * PAIR + SEG][:, :SEG]
        bias = bias - jnp.max(bias, axis=0, keepdims=True)
        e = jnp.exp2(dot(keys, queries, 1, 1) * (FACTOR * LOG2E) + bias)
        dp = dot(kvx[1, h, BEFORE:ROWS], qd0[1, h], 1, 1)
        inv = 1.0 / jnp.sum(e, axis=0, keepdims=True)
        delta = jnp.sum(e * dp, axis=0, keepdims=True) * inv
        prob = e * inv
        d_score = prob * (dp - delta)
        d_low = d_score.astype(BF16)
        dk = dot(d_low, queries, 1, 0)
        dq = dot(d_low, keys, 0, 0)
        from_before[0, h] = (dk * FACTOR).astype(BF16)
        from_before[1, h] = dot(prob.astype(BF16), qd0[1, h], 1, 0).astype(BF16)
        dq_from_before[:, h * HEAD_DIM:(h + 1) * HEAD_DIM] = query_rows(dq, u, r)
        at_tile = slice(2 * PAIR, 2 * PAIR + SEG)
        d_v[h, at_tile] = d_v[h, at_tile] + jnp.concatenate([d_score, jnp.zeros((SEG, SEG), F32)], axis=1)
        extra_gains[0:1] = extra_gains[0:1] + jnp.sum(dq * u, axis=0, keepdims=True)
        extra_gains[1:2] = extra_gains[1:2] + jnp.sum(dk * ku[h, BEFORE:ROWS], axis=0, keepdims=True)

    sublane = lax.broadcasted_iota(jnp.int32, (8, PAIR), 0)

    def skewed_sum(tile, right):
        parts = [pltpu.roll(tile[first:first + 8], (right - first) % PAIR, 1) for first in range(0, PAIR, 8)]
        while len(parts) > 1:
            parts = [a + b for a, b in zip(parts[::2], parts[1::2])]
        total = parts[0]
        for bit in range(1, 8):
            total = jnp.where(sublane == bit, pltpu.roll(parts[0], PAIR - bit, 1), total)
        return jnp.sum(total, axis=0, keepdims=True)

    def fold_table(h, d_score):
        d0, d1, d2 = (d_score[b * PAIR:(b + 1) * PAIR] for b in range(3))
        mixed = jnp.where(past, d2, d1)
        ahead = jnp.where(past, 0.0, d2)
        rest = d0 + jnp.where(past, d1, 0.0)
        behind_row, ahead_row = skewed_sum(mixed, SEG - 1), skewed_sum(ahead, SEG - 1)
        high_row = skewed_sum(mixed, SEG - 1 + SEG) if h else behind_row
        rest_sum = jnp.sum(jnp.sum(rest, axis=0, keepdims=True), axis=1, keepdims=True)
        table_v2[h, 0] = jnp.where(lane < SEG - 1, ahead_row, behind_row)
        table_v2[h, 1] = jnp.where(lane == SEG - 1 + h * SEG, rest_sum, high_row)

    for h in range(HEADS):
        block(h, 0, 2)

    @pl.when(tp == 1)
    def _():
        pl.semaphore_wait(round1, len(close))
        signal(row_sem, (z, y, x, 0))
        for a, n in enumerate(sizes[:2]):
            if n > 5:
                for o in near(n, 2):
                    signal(round2, along(a, o))

    def wait_left(piece):
        @pl.when(place > 0)
        def _():
            forth[piece].wait_recv()

    def wait_right(h):
        @pl.when(place < total - 1)
        def _():
            wait_bytes(kvx.at[:, h, :PAIR], right_recv.at[h])

    def greet_far():
        @pl.when(tp == 1)
        def _():
            count = sum(len(near(n, 2)) for n in sizes[:2] if n > 5)
            if count:
                pl.semaphore_wait(round2, count)
            if nz > 9:
                for o in near(nz, 3):
                    signal(round3, along(0, o))

    def do_first(h):
        @pl.when(is_first)
        def _():
            first_segment(h)

    def from_left_near(h):
        norm_keys(h, PAIR, SEG)
        block(h, 0, 1)

    def from_left_far(h):
        norm_keys(h, 0, PAIR)
        block(h, 0, 0)

    def from_right(h):
        norm_keys(h, BEFORE + ROWS, SEG)
        norm_queries(h, BEFORE, SEG)
        block(h, 1, 1)
        block(h, 1, 2)

    @pl.when(x == nx - 1)
    def _():
        wait_left(0)
        for h in range(HEADS):
            from_left_near(h)
        for h in range(HEADS):
            wait_left(1 + h)
            from_left_far(h)
            finish(h, 0, False)
            if nx == 1:
                do_first(h)
        greet_far()
        for h in range(HEADS):
            wait_right(h)
            from_right(h)
            block(h, 1, 0)
            fold_table(h, finish(h, 1, True))

    if nx > 1:
        @pl.when(x == 0)
        def _():
            for h in range(HEADS):
                wait_right(h)
            for h in range(HEADS):
                from_right(h)
            wait_left(0)
            for h in range(HEADS):
                from_left_near(h)
                block(h, 1, 0)
                finish(h, 1, False)
            for h in range(HEADS):
                do_first(h)
            greet_far()
            for h in range(HEADS):
                wait_left(1 + h)
                from_left_far(h)
                fold_table(h, finish(h, 0, True))

    if nx > 2:
        @pl.when(jnp.logical_and(x > 0, x < nx - 1))
        def _():
            wait_left(0)
            for h in range(HEADS):
                from_left_near(h)
            for h in range(HEADS):
                wait_right(h)
                from_right(h)
                block(h, 1, 0)
                finish(h, 1, False)
                if h:
                    greet_far()
                wait_left(1 + h)
                from_left_far(h)
                fold_table(h, finish(h, 0, True))

    row = lax.broadcasted_iota(jnp.int32, (8, HEAD_DIM), 0)
    vec = jnp.zeros((8, HEAD_DIM), F32)
    second = jnp.where(lane < SEG, table_v2[0, 1], table_v2[1, 1])
    for j, part in enumerate((table_v2[0, 0], table_v2[1, 0], second)):
        vec = jnp.where(row == 3 * tp + j, part, vec)
    for j in range(2):
        part = gain_v[0, 0, j] + gain_v[0, 1, j] + gain_v[1, 0, j] + gain_v[1, 1, j]
        part = part + jnp.where(is_first, extra_gains[j:j + 1], 0.0)
        vec = jnp.where(row == 6 + j, part * FACTOR, vec)
    mine = 2 * x + tp
    lines[mine] = vec

    to_neighbours = [
        remote(to_before.at[:, h], from_after.at[:, h], back_send.at[0], after_recv.at[h], before) for h in range(HEADS)]
    to_next = [
        remote(to_after, from_before, back_send.at[1], before_recv, after),
        remote(dq_to_after, dq_from_before, back_send.at[1], before_recv, after)]

    def stage_results():
        for h in range(HEADS):
            low, high_tile = (dot(prob_v[h, p], qdx[1, h, p * PAIR:(p + 1) * PAIR], 1, 0) for p in range(2))
            dvx[h, :PAIR] = low[:PAIR]
            dvx[h, PAIR:3 * PAIR] = low[PAIR:] + high_tile[:2 * PAIR]
            dvx[h, 3 * PAIR:] = high_tile[2 * PAIR:]
            lanes = slice(h * HEAD_DIM, (h + 1) * HEAD_DIM)
            to_before[0, h] = (dkx[h, :BEFORE] * FACTOR).astype(BF16)
            to_before[1, h] = dvx[h, :BEFORE].astype(BF16)
            to_after[0, h] = (dkx[h, BEFORE + ROWS:] * FACTOR).astype(BF16)
            to_after[1, h] = dvx[h, BEFORE + ROWS:].astype(BF16)
            rows = query_rows(dqx[h], qu[h], qr[h])
            dq_v[SEG:, lanes] = rows[:BEFORE]
            dq_to_after[:, lanes] = rows[BEFORE:]

    def send_results(when):
        @pl.when(jnp.logical_and(when, place > 0))
        def _():
            for copy in to_neighbours:
                copy.start()

        @pl.when(jnp.logical_and(when, place < total - 1))
        def _():
            for copy in to_next:
                copy.start()

    def line_sum(first, count):
        part = lines[first]
        for n in range(first + 1, first + count):
            part = part + lines[n]
        return part

    ys, zs = 2 * nx, 2 * nx + ny
    at_end = jnp.logical_or(x == 0, x == nx - 1)

    @pl.when(tp == 1)
    def _():
        for o in far_first(nx):
            remote(lines.at[mine], lines.at[mine], xy_send, x_recv, along(2, o)).start()
        stage_results()
        send_results(jnp.logical_not(at_end))
        wait_bytes(lines.at[:2 * nx - 1], x_recv)
        lines[ys + y] = line_sum(0, 2 * nx)
        for o in far_first(ny):
            remote(lines.at[ys + y], lines.at[ys + y], xy_send, y_recv, along(1, o)).start()
        send_results(at_end)
        if ny > 1:
            wait_bytes(lines.at[:ny - 1], y_recv)
        part = line_sum(ys, ny)
        for core in range(2):
            zout[core, :3] = part[3 * core:3 * core + 3]
            zout[core, 3:] = part[6:]
        zbuf[z] = zout[1]
        if nz > 9:
            pl.semaphore_wait(round3, len(near(nz, 3)))
        for o in [*far_first(nz), 0]:
            for core in range(2 if o else 1):
                remote(zout.at[core], zbuf.at[z], z_send, z_recv, along(0, o, core)).start()

    @pl.when(tp == 0)
    def _():
        pl.semaphore_wait(row_sem, 1)
        for o in [*far_first(nx), 0]:
            remote(lines.at[mine], lines.at[mine], xy_send, x_recv, along(2, o)).start()
        stage_results()
        send_results(place >= 0)

    @pl.when(place > 0)
    def _():
        wait_bytes(from_after.at[:, 0], before_recv)

    dq_v[:SEG] = dq_from_before[...]
    for h in range(HEADS):
        @pl.when(place < total - 1)
        def _(h=h):
            to_neighbours[h].wait_recv()

        lanes = slice(h * HEAD_DIM, (h + 1) * HEAD_DIM)
        sums_in = [
            jnp.concatenate([from_before[n, h].astype(F32), from_after[n, h].astype(F32)], axis=0) for n in range(2)]
        g = (dkx[h, BEFORE:BEFORE + ROWS] * FACTOR + sums_in[0]) * gain_k
        u = ku[h, BEFORE:BEFORE + ROWS]
        dk_v[:, lanes] = (kr[h] * (g - u * jnp.mean(g * u, axis=-1, keepdims=True))).astype(BF16)
        dv_v[:, lanes] = (dvx[h, BEFORE:BEFORE + ROWS] + sums_in[1]).astype(BF16)

    @pl.when(place < total - 1)
    def _():
        wait_bytes(kvx.at[:, :, :BEFORE], halo_send.at[0])
        wait_bytes(from_after.at[:, 0], back_send.at[1])

    @pl.when(place > 0)
    def _():
        wait_bytes(kvx.at[:, :, :PAIR], halo_send.at[1])
        wait_bytes(from_after, back_send.at[0])

    @pl.when(tp == 1)
    def _():
        if nx + ny > 2:
            wait_bytes(lines.at[:nx + ny - 2], xy_send)
        wait_bytes(zbuf.at[:2 * nz - 1], z_send)
        if nz > 1:
            wait_bytes(zbuf.at[:nz - 1], z_recv)

    @pl.when(tp == 0)
    def _():
        wait_bytes(lines.at[:nx], xy_send)
        wait_bytes(zbuf.at[:nz], z_recv)

    result = zbuf[0]
    for n in range(1, nz):
        result = result + zbuf[n]
    for j in range(HEADS):
        dtab_v[j:j + 1, :PAIR] = result[j:j + 1]
        dtab_v[j:j + 1, PAIR:] = result[2:3, j * SEG:(j + 1) * SEG]
    dgain_v[...] = result[3:]


def write_out(*refs):
    count = len(refs) // 2
    copies = [pltpu.make_async_copy(refs[n], refs[count + n], refs[-1].at[n]) for n in range(count)]
    for copy in copies:
        copy.start()
    for copy in copies:
        copy.wait()


def local(sizes, queries, keys, values, gains, bias_table, d_out):
    nz, ny, nx = sizes
    width = HEADS * HEAD_DIM
    hbm_spec = pl.BlockSpec(memory_space=pltpu.HBM)
    vmem_spec = pl.BlockSpec(memory_space=pltpu.VMEM)
    first = (HEADS, SEG, HEAD_DIM)
    tile = (HEADS, ROWS, HEAD_DIM)
    wide = (HEADS, 2 * ROWS, HEAD_DIM)
    pairs = (HEADS, 2, 3 * PAIR, PAIR)
    dma, regular = pltpu.SemaphoreType.DMA, pltpu.SemaphoreType.REGULAR
    vmem = pltpu.VMEM
    outs = [((ROWS, width), BF16)] * 3 + [((HEADS, ENTRIES), F32), ((2, HEAD_DIM), F32)]
    out = pl.pallas_call(
        functools.partial(kernel, sizes),
        out_shape=tuple(vmem(*o) for o in outs),
        in_specs=[hbm_spec] * 6,
        out_specs=(vmem_spec,) * 5,
        scratch_shapes=[
            vmem((2, *tile), BF16), vmem((2, *first), BF16), vmem((2, *wide), BF16),
            vmem((2, HEAD_DIM), F32), vmem((HEADS, ENTRIES), F32),
            vmem(tile, BF16), vmem(tile, F32), vmem(tile, F32),
            vmem(wide, BF16), vmem(wide, F32), vmem(tile, F32),
            vmem(pairs, F32), vmem(pairs, F32), vmem(pairs, F32),
            vmem(wide, F32), vmem(wide, F32), vmem(tile, F32), vmem((HEADS, 3 * PAIR, PAIR), F32),
            vmem(pairs, BF16), vmem((HEADS, 2, 6, 1, PAIR), F32), vmem((HEADS, 2, 2, 1, PAIR), F32), vmem((HEADS, 2, 1, PAIR), F32), vmem((2, HEAD_DIM), F32),
            vmem((2, HEADS, BEFORE, HEAD_DIM), BF16), vmem((2, HEADS, BEFORE, HEAD_DIM), BF16),
            vmem((2, *first), BF16), vmem((2, *first), BF16), vmem((SEG, width), BF16), vmem((SEG, width), BF16),
            vmem((2 * nx + ny, 8, HEAD_DIM), F32), vmem((2, 5, HEAD_DIM), F32), vmem((2 * nz, 5, HEAD_DIM), F32),
            dma((2,)), dma, dma, dma((2,)), dma((HEADS + 1,)), dma((HEADS,)), dma((2,)), dma((HEADS,)), dma,
            dma, dma, dma, dma, dma, regular, regular, regular, regular,
        ],
        compiler_params=pltpu.CompilerParams(
            collective_id=0, has_side_effects=True, vmem_limit_bytes=32 * 1024 * 1024),
        name="segment_attention_grad",
    )(*(pltpu.with_memory_space_constraint(a, pltpu.HBM) for a in (queries, keys, values, d_out, gains, bias_table.T)))
    d_queries, d_keys, d_values, d_table, d_gains = pl.pallas_call(
        write_out,
        out_shape=tuple(jax.ShapeDtypeStruct(*o) for o in outs),
        in_specs=[vmem_spec] * 5,
        out_specs=(hbm_spec,) * 5,
        scratch_shapes=[dma((5,))],
        name="write_out",
    )(*(pltpu.with_memory_space_constraint(o, pltpu.VMEM) for o in out))
    return d_queries, d_keys, d_values, d_table.T, d_gains


def solution(mesh):
    shape = (12, 8, 4)
    if mesh.shape["sp"] != int(np.prod(shape)):
        shape = mesh.small_shape
    split = Mesh(mesh.devices.reshape(*shape, mesh.shape["tp"]), AXES)
    placed = (P(SP, "tp"), P(SP, "tp"), P(SP, "tp"), P(), P(None, "tp"), P(SP, "tp"))
    return jax.shard_map(
        functools.partial(local, shape),
        mesh=split,
        in_specs=placed,
        out_specs=(P(SP, "tp"), P(SP, "tp"), P(SP, "tp"), P(None, "tp"), P()),
        check_vma=False,
    )
```

```python
import functools

import jax
import jax.numpy as jnp
import numpy as np
from jax import lax
from jax.experimental import pallas as pl
from jax.experimental.pallas import tpu as pltpu
from jax.sharding import Mesh
from jax.sharding import PartitionSpec as P

HEAD_DIM = 128
SEG = 64
LEFT = 4
MAX_REL = 128
ENTRIES = MAX_REL + SEG
ROWS = LEFT * SEG
HEADS = 2
PAIR = 2 * SEG
BEFORE = 3 * SEG
AXES = ("sp_0", "sp_1", "sp_2", "tp")
SP = AXES[:3]

EPSILON = 1e-06
FACTOR = HEAD_DIM ** (-0.5)
LOG2E = 1.4426950408889634
MASKED = -1e30
F32, BF16 = jnp.float32, jnp.bfloat16


def dot(a, b, a_dim, b_dim):
    return lax.dot_general(a, b, (((a_dim,), (b_dim,)), ((), ())), preferred_element_type=F32)


def near(size, step=1):
    return sorted({step % size, -step % size} - {0})


def far_first(size):
    return sorted(range(1, size), key=lambda d: -min(d, size - d))


def unit(raw):
    wide = raw.astype(F32)
    inv_rms = lax.rsqrt(jnp.mean(wide * wide, axis=-1, keepdims=True) + EPSILON)
    return wide * inv_rms, inv_rms


def kernel(sizes, q_hbm, k_hbm, v_hbm, do_hbm, gains_hbm, table_hbm,
           dq_v, dk_v, dv_v, dtab_v, dgain_v,
           q_raw, k_raw, qdx, qd0, kvx, first_kv, gains_v, table_v,
           qu, qr, ku, kr, bias_v, e_v, dp_v,
           dkx, dvx, dqx, d_v, prob_v, d_low_v, sum_v, gain_v, table_v2, extra_gain, extra_dv,
           to_before, from_after, to_after, from_before, dq_from_before, to_before_first, from_after_first,
           lines, zout, zbuf,
           load_sem, gains_sem, table_sem, halo_send, left_recv, right_recv, back_send, after_recv, before_recv, first_recv,
           xy_send, x_recv, y_recv, z_send, z_recv, round1, round2, round3, row_sem):
    nz, ny, nx = sizes
    z, y, x, tp = (lax.axis_index(a) for a in AXES)
    place = (z * ny + y) * nx + x
    total = nz * ny * nx
    is_first, is_last = place == 0, place == total - 1
    opens, closes = jnp.logical_and(x == 0, y == 0), jnp.logical_and(x == nx - 1, y == ny - 1)
    opens_later, closes_early = jnp.logical_and(opens, place > 0), jnp.logical_and(closes, place < total - 1)
    takes_back, takes_next = jnp.logical_not(opens), jnp.logical_not(closes)

    def at(number, core):
        return (number // (ny * nx), (number // nx) % ny, number % nx, core)

    after = at(jnp.minimum(place + 1, total - 1), tp)
    before = at(jnp.maximum(place - 1, 0), tp)

    def along(axis, offset, core=1):
        if axis == 0:
            return (lax.rem(z + offset, nz), y, x, core)
        if axis == 1:
            return (z, lax.rem(y + offset, ny), x, core)
        return (z, y, lax.rem(x + offset, nx), core)

    def signal(sem, target):
        pl.semaphore_signal(sem, inc=1, device_id=target, device_id_type=pl.DeviceIdType.MESH)

    def remote(src, dst, send, recv, target):
        return pltpu.make_async_remote_copy(
            src_ref=src, dst_ref=dst, send_sem=send, recv_sem=recv,
            device_id=target, device_id_type=pl.DeviceIdType.MESH)

    def wait_bytes(ref, sem):
        pltpu.make_async_copy(ref, ref, sem).wait()

    barrier = pltpu.get_barrier_semaphore()

    @pl.when(place > 0)
    def _():
        signal(barrier, before)

    @pl.when(place < total - 1)
    def _():
        signal(barrier, after)

    sides = jnp.where(is_first, 0, 1) + jnp.where(is_last, 0, 1)
    small_loads = [pltpu.make_async_copy(gains_hbm, gains_v, gains_sem), pltpu.make_async_copy(table_hbm, table_v, table_sem)]
    for load in small_loads:
        load.start()
    for h in range(HEADS):
        lanes = slice(h * HEAD_DIM, (h + 1) * HEAD_DIM)
        pltpu.make_async_copy(k_hbm.at[:, lanes], k_raw.at[h], load_sem.at[0]).start()
        pltpu.make_async_copy(q_hbm.at[:, lanes], q_raw.at[h], load_sem.at[0]).start()
        pltpu.make_async_copy(v_hbm.at[:, lanes], kvx.at[1, h, BEFORE:BEFORE + ROWS], load_sem.at[0]).start()
        pltpu.make_async_copy(do_hbm.at[:SEG, lanes], qd0.at[1, h], load_sem.at[0]).start()
        pltpu.make_async_copy(do_hbm.at[SEG:, lanes], qdx.at[1, h, :BEFORE], load_sem.at[1]).start()

    close = [(a, o) for a, n in enumerate(sizes) for o in near(n)]

    @pl.when(tp == 1)
    def _():
        for a, o in close:
            signal(barrier, along(a, o))
        signal(barrier, (z, y, x, 0))

    @pl.when(tp == 0)
    def _():
        signal(barrier, (z, y, x, 1))

    for load in small_loads:
        load.wait()
    gains = gains_v[...]
    gain_q, gain_k = gains[0:1, :], gains[1:2, :]
    wait_bytes(kvx.at[:, :, :ROWS + PAIR + SEG // 2], load_sem.at[0])
    def norm_keys(first, size):
        for h in range(HEADS):
            u, r = unit(k_raw[h, first:first + size])
            ku[h, first:first + size] = u
            kr[h, first:first + size] = jnp.broadcast_to(r, u.shape)
            kvx[0, h, BEFORE + first:BEFORE + first + size] = (u * gain_k).astype(BF16)

    def norm_queries(first, size, out):
        for h in range(HEADS):
            u, r = unit(q_raw[h, first:first + size])
            qu[h, first:first + size] = u
            qr[h, first:first + size] = jnp.broadcast_to(r, u.shape)
            out[h] = (u * gain_q).astype(BF16)

    forth = [remote(
        kvx.at[:, :, ROWS + PAIR:ROWS + BEFORE], kvx.at[:, :, PAIR:BEFORE], halo_send.at[0], left_recv.at[HEADS], after)]
    back = {}
    for h in range(HEADS):
        forth.append(remote(
            kvx.at[:, h, ROWS:ROWS + PAIR], kvx.at[:, h, :PAIR], halo_send.at[0], left_recv.at[h], after))
        back[h] = [
            remote(kvx.at[:, h, BEFORE:ROWS], kvx.at[:, h, BEFORE + ROWS:], halo_send.at[1], right_recv.at[h], before),
            remote(qd0.at[:, h], qdx.at[:, h, BEFORE:], halo_send.at[1], right_recv.at[h], before)]

    plane_piece = remote(kvx.at[:, :, BEFORE:ROWS], first_kv, halo_send.at[0], left_recv.at[HEADS + 1], after)

    def go_on(pieces, when=place < total - 1):
        @pl.when(when)
        def _():
            for copy in pieces:
                copy.start()

    norm_keys(BEFORE, SEG)
    pl.semaphore_wait(barrier, sides + jnp.where(tp == 1, 1 + len(close), 1))
    go_on(forth[:1])
    norm_keys(0, SEG)
    norm_queries(0, SEG, qd0.at[0])

    go_on([copy for h in range(HEADS) for copy in back[h]], takes_back)
    norm_keys(SEG, PAIR)
    go_on(forth[1:])
    go_on([plane_piece], closes_early)
    norm_queries(SEG, BEFORE, qdx.at[0, :, :BEFORE])

    @pl.when(tp == 1)
    def _():
        for a, o in close:
            signal(round1, along(a, o))

    wait_bytes(qdx.at[1, :, :BEFORE], load_sem.at[1])

    @pl.when(is_first)
    def _():
        for h in range(HEADS):
            for n in range(2):
                kvx[n, h, :BEFORE] = kvx[n, h, BEFORE:2 * BEFORE]
                first_kv[n, h] = kvx[n, h, BEFORE:ROWS]

    @pl.when(opens)
    def _():
        extra_gain[...] = jnp.zeros((1, HEAD_DIM), F32)

    @pl.when(closes)
    def _():
        for h in range(HEADS):
            for n in range(2):
                kvx[n, h, BEFORE + ROWS:] = kvx[n, h, BEFORE:ROWS]
            qdx[0, h, BEFORE:] = qd0[0, h]
            qdx[1, h, BEFORE:] = jnp.zeros((SEG, HEAD_DIM), BF16)

    @pl.when(is_last)
    def _():
        for h in range(HEADS):
            for n in range(2):
                from_after[n, h] = jnp.zeros((BEFORE, HEAD_DIM), BF16)

    key_at = lax.broadcasted_iota(jnp.int32, (PAIR, PAIR), 0)
    query_at = lax.broadcasted_iota(jnp.int32, (PAIR, PAIR), 1)
    past = query_at >= key_at
    early = query_at < SEG
    high = key_at >= SEG
    lane = lax.broadcasted_iota(jnp.int32, (1, PAIR), 1)
    table = table_v[...]
    low_part = table[:, :PAIR]
    high_part = jnp.concatenate([table[:, PAIR:], jnp.zeros((HEADS, 2 * PAIR - ENTRIES), F32)], axis=1)
    low_rolled = pltpu.roll(low_part, PAIR - SEG + 1, 1)
    high_rolled = pltpu.roll(high_part, PAIR - SEG + 1, 1)
    for h in range(HEADS):
        last = table[h:h + 1, ENTRIES - 1:ENTRIES]
        dist_low = low_rolled[h:h + 1]
        dist_row = jnp.where(lane <= SEG, dist_low, high_rolled[h:h + 1])
        ahead = pltpu.roll(jnp.broadcast_to(dist_low, (PAIR, PAIR)), 0, 1, stride=1, stride_axis=0)
        behind = pltpu.roll(jnp.broadcast_to(dist_row, (PAIR, PAIR)), 0, 1, stride=1, stride_axis=0)
        tile0 = jnp.where(jnp.logical_or(early, high), last, MASKED)
        tile1 = jnp.where(past, last, behind)
        tile2 = jnp.where(jnp.logical_and(early, high), MASKED, jnp.where(past, behind, ahead))
        none, low = (jnp.where(is_first, MASKED, t) for t in (tile0, tile1))
        for p, tiles in enumerate((
                (none, jnp.where(high, tile1, low), tile2),
                (jnp.where(high, tile0, none), tile1, tile2))):
            top = jnp.max(jnp.maximum(jnp.maximum(tiles[0], tiles[1]), tiles[2]), axis=0, keepdims=True)
            for b, tile in enumerate(tiles):
                bias_v[h, p, b * PAIR:(b + 1) * PAIR] = (tile - top) * LOG2E

    def block(h, p, b):
        first = (p + b) * PAIR
        own = slice(p * PAIR, (p + 1) * PAIR)
        s = dot(kvx[0, h, first:first + PAIR], qdx[0, h, own], 1, 1)
        e = jnp.exp2(s * (FACTOR * LOG2E) + bias_v[h, p, b * PAIR:(b + 1) * PAIR])
        dp = dot(kvx[1, h, first:first + PAIR], qdx[1, h, own], 1, 1)
        e_v[h, p, b * PAIR:(b + 1) * PAIR] = e
        dp_v[h, p, b * PAIR:(b + 1) * PAIR] = dp
        sum_v[h, p, b] = jnp.sum(e, axis=0, keepdims=True)
        sum_v[h, p, 3 + b] = jnp.sum(e * dp, axis=0, keepdims=True)

    def finish(h, p, again):
        inv = 1.0 / (sum_v[h, p, 0] + sum_v[h, p, 1] + sum_v[h, p, 2])
        delta = (sum_v[h, p, 3] + sum_v[h, p, 4] + sum_v[h, p, 5]) * inv
        own = slice(p * PAIR, (p + 1) * PAIR)
        keys = slice(p * PAIR, (p + 3) * PAIR)
        prob = e_v[h, p] * inv
        d_score = prob * (dp_v[h, p] - delta)
        prob_low = prob.astype(BF16)
        d_low = d_score.astype(BF16)
        prob_v[h, p] = prob_low
        d_low_v[h, p] = d_low
        dk = dot(d_low, qdx[0, h, own], 1, 0)
        gain_v[h, p] = jnp.sum(dk * kvx[0, h, keys].astype(F32), axis=0, keepdims=True)
        if again:
            shared, alone = slice(PAIR, 3 * PAIR), slice(3 * p * PAIR, (3 * p + 1) * PAIR)
            ours = slice((1 - p) * PAIR, (3 - p) * PAIR)
            rest = slice(2 * p * PAIR, (2 * p + 1) * PAIR)
            dkx[h, alone] = dk[rest]
            dkx[h, shared] = dkx[h, shared] + dk[ours]
            return d_v[h] + d_score
        dkx[h, keys] = dk
        d_v[h] = d_score

    def query_rows(g, u, r):
        g = g * FACTOR * gain_q
        return (r * (g - u * jnp.mean(g * u, axis=-1, keepdims=True))).astype(BF16)

    sublane = lax.broadcasted_iota(jnp.int32, (8, PAIR), 0)

    def skewed_sum(tile, right):
        parts = [pltpu.roll(tile[first:first + 8], (right - first) % PAIR, 1) for first in range(0, PAIR, 8)]
        while len(parts) > 1:
            parts = [a + b for a, b in zip(parts[::2], parts[1::2])]
        total = parts[0]
        for bit in range(1, 8):
            total = jnp.where(sublane == bit, pltpu.roll(parts[0], PAIR - bit, 1), total)
        return jnp.sum(total, axis=0, keepdims=True)

    def fold_rows(h, d_score):
        d0, d1, d2 = (d_score[b * PAIR:(b + 1) * PAIR] for b in range(3))
        mixed = jnp.where(past, d2, d1)
        ahead = jnp.where(past, 0.0, d2)
        rest = d0 + jnp.where(past, d1, 0.0)
        behind_row, ahead_row = skewed_sum(mixed, SEG - 1), skewed_sum(ahead, SEG - 1)
        high_row = skewed_sum(mixed, SEG - 1 + SEG) if h else behind_row
        rest_sum = jnp.sum(jnp.sum(rest, axis=0, keepdims=True), axis=1, keepdims=True)
        return (
            jnp.where(lane < SEG - 1, ahead_row, behind_row),
            jnp.where(lane == SEG - 1 + h * SEG, rest_sum, high_row))

    def fold_table(h, d_score):
        table_v2[h, 0], table_v2[h, 1] = fold_rows(h, d_score)

    def first_segment(h):
        queries, cotangents = qd0[0, h], qd0[1, h]
        keys, rest = first_kv[0, h], kvx[0, h, :ROWS]
        key_number = lax.broadcasted_iota(jnp.int32, (ROWS + SEG, SEG), 0)
        bias = bias_v[h, 0, :ROWS + SEG][:, :SEG]
        bias = jnp.where(jnp.logical_and(is_first, key_number < ROWS), MASKED, bias)
        bias = bias - jnp.max(bias, axis=0, keepdims=True)
        s = jnp.concatenate([dot(keys, queries, 1, 1), dot(rest, queries, 1, 1)], axis=0)
        e = jnp.exp2(s * (FACTOR * LOG2E) + bias)
        dp = jnp.concatenate([dot(first_kv[1, h], cotangents, 1, 1), dot(kvx[1, h, :ROWS], cotangents, 1, 1)], axis=0)
        inv = 1.0 / jnp.sum(e, axis=0, keepdims=True)
        delta = jnp.sum(e * dp, axis=0, keepdims=True) * inv
        prob = e * inv
        d_score = prob * (dp - delta)
        d_low = d_score.astype(BF16)
        dk = dot(d_low, queries, 1, 0)
        dv = dot(prob.astype(BF16), cotangents, 1, 0)
        dq_from_before[h] = dot(d_low[:SEG], keys, 0, 0) + dot(d_low[SEG:], rest, 0, 0)
        for n, part in enumerate((dk * FACTOR, dv)):
            to_before_first[n, h] = part[:SEG].astype(BF16)
            from_before[n, h] = part[ROWS:].astype(BF16)
        dkx[h, :BEFORE] = dkx[h, :BEFORE] + dk[SEG:ROWS]
        extra_dv[h] = dv[SEG:ROWS]
        extra_gain[...] = extra_gain[...] + (
            jnp.sum(dk[:SEG] * keys.astype(F32), axis=0, keepdims=True)
            + jnp.sum(dk[SEG:] * rest.astype(F32), axis=0, keepdims=True))
        tile = jnp.concatenate([d_score, jnp.zeros((ROWS + SEG, SEG), F32)], axis=1)
        rows = fold_rows(h, jnp.concatenate([tile, jnp.zeros((SEG, PAIR), F32)], axis=0))
        for j in range(2):
            table_v2[h, j] = table_v2[h, j] + rows[j]

    for h in range(HEADS):
        block(h, 0, 2)

    @pl.when(tp == 1)
    def _():
        pl.semaphore_wait(round1, len(close))
        signal(row_sem, (z, y, x, 0))
        for a, n in enumerate(sizes[:2]):
            if n > 5:
                for o in near(n, 2):
                    signal(round2, along(a, o))

    def wait_left(piece):
        @pl.when(place > 0)
        def _():
            forth[piece].wait_recv()

    def wait_right(h):
        @pl.when(takes_next)
        def _():
            wait_bytes(kvx.at[:, h, :PAIR], right_recv.at[h])

    def greet_far():
        @pl.when(tp == 1)
        def _():
            count = sum(len(near(n, 2)) for n in sizes[:2] if n > 5)
            if count:
                pl.semaphore_wait(round2, count)
            if nz > 9:
                for o in near(nz, 3):
                    signal(round3, along(0, o))

    def do_first():
        @pl.when(opens)
        def _():
            @pl.when(place > 0)
            def _():
                plane_piece.wait_recv()

            for h in range(HEADS):
                first_segment(h)

    @pl.when(x == nx - 1)
    def _():
        wait_left(0)
        for h in range(HEADS):
            block(h, 0, 1)
        for h in range(HEADS):
            wait_left(1 + h)
            block(h, 0, 0)
            finish(h, 0, False)
        greet_far()
        for h in range(HEADS):
            wait_right(h)
            block(h, 1, 1)
            block(h, 1, 2)
            block(h, 1, 0)
            fold_table(h, finish(h, 1, True))
        if nx == 1:
            do_first()

    if nx > 1:
        @pl.when(x == 0)
        def _():
            for h in range(HEADS):
                wait_right(h)
            for h in range(HEADS):
                block(h, 1, 1)
                block(h, 1, 2)
            wait_left(0)
            for h in range(HEADS):
                block(h, 0, 1)
                block(h, 1, 0)
                finish(h, 1, False)
            greet_far()
            for h in range(HEADS):
                wait_left(1 + h)
                block(h, 0, 0)
                fold_table(h, finish(h, 0, True))
            do_first()

    if nx > 2:
        @pl.when(jnp.logical_and(x > 0, x < nx - 1))
        def _():
            wait_left(0)
            for h in range(HEADS):
                block(h, 0, 1)
            for h in range(HEADS):
                wait_right(h)
                block(h, 1, 1)
                block(h, 1, 2)
                block(h, 1, 0)
                finish(h, 1, False)
                if h:
                    greet_far()
                wait_left(1 + h)
                block(h, 0, 0)
                fold_table(h, finish(h, 0, True))

    row = lax.broadcasted_iota(jnp.int32, (8, HEAD_DIM), 0)
    vec = jnp.zeros((8, HEAD_DIM), F32)
    second = jnp.where(lane < SEG, table_v2[0, 1], table_v2[1, 1])
    for j, part in enumerate((table_v2[0, 0], table_v2[1, 0], second)):
        vec = jnp.where(row == 3 * tp + j, part, vec)
    part = gain_v[0, 0] + gain_v[0, 1] + gain_v[1, 0] + gain_v[1, 1] + jnp.where(opens, extra_gain[...], 0.0)
    vec = jnp.where(row == 6, part * FACTOR, vec)
    mine = 2 * x + tp
    lines[mine] = vec[:7]

    to_neighbours = [
        remote(to_before.at[:, h], from_after.at[:, h], back_send.at[0], after_recv.at[h], before) for h in range(HEADS)]
    to_next = [
        remote(to_after, from_before, back_send.at[1], before_recv, after),
        remote(dqx.at[:, BEFORE:], dq_from_before, back_send.at[1], before_recv, after)]
    to_plane_before = remote(to_before_first, from_after_first, back_send.at[0], first_recv, before)

    def stage_results():
        for h in range(HEADS):
            low, high_tile = (dot(prob_v[h, p], qdx[1, h, p * PAIR:(p + 1) * PAIR], 1, 0) for p in range(2))
            dvx[h, :PAIR] = low[:PAIR]
            dvx[h, PAIR:3 * PAIR] = low[PAIR:] + high_tile[:2 * PAIR]
            dvx[h, 3 * PAIR:] = high_tile[2 * PAIR:]

            @pl.when(opens)
            def _(h=h):
                dvx[h, :BEFORE] = dvx[h, :BEFORE] + extra_dv[h]

            lanes = slice(h * HEAD_DIM, (h + 1) * HEAD_DIM)
            to_before[0, h] = (dkx[h, :BEFORE] * FACTOR).astype(BF16)
            to_before[1, h] = dvx[h, :BEFORE].astype(BF16)
            to_after[0, h] = (dkx[h, BEFORE + ROWS:] * FACTOR).astype(BF16)
            to_after[1, h] = dvx[h, BEFORE + ROWS:].astype(BF16)
            for p in range(2):
                dqx[h, p * PAIR:(p + 1) * PAIR] = dot(d_low_v[h, p], kvx[0, h, p * PAIR:(p + 3) * PAIR], 0, 0)
            dq_v[SEG:, lanes] = query_rows(dqx[h, :BEFORE], qu[h, SEG:], qr[h, SEG:])

    def send_results(when):
        @pl.when(jnp.logical_and(when, place > 0))
        def _():
            for copy in to_neighbours:
                copy.start()

        @pl.when(jnp.logical_and(when, opens_later))
        def _():
            to_plane_before.start()

        @pl.when(jnp.logical_and(when, takes_next))
        def _():
            for copy in to_next:
                copy.start()

    def line_sum(first, count):
        part = lines[first]
        for n in range(first + 1, first + count):
            part = part + lines[n]
        return part

    ys, zs = 2 * nx, 2 * nx + ny
    at_end = jnp.logical_or(x == 0, x == nx - 1)

    @pl.when(tp == 1)
    def _():
        for o in far_first(nx):
            remote(lines.at[mine], lines.at[mine], xy_send, x_recv, along(2, o)).start()
        stage_results()
        send_results(jnp.logical_not(at_end))
        wait_bytes(lines.at[:2 * nx - 1], x_recv)
        lines[ys + y] = line_sum(0, 2 * nx)
        for o in far_first(ny):
            remote(lines.at[ys + y], lines.at[ys + y], xy_send, y_recv, along(1, o)).start()
        send_results(at_end)
        if ny > 1:
            wait_bytes(lines.at[:ny - 1], y_recv)
        part = line_sum(ys, ny)
        for core in range(2):
            zout[core, :3] = part[3 * core:3 * core + 3]
            zout[core, 3:] = part[6:]
        zbuf[z] = zout[1]
        if nz > 9:
            pl.semaphore_wait(round3, len(near(nz, 3)))
        for o in [*far_first(nz), 0]:
            for core in range(2 if o else 1):
                remote(zout.at[core], zbuf.at[z], z_send, z_recv, along(0, o, core)).start()

    @pl.when(tp == 0)
    def _():
        pl.semaphore_wait(row_sem, 1)
        for o in [*far_first(nx), 0]:
            remote(lines.at[mine], lines.at[mine], xy_send, x_recv, along(2, o)).start()
        stage_results()
        send_results(place >= 0)

    @pl.when(takes_back)
    def _():
        wait_bytes(kvx.at[:, :, :PAIR], before_recv)

    @pl.when(closes_early)
    def _():
        to_plane_before.wait_recv()

    for h in range(HEADS):
        dq_v[:SEG, h * HEAD_DIM:(h + 1) * HEAD_DIM] = query_rows(dq_from_before[h], qu[h, :SEG], qr[h, :SEG])

    for h in range(HEADS):
        @pl.when(place < total - 1)
        def _(h=h):
            to_neighbours[h].wait_recv()

        lanes = slice(h * HEAD_DIM, (h + 1) * HEAD_DIM)
        sums_in = [
            jnp.concatenate([
                jnp.where(takes_next, 0.0, jnp.where(is_last, 0.0, from_after_first[n, h].astype(F32)))
                + from_before[n, h].astype(F32), from_after[n, h].astype(F32)], axis=0) for n in range(2)]
        g = (dkx[h, BEFORE:BEFORE + ROWS] * FACTOR + sums_in[0]) * gain_k
        u = ku[h]
        dk_v[:, lanes] = (kr[h] * (g - u * jnp.mean(g * u, axis=-1, keepdims=True))).astype(BF16)
        dv_v[:, lanes] = (dvx[h, BEFORE:BEFORE + ROWS] + sums_in[1]).astype(BF16)

    @pl.when(takes_next)
    def _():
        wait_bytes(kvx.at[:, :, :BEFORE], halo_send.at[0])
        wait_bytes(kvx.at[:, :, :PAIR], back_send.at[1])

    @pl.when(closes_early)
    def _():
        wait_bytes(kvx.at[:, :, :ROWS], halo_send.at[0])

    @pl.when(takes_back)
    def _():
        wait_bytes(kvx.at[:, :, :PAIR], halo_send.at[1])
        wait_bytes(from_after, back_send.at[0])

    @pl.when(opens_later)
    def _():
        wait_bytes(kvx.at[:, :, :ROWS], back_send.at[0])

    @pl.when(tp == 1)
    def _():
        if nx + ny > 2:
            wait_bytes(lines.at[:nx + ny - 2], xy_send)
        wait_bytes(zbuf.at[:2 * nz - 1], z_send)
        if nz > 1:
            wait_bytes(zbuf.at[:nz - 1], z_recv)

    @pl.when(tp == 0)
    def _():
        wait_bytes(lines.at[:nx], xy_send)
        wait_bytes(zbuf.at[:nz], z_recv)

    result = zbuf[0]
    for n in range(1, nz):
        result = result + zbuf[n]
    for j in range(HEADS):
        dtab_v[j:j + 1, :PAIR] = result[j:j + 1]
        dtab_v[j:j + 1, PAIR:] = result[2:3, j * SEG:(j + 1) * SEG]
    dgain_v[0:1] = result[3:] / gain_q
    dgain_v[1:2] = result[3:] / gain_k


def write_out(*refs):
    count = len(refs) // 2
    copies = [pltpu.make_async_copy(refs[n], refs[count + n], refs[-1].at[n]) for n in range(count)]
    for copy in copies:
        copy.start()
    for copy in copies:
        copy.wait()


def local(sizes, queries, keys, values, gains, bias_table, d_out):
    nz, ny, nx = sizes
    width = HEADS * HEAD_DIM
    hbm_spec = pl.BlockSpec(memory_space=pltpu.HBM)
    vmem_spec = pl.BlockSpec(memory_space=pltpu.VMEM)
    first = (HEADS, SEG, HEAD_DIM)
    tile = (HEADS, ROWS, HEAD_DIM)
    wide = (HEADS, 2 * ROWS, HEAD_DIM)
    pairs = (HEADS, 2, 3 * PAIR, PAIR)
    dma, regular = pltpu.SemaphoreType.DMA, pltpu.SemaphoreType.REGULAR
    vmem = pltpu.VMEM
    outs = [((ROWS, width), BF16)] * 3 + [((HEADS, ENTRIES), F32), ((2, HEAD_DIM), F32)]
    out = pl.pallas_call(
        functools.partial(kernel, sizes),
        out_shape=tuple(vmem(*o) for o in outs),
        in_specs=[hbm_spec] * 6,
        out_specs=(vmem_spec,) * 5,
        scratch_shapes=[
            vmem(tile, BF16), vmem(tile, BF16), vmem((2, *tile), BF16), vmem((2, *first), BF16), vmem((2, *wide), BF16), vmem((2, *first), BF16),
            vmem((2, HEAD_DIM), F32), vmem((HEADS, ENTRIES), F32),
            vmem(tile, F32), vmem(tile, F32), vmem(tile, F32), vmem(tile, F32),
            vmem(pairs, F32), vmem(pairs, F32), vmem(pairs, F32),
            vmem(wide, F32), vmem(wide, F32), vmem(tile, F32), vmem((HEADS, 3 * PAIR, PAIR), F32),
            vmem(pairs, BF16), vmem(pairs, BF16), vmem((HEADS, 2, 6, 1, PAIR), F32), vmem((HEADS, 2, 1, PAIR), F32),
            vmem((HEADS, 2, 1, PAIR), F32), vmem((1, HEAD_DIM), F32), vmem((HEADS, BEFORE, HEAD_DIM), F32),
            vmem((2, HEADS, BEFORE, HEAD_DIM), BF16), vmem((2, HEADS, BEFORE, HEAD_DIM), BF16),
            vmem((2, *first), BF16), vmem((2, *first), BF16), vmem(first, F32), vmem((2, *first), BF16), vmem((2, *first), BF16),
            vmem((2 * nx + ny, 7, HEAD_DIM), F32), vmem((2, 4, HEAD_DIM), F32), vmem((2 * nz, 4, HEAD_DIM), F32),
            dma((2,)), dma, dma, dma((2,)), dma((HEADS + 2,)), dma((HEADS,)), dma((2,)), dma((HEADS,)), dma, dma,
            dma, dma, dma, dma, dma, regular, regular, regular, regular,
        ],
        compiler_params=pltpu.CompilerParams(
            collective_id=0, has_side_effects=True, vmem_limit_bytes=32 * 1024 * 1024),
        name="segment_attention_grad",
    )(*(pltpu.with_memory_space_constraint(a, pltpu.HBM) for a in (queries, keys, values, d_out, gains, bias_table.T)))
    d_queries, d_keys, d_values, d_table, d_gains = pl.pallas_call(
        write_out,
        out_shape=tuple(jax.ShapeDtypeStruct(*o) for o in outs),
        in_specs=[vmem_spec] * 5,
        out_specs=(hbm_spec,) * 5,
        scratch_shapes=[dma((5,))],
        name="write_out",
    )(*(pltpu.with_memory_space_constraint(o, pltpu.VMEM) for o in out))
    return d_queries, d_keys, d_values, d_table.T, d_gains


def solution(mesh):
    shape = (12, 8, 4)
    if mesh.shape["sp"] != int(np.prod(shape)):
        shape = mesh.small_shape
    split = Mesh(mesh.devices.reshape(*shape, mesh.shape["tp"]), AXES)
    placed = (P(SP, "tp"), P(SP, "tp"), P(SP, "tp"), P(), P(None, "tp"), P(SP, "tp"))
    return jax.shard_map(
        functools.partial(local, shape),
        mesh=split,
        in_specs=placed,
        out_specs=(P(SP, "tp"), P(SP, "tp"), P(SP, "tp"), P(None, "tp"), P()),
        check_vma=False,
    )
```

```python
import functools

import jax
import jax.numpy as jnp
import numpy as np
from jax import lax
from jax.experimental import pallas as pl
from jax.experimental.pallas import tpu as pltpu
from jax.sharding import Mesh
from jax.sharding import PartitionSpec as P

HEAD_DIM = 128
SEG = 64
LEFT = 4
MAX_REL = 128
ENTRIES = MAX_REL + SEG
ROWS = LEFT * SEG
HEADS = 2
PAIR = 2 * SEG
BEFORE = 3 * SEG
AXES = ("sp_0", "sp_1", "sp_2", "tp")
SP = AXES[:3]

EPSILON = 1e-06
FACTOR = HEAD_DIM ** (-0.5)
LOG2E = 1.4426950408889634
MASKED = -1e30
F32, BF16 = jnp.float32, jnp.bfloat16


def dot(a, b, a_dim, b_dim):
    return lax.dot_general(a, b, (((a_dim,), (b_dim,)), ((), ())), preferred_element_type=F32)


def near(size, step=1):
    return sorted({step % size, -step % size} - {0})


def far_first(size):
    return sorted(range(1, size), key=lambda d: -min(d, size - d))


def unit(raw):
    wide = raw.astype(F32)
    inv_rms = lax.rsqrt(jnp.mean(wide * wide, axis=-1, keepdims=True) + EPSILON)
    return wide * inv_rms, inv_rms


def kernel(sizes, q_hbm, k_hbm, v_hbm, do_hbm, gains_hbm, table_hbm,
           dq_v, dk_v, dv_v, dtab_v, dgain_v,
           q_raw, k_raw, qdx, qd0, kvx, first_kv, gains_v, table_v,
           qu, qr, ku, kr, bias_v, e_v, dp_v,
           dkx, dvx, dqx, d_v, prob_v, d_low_v, sum_v, gain_v, table_v2, extra_gain, extra_dv,
           to_before, from_after, to_after, from_before, dq_from_before, to_before_first, from_after_first,
           lines, zout, zbuf,
           load_sem, gains_sem, table_sem, halo_send, left_recv, right_recv, back_send, after_recv, before_recv, first_recv,
           xy_send, x_recv, y_recv, z_send, z_recv, round1, round2, round3, row_sem):
    nz, ny, nx = sizes
    z, y, x, tp = (lax.axis_index(a) for a in AXES)
    place = (z * ny + y) * nx + x
    total = nz * ny * nx
    is_first, is_last = place == 0, place == total - 1
    opens, closes = jnp.logical_and(x == 0, y == 0), jnp.logical_and(x == nx - 1, y == ny - 1)
    opens_later, closes_early = jnp.logical_and(opens, place > 0), jnp.logical_and(closes, place < total - 1)
    takes_back, takes_next = jnp.logical_not(opens), jnp.logical_not(closes)

    def at(number, core):
        return (number // (ny * nx), (number // nx) % ny, number % nx, core)

    after = at(jnp.minimum(place + 1, total - 1), tp)
    before = at(jnp.maximum(place - 1, 0), tp)

    def along(axis, offset, core=1):
        if axis == 0:
            return (lax.rem(z + offset, nz), y, x, core)
        if axis == 1:
            return (z, lax.rem(y + offset, ny), x, core)
        return (z, y, lax.rem(x + offset, nx), core)

    def signal(sem, target):
        pl.semaphore_signal(sem, inc=1, device_id=target, device_id_type=pl.DeviceIdType.MESH)

    def remote(src, dst, send, recv, target):
        return pltpu.make_async_remote_copy(
            src_ref=src, dst_ref=dst, send_sem=send, recv_sem=recv,
            device_id=target, device_id_type=pl.DeviceIdType.MESH)

    def wait_bytes(ref, sem):
        pltpu.make_async_copy(ref, ref, sem).wait()

    barrier = pltpu.get_barrier_semaphore()

    @pl.when(place > 0)
    def _():
        signal(barrier, before)

    @pl.when(place < total - 1)
    def _():
        signal(barrier, after)

    sides = jnp.where(is_first, 0, 1) + jnp.where(is_last, 0, 1)
    small_loads = [pltpu.make_async_copy(gains_hbm, gains_v, gains_sem), pltpu.make_async_copy(table_hbm, table_v, table_sem)]
    for load in small_loads:
        load.start()
    for h in range(HEADS):
        lanes = slice(h * HEAD_DIM, (h + 1) * HEAD_DIM)
        pltpu.make_async_copy(k_hbm.at[:, lanes], k_raw.at[h], load_sem.at[0]).start()
        pltpu.make_async_copy(q_hbm.at[:, lanes], q_raw.at[h], load_sem.at[0]).start()
        pltpu.make_async_copy(v_hbm.at[:, lanes], kvx.at[1, h, BEFORE:BEFORE + ROWS], load_sem.at[0]).start()
        pltpu.make_async_copy(do_hbm.at[:SEG, lanes], qd0.at[1, h], load_sem.at[0]).start()
        pltpu.make_async_copy(do_hbm.at[SEG:, lanes], qdx.at[1, h, :BEFORE], load_sem.at[1]).start()

    close = [(a, o) for a, n in enumerate(sizes) for o in near(n)]

    @pl.when(tp == 1)
    def _():
        for a, o in close:
            signal(barrier, along(a, o))
        signal(barrier, (z, y, x, 0))

    @pl.when(tp == 0)
    def _():
        signal(barrier, (z, y, x, 1))

    for load in small_loads:
        load.wait()
    gains = gains_v[...]
    gain_q, gain_k = gains[0:1, :], gains[1:2, :]
    wait_bytes(kvx.at[:, :, :ROWS + PAIR + SEG // 2], load_sem.at[0])
    def norm_keys(first, size):
        for h in range(HEADS):
            u, r = unit(k_raw[h, first:first + size])
            ku[h, first:first + size] = u
            kr[h, first:first + size] = jnp.broadcast_to(r, u.shape)
            kvx[0, h, BEFORE + first:BEFORE + first + size] = (u * gain_k).astype(BF16)

    def norm_queries(first, size, out):
        for h in range(HEADS):
            u, r = unit(q_raw[h, first:first + size])
            qu[h, first:first + size] = u
            qr[h, first:first + size] = jnp.broadcast_to(r, u.shape)
            out[h] = (u * gain_q).astype(BF16)

    forth = [remote(
        kvx.at[:, :, ROWS + PAIR:ROWS + BEFORE], kvx.at[:, :, PAIR:BEFORE], halo_send.at[0], left_recv.at[HEADS], after)]
    back = {}
    for h in range(HEADS):
        forth.append(remote(
            kvx.at[:, h, ROWS:ROWS + PAIR], kvx.at[:, h, :PAIR], halo_send.at[0], left_recv.at[h], after))
        back[h] = [
            remote(kvx.at[:, h, BEFORE:ROWS], kvx.at[:, h, BEFORE + ROWS:], halo_send.at[1], right_recv.at[h], before),
            remote(qd0.at[:, h], qdx.at[:, h, BEFORE:], halo_send.at[1], right_recv.at[h], before)]

    plane_piece = remote(kvx.at[:, :, BEFORE:ROWS], first_kv, halo_send.at[0], left_recv.at[HEADS + 1], after)

    def go_on(pieces, when=place < total - 1):
        @pl.when(when)
        def _():
            for copy in pieces:
                copy.start()

    norm_keys(BEFORE, SEG)
    pl.semaphore_wait(barrier, sides + jnp.where(tp == 1, 1 + len(close), 1))
    go_on(forth[:1])
    norm_keys(0, SEG)
    norm_queries(0, SEG, qd0.at[0])

    go_on([copy for h in range(HEADS) for copy in back[h]], takes_back)
    norm_keys(SEG, PAIR)
    go_on(forth[1:], jnp.logical_and(tp == 0, place < total - 1))
    go_on(forth[1:2], jnp.logical_and(tp == 1, place < total - 1))
    go_on([plane_piece], closes_early)
    norm_queries(SEG, BEFORE, qdx.at[0, :, :BEFORE])

    @pl.when(tp == 1)
    def _():
        for a, o in close:
            signal(round1, along(a, o))

    wait_bytes(qdx.at[1, :, :BEFORE], load_sem.at[1])

    @pl.when(is_first)
    def _():
        for h in range(HEADS):
            for n in range(2):
                kvx[n, h, :BEFORE] = kvx[n, h, BEFORE:2 * BEFORE]
                first_kv[n, h] = kvx[n, h, BEFORE:ROWS]

    @pl.when(opens)
    def _():
        extra_gain[...] = jnp.zeros((1, HEAD_DIM), F32)

    @pl.when(closes)
    def _():
        for h in range(HEADS):
            for n in range(2):
                kvx[n, h, BEFORE + ROWS:] = kvx[n, h, BEFORE:ROWS]
            qdx[0, h, BEFORE:] = qd0[0, h]
            qdx[1, h, BEFORE:] = jnp.zeros((SEG, HEAD_DIM), BF16)

    @pl.when(is_last)
    def _():
        for h in range(HEADS):
            for n in range(2):
                from_after[n, h] = jnp.zeros((BEFORE, HEAD_DIM), BF16)

    key_at = lax.broadcasted_iota(jnp.int32, (PAIR, PAIR), 0)
    query_at = lax.broadcasted_iota(jnp.int32, (PAIR, PAIR), 1)
    past = query_at >= key_at
    early = query_at < SEG
    high = key_at >= SEG
    lane = lax.broadcasted_iota(jnp.int32, (1, PAIR), 1)
    table = table_v[...]
    low_part = table[:, :PAIR]
    high_part = jnp.concatenate([table[:, PAIR:], jnp.zeros((HEADS, 2 * PAIR - ENTRIES), F32)], axis=1)
    low_rolled = pltpu.roll(low_part, PAIR - SEG + 1, 1)
    high_rolled = pltpu.roll(high_part, PAIR - SEG + 1, 1)
    for h in range(HEADS):
        last = table[h:h + 1, ENTRIES - 1:ENTRIES]
        dist_low = low_rolled[h:h + 1]
        dist_row = jnp.where(lane <= SEG, dist_low, high_rolled[h:h + 1])
        ahead = pltpu.roll(jnp.broadcast_to(dist_low, (PAIR, PAIR)), 0, 1, stride=1, stride_axis=0)
        behind = pltpu.roll(jnp.broadcast_to(dist_row, (PAIR, PAIR)), 0, 1, stride=1, stride_axis=0)
        tile0 = jnp.where(jnp.logical_or(early, high), last, MASKED)
        tile1 = jnp.where(past, last, behind)
        tile2 = jnp.where(jnp.logical_and(early, high), MASKED, jnp.where(past, behind, ahead))
        none, low = (jnp.where(is_first, MASKED, t) for t in (tile0, tile1))
        for p, tiles in enumerate((
                (none, jnp.where(high, tile1, low), tile2),
                (jnp.where(high, tile0, none), tile1, tile2))):
            top = jnp.max(jnp.maximum(jnp.maximum(tiles[0], tiles[1]), tiles[2]), axis=0, keepdims=True)
            for b, tile in enumerate(tiles):
                bias_v[h, p, b * PAIR:(b + 1) * PAIR] = (tile - top) * LOG2E

    def work(blocks, tiles=()):
        at_keys = {(p, b): slice((p + b) * PAIR, (p + b + 1) * PAIR) for h, p, b in blocks}
        at_queries = [slice(p * PAIR, (p + 1) * PAIR) for p in range(2)]
        at_rows = [slice(b * PAIR, (b + 1) * PAIR) for b in range(3)]
        scores = [dot(kvx[0, h, at_keys[p, b]], qdx[0, h, at_queries[p]], 1, 1) for h, p, b in blocks]
        d_probs = [dot(kvx[1, h, at_keys[p, b]], qdx[1, h, at_queries[p]], 1, 1) for h, p, b in blocks]
        for (h, p, b), s, dp in zip(blocks, scores, d_probs):
            e = jnp.exp2(s * (FACTOR * LOG2E) + bias_v[h, p, at_rows[b]])
            e_v[h, p, at_rows[b]] = e
            dp_v[h, p, at_rows[b]] = dp
            sum_v[h, p, b] = jnp.sum(e, axis=0, keepdims=True)
            sum_v[h, p, 3 + b] = jnp.sum(e * dp, axis=0, keepdims=True)
        d_scores, products = [], []
        for h, p, _ in tiles:
            inv = 1.0 / (sum_v[h, p, 0] + sum_v[h, p, 1] + sum_v[h, p, 2])
            delta = (sum_v[h, p, 3] + sum_v[h, p, 4] + sum_v[h, p, 5]) * inv
            prob = e_v[h, p] * inv
            d_score = prob * (dp_v[h, p] - delta)
            d_low = d_score.astype(BF16)
            prob_v[h, p] = prob.astype(BF16)
            d_low_v[h, p] = d_low
            d_scores.append(d_score)
            products.append(dot(d_low, qdx[0, h, at_queries[p]], 1, 0))
        for (h, p, again), d_score in zip(tiles, d_scores):
            if again:
                fold_table(h, d_v[h] + d_score)
            else:
                d_v[h] = d_score
        for (h, p, again), dk in zip(tiles, products):
            keys = slice(p * PAIR, (p + 3) * PAIR)
            gain_v[h, p] = jnp.sum(dk * kvx[0, h, keys].astype(F32), axis=0, keepdims=True)
            if again:
                shared, alone = slice(PAIR, 3 * PAIR), slice(3 * p * PAIR, (3 * p + 1) * PAIR)
                dkx[h, alone] = dk[2 * p * PAIR:(2 * p + 1) * PAIR]
                dkx[h, shared] = dkx[h, shared] + dk[(1 - p) * PAIR:(3 - p) * PAIR]
            else:
                dkx[h, keys] = dk

    def query_rows(g, u, r):
        g = g * FACTOR * gain_q
        return (r * (g - u * jnp.mean(g * u, axis=-1, keepdims=True))).astype(BF16)

    sublane = lax.broadcasted_iota(jnp.int32, (8, PAIR), 0)

    def skewed_sum(tile, right):
        parts = [pltpu.roll(tile[first:first + 8], (right - first) % PAIR, 1) for first in range(0, PAIR, 8)]
        while len(parts) > 1:
            parts = [a + b for a, b in zip(parts[::2], parts[1::2])]
        total = parts[0]
        for bit in range(1, 8):
            total = jnp.where(sublane == bit, pltpu.roll(parts[0], PAIR - bit, 1), total)
        return jnp.sum(total, axis=0, keepdims=True)

    def fold_rows(h, d_score):
        d0, d1, d2 = (d_score[b * PAIR:(b + 1) * PAIR] for b in range(3))
        mixed = jnp.where(past, d2, d1)
        ahead = jnp.where(past, 0.0, d2)
        rest = d0 + jnp.where(past, d1, 0.0)
        behind_row, ahead_row = skewed_sum(mixed, SEG - 1), skewed_sum(ahead, SEG - 1)
        high_row = skewed_sum(mixed, SEG - 1 + SEG) if h else behind_row
        rest_sum = jnp.sum(jnp.sum(rest, axis=0, keepdims=True), axis=1, keepdims=True)
        return (
            jnp.where(lane < SEG - 1, ahead_row, behind_row),
            jnp.where(lane == SEG - 1 + h * SEG, rest_sum, high_row))

    def fold_table(h, d_score):
        table_v2[h, 0], table_v2[h, 1] = fold_rows(h, d_score)

    def first_segment(h):
        queries, cotangents = qd0[0, h], qd0[1, h]
        keys, rest = first_kv[0, h], kvx[0, h, :ROWS]
        key_number = lax.broadcasted_iota(jnp.int32, (ROWS + SEG, SEG), 0)
        bias = bias_v[h, 0, :ROWS + SEG][:, :SEG]
        bias = jnp.where(jnp.logical_and(is_first, key_number < ROWS), MASKED, bias)
        bias = bias - jnp.max(bias, axis=0, keepdims=True)
        s = jnp.concatenate([dot(keys, queries, 1, 1), dot(rest, queries, 1, 1)], axis=0)
        e = jnp.exp2(s * (FACTOR * LOG2E) + bias)
        dp = jnp.concatenate([dot(first_kv[1, h], cotangents, 1, 1), dot(kvx[1, h, :ROWS], cotangents, 1, 1)], axis=0)
        inv = 1.0 / jnp.sum(e, axis=0, keepdims=True)
        delta = jnp.sum(e * dp, axis=0, keepdims=True) * inv
        prob = e * inv
        d_score = prob * (dp - delta)
        d_low = d_score.astype(BF16)
        dk = dot(d_low, queries, 1, 0)
        dv = dot(prob.astype(BF16), cotangents, 1, 0)
        dq_from_before[h] = dot(d_low[:SEG], keys, 0, 0) + dot(d_low[SEG:], rest, 0, 0)
        for n, part in enumerate((dk * FACTOR, dv)):
            to_before_first[n, h] = part[:SEG].astype(BF16)
            from_before[n, h] = part[ROWS:].astype(BF16)
        dkx[h, :BEFORE] = dkx[h, :BEFORE] + dk[SEG:ROWS]
        extra_dv[h] = dv[SEG:ROWS]
        extra_gain[...] = extra_gain[...] + (
            jnp.sum(dk[:SEG] * keys.astype(F32), axis=0, keepdims=True)
            + jnp.sum(dk[SEG:] * rest.astype(F32), axis=0, keepdims=True))
        tile = jnp.concatenate([d_score, jnp.zeros((ROWS + SEG, SEG), F32)], axis=1)
        rows = fold_rows(h, jnp.concatenate([tile, jnp.zeros((SEG, PAIR), F32)], axis=0))
        for j in range(2):
            table_v2[h, j] = table_v2[h, j] + rows[j]

    heads = range(HEADS)
    work([(h, 0, 2) for h in heads])

    go_on(forth[2:], jnp.logical_and(tp == 1, place < total - 1))
    @pl.when(tp == 1)
    def _():
        pl.semaphore_wait(round1, len(close))
        signal(row_sem, (z, y, x, 0))
        for a, n in enumerate(sizes[:2]):
            if n > 5:
                for o in near(n, 2):
                    signal(round2, along(a, o))

    def wait_left(piece):
        @pl.when(place > 0)
        def _():
            forth[piece].wait_recv()

    def wait_right(h):
        @pl.when(takes_next)
        def _():
            wait_bytes(kvx.at[:, h, :PAIR], right_recv.at[h])

    def greet_far():
        @pl.when(tp == 1)
        def _():
            count = sum(len(near(n, 2)) for n in sizes[:2] if n > 5)
            if count:
                pl.semaphore_wait(round2, count)
            if nz > 9:
                for o in near(nz, 3):
                    signal(round3, along(0, o))

    def do_first():
        @pl.when(opens)
        def _():
            @pl.when(place > 0)
            def _():
                plane_piece.wait_recv()

            for h in range(HEADS):
                first_segment(h)

    @pl.when(x == nx - 1)
    def _():
        wait_left(0)
        work([(h, 0, 1) for h in heads])
        for h in heads:
            wait_left(1 + h)
            work([(h, 0, 0)], [(h, 0, False)])
        greet_far()
        for h in heads:
            wait_right(h)
        work([(h, 1, b) for b in range(3) for h in heads], [(h, 1, True) for h in heads])
        if nx == 1:
            do_first()

    if nx > 1:
        @pl.when(x == 0)
        def _():
            for h in heads:
                wait_right(h)
            work([(h, 1, b) for b in (1, 2) for h in heads])
            wait_left(0)
            work([(h, p, 1 - p) for p in (1, 0) for h in heads], [(h, 1, False) for h in heads])
            greet_far()
            for h in heads:
                wait_left(1 + h)
                work([(h, 0, 0)], [(h, 0, True)])
            do_first()

    if nx > 2:
        @pl.when(jnp.logical_and(x > 0, x < nx - 1))
        def _():
            wait_left(0)
            work([(h, 0, 1) for h in heads])
            for h in heads:
                wait_right(h)
            work([(h, 1, b) for b in range(3) for h in heads], [(h, 1, False) for h in heads])
            greet_far()
            for h in heads:
                wait_left(1 + h)
                work([(h, 0, 0)], [(h, 0, True)])

    row = lax.broadcasted_iota(jnp.int32, (8, HEAD_DIM), 0)
    vec = jnp.zeros((8, HEAD_DIM), F32)
    second = jnp.where(lane < SEG, table_v2[0, 1], table_v2[1, 1])
    for j, part in enumerate((table_v2[0, 0], table_v2[1, 0], second)):
        vec = jnp.where(row == 3 * tp + j, part, vec)
    part = gain_v[0, 0] + gain_v[0, 1] + gain_v[1, 0] + gain_v[1, 1] + jnp.where(opens, extra_gain[...], 0.0)
    vec = jnp.where(row == 6, part * FACTOR, vec)
    mine = 2 * x + tp
    lines[mine] = vec[:7]

    to_neighbours = [
        remote(to_before.at[:, h], from_after.at[:, h], back_send.at[0], after_recv.at[h], before) for h in range(HEADS)]
    to_next = [
        remote(to_after, from_before, back_send.at[1], before_recv, after),
        remote(dqx.at[:, BEFORE:], dq_from_before, back_send.at[1], before_recv, after)]
    to_plane_before = remote(to_before_first, from_after_first, back_send.at[0], first_recv, before)

    def stage_results():
        for h in range(HEADS):
            low, high_tile = (dot(prob_v[h, p], qdx[1, h, p * PAIR:(p + 1) * PAIR], 1, 0) for p in range(2))
            dvx[h, :PAIR] = low[:PAIR]
            dvx[h, PAIR:3 * PAIR] = low[PAIR:] + high_tile[:2 * PAIR]
            dvx[h, 3 * PAIR:] = high_tile[2 * PAIR:]

            @pl.when(opens)
            def _(h=h):
                dvx[h, :BEFORE] = dvx[h, :BEFORE] + extra_dv[h]

            lanes = slice(h * HEAD_DIM, (h + 1) * HEAD_DIM)
            to_before[0, h] = (dkx[h, :BEFORE] * FACTOR).astype(BF16)
            to_before[1, h] = dvx[h, :BEFORE].astype(BF16)
            to_after[0, h] = (dkx[h, BEFORE + ROWS:] * FACTOR).astype(BF16)
            to_after[1, h] = dvx[h, BEFORE + ROWS:].astype(BF16)
            for p in range(2):
                dqx[h, p * PAIR:(p + 1) * PAIR] = dot(d_low_v[h, p], kvx[0, h, p * PAIR:(p + 3) * PAIR], 0, 0)
            dq_v[SEG:, lanes] = query_rows(dqx[h, :BEFORE], qu[h, SEG:], qr[h, SEG:])

    def send_results(when):
        @pl.when(jnp.logical_and(when, place > 0))
        def _():
            for copy in to_neighbours:
                copy.start()

        @pl.when(jnp.logical_and(when, opens_later))
        def _():
            to_plane_before.start()

        @pl.when(jnp.logical_and(when, takes_next))
        def _():
            for copy in to_next:
                copy.start()

    def line_sum(first, count):
        part = lines[first]
        for n in range(first + 1, first + count):
            part = part + lines[n]
        return part

    ys, zs = 2 * nx, 2 * nx + ny
    at_end = jnp.logical_or(x == 0, x == nx - 1)

    @pl.when(tp == 1)
    def _():
        for o in far_first(nx):
            remote(lines.at[mine], lines.at[mine], xy_send, x_recv, along(2, o)).start()
        stage_results()
        wait_bytes(lines.at[:2 * nx - 1], x_recv)
        lines[ys + y] = line_sum(0, 2 * nx)
        for o in far_first(ny):
            remote(lines.at[ys + y], lines.at[ys + y], xy_send, y_recv, along(1, o)).start()
        if ny > 1:
            wait_bytes(lines.at[:ny - 1], y_recv)
        part = line_sum(ys, ny)
        for core in range(2):
            zout[core, :3] = part[3 * core:3 * core + 3]
            zout[core, 3:] = part[6:]
        zbuf[z] = zout[1]
        if nz > 9:
            pl.semaphore_wait(round3, len(near(nz, 3)))
        for o in [*far_first(nz), 0]:
            for core in range(2 if o else 1):
                remote(zout.at[core], zbuf.at[z], z_send, z_recv, along(0, o, core)).start()
        send_results(place >= 0)
        signal(row_sem, (z, y, x, 0))

    @pl.when(tp == 0)
    def _():
        pl.semaphore_wait(row_sem, 1)
        for o in [*far_first(nx), 0]:
            remote(lines.at[mine], lines.at[mine], xy_send, x_recv, along(2, o)).start()
        stage_results()
        pl.semaphore_wait(row_sem, 1)
        send_results(place >= 0)

    @pl.when(takes_back)
    def _():
        wait_bytes(kvx.at[:, :, :PAIR], before_recv)

    @pl.when(closes_early)
    def _():
        to_plane_before.wait_recv()

    for h in range(HEADS):
        dq_v[:SEG, h * HEAD_DIM:(h + 1) * HEAD_DIM] = query_rows(dq_from_before[h], qu[h, :SEG], qr[h, :SEG])

    for h in range(HEADS):
        @pl.when(place < total - 1)
        def _(h=h):
            to_neighbours[h].wait_recv()

        lanes = slice(h * HEAD_DIM, (h + 1) * HEAD_DIM)
        sums_in = [
            jnp.concatenate([
                jnp.where(takes_next, 0.0, jnp.where(is_last, 0.0, from_after_first[n, h].astype(F32)))
                + from_before[n, h].astype(F32), from_after[n, h].astype(F32)], axis=0) for n in range(2)]
        g = (dkx[h, BEFORE:BEFORE + ROWS] * FACTOR + sums_in[0]) * gain_k
        u = ku[h]
        dk_v[:, lanes] = (kr[h] * (g - u * jnp.mean(g * u, axis=-1, keepdims=True))).astype(BF16)
        dv_v[:, lanes] = (dvx[h, BEFORE:BEFORE + ROWS] + sums_in[1]).astype(BF16)

    @pl.when(takes_next)
    def _():
        wait_bytes(kvx.at[:, :, :BEFORE], halo_send.at[0])
        wait_bytes(kvx.at[:, :, :PAIR], back_send.at[1])

    @pl.when(closes_early)
    def _():
        wait_bytes(kvx.at[:, :, :ROWS], halo_send.at[0])

    @pl.when(takes_back)
    def _():
        wait_bytes(kvx.at[:, :, :PAIR], halo_send.at[1])
        wait_bytes(from_after, back_send.at[0])

    @pl.when(opens_later)
    def _():
        wait_bytes(kvx.at[:, :, :ROWS], back_send.at[0])

    @pl.when(tp == 1)
    def _():
        if nx + ny > 2:
            wait_bytes(lines.at[:nx + ny - 2], xy_send)
        wait_bytes(zbuf.at[:2 * nz - 1], z_send)
        if nz > 1:
            wait_bytes(zbuf.at[:nz - 1], z_recv)

    @pl.when(tp == 0)
    def _():
        wait_bytes(lines.at[:nx], xy_send)
        wait_bytes(zbuf.at[:nz], z_recv)

    result = zbuf[0]
    for n in range(1, nz):
        result = result + zbuf[n]
    for j in range(HEADS):
        dtab_v[j:j + 1, :PAIR] = result[j:j + 1]
        dtab_v[j:j + 1, PAIR:] = result[2:3, j * SEG:(j + 1) * SEG]
    dgain_v[0:1] = result[3:] / gain_q
    dgain_v[1:2] = result[3:] / gain_k


def write_out(*refs):
    count = len(refs) // 2
    copies = [pltpu.make_async_copy(refs[n], refs[count + n], refs[-1].at[n]) for n in range(count)]
    for copy in copies:
        copy.start()
    for copy in copies:
        copy.wait()


def local(sizes, queries, keys, values, gains, bias_table, d_out):
    nz, ny, nx = sizes
    width = HEADS * HEAD_DIM
    hbm_spec = pl.BlockSpec(memory_space=pltpu.HBM)
    vmem_spec = pl.BlockSpec(memory_space=pltpu.VMEM)
    first = (HEADS, SEG, HEAD_DIM)
    tile = (HEADS, ROWS, HEAD_DIM)
    wide = (HEADS, 2 * ROWS, HEAD_DIM)
    pairs = (HEADS, 2, 3 * PAIR, PAIR)
    dma, regular = pltpu.SemaphoreType.DMA, pltpu.SemaphoreType.REGULAR
    vmem = pltpu.VMEM
    outs = [((ROWS, width), BF16)] * 3 + [((HEADS, ENTRIES), F32), ((2, HEAD_DIM), F32)]
    out = pl.pallas_call(
        functools.partial(kernel, sizes),
        out_shape=tuple(vmem(*o) for o in outs),
        in_specs=[hbm_spec] * 6,
        out_specs=(vmem_spec,) * 5,
        scratch_shapes=[
            vmem(tile, BF16), vmem(tile, BF16), vmem((2, *tile), BF16), vmem((2, *first), BF16), vmem((2, *wide), BF16), vmem((2, *first), BF16),
            vmem((2, HEAD_DIM), F32), vmem((HEADS, ENTRIES), F32),
            vmem(tile, F32), vmem(tile, F32), vmem(tile, F32), vmem(tile, F32),
            vmem(pairs, F32), vmem(pairs, F32), vmem(pairs, F32),
            vmem(wide, F32), vmem(wide, F32), vmem(tile, F32), vmem((HEADS, 3 * PAIR, PAIR), F32),
            vmem(pairs, BF16), vmem(pairs, BF16), vmem((HEADS, 2, 6, 1, PAIR), F32), vmem((HEADS, 2, 1, PAIR), F32),
            vmem((HEADS, 2, 1, PAIR), F32), vmem((1, HEAD_DIM), F32), vmem((HEADS, BEFORE, HEAD_DIM), F32),
            vmem((2, HEADS, BEFORE, HEAD_DIM), BF16), vmem((2, HEADS, BEFORE, HEAD_DIM), BF16),
            vmem((2, *first), BF16), vmem((2, *first), BF16), vmem(first, F32), vmem((2, *first), BF16), vmem((2, *first), BF16),
            vmem((2 * nx + ny, 7, HEAD_DIM), F32), vmem((2, 4, HEAD_DIM), F32), vmem((2 * nz, 4, HEAD_DIM), F32),
            dma((2,)), dma, dma, dma((2,)), dma((HEADS + 2,)), dma((HEADS,)), dma((2,)), dma((HEADS,)), dma, dma,
            dma, dma, dma, dma, dma, regular, regular, regular, regular,
        ],
        compiler_params=pltpu.CompilerParams(
            collective_id=0, has_side_effects=True, vmem_limit_bytes=32 * 1024 * 1024),
        name="segment_attention_grad",
    )(*(pltpu.with_memory_space_constraint(a, pltpu.HBM) for a in (queries, keys, values, d_out, gains, bias_table.T)))
    d_queries, d_keys, d_values, d_table, d_gains = pl.pallas_call(
        write_out,
        out_shape=tuple(jax.ShapeDtypeStruct(*o) for o in outs),
        in_specs=[vmem_spec] * 5,
        out_specs=(hbm_spec,) * 5,
        scratch_shapes=[dma((5,))],
        name="write_out",
    )(*(pltpu.with_memory_space_constraint(o, pltpu.VMEM) for o in out))
    return d_queries, d_keys, d_values, d_table.T, d_gains


def solution(mesh):
    shape = (12, 8, 4)
    if mesh.shape["sp"] != int(np.prod(shape)):
        shape = mesh.small_shape
    split = Mesh(mesh.devices.reshape(*shape, mesh.shape["tp"]), AXES)
    placed = (P(SP, "tp"), P(SP, "tp"), P(SP, "tp"), P(), P(None, "tp"), P(SP, "tp"))
    return jax.shard_map(
        functools.partial(local, shape),
        mesh=split,
        in_specs=placed,
        out_specs=(P(SP, "tp"), P(SP, "tp"), P(SP, "tp"), P(None, "tp"), P()),
        check_vma=False,
    )
```

```python
import functools

import jax
import jax.numpy as jnp
import numpy as np
from jax import lax
from jax.experimental import pallas as pl
from jax.experimental.pallas import tpu as pltpu
from jax.sharding import Mesh
from jax.sharding import PartitionSpec as P

HEAD_DIM = 128
SEG = 64
LEFT = 4
MAX_REL = 128
ENTRIES = MAX_REL + SEG
ROWS = LEFT * SEG
HEADS = 2
PAIR = 2 * SEG
BEFORE = 3 * SEG
AXES = ("sp_0", "sp_1", "sp_2", "tp")
SP = AXES[:3]

EPSILON = 1e-06
FACTOR = HEAD_DIM ** (-0.5)
LOG2E = 1.4426950408889634
MASKED = -1e30
F32, BF16 = jnp.float32, jnp.bfloat16


def dot(a, b, a_dim, b_dim):
    return lax.dot_general(a, b, (((a_dim,), (b_dim,)), ((), ())), preferred_element_type=F32)


def near(size, step=1):
    return sorted({step % size, -step % size} - {0})


def far_first(size):
    return sorted(range(1, size), key=lambda d: -min(d, size - d))


def unit(raw):
    wide = raw.astype(F32)
    inv_rms = lax.rsqrt(jnp.mean(wide * wide, axis=-1, keepdims=True) + EPSILON)
    return wide * inv_rms, inv_rms


def kernel(sizes, q_hbm, k_hbm, v_hbm, do_hbm, gains_hbm, table_hbm,
           dq_v, dk_v, dv_v, dtab_v, dgain_v,
           q_raw, k_raw, qdx, qd0, kvx, first_kv, gains_v, table_v,
           qu, qr, ku, kr, bias_v, e_v, dp_v,
           dkx, dvx, dqx, d_v, prob_v, d_low_v, sum_v, gain_v, table_v2, extra_gain, extra_dv,
           to_before, from_after, to_after, from_before, dq_from_before, to_before_first, from_after_first,
           lines, plane, zout, zbuf,
           load_sem, gains_sem, table_sem, halo_send, left_recv, right_recv, back_send, after_recv, before_recv, first_recv,
           xy_send, x_recv, y_recv, plane_recv, z_send, z_recv, round1, round2, round3, plane_round):
    nz, ny, nx = sizes
    z, y, x, tp = (lax.axis_index(a) for a in AXES)
    place = (z * ny + y) * nx + x
    total = nz * ny * nx
    is_first, is_last = place == 0, place == total - 1
    opens, closes = jnp.logical_and(x == 0, y == 0), jnp.logical_and(x == nx - 1, y == ny - 1)
    opens_later, closes_early = jnp.logical_and(opens, place > 0), jnp.logical_and(closes, place < total - 1)
    takes_back, takes_next = jnp.logical_not(opens), jnp.logical_not(closes)

    def at(number, core):
        return (number // (ny * nx), (number // nx) % ny, number % nx, core)

    after = at(jnp.minimum(place + 1, total - 1), tp)
    before = at(jnp.maximum(place - 1, 0), tp)

    def along(axis, offset, core=1):
        if axis == 0:
            return (lax.rem(z + offset, nz), y, x, core)
        if axis == 1:
            return (z, lax.rem(y + offset, ny), x, core)
        return (z, y, lax.rem(x + offset, nx), core)

    def signal(sem, target):
        pl.semaphore_signal(sem, inc=1, device_id=target, device_id_type=pl.DeviceIdType.MESH)

    def remote(src, dst, send, recv, target):
        return pltpu.make_async_remote_copy(
            src_ref=src, dst_ref=dst, send_sem=send, recv_sem=recv,
            device_id=target, device_id_type=pl.DeviceIdType.MESH)

    def wait_bytes(ref, sem):
        pltpu.make_async_copy(ref, ref, sem).wait()

    barrier = pltpu.get_barrier_semaphore()

    @pl.when(place > 0)
    def _():
        signal(barrier, before)

    @pl.when(place < total - 1)
    def _():
        signal(barrier, after)

    sides = jnp.where(is_first, 0, 1) + jnp.where(is_last, 0, 1)
    small_loads = [pltpu.make_async_copy(gains_hbm, gains_v, gains_sem), pltpu.make_async_copy(table_hbm, table_v, table_sem)]
    for load in small_loads:
        load.start()
    for h in range(HEADS):
        lanes = slice(h * HEAD_DIM, (h + 1) * HEAD_DIM)
        pltpu.make_async_copy(k_hbm.at[:, lanes], k_raw.at[h], load_sem.at[0]).start()
        pltpu.make_async_copy(q_hbm.at[:, lanes], q_raw.at[h], load_sem.at[0]).start()
        pltpu.make_async_copy(v_hbm.at[:, lanes], kvx.at[1, h, BEFORE:BEFORE + ROWS], load_sem.at[0]).start()
        pltpu.make_async_copy(do_hbm.at[:SEG, lanes], qd0.at[1, h], load_sem.at[0]).start()
        pltpu.make_async_copy(do_hbm.at[SEG:, lanes], qdx.at[1, h, :BEFORE], load_sem.at[1]).start()

    close = [(a, o) for a, n in enumerate(sizes) for o in near(n)]

    @pl.when(tp == 1)
    def _():
        for a, o in close:
            signal(barrier, along(a, o))
        signal(barrier, (z, y, x, 0))

    @pl.when(tp == 0)
    def _():
        signal(barrier, (z, y, x, 1))

    for load in small_loads:
        load.wait()
    gains = gains_v[...]
    gain_q, gain_k = gains[0:1, :], gains[1:2, :]
    wait_bytes(kvx.at[:, :, :ROWS + PAIR + SEG // 2], load_sem.at[0])
    def norm_keys(first, size):
        for h in range(HEADS):
            u, r = unit(k_raw[h, first:first + size])
            ku[h, first:first + size] = u
            kr[h, first:first + size] = jnp.broadcast_to(r, u.shape)
            kvx[0, h, BEFORE + first:BEFORE + first + size] = (u * gain_k).astype(BF16)

    def norm_queries(first, size, out):
        for h in range(HEADS):
            u, r = unit(q_raw[h, first:first + size])
            qu[h, first:first + size] = u
            qr[h, first:first + size] = jnp.broadcast_to(r, u.shape)
            out[h] = (u * gain_q).astype(BF16)

    forth = [remote(
        kvx.at[:, :, ROWS + PAIR:ROWS + BEFORE], kvx.at[:, :, PAIR:BEFORE], halo_send.at[0], left_recv.at[HEADS], after)]
    back = {}
    for h in range(HEADS):
        forth.append(remote(
            kvx.at[:, h, ROWS:ROWS + PAIR], kvx.at[:, h, :PAIR], halo_send.at[0], left_recv.at[h], after))
        back[h] = [
            remote(kvx.at[:, h, BEFORE:ROWS], kvx.at[:, h, BEFORE + ROWS:], halo_send.at[1], right_recv.at[h], before),
            remote(qd0.at[:, h], qdx.at[:, h, BEFORE:], halo_send.at[1], right_recv.at[h], before)]

    plane_piece = remote(kvx.at[:, :, BEFORE:ROWS], first_kv, halo_send.at[0], left_recv.at[HEADS + 1], after)

    def go_on(pieces, when=place < total - 1):
        @pl.when(when)
        def _():
            for copy in pieces:
                copy.start()

    norm_keys(BEFORE, SEG)
    pl.semaphore_wait(barrier, sides + jnp.where(tp == 1, 1 + len(close), 1))
    go_on(forth[:1])
    norm_keys(0, SEG)
    norm_queries(0, SEG, qd0.at[0])

    go_on([copy for h in range(HEADS) for copy in back[h]], takes_back)
    norm_keys(SEG, PAIR)
    go_on(forth[1:], jnp.logical_and(tp == 0, place < total - 1))
    go_on(forth[1:2], jnp.logical_and(tp == 1, place < total - 1))
    go_on([plane_piece], closes_early)
    norm_queries(SEG, BEFORE, qdx.at[0, :, :BEFORE])

    @pl.when(tp == 1)
    def _():
        for a, o in close:
            signal(round1, along(a, o))

    wait_bytes(qdx.at[1, :, :BEFORE], load_sem.at[1])

    @pl.when(is_first)
    def _():
        for h in range(HEADS):
            for n in range(2):
                kvx[n, h, :BEFORE] = kvx[n, h, BEFORE:2 * BEFORE]
                first_kv[n, h] = kvx[n, h, BEFORE:ROWS]

    @pl.when(opens)
    def _():
        extra_gain[...] = jnp.zeros((1, HEAD_DIM), F32)

    @pl.when(closes)
    def _():
        for h in range(HEADS):
            for n in range(2):
                kvx[n, h, BEFORE + ROWS:] = kvx[n, h, BEFORE:ROWS]
            qdx[0, h, BEFORE:] = qd0[0, h]
            qdx[1, h, BEFORE:] = jnp.zeros((SEG, HEAD_DIM), BF16)

    @pl.when(is_last)
    def _():
        for h in range(HEADS):
            for n in range(2):
                from_after[n, h] = jnp.zeros((BEFORE, HEAD_DIM), BF16)

    key_at = lax.broadcasted_iota(jnp.int32, (PAIR, PAIR), 0)
    query_at = lax.broadcasted_iota(jnp.int32, (PAIR, PAIR), 1)
    past = query_at >= key_at
    early = query_at < SEG
    high = key_at >= SEG
    lane = lax.broadcasted_iota(jnp.int32, (1, PAIR), 1)
    table = table_v[...]
    low_part = table[:, :PAIR]
    high_part = jnp.concatenate([table[:, PAIR:], jnp.zeros((HEADS, 2 * PAIR - ENTRIES), F32)], axis=1)
    low_rolled = pltpu.roll(low_part, PAIR - SEG + 1, 1)
    high_rolled = pltpu.roll(high_part, PAIR - SEG + 1, 1)
    for h in range(HEADS):
        last = table[h:h + 1, ENTRIES - 1:ENTRIES]
        dist_low = low_rolled[h:h + 1]
        dist_row = jnp.where(lane <= SEG, dist_low, high_rolled[h:h + 1])
        ahead = pltpu.roll(jnp.broadcast_to(dist_low, (PAIR, PAIR)), 0, 1, stride=1, stride_axis=0)
        behind = pltpu.roll(jnp.broadcast_to(dist_row, (PAIR, PAIR)), 0, 1, stride=1, stride_axis=0)
        tile0 = jnp.where(jnp.logical_or(early, high), last, MASKED)
        tile1 = jnp.where(past, last, behind)
        tile2 = jnp.where(jnp.logical_and(early, high), MASKED, jnp.where(past, behind, ahead))
        none, low = (jnp.where(is_first, MASKED, t) for t in (tile0, tile1))
        for p, tiles in enumerate((
                (none, jnp.where(high, tile1, low), tile2),
                (jnp.where(high, tile0, none), tile1, tile2))):
            top = jnp.max(jnp.maximum(jnp.maximum(tiles[0], tiles[1]), tiles[2]), axis=0, keepdims=True)
            for b, tile in enumerate(tiles):
                bias_v[h, p, b * PAIR:(b + 1) * PAIR] = (tile - top) * LOG2E

    def work(blocks, tiles=()):
        at_keys = {(p, b): slice((p + b) * PAIR, (p + b + 1) * PAIR) for h, p, b in blocks}
        at_queries = [slice(p * PAIR, (p + 1) * PAIR) for p in range(2)]
        at_rows = [slice(b * PAIR, (b + 1) * PAIR) for b in range(3)]
        scores = [dot(kvx[0, h, at_keys[p, b]], qdx[0, h, at_queries[p]], 1, 1) for h, p, b in blocks]
        d_probs = [dot(kvx[1, h, at_keys[p, b]], qdx[1, h, at_queries[p]], 1, 1) for h, p, b in blocks]
        for (h, p, b), s, dp in zip(blocks, scores, d_probs):
            e = jnp.exp2(s * (FACTOR * LOG2E) + bias_v[h, p, at_rows[b]])
            e_v[h, p, at_rows[b]] = e
            dp_v[h, p, at_rows[b]] = dp
            sum_v[h, p, b] = jnp.sum(e, axis=0, keepdims=True)
            sum_v[h, p, 3 + b] = jnp.sum(e * dp, axis=0, keepdims=True)
        d_scores, products = [], []
        for h, p, _ in tiles:
            inv = 1.0 / (sum_v[h, p, 0] + sum_v[h, p, 1] + sum_v[h, p, 2])
            delta = (sum_v[h, p, 3] + sum_v[h, p, 4] + sum_v[h, p, 5]) * inv
            prob = e_v[h, p] * inv
            d_score = prob * (dp_v[h, p] - delta)
            d_low = d_score.astype(BF16)
            prob_v[h, p] = prob.astype(BF16)
            d_low_v[h, p] = d_low
            d_scores.append(d_score)
            products.append(dot(d_low, qdx[0, h, at_queries[p]], 1, 0))
        for (h, p, again), d_score in zip(tiles, d_scores):
            if again:
                fold_table(h, d_v[h] + d_score)
            else:
                d_v[h] = d_score
        for (h, p, again), dk in zip(tiles, products):
            keys = slice(p * PAIR, (p + 3) * PAIR)
            gain_v[h, p] = jnp.sum(dk * kvx[0, h, keys].astype(F32), axis=0, keepdims=True)
            if again:
                shared, alone = slice(PAIR, 3 * PAIR), slice(3 * p * PAIR, (3 * p + 1) * PAIR)
                dkx[h, alone] = dk[2 * p * PAIR:(2 * p + 1) * PAIR]
                dkx[h, shared] = dkx[h, shared] + dk[(1 - p) * PAIR:(3 - p) * PAIR]
            else:
                dkx[h, keys] = dk

    def query_rows(g, u, r):
        g = g * FACTOR * gain_q
        return (r * (g - u * jnp.mean(g * u, axis=-1, keepdims=True))).astype(BF16)

    sublane = lax.broadcasted_iota(jnp.int32, (8, PAIR), 0)

    def skewed_sum(tile, right):
        parts = [pltpu.roll(tile[first:first + 8], (right - first) % PAIR, 1) for first in range(0, PAIR, 8)]
        while len(parts) > 1:
            parts = [a + b for a, b in zip(parts[::2], parts[1::2])]
        total = parts[0]
        for bit in range(1, 8):
            total = jnp.where(sublane == bit, pltpu.roll(parts[0], PAIR - bit, 1), total)
        return jnp.sum(total, axis=0, keepdims=True)

    def fold_rows(h, d_score):
        d0, d1, d2 = (d_score[b * PAIR:(b + 1) * PAIR] for b in range(3))
        mixed = jnp.where(past, d2, d1)
        ahead = jnp.where(past, 0.0, d2)
        rest = d0 + jnp.where(past, d1, 0.0)
        behind_row, ahead_row = skewed_sum(mixed, SEG - 1), skewed_sum(ahead, SEG - 1)
        high_row = skewed_sum(mixed, SEG - 1 + SEG) if h else behind_row
        rest_sum = jnp.sum(jnp.sum(rest, axis=0, keepdims=True), axis=1, keepdims=True)
        return (
            jnp.where(lane < SEG - 1, ahead_row, behind_row),
            jnp.where(lane == SEG - 1 + h * SEG, rest_sum, high_row))

    def fold_table(h, d_score):
        table_v2[h, 0], table_v2[h, 1] = fold_rows(h, d_score)

    def first_segment(h):
        queries, cotangents = qd0[0, h], qd0[1, h]
        keys, rest = first_kv[0, h], kvx[0, h, :ROWS]
        key_number = lax.broadcasted_iota(jnp.int32, (ROWS + SEG, SEG), 0)
        bias = bias_v[h, 0, :ROWS + SEG][:, :SEG]
        bias = jnp.where(jnp.logical_and(is_first, key_number < ROWS), MASKED, bias)
        bias = bias - jnp.max(bias, axis=0, keepdims=True)
        s = jnp.concatenate([dot(keys, queries, 1, 1), dot(rest, queries, 1, 1)], axis=0)
        e = jnp.exp2(s * (FACTOR * LOG2E) + bias)
        dp = jnp.concatenate([dot(first_kv[1, h], cotangents, 1, 1), dot(kvx[1, h, :ROWS], cotangents, 1, 1)], axis=0)
        inv = 1.0 / jnp.sum(e, axis=0, keepdims=True)
        delta = jnp.sum(e * dp, axis=0, keepdims=True) * inv
        prob = e * inv
        d_score = prob * (dp - delta)
        d_low = d_score.astype(BF16)
        dk = dot(d_low, queries, 1, 0)
        dv = dot(prob.astype(BF16), cotangents, 1, 0)
        dq_from_before[h] = dot(d_low[:SEG], keys, 0, 0) + dot(d_low[SEG:], rest, 0, 0)
        for n, part in enumerate((dk * FACTOR, dv)):
            to_before_first[n, h] = part[:SEG].astype(BF16)
            from_before[n, h] = part[ROWS:].astype(BF16)
        dkx[h, :BEFORE] = dkx[h, :BEFORE] + dk[SEG:ROWS]
        extra_dv[h] = dv[SEG:ROWS]
        extra_gain[...] = extra_gain[...] + (
            jnp.sum(dk[:SEG] * keys.astype(F32), axis=0, keepdims=True)
            + jnp.sum(dk[SEG:] * rest.astype(F32), axis=0, keepdims=True))
        tile = jnp.concatenate([d_score, jnp.zeros((ROWS + SEG, SEG), F32)], axis=1)
        rows = fold_rows(h, jnp.concatenate([tile, jnp.zeros((SEG, PAIR), F32)], axis=0))
        for j in range(2):
            table_v2[h, j] = table_v2[h, j] + rows[j]

    heads = range(HEADS)
    work([(h, 0, 2) for h in heads])

    go_on(forth[2:], jnp.logical_and(tp == 1, place < total - 1))
    @pl.when(tp == 1)
    def _():
        pl.semaphore_wait(round1, len(close))
        for a, n in enumerate(sizes[:2]):
            if n > 5:
                for o in near(n, 2):
                    signal(round2, along(a, o))

    def wait_left(piece):
        @pl.when(place > 0)
        def _():
            forth[piece].wait_recv()

    def wait_right(h):
        @pl.when(takes_next)
        def _():
            wait_bytes(kvx.at[:, h, :PAIR], right_recv.at[h])

    beside = sorted({*near(ny), *near(ny, 2)})

    def greet_far():
        @pl.when(tp == 1)
        def _():
            count = sum(len(near(n, 2)) for n in sizes[:2] if n > 5)
            if count:
                pl.semaphore_wait(round2, count)
            for o in beside:
                signal(plane_round, along(1, o))
            if nz > 9:
                for o in near(nz, 3):
                    signal(round3, along(0, o))

    def do_first():
        @pl.when(opens)
        def _():
            @pl.when(place > 0)
            def _():
                plane_piece.wait_recv()

            for h in range(HEADS):
                first_segment(h)

    @pl.when(x == nx - 1)
    def _():
        wait_left(0)
        work([(h, 0, 1) for h in heads])
        for h in heads:
            wait_left(1 + h)
            work([(h, 0, 0)], [(h, 0, False)])
            if not h:
                greet_far()
        for h in heads:
            wait_right(h)
        work([(h, 1, b) for b in range(3) for h in heads], [(h, 1, True) for h in heads])
        if nx == 1:
            do_first()

    if nx > 1:
        @pl.when(x == 0)
        def _():
            for h in heads:
                wait_right(h)
            work([(h, 1, b) for b in (1, 2) for h in heads])
            greet_far()
            wait_left(0)
            work([(h, p, 1 - p) for p in (1, 0) for h in heads], [(h, 1, False) for h in heads])
            for h in heads:
                wait_left(1 + h)
                work([(h, 0, 0)], [(h, 0, True)])
            do_first()

    if nx > 2:
        @pl.when(jnp.logical_and(x > 0, x < nx - 1))
        def _():
            wait_left(0)
            work([(h, 0, 1) for h in heads])
            for h in heads:
                wait_right(h)
            work([(h, 1, b) for b in range(3) for h in heads], [(h, 1, False) for h in heads])
            greet_far()
            for h in heads:
                wait_left(1 + h)
                work([(h, 0, 0)], [(h, 0, True)])

    gain = gain_v[0, 0] + gain_v[0, 1] + gain_v[1, 0] + gain_v[1, 1] + jnp.where(opens, extra_gain[...], 0.0)
    second = jnp.where(lane < SEG, table_v2[0, 1], table_v2[1, 1])
    vec = jnp.concatenate([table_v2[0, 0], table_v2[1, 0], second, gain * FACTOR], axis=0)
    chip = y * nx + x

    to_neighbours = [
        remote(to_before.at[:, h], from_after.at[:, h], back_send.at[0], after_recv.at[h], before) for h in range(HEADS)]
    to_next = [
        remote(to_after, from_before, back_send.at[1], before_recv, after),
        remote(dqx.at[:, BEFORE:], dq_from_before, back_send.at[1], before_recv, after)]
    to_plane_before = remote(to_before_first, from_after_first, back_send.at[0], first_recv, before)

    def stage_results():
        for h in range(HEADS):
            low, high_tile = (dot(prob_v[h, p], qdx[1, h, p * PAIR:(p + 1) * PAIR], 1, 0) for p in range(2))
            dvx[h, :PAIR] = low[:PAIR]
            dvx[h, PAIR:3 * PAIR] = low[PAIR:] + high_tile[:2 * PAIR]
            dvx[h, 3 * PAIR:] = high_tile[2 * PAIR:]

            @pl.when(opens)
            def _(h=h):
                dvx[h, :BEFORE] = dvx[h, :BEFORE] + extra_dv[h]

            lanes = slice(h * HEAD_DIM, (h + 1) * HEAD_DIM)
            to_before[0, h] = (dkx[h, :BEFORE] * FACTOR).astype(BF16)
            to_before[1, h] = dvx[h, :BEFORE].astype(BF16)
            to_after[0, h] = (dkx[h, BEFORE + ROWS:] * FACTOR).astype(BF16)
            to_after[1, h] = dvx[h, BEFORE + ROWS:].astype(BF16)
            for p in range(2):
                dqx[h, p * PAIR:(p + 1) * PAIR] = dot(d_low_v[h, p], kvx[0, h, p * PAIR:(p + 3) * PAIR], 0, 0)
            dq_v[SEG:, lanes] = query_rows(dqx[h, :BEFORE], qu[h, SEG:], qr[h, SEG:])

    def send_results(when):
        @pl.when(jnp.logical_and(when, place > 0))
        def _():
            for copy in to_neighbours:
                copy.start()

        @pl.when(jnp.logical_and(when, opens_later))
        def _():
            to_plane_before.start()

        @pl.when(jnp.logical_and(when, takes_next))
        def _():
            for copy in to_next:
                copy.start()

    def sum_of(ref, first, count):
        parts = [ref[n] for n in range(first, first + count)]
        while len(parts) > 1:
            parts = [sum(parts[n:n + 2]) for n in range(0, len(parts), 2)]
        return parts[0]

    @pl.when(tp == 1)
    def _():
        lines[x] = vec
        for o in far_first(nx):
            remote(lines.at[x], lines.at[x], xy_send, x_recv, along(2, o)).start()
        if beside:
            pl.semaphore_wait(plane_round, len(beside))
        signal(round1, (z, y, x, 0))
        stage_results()
        if nx > 1:
            wait_bytes(lines.at[:nx - 1], x_recv)
        lines[nx + y] = sum_of(lines, 0, nx)
        for o in far_first(ny):
            remote(lines.at[nx + y], lines.at[nx + y], xy_send, y_recv, along(1, o)).start()
        wait_bytes(plane, plane_recv)
        others = sum_of(plane, 0, nx * ny)
        if ny > 1:
            wait_bytes(lines.at[:ny - 1], y_recv)
        part = sum_of(lines, nx, ny)
        gain = part[3:] + others[3:]
        for core, rows in enumerate((others, part)):
            zout[core, :3] = rows[:3]
            zout[core, 3:] = gain
        zbuf[z] = zout[1]
        if nz > 9:
            pl.semaphore_wait(round3, len(near(nz, 3)))
        for o in [*far_first(nz), 0]:
            for core in range(2 if o else 1):
                remote(zout.at[core], zbuf.at[z], z_send, z_recv, along(0, o, core)).start()
        send_results(place >= 0)
        signal(round2, (z, y, x, 0))

    @pl.when(tp == 0)
    def _():
        plane[chip] = vec
        pl.semaphore_wait(round1, 1)
        for oy, ox in sorted(
                ((oy, ox) for oy in range(ny) for ox in range(nx)),
                key=lambda o: -min(o[0], ny - o[0]) - min(o[1], nx - o[1])):
            remote(
                plane.at[chip], plane.at[chip], xy_send, plane_recv,
                (z, lax.rem(y + oy, ny), lax.rem(x + ox, nx), 1)).start()
        stage_results()
        pl.semaphore_wait(round2, 1)
        send_results(place >= 0)

    @pl.when(takes_back)
    def _():
        wait_bytes(kvx.at[:, :, :PAIR], before_recv)

    @pl.when(closes_early)
    def _():
        to_plane_before.wait_recv()

    for h in range(HEADS):
        dq_v[:SEG, h * HEAD_DIM:(h + 1) * HEAD_DIM] = query_rows(dq_from_before[h], qu[h, :SEG], qr[h, :SEG])

    for h in range(HEADS):
        @pl.when(place < total - 1)
        def _(h=h):
            to_neighbours[h].wait_recv()

        lanes = slice(h * HEAD_DIM, (h + 1) * HEAD_DIM)
        sums_in = [
            jnp.concatenate([
                jnp.where(takes_next, 0.0, jnp.where(is_last, 0.0, from_after_first[n, h].astype(F32)))
                + from_before[n, h].astype(F32), from_after[n, h].astype(F32)], axis=0) for n in range(2)]
        g = (dkx[h, BEFORE:BEFORE + ROWS] * FACTOR + sums_in[0]) * gain_k
        u = ku[h]
        dk_v[:, lanes] = (kr[h] * (g - u * jnp.mean(g * u, axis=-1, keepdims=True))).astype(BF16)
        dv_v[:, lanes] = (dvx[h, BEFORE:BEFORE + ROWS] + sums_in[1]).astype(BF16)

    @pl.when(takes_next)
    def _():
        wait_bytes(kvx.at[:, :, :BEFORE], halo_send.at[0])
        wait_bytes(kvx.at[:, :, :PAIR], back_send.at[1])

    @pl.when(closes_early)
    def _():
        wait_bytes(kvx.at[:, :, :ROWS], halo_send.at[0])

    @pl.when(takes_back)
    def _():
        wait_bytes(kvx.at[:, :, :PAIR], halo_send.at[1])
        wait_bytes(from_after, back_send.at[0])

    @pl.when(opens_later)
    def _():
        wait_bytes(kvx.at[:, :, :ROWS], back_send.at[0])

    @pl.when(tp == 1)
    def _():
        if nx + ny > 2:
            wait_bytes(lines.at[:nx + ny - 2], xy_send)
        wait_bytes(zbuf.at[:2 * nz - 1], z_send)
        if nz > 1:
            wait_bytes(zbuf.at[:nz - 1], z_recv)

    @pl.when(tp == 0)
    def _():
        wait_bytes(plane, xy_send)
        wait_bytes(zbuf.at[:nz], z_recv)

    result = zbuf[0]
    for n in range(1, nz):
        result = result + zbuf[n]
    for j in range(HEADS):
        dtab_v[j:j + 1, :PAIR] = result[j:j + 1]
        dtab_v[j:j + 1, PAIR:] = result[2:3, j * SEG:(j + 1) * SEG]
    dgain_v[0:1] = result[3:] / gain_q
    dgain_v[1:2] = result[3:] / gain_k


def write_out(*refs):
    count = len(refs) // 2
    copies = [pltpu.make_async_copy(refs[n], refs[count + n], refs[-1].at[n]) for n in range(count)]
    for copy in copies:
        copy.start()
    for copy in copies:
        copy.wait()


def local(sizes, queries, keys, values, gains, bias_table, d_out):
    nz, ny, nx = sizes
    width = HEADS * HEAD_DIM
    hbm_spec = pl.BlockSpec(memory_space=pltpu.HBM)
    vmem_spec = pl.BlockSpec(memory_space=pltpu.VMEM)
    first = (HEADS, SEG, HEAD_DIM)
    tile = (HEADS, ROWS, HEAD_DIM)
    wide = (HEADS, 2 * ROWS, HEAD_DIM)
    pairs = (HEADS, 2, 3 * PAIR, PAIR)
    dma, regular = pltpu.SemaphoreType.DMA, pltpu.SemaphoreType.REGULAR
    vmem = pltpu.VMEM
    outs = [((ROWS, width), BF16)] * 3 + [((HEADS, ENTRIES), F32), ((2, HEAD_DIM), F32)]
    out = pl.pallas_call(
        functools.partial(kernel, sizes),
        out_shape=tuple(vmem(*o) for o in outs),
        in_specs=[hbm_spec] * 6,
        out_specs=(vmem_spec,) * 5,
        scratch_shapes=[
            vmem(tile, BF16), vmem(tile, BF16), vmem((2, *tile), BF16), vmem((2, *first), BF16), vmem((2, *wide), BF16), vmem((2, *first), BF16),
            vmem((2, HEAD_DIM), F32), vmem((HEADS, ENTRIES), F32),
            vmem(tile, F32), vmem(tile, F32), vmem(tile, F32), vmem(tile, F32),
            vmem(pairs, F32), vmem(pairs, F32), vmem(pairs, F32),
            vmem(wide, F32), vmem(wide, F32), vmem(tile, F32), vmem((HEADS, 3 * PAIR, PAIR), F32),
            vmem(pairs, BF16), vmem(pairs, BF16), vmem((HEADS, 2, 6, 1, PAIR), F32), vmem((HEADS, 2, 1, PAIR), F32),
            vmem((HEADS, 2, 1, PAIR), F32), vmem((1, HEAD_DIM), F32), vmem((HEADS, BEFORE, HEAD_DIM), F32),
            vmem((2, HEADS, BEFORE, HEAD_DIM), BF16), vmem((2, HEADS, BEFORE, HEAD_DIM), BF16),
            vmem((2, *first), BF16), vmem((2, *first), BF16), vmem(first, F32), vmem((2, *first), BF16), vmem((2, *first), BF16),
            vmem((nx + ny, 4, HEAD_DIM), F32), vmem((nx * ny, 4, HEAD_DIM), F32), vmem((2, 4, HEAD_DIM), F32), vmem((2 * nz, 4, HEAD_DIM), F32),
            dma((2,)), dma, dma, dma((2,)), dma((HEADS + 2,)), dma((HEADS,)), dma((2,)), dma((HEADS,)), dma, dma,
            dma, dma, dma, dma, dma, dma, regular, regular, regular, regular,
        ],
        compiler_params=pltpu.CompilerParams(
            collective_id=0, has_side_effects=True, vmem_limit_bytes=32 * 1024 * 1024),
        name="segment_attention_grad",
    )(*(pltpu.with_memory_space_constraint(a, pltpu.HBM) for a in (queries, keys, values, d_out, gains, bias_table.T)))
    d_queries, d_keys, d_values, d_table, d_gains = pl.pallas_call(
        write_out,
        out_shape=tuple(jax.ShapeDtypeStruct(*o) for o in outs),
        in_specs=[vmem_spec] * 5,
        out_specs=(hbm_spec,) * 5,
        scratch_shapes=[dma((5,))],
        name="write_out",
    )(*(pltpu.with_memory_space_constraint(o, pltpu.VMEM) for o in out))
    return d_queries, d_keys, d_values, d_table.T, d_gains


def solution(mesh):
    shape = (12, 8, 4)
    if mesh.shape["sp"] != int(np.prod(shape)):
        shape = mesh.small_shape
    split = Mesh(mesh.devices.reshape(*shape, mesh.shape["tp"]), AXES)
    placed = (P(SP, "tp"), P(SP, "tp"), P(SP, "tp"), P(), P(None, "tp"), P(SP, "tp"))
    return jax.shard_map(
        functools.partial(local, shape),
        mesh=split,
        in_specs=placed,
        out_specs=(P(SP, "tp"), P(SP, "tp"), P(SP, "tp"), P(None, "tp"), P()),
        check_vma=False,
    )
```

```python
import functools

import jax
import jax.numpy as jnp
import numpy as np
from jax import lax
from jax.experimental import pallas as pl
from jax.experimental.pallas import tpu as pltpu
from jax.sharding import Mesh
from jax.sharding import PartitionSpec as P

HEAD_DIM = 128
SEG = 64
LEFT = 4
MAX_REL = 128
ENTRIES = MAX_REL + SEG
ROWS = LEFT * SEG
HEADS = 2
PAIR = 2 * SEG
BEFORE = 3 * SEG
AXES = ("sp_0", "sp_1", "sp_2", "tp")
SP = AXES[:3]

EPSILON = 1e-06
FACTOR = HEAD_DIM ** (-0.5)
LOG2E = 1.4426950408889634
MASKED = -1e30
F32, BF16 = jnp.float32, jnp.bfloat16


def dot(a, b, a_dim, b_dim):
    return lax.dot_general(a, b, (((a_dim,), (b_dim,)), ((), ())), preferred_element_type=F32)


def near(size, step=1):
    return sorted({step % size, -step % size} - {0})


def far_first(size):
    return sorted(range(1, size), key=lambda d: -min(d, size - d))


def unit(raw):
    wide = raw.astype(F32)
    inv_rms = lax.rsqrt(jnp.mean(wide * wide, axis=-1, keepdims=True) + EPSILON)
    return wide * inv_rms, inv_rms


def kernel(sizes, q_hbm, k_hbm, v_hbm, do_hbm, gains_hbm, table_hbm,
           dq_v, dk_v, dv_v, dtab_v, dgain_v,
           q_raw, k_raw, qdx, qd0, kvx, first_kv, gains_v, table_v,
           qu, qr, ku, kr, bias_v, e_v, dp_v,
           dkx, dvx, dqx, d_v, prob_v, d_low_v, sum_v, gain_v, table_v2, extra_gain, extra_dv,
           to_before, from_after, to_after, from_before, dq_from_before, to_before_first, from_after_first,
           lines, plane, zout, zbuf,
           load_sem, gains_sem, table_sem, halo_send, left_recv, right_recv, back_send, after_recv, before_recv, first_recv,
           xy_send, x_recv, y_recv, plane_recv, z_send, z_recv, round1, round2, round3, plane_round):
    nz, ny, nx = sizes
    z, y, x, tp = (lax.axis_index(a) for a in AXES)
    place = (z * ny + y) * nx + x
    total = nz * ny * nx
    is_first, is_last = place == 0, place == total - 1
    opens, closes = jnp.logical_and(x == 0, y == 0), jnp.logical_and(x == nx - 1, y == ny - 1)
    opens_later, closes_early = jnp.logical_and(opens, place > 0), jnp.logical_and(closes, place < total - 1)
    takes_back, takes_next = jnp.logical_not(opens), jnp.logical_not(closes)

    def at(number, core):
        return (number // (ny * nx), (number // nx) % ny, number % nx, core)

    after = at(jnp.minimum(place + 1, total - 1), tp)
    before = at(jnp.maximum(place - 1, 0), tp)

    def along(axis, offset, core=1):
        if axis == 0:
            return (lax.rem(z + offset, nz), y, x, core)
        if axis == 1:
            return (z, lax.rem(y + offset, ny), x, core)
        return (z, y, lax.rem(x + offset, nx), core)

    def signal(sem, target):
        pl.semaphore_signal(sem, inc=1, device_id=target, device_id_type=pl.DeviceIdType.MESH)

    def remote(src, dst, send, recv, target):
        return pltpu.make_async_remote_copy(
            src_ref=src, dst_ref=dst, send_sem=send, recv_sem=recv,
            device_id=target, device_id_type=pl.DeviceIdType.MESH)

    def wait_bytes(ref, sem):
        pltpu.make_async_copy(ref, ref, sem).wait()

    barrier = pltpu.get_barrier_semaphore()

    @pl.when(place > 0)
    def _():
        signal(barrier, before)

    @pl.when(place < total - 1)
    def _():
        signal(barrier, after)

    sides = jnp.where(is_first, 0, 1) + jnp.where(is_last, 0, 1)
    small_loads = [pltpu.make_async_copy(gains_hbm, gains_v, gains_sem), pltpu.make_async_copy(table_hbm, table_v, table_sem)]
    for load in small_loads:
        load.start()
    for h in range(HEADS):
        lanes = slice(h * HEAD_DIM, (h + 1) * HEAD_DIM)
        pltpu.make_async_copy(k_hbm.at[:, lanes], k_raw.at[h], load_sem.at[0]).start()
        pltpu.make_async_copy(q_hbm.at[:, lanes], q_raw.at[h], load_sem.at[0]).start()
        pltpu.make_async_copy(v_hbm.at[:, lanes], kvx.at[1, h, BEFORE:BEFORE + ROWS], load_sem.at[0]).start()
        pltpu.make_async_copy(do_hbm.at[:SEG, lanes], qd0.at[1, h], load_sem.at[0]).start()
        pltpu.make_async_copy(do_hbm.at[SEG:, lanes], qdx.at[1, h, :BEFORE], load_sem.at[1]).start()

    close = [(a, o) for a, n in enumerate(sizes) for o in near(n)]

    @pl.when(tp == 1)
    def _():
        for a, o in close:
            signal(barrier, along(a, o))
        signal(barrier, (z, y, x, 0))

    @pl.when(tp == 0)
    def _():
        signal(barrier, (z, y, x, 1))

    for load in small_loads:
        load.wait()
    gains = gains_v[...]
    gain_q, gain_k = gains[0:1, :], gains[1:2, :]
    wait_bytes(kvx.at[:, :, :ROWS + PAIR + SEG // 2], load_sem.at[0])
    def norm_keys(first, size):
        for h in range(HEADS):
            u, r = unit(k_raw[h, first:first + size])
            ku[h, first:first + size] = u
            kr[h, first:first + size] = jnp.broadcast_to(r, u.shape)
            kvx[0, h, BEFORE + first:BEFORE + first + size] = (u * gain_k).astype(BF16)

    def norm_queries(first, size, out):
        for h in range(HEADS):
            u, r = unit(q_raw[h, first:first + size])
            qu[h, first:first + size] = u
            qr[h, first:first + size] = jnp.broadcast_to(r, u.shape)
            out[h] = (u * gain_q).astype(BF16)

    forth = [remote(
        kvx.at[:, :, ROWS + PAIR:ROWS + BEFORE], kvx.at[:, :, PAIR:BEFORE], halo_send.at[0], left_recv.at[HEADS], after)]
    back = {}
    for h in range(HEADS):
        forth.append(remote(
            kvx.at[:, h, ROWS:ROWS + PAIR], kvx.at[:, h, :PAIR], halo_send.at[0], left_recv.at[h], after))
        back[h] = [
            remote(kvx.at[:, h, BEFORE:ROWS], kvx.at[:, h, BEFORE + ROWS:], halo_send.at[1], right_recv.at[h], before),
            remote(qd0.at[:, h], qdx.at[:, h, BEFORE:], halo_send.at[1], right_recv.at[h], before)]

    plane_piece = remote(kvx.at[:, :, BEFORE:ROWS], first_kv, halo_send.at[0], left_recv.at[HEADS + 1], after)

    def go_on(pieces, when=place < total - 1):
        @pl.when(when)
        def _():
            for copy in pieces:
                copy.start()

    norm_keys(BEFORE, SEG)
    pl.semaphore_wait(barrier, sides + jnp.where(tp == 1, 1 + len(close), 1))
    go_on(forth[:1])
    norm_keys(0, SEG)
    norm_queries(0, SEG, qd0.at[0])

    go_on([copy for h in range(HEADS) for copy in back[h]], takes_back)
    norm_keys(SEG, PAIR)
    go_on(forth[1:], jnp.logical_and(tp == 0, place < total - 1))
    go_on(forth[1:2], jnp.logical_and(tp == 1, place < total - 1))
    go_on([plane_piece], closes_early)
    norm_queries(SEG, BEFORE, qdx.at[0, :, :BEFORE])

    @pl.when(tp == 1)
    def _():
        for a, o in close:
            signal(round1, along(a, o))

    wait_bytes(qdx.at[1, :, :BEFORE], load_sem.at[1])

    @pl.when(is_first)
    def _():
        for h in range(HEADS):
            for n in range(2):
                kvx[n, h, :BEFORE] = kvx[n, h, BEFORE:2 * BEFORE]
                first_kv[n, h] = kvx[n, h, BEFORE:ROWS]

    @pl.when(opens)
    def _():
        extra_gain[...] = jnp.zeros((1, HEAD_DIM), F32)

    @pl.when(closes)
    def _():
        for h in range(HEADS):
            for n in range(2):
                kvx[n, h, BEFORE + ROWS:] = kvx[n, h, BEFORE:ROWS]
            qdx[0, h, BEFORE:] = qd0[0, h]
            qdx[1, h, BEFORE:] = jnp.zeros((SEG, HEAD_DIM), BF16)

    @pl.when(is_last)
    def _():
        for h in range(HEADS):
            for n in range(2):
                from_after[n, h] = jnp.zeros((BEFORE, HEAD_DIM), BF16)

    key_at = lax.broadcasted_iota(jnp.int32, (PAIR, PAIR), 0)
    query_at = lax.broadcasted_iota(jnp.int32, (PAIR, PAIR), 1)
    past = query_at >= key_at
    early = query_at < SEG
    high = key_at >= SEG
    lane = lax.broadcasted_iota(jnp.int32, (1, PAIR), 1)
    table = table_v[...]
    low_part = table[:, :PAIR]
    high_part = jnp.concatenate([table[:, PAIR:], jnp.zeros((HEADS, 2 * PAIR - ENTRIES), F32)], axis=1)
    low_rolled = pltpu.roll(low_part, PAIR - SEG + 1, 1)
    high_rolled = pltpu.roll(high_part, PAIR - SEG + 1, 1)
    for h in range(HEADS):
        last = table[h:h + 1, ENTRIES - 1:ENTRIES]
        dist_low = low_rolled[h:h + 1]
        dist_row = jnp.where(lane <= SEG, dist_low, high_rolled[h:h + 1])
        ahead = pltpu.roll(jnp.broadcast_to(dist_low, (PAIR, PAIR)), 0, 1, stride=1, stride_axis=0)
        behind = pltpu.roll(jnp.broadcast_to(dist_row, (PAIR, PAIR)), 0, 1, stride=1, stride_axis=0)
        tile0 = jnp.where(jnp.logical_or(early, high), last, MASKED)
        tile1 = jnp.where(past, last, behind)
        tile2 = jnp.where(jnp.logical_and(early, high), MASKED, jnp.where(past, behind, ahead))
        none, low = (jnp.where(is_first, MASKED, t) for t in (tile0, tile1))
        for p, tiles in enumerate((
                (none, jnp.where(high, tile1, low), tile2),
                (jnp.where(high, tile0, none), tile1, tile2))):
            top = jnp.max(jnp.maximum(jnp.maximum(tiles[0], tiles[1]), tiles[2]), axis=0, keepdims=True)
            for b, tile in enumerate(tiles):
                bias_v[h, p, b * PAIR:(b + 1) * PAIR] = (tile - top) * LOG2E

    def work(blocks, tiles=()):
        at_keys = {(p, b): slice((p + b) * PAIR, (p + b + 1) * PAIR) for h, p, b in blocks}
        at_queries = [slice(p * PAIR, (p + 1) * PAIR) for p in range(2)]
        at_rows = [slice(b * PAIR, (b + 1) * PAIR) for b in range(3)]
        scores = [dot(kvx[0, h, at_keys[p, b]], qdx[0, h, at_queries[p]], 1, 1) for h, p, b in blocks]
        d_probs = [dot(kvx[1, h, at_keys[p, b]], qdx[1, h, at_queries[p]], 1, 1) for h, p, b in blocks]
        for (h, p, b), s, dp in zip(blocks, scores, d_probs):
            e = jnp.exp2(s * (FACTOR * LOG2E) + bias_v[h, p, at_rows[b]])
            e_v[h, p, at_rows[b]] = e
            dp_v[h, p, at_rows[b]] = dp
            sum_v[h, p, b] = jnp.sum(e, axis=0, keepdims=True)
            sum_v[h, p, 3 + b] = jnp.sum(e * dp, axis=0, keepdims=True)
        d_scores, products = [], []
        for h, p, _ in tiles:
            inv = 1.0 / (sum_v[h, p, 0] + sum_v[h, p, 1] + sum_v[h, p, 2])
            delta = (sum_v[h, p, 3] + sum_v[h, p, 4] + sum_v[h, p, 5]) * inv
            prob = e_v[h, p] * inv
            d_score = prob * (dp_v[h, p] - delta)
            d_low = d_score.astype(BF16)
            prob_v[h, p] = prob.astype(BF16)
            d_low_v[h, p] = d_low
            d_scores.append(d_score)
            products.append(dot(d_low, qdx[0, h, at_queries[p]], 1, 0))
        for (h, p, again), d_score in zip(tiles, d_scores):
            if again:
                fold_table(h, d_v[h] + d_score)
            else:
                d_v[h] = d_score
        for (h, p, again), dk in zip(tiles, products):
            keys = slice(p * PAIR, (p + 3) * PAIR)
            gain_v[h, p] = jnp.sum(dk * kvx[0, h, keys].astype(F32), axis=0, keepdims=True)
            if again:
                shared, alone = slice(PAIR, 3 * PAIR), slice(3 * p * PAIR, (3 * p + 1) * PAIR)
                dkx[h, alone] = dk[2 * p * PAIR:(2 * p + 1) * PAIR]
                dkx[h, shared] = dkx[h, shared] + dk[(1 - p) * PAIR:(3 - p) * PAIR]
            else:
                dkx[h, keys] = dk

    def query_rows(g, u, r):
        g = g * FACTOR * gain_q
        return (r * (g - u * jnp.mean(g * u, axis=-1, keepdims=True))).astype(BF16)

    sublane = lax.broadcasted_iota(jnp.int32, (8, PAIR), 0)

    def skewed_sum(tile, right):
        parts = [pltpu.roll(tile[first:first + 8], (right - first) % PAIR, 1) for first in range(0, PAIR, 8)]
        while len(parts) > 1:
            parts = [a + b for a, b in zip(parts[::2], parts[1::2])]
        total = parts[0]
        for bit in range(1, 8):
            total = jnp.where(sublane == bit, pltpu.roll(parts[0], PAIR - bit, 1), total)
        return jnp.sum(total, axis=0, keepdims=True)

    def fold_rows(h, d_score):
        d0, d1, d2 = (d_score[b * PAIR:(b + 1) * PAIR] for b in range(3))
        mixed = jnp.where(past, d2, d1)
        ahead = jnp.where(past, 0.0, d2)
        rest = d0 + jnp.where(past, d1, 0.0)
        behind_row, ahead_row = skewed_sum(mixed, SEG - 1), skewed_sum(ahead, SEG - 1)
        high_row = skewed_sum(mixed, SEG - 1 + SEG) if h else behind_row
        rest_sum = jnp.sum(jnp.sum(rest, axis=0, keepdims=True), axis=1, keepdims=True)
        return (
            jnp.where(lane < SEG - 1, ahead_row, behind_row),
            jnp.where(lane == SEG - 1 + h * SEG, rest_sum, high_row))

    def fold_table(h, d_score):
        table_v2[h, 0], table_v2[h, 1] = fold_rows(h, d_score)

    def first_segment(h):
        queries, cotangents = qd0[0, h], qd0[1, h]
        keys, rest = first_kv[0, h], kvx[0, h, :ROWS]
        key_number = lax.broadcasted_iota(jnp.int32, (ROWS + SEG, SEG), 0)
        bias = bias_v[h, 0, :ROWS + SEG][:, :SEG]
        bias = jnp.where(jnp.logical_and(is_first, key_number < ROWS), MASKED, bias)
        bias = bias - jnp.max(bias, axis=0, keepdims=True)
        s = jnp.concatenate([dot(keys, queries, 1, 1), dot(rest, queries, 1, 1)], axis=0)
        e = jnp.exp2(s * (FACTOR * LOG2E) + bias)
        dp = jnp.concatenate([dot(first_kv[1, h], cotangents, 1, 1), dot(kvx[1, h, :ROWS], cotangents, 1, 1)], axis=0)
        inv = 1.0 / jnp.sum(e, axis=0, keepdims=True)
        delta = jnp.sum(e * dp, axis=0, keepdims=True) * inv
        prob = e * inv
        d_score = prob * (dp - delta)
        d_low = d_score.astype(BF16)
        dk = dot(d_low, queries, 1, 0)
        dv = dot(prob.astype(BF16), cotangents, 1, 0)
        dq_from_before[h] = dot(d_low[:SEG], keys, 0, 0) + dot(d_low[SEG:], rest, 0, 0)
        for n, part in enumerate((dk * FACTOR, dv)):
            to_before_first[n, h] = part[:SEG].astype(BF16)
            from_before[n, h] = part[ROWS:].astype(BF16)
        dkx[h, :BEFORE] = dkx[h, :BEFORE] + dk[SEG:ROWS]
        extra_dv[h] = dv[SEG:ROWS]
        extra_gain[...] = extra_gain[...] + (
            jnp.sum(dk[:SEG] * keys.astype(F32), axis=0, keepdims=True)
            + jnp.sum(dk[SEG:] * rest.astype(F32), axis=0, keepdims=True))
        tile = jnp.concatenate([d_score, jnp.zeros((ROWS + SEG, SEG), F32)], axis=1)
        rows = fold_rows(h, jnp.concatenate([tile, jnp.zeros((SEG, PAIR), F32)], axis=0))
        for j in range(2):
            table_v2[h, j] = table_v2[h, j] + rows[j]

    heads = range(HEADS)
    work([(h, 0, 2) for h in heads])

    go_on(forth[2:], jnp.logical_and(tp == 1, place < total - 1))
    @pl.when(tp == 1)
    def _():
        pl.semaphore_wait(round1, len(close))
        for a, n in enumerate(sizes[:2]):
            if n > 5:
                for o in near(n, 2):
                    signal(round2, along(a, o))

    def wait_left(piece):
        @pl.when(place > 0)
        def _():
            forth[piece].wait_recv()

    def wait_right(h):
        @pl.when(takes_next)
        def _():
            wait_bytes(kvx.at[:, h, :PAIR], right_recv.at[h])

    beside = sorted({*near(ny), *near(ny, 2)})

    def greet_far():
        @pl.when(tp == 1)
        def _():
            count = sum(len(near(n, 2)) for n in sizes[:2] if n > 5)
            if count:
                pl.semaphore_wait(round2, count)
            for o in beside:
                signal(plane_round, along(1, o))
            if nz > 9:
                for o in near(nz, 3):
                    signal(round3, along(0, o))

    def do_first():
        @pl.when(opens)
        def _():
            @pl.when(place > 0)
            def _():
                plane_piece.wait_recv()

            for h in range(HEADS):
                first_segment(h)

    @pl.when(x == nx - 1)
    def _():
        wait_left(0)
        work([(h, 0, 1) for h in heads])
        for h in heads:
            wait_left(1 + h)
            work([(h, 0, 0)], [(h, 0, False)])
            if not h:
                greet_far()
        for h in heads:
            wait_right(h)
        work([(h, 1, b) for b in range(3) for h in heads], [(h, 1, True) for h in heads])
        if nx == 1:
            do_first()

    if nx > 1:
        @pl.when(x == 0)
        def _():
            for h in heads:
                wait_right(h)
            work([(h, 1, b) for b in (1, 2) for h in heads])
            greet_far()
            wait_left(0)
            work([(h, p, 1 - p) for p in (1, 0) for h in heads], [(h, 1, False) for h in heads])
            for h in heads:
                wait_left(1 + h)
                work([(h, 0, 0)], [(h, 0, True)])
            do_first()

    if nx > 2:
        @pl.when(jnp.logical_and(x > 0, x < nx - 1))
        def _():
            wait_left(0)
            work([(h, 0, 1) for h in heads])
            for h in heads:
                wait_right(h)
            work([(h, 1, b) for b in range(3) for h in heads], [(h, 1, False) for h in heads])
            greet_far()
            for h in heads:
                wait_left(1 + h)
                work([(h, 0, 0)], [(h, 0, True)])

    gain = gain_v[0, 0] + gain_v[0, 1] + gain_v[1, 0] + gain_v[1, 1] + jnp.where(opens, extra_gain[...], 0.0)
    second = jnp.where(lane < SEG, table_v2[0, 1], table_v2[1, 1])
    vec = jnp.concatenate([table_v2[0, 0], table_v2[1, 0], second, gain * FACTOR], axis=0)
    chip = y * nx + x

    to_neighbours = [
        remote(to_before.at[:, h], from_after.at[:, h], back_send.at[0], after_recv.at[h], before) for h in range(HEADS)]
    to_next = [
        remote(to_after, from_before, back_send.at[1], before_recv, after),
        remote(dqx.at[:, BEFORE:], dq_from_before, back_send.at[1], before_recv, after)]
    to_plane_before = remote(to_before_first, from_after_first, back_send.at[0], first_recv, before)

    def stage_results():
        for h in range(HEADS):
            low, high_tile = (dot(prob_v[h, p], qdx[1, h, p * PAIR:(p + 1) * PAIR], 1, 0) for p in range(2))
            dvx[h, :PAIR] = low[:PAIR]
            dvx[h, PAIR:3 * PAIR] = low[PAIR:] + high_tile[:2 * PAIR]
            dvx[h, 3 * PAIR:] = high_tile[2 * PAIR:]

            @pl.when(opens)
            def _(h=h):
                dvx[h, :BEFORE] = dvx[h, :BEFORE] + extra_dv[h]

            lanes = slice(h * HEAD_DIM, (h + 1) * HEAD_DIM)
            to_before[0, h] = (dkx[h, :BEFORE] * FACTOR).astype(BF16)
            to_before[1, h] = dvx[h, :BEFORE].astype(BF16)
            to_after[0, h] = (dkx[h, BEFORE + ROWS:] * FACTOR).astype(BF16)
            to_after[1, h] = dvx[h, BEFORE + ROWS:].astype(BF16)
            for p in range(2):
                dqx[h, p * PAIR:(p + 1) * PAIR] = dot(d_low_v[h, p], kvx[0, h, p * PAIR:(p + 3) * PAIR], 0, 0)
            dq_v[SEG:, lanes] = query_rows(dqx[h, :BEFORE], qu[h, SEG:], qr[h, SEG:])

    def send_results(when):
        @pl.when(jnp.logical_and(when, place > 0))
        def _():
            for copy in to_neighbours:
                copy.start()

        @pl.when(jnp.logical_and(when, opens_later))
        def _():
            to_plane_before.start()

        @pl.when(jnp.logical_and(when, takes_next))
        def _():
            for copy in to_next:
                copy.start()

    def sum_of(ref, first, count):
        parts = [ref[n] for n in range(first, first + count)]
        while len(parts) > 1:
            parts = [sum(parts[n:n + 2]) for n in range(0, len(parts), 2)]
        return parts[0]

    @pl.when(tp == 1)
    def _():
        lines[x] = vec
        for o in far_first(nx):
            remote(lines.at[x], lines.at[x], xy_send, x_recv, along(2, o)).start()
        if beside:
            pl.semaphore_wait(plane_round, len(beside))
        signal(round1, (z, y, x, 0))
        stage_results()
        send_results(jnp.logical_and(x > 0, x < nx - 1))
        if nx > 1:
            wait_bytes(lines.at[:nx - 1], x_recv)
        lines[nx + y] = sum_of(lines, 0, nx)
        for o in far_first(ny):
            remote(lines.at[nx + y], lines.at[nx + y], xy_send, y_recv, along(1, o)).start()
        wait_bytes(plane, plane_recv)
        others = sum_of(plane, 0, nx * ny)
        if ny > 1:
            wait_bytes(lines.at[:ny - 1], y_recv)
        part = sum_of(lines, nx, ny)
        gain = part[3:] + others[3:]
        for core, rows in enumerate((others, part)):
            zout[core, :3] = rows[:3]
            zout[core, 3:] = gain
        zbuf[z] = zout[1]
        if nz > 9:
            pl.semaphore_wait(round3, len(near(nz, 3)))
        for o in [*far_first(nz), 0]:
            for core in range(2 if o else 1):
                remote(zout.at[core], zbuf.at[z], z_send, z_recv, along(0, o, core)).start()
        send_results(jnp.logical_or(x == 0, x == nx - 1))
        signal(round2, (z, y, x, 0))

    @pl.when(tp == 0)
    def _():
        plane[chip] = vec
        pl.semaphore_wait(round1, 1)
        for oy, ox in sorted(
                ((oy, ox) for oy in range(ny) for ox in range(nx)),
                key=lambda o: -min(o[0], ny - o[0]) - min(o[1], nx - o[1])):
            remote(
                plane.at[chip], plane.at[chip], xy_send, plane_recv,
                (z, lax.rem(y + oy, ny), lax.rem(x + ox, nx), 1)).start()
        stage_results()
        send_results(jnp.logical_or(opens, jnp.logical_and(x > 0, x < nx - 1)))
        pl.semaphore_wait(round2, 1)
        send_results(jnp.logical_and(jnp.logical_not(opens), jnp.logical_or(x == 0, x == nx - 1)))

    @pl.when(takes_back)
    def _():
        wait_bytes(kvx.at[:, :, :PAIR], before_recv)

    @pl.when(closes_early)
    def _():
        to_plane_before.wait_recv()

    for h in range(HEADS):
        dq_v[:SEG, h * HEAD_DIM:(h + 1) * HEAD_DIM] = query_rows(dq_from_before[h], qu[h, :SEG], qr[h, :SEG])

    for h in range(HEADS):
        @pl.when(place < total - 1)
        def _(h=h):
            to_neighbours[h].wait_recv()

        lanes = slice(h * HEAD_DIM, (h + 1) * HEAD_DIM)
        sums_in = [
            jnp.concatenate([
                jnp.where(takes_next, 0.0, jnp.where(is_last, 0.0, from_after_first[n, h].astype(F32)))
                + from_before[n, h].astype(F32), from_after[n, h].astype(F32)], axis=0) for n in range(2)]
        g = (dkx[h, BEFORE:BEFORE + ROWS] * FACTOR + sums_in[0]) * gain_k
        u = ku[h]
        dk_v[:, lanes] = (kr[h] * (g - u * jnp.mean(g * u, axis=-1, keepdims=True))).astype(BF16)
        dv_v[:, lanes] = (dvx[h, BEFORE:BEFORE + ROWS] + sums_in[1]).astype(BF16)

    @pl.when(takes_next)
    def _():
        wait_bytes(kvx.at[:, :, :BEFORE], halo_send.at[0])
        wait_bytes(kvx.at[:, :, :PAIR], back_send.at[1])

    @pl.when(closes_early)
    def _():
        wait_bytes(kvx.at[:, :, :ROWS], halo_send.at[0])

    @pl.when(takes_back)
    def _():
        wait_bytes(kvx.at[:, :, :PAIR], halo_send.at[1])
        wait_bytes(from_after, back_send.at[0])

    @pl.when(opens_later)
    def _():
        wait_bytes(kvx.at[:, :, :ROWS], back_send.at[0])

    @pl.when(tp == 1)
    def _():
        if nx + ny > 2:
            wait_bytes(lines.at[:nx + ny - 2], xy_send)
        wait_bytes(zbuf.at[:2 * nz - 1], z_send)
        if nz > 1:
            wait_bytes(zbuf.at[:nz - 1], z_recv)

    @pl.when(tp == 0)
    def _():
        wait_bytes(plane, xy_send)
        wait_bytes(zbuf.at[:nz], z_recv)

    result = zbuf[0]
    for n in range(1, nz):
        result = result + zbuf[n]
    for j in range(HEADS):
        dtab_v[j:j + 1, :PAIR] = result[j:j + 1]
        dtab_v[j:j + 1, PAIR:] = result[2:3, j * SEG:(j + 1) * SEG]
    dgain_v[0:1] = result[3:] / gain_q
    dgain_v[1:2] = result[3:] / gain_k


def write_out(*refs):
    count = len(refs) // 2
    copies = [pltpu.make_async_copy(refs[n], refs[count + n], refs[-1].at[n]) for n in range(count)]
    for copy in copies:
        copy.start()
    for copy in copies:
        copy.wait()


def local(sizes, queries, keys, values, gains, bias_table, d_out):
    nz, ny, nx = sizes
    width = HEADS * HEAD_DIM
    hbm_spec = pl.BlockSpec(memory_space=pltpu.HBM)
    vmem_spec = pl.BlockSpec(memory_space=pltpu.VMEM)
    first = (HEADS, SEG, HEAD_DIM)
    tile = (HEADS, ROWS, HEAD_DIM)
    wide = (HEADS, 2 * ROWS, HEAD_DIM)
    pairs = (HEADS, 2, 3 * PAIR, PAIR)
    dma, regular = pltpu.SemaphoreType.DMA, pltpu.SemaphoreType.REGULAR
    vmem = pltpu.VMEM
    outs = [((ROWS, width), BF16)] * 3 + [((HEADS, ENTRIES), F32), ((2, HEAD_DIM), F32)]
    out = pl.pallas_call(
        functools.partial(kernel, sizes),
        out_shape=tuple(vmem(*o) for o in outs),
        in_specs=[hbm_spec] * 6,
        out_specs=(vmem_spec,) * 5,
        scratch_shapes=[
            vmem(tile, BF16), vmem(tile, BF16), vmem((2, *tile), BF16), vmem((2, *first), BF16), vmem((2, *wide), BF16), vmem((2, *first), BF16),
            vmem((2, HEAD_DIM), F32), vmem((HEADS, ENTRIES), F32),
            vmem(tile, F32), vmem(tile, F32), vmem(tile, F32), vmem(tile, F32),
            vmem(pairs, F32), vmem(pairs, F32), vmem(pairs, F32),
            vmem(wide, F32), vmem(wide, F32), vmem(tile, F32), vmem((HEADS, 3 * PAIR, PAIR), F32),
            vmem(pairs, BF16), vmem(pairs, BF16), vmem((HEADS, 2, 6, 1, PAIR), F32), vmem((HEADS, 2, 1, PAIR), F32),
            vmem((HEADS, 2, 1, PAIR), F32), vmem((1, HEAD_DIM), F32), vmem((HEADS, BEFORE, HEAD_DIM), F32),
            vmem((2, HEADS, BEFORE, HEAD_DIM), BF16), vmem((2, HEADS, BEFORE, HEAD_DIM), BF16),
            vmem((2, *first), BF16), vmem((2, *first), BF16), vmem(first, F32), vmem((2, *first), BF16), vmem((2, *first), BF16),
            vmem((nx + ny, 4, HEAD_DIM), F32), vmem((nx * ny, 4, HEAD_DIM), F32), vmem((2, 4, HEAD_DIM), F32), vmem((2 * nz, 4, HEAD_DIM), F32),
            dma((2,)), dma, dma, dma((2,)), dma((HEADS + 2,)), dma((HEADS,)), dma((2,)), dma((HEADS,)), dma, dma,
            dma, dma, dma, dma, dma, dma, regular, regular, regular, regular,
        ],
        compiler_params=pltpu.CompilerParams(
            collective_id=0, has_side_effects=True, vmem_limit_bytes=32 * 1024 * 1024),
        name="segment_attention_grad",
    )(*(pltpu.with_memory_space_constraint(a, pltpu.HBM) for a in (queries, keys, values, d_out, gains, bias_table.T)))
    d_queries, d_keys, d_values, d_table, d_gains = pl.pallas_call(
        write_out,
        out_shape=tuple(jax.ShapeDtypeStruct(*o) for o in outs),
        in_specs=[vmem_spec] * 5,
        out_specs=(hbm_spec,) * 5,
        scratch_shapes=[dma((5,))],
        name="write_out",
    )(*(pltpu.with_memory_space_constraint(o, pltpu.VMEM) for o in out))
    return d_queries, d_keys, d_values, d_table.T, d_gains


def solution(mesh):
    shape = (12, 8, 4)
    if mesh.shape["sp"] != int(np.prod(shape)):
        shape = mesh.small_shape
    split = Mesh(mesh.devices.reshape(*shape, mesh.shape["tp"]), AXES)
    placed = (P(SP, "tp"), P(SP, "tp"), P(SP, "tp"), P(), P(None, "tp"), P(SP, "tp"))
    return jax.shard_map(
        functools.partial(local, shape),
        mesh=split,
        in_specs=placed,
        out_specs=(P(SP, "tp"), P(SP, "tp"), P(SP, "tp"), P(None, "tp"), P()),
        check_vma=False,
    )
```

```python
import functools

import jax
import jax.numpy as jnp
import numpy as np
from jax import lax
from jax.experimental import pallas as pl
from jax.experimental.pallas import tpu as pltpu
from jax.sharding import Mesh
from jax.sharding import PartitionSpec as P

HEAD_DIM = 128
SEG = 64
LEFT = 4
MAX_REL = 128
ENTRIES = MAX_REL + SEG
ROWS = LEFT * SEG
HEADS = 2
PAIR = 2 * SEG
BEFORE = 3 * SEG
AXES = ("sp_0", "sp_1", "sp_2", "tp")
SP = AXES[:3]

EPSILON = 1e-06
FACTOR = HEAD_DIM ** (-0.5)
LOG2E = 1.4426950408889634
MASKED = -1e30
F32, BF16 = jnp.float32, jnp.bfloat16


def dot(a, b, a_dim, b_dim):
    return lax.dot_general(a, b, (((a_dim,), (b_dim,)), ((), ())), preferred_element_type=F32)


def near(size, step=1):
    return sorted({step % size, -step % size} - {0})


def far_first(size):
    return sorted(range(1, size), key=lambda d: -min(d, size - d))


def unit(raw):
    wide = raw.astype(F32)
    inv_rms = lax.rsqrt(jnp.mean(wide * wide, axis=-1, keepdims=True) + EPSILON)
    return wide * inv_rms, inv_rms


def kernel(sizes, q_hbm, k_hbm, v_hbm, do_hbm, gains_hbm, table_hbm,
           dq_v, dk_v, dv_v, dtab_v, dgain_v,
           q_raw, k_raw, qdx, qd0, kvx, first_kv, gains_v, table_v,
           qu, qr, ku, kr, bias_v, e_v, dp_v,
           dkx, dvx, dqx, d_v, prob_v, d_low_v, sum_v, gain_v, table_v2, extra_gain, first_prob, first_d_low, first_dk,
           to_before, from_after, to_after, from_before, dq_from_before, to_before_first, from_after_first,
           rows_x, plane, zout, zbuf,
           load_sem, more_sem, gains_sem, table_sem, left_recv, right_recv, after_recv, before_recv,
           sum_send, x_recv, plane_recv, z_recv, round1, round2, round3, plane_round):
    nz, ny, nx = sizes
    z, y, x, tp = (lax.axis_index(a) for a in AXES)
    place = (z * ny + y) * nx + x
    total = nz * ny * nx
    is_first, is_last = place == 0, place == total - 1
    opens, closes = jnp.logical_and(x == 0, y == 0), jnp.logical_and(x == nx - 1, y == ny - 1)
    opens_later, closes_early = jnp.logical_and(opens, place > 0), jnp.logical_and(closes, place < total - 1)
    takes_back, takes_next = jnp.logical_not(opens), jnp.logical_not(closes)

    def at(number, core):
        return (number // (ny * nx), (number // nx) % ny, number % nx, core)

    after = at(jnp.minimum(place + 1, total - 1), tp)
    before = at(jnp.maximum(place - 1, 0), tp)

    def along(axis, offset, core=1):
        if axis == 0:
            return (lax.rem(z + offset, nz), y, x, core)
        if axis == 1:
            return (z, lax.rem(y + offset, ny), x, core)
        return (z, y, lax.rem(x + offset, nx), core)

    def signal(sem, target):
        pl.semaphore_signal(sem, inc=1, device_id=target, device_id_type=pl.DeviceIdType.MESH)

    def remote(src, dst, send, recv, target):
        return pltpu.make_async_remote_copy(
            src_ref=src, dst_ref=dst, send_sem=send, recv_sem=recv,
            device_id=target, device_id_type=pl.DeviceIdType.MESH)

    def wait_bytes(ref, sem):
        pltpu.make_async_copy(ref, ref, sem).wait()

    barrier = pltpu.get_barrier_semaphore()

    @pl.when(place > 0)
    def _():
        signal(barrier, before)

    @pl.when(place < total - 1)
    def _():
        signal(barrier, after)

    sides = jnp.where(is_first, 0, 1) + jnp.where(is_last, 0, 1)
    small_loads = [pltpu.make_async_copy(gains_hbm, gains_v, gains_sem), pltpu.make_async_copy(table_hbm, table_v, table_sem)]
    for load in small_loads:
        load.start()
    for h in range(HEADS):
        lanes = slice(h * HEAD_DIM, (h + 1) * HEAD_DIM)
        pltpu.make_async_copy(k_hbm.at[:, lanes], k_raw.at[h], load_sem).start()
        pltpu.make_async_copy(q_hbm.at[:, lanes], q_raw.at[h], load_sem).start()
        pltpu.make_async_copy(v_hbm.at[:, lanes], kvx.at[1, h, BEFORE:BEFORE + ROWS], load_sem).start()
        pltpu.make_async_copy(do_hbm.at[:SEG, lanes], qd0.at[1, h], load_sem).start()
        pltpu.make_async_copy(do_hbm.at[SEG:, lanes], qdx.at[1, h, :BEFORE], more_sem).start()

    close = [(a, o) for a, n in enumerate(sizes) for o in near(n)]

    @pl.when(tp == 1)
    def _():
        for a, o in close:
            signal(barrier, along(a, o))
        signal(barrier, (z, y, x, 0))

    @pl.when(tp == 0)
    def _():
        signal(barrier, (z, y, x, 1))

    for load in small_loads:
        load.wait()
    gains = gains_v[...]
    gain_q, gain_k = gains[0:1, :], gains[1:2, :]
    wait_bytes(kvx.at[:, :, :ROWS + PAIR + SEG // 2], load_sem)
    def norm_keys(first, size):
        for h in range(HEADS):
            u, r = unit(k_raw[h, first:first + size])
            ku[h, first:first + size] = u
            kr[h, first:first + size] = jnp.broadcast_to(r, u.shape)
            kvx[0, h, BEFORE + first:BEFORE + first + size] = (u * gain_k).astype(BF16)

    def norm_queries(first, size, out):
        for h in range(HEADS):
            u, r = unit(q_raw[h, first:first + size])
            qu[h, first:first + size] = u
            qr[h, first:first + size] = jnp.broadcast_to(r, u.shape)
            out[h] = (u * gain_q).astype(BF16)

    forth = [remote(
        kvx.at[:, :, ROWS + PAIR:ROWS + BEFORE], kvx.at[:, :, PAIR:BEFORE], load_sem, left_recv.at[HEADS], after)]
    back = {}
    for h in range(HEADS):
        forth.append(remote(
            kvx.at[:, h, ROWS:ROWS + PAIR], kvx.at[:, h, :PAIR], load_sem, left_recv.at[h], after))
        back[h] = [
            remote(kvx.at[:, h, BEFORE:ROWS], kvx.at[:, h, BEFORE + ROWS:], gains_sem, right_recv, before),
            remote(qd0.at[:, h], qdx.at[:, h, BEFORE:], gains_sem, right_recv, before)]

    plane_piece = remote(kvx.at[:, :, BEFORE:ROWS], first_kv, load_sem, left_recv.at[HEADS - 1], after)

    def go_on(pieces, when=place < total - 1):
        @pl.when(when)
        def _():
            for copy in pieces:
                copy.start()

    norm_keys(BEFORE, SEG)
    pl.semaphore_wait(barrier, sides + jnp.where(tp == 1, 1 + len(close), 1))
    go_on(forth[:1])
    norm_keys(0, SEG)
    norm_queries(0, SEG, qd0.at[0])

    go_on([copy for h in range(HEADS) for copy in back[h]], takes_back)
    norm_keys(SEG, PAIR)
    go_on(forth[1:], jnp.logical_and(tp == 0, place < total - 1))
    go_on(forth[1:2], jnp.logical_and(tp == 1, place < total - 1))
    go_on([plane_piece], closes_early)
    norm_queries(SEG, BEFORE, qdx.at[0, :, :BEFORE])

    @pl.when(tp == 1)
    def _():
        for a, o in close:
            signal(round1, along(a, o))

    wait_bytes(qdx.at[1, :, :BEFORE], more_sem)

    @pl.when(is_first)
    def _():
        for h in range(HEADS):
            for n in range(2):
                kvx[n, h, :BEFORE] = kvx[n, h, BEFORE:2 * BEFORE]
                first_kv[n, h] = kvx[n, h, BEFORE:ROWS]

    @pl.when(closes)
    def _():
        for h in range(HEADS):
            for n in range(2):
                kvx[n, h, BEFORE + ROWS:] = kvx[n, h, BEFORE:ROWS]
            qdx[0, h, BEFORE:] = qd0[0, h]
            qdx[1, h, BEFORE:] = jnp.zeros((SEG, HEAD_DIM), BF16)

    @pl.when(is_last)
    def _():
        for h in range(HEADS):
            for n in range(2):
                from_after[n, h] = jnp.zeros((BEFORE, HEAD_DIM), BF16)

    key_at = lax.broadcasted_iota(jnp.int32, (PAIR, PAIR), 0)
    query_at = lax.broadcasted_iota(jnp.int32, (PAIR, PAIR), 1)
    past = query_at >= key_at
    early = query_at < SEG
    high = key_at >= SEG
    lane = lax.broadcasted_iota(jnp.int32, (1, PAIR), 1)
    table = table_v[...]
    low_part = table[:, :PAIR]
    high_part = jnp.concatenate([table[:, PAIR:], jnp.zeros((HEADS, 2 * PAIR - ENTRIES), F32)], axis=1)
    low_rolled = pltpu.roll(low_part, PAIR - SEG + 1, 1)
    high_rolled = pltpu.roll(high_part, PAIR - SEG + 1, 1)
    for h in range(HEADS):
        last = table[h:h + 1, ENTRIES - 1:ENTRIES]
        dist_low = low_rolled[h:h + 1]
        dist_row = jnp.where(lane <= SEG, dist_low, high_rolled[h:h + 1])
        ahead = pltpu.roll(jnp.broadcast_to(dist_low, (PAIR, PAIR)), 0, 1, stride=1, stride_axis=0)
        behind = pltpu.roll(jnp.broadcast_to(dist_row, (PAIR, PAIR)), 0, 1, stride=1, stride_axis=0)
        tile0 = jnp.where(jnp.logical_or(early, high), last, MASKED)
        tile1 = jnp.where(past, last, behind)
        tile2 = jnp.where(jnp.logical_and(early, high), MASKED, jnp.where(past, behind, ahead))
        none, low = (jnp.where(is_first, MASKED, t) for t in (tile0, tile1))
        for p, tiles in enumerate((
                (none, jnp.where(high, tile1, low), tile2),
                (jnp.where(high, tile0, none), tile1, tile2))):
            top = jnp.max(jnp.maximum(jnp.maximum(tiles[0], tiles[1]), tiles[2]), axis=0, keepdims=True)
            for b, tile in enumerate(tiles):
                bias_v[h, p, b * PAIR:(b + 1) * PAIR] = (tile - top) * LOG2E

    def work(blocks, tiles=()):
        at_keys = {(p, b): slice((p + b) * PAIR, (p + b + 1) * PAIR) for h, p, b in blocks}
        at_queries = [slice(p * PAIR, (p + 1) * PAIR) for p in range(2)]
        at_rows = [slice(b * PAIR, (b + 1) * PAIR) for b in range(3)]
        scores = [dot(kvx[0, h, at_keys[p, b]], qdx[0, h, at_queries[p]], 1, 1) for h, p, b in blocks]
        d_probs = [dot(kvx[1, h, at_keys[p, b]], qdx[1, h, at_queries[p]], 1, 1) for h, p, b in blocks]
        for (h, p, b), s, dp in zip(blocks, scores, d_probs):
            e = jnp.exp2(s * (FACTOR * LOG2E) + bias_v[h, p, at_rows[b]])
            e_v[h, p, at_rows[b]] = e
            dp_v[h, p, at_rows[b]] = dp
            sum_v[h, p, b] = jnp.sum(e, axis=0, keepdims=True)
            sum_v[h, p, 3 + b] = jnp.sum(e * dp, axis=0, keepdims=True)
        d_scores, products = [], []
        for h, p, _ in tiles:
            inv = 1.0 / (sum_v[h, p, 0] + sum_v[h, p, 1] + sum_v[h, p, 2])
            delta = (sum_v[h, p, 3] + sum_v[h, p, 4] + sum_v[h, p, 5]) * inv
            prob = e_v[h, p] * inv
            d_score = prob * (dp_v[h, p] - delta)
            d_low = d_score.astype(BF16)
            prob_v[h, p] = prob.astype(BF16)
            d_low_v[h, p] = d_low
            d_scores.append(d_score)
            products.append(dot(d_low, qdx[0, h, at_queries[p]], 1, 0))
        for (h, p, again), d_score in zip(tiles, d_scores):
            if again:
                fold_table(h, d_v[h] + d_score)
            else:
                d_v[h] = d_score
        for (h, p, again), dk in zip(tiles, products):
            keys = slice(p * PAIR, (p + 3) * PAIR)
            gain_v[h, p] = jnp.sum(dk * kvx[0, h, keys].astype(F32), axis=0, keepdims=True)
            if again:
                shared, alone = slice(PAIR, 3 * PAIR), slice(3 * p * PAIR, (3 * p + 1) * PAIR)
                dkx[h, alone] = dk[2 * p * PAIR:(2 * p + 1) * PAIR]
                dkx[h, shared] = dkx[h, shared] + dk[(1 - p) * PAIR:(3 - p) * PAIR]
            else:
                dkx[h, keys] = dk

    def query_rows(g, u, r):
        g = g * FACTOR * gain_q
        return (r * (g - u * jnp.mean(g * u, axis=-1, keepdims=True))).astype(BF16)

    sublane = lax.broadcasted_iota(jnp.int32, (8, PAIR), 0)

    def skewed_sum(tile, right):
        parts = [pltpu.roll(tile[first:first + 8], (right - first) % PAIR, 1) for first in range(0, PAIR, 8)]
        while len(parts) > 1:
            parts = [a + b for a, b in zip(parts[::2], parts[1::2])]
        total = parts[0]
        for bit in range(1, 8):
            total = jnp.where(sublane == bit, pltpu.roll(parts[0], PAIR - bit, 1), total)
        return jnp.sum(total, axis=0, keepdims=True)

    def fold_rows(h, d_score):
        d0, d1, d2 = (d_score[b * PAIR:(b + 1) * PAIR] for b in range(3))
        mixed = jnp.where(past, d2, d1)
        ahead = jnp.where(past, 0.0, d2)
        rest = d0 + jnp.where(past, d1, 0.0)
        behind_row, ahead_row = skewed_sum(mixed, SEG - 1), skewed_sum(ahead, SEG - 1)
        high_row = skewed_sum(mixed, SEG - 1 + SEG) if h else behind_row
        rest_sum = jnp.sum(jnp.sum(rest, axis=0, keepdims=True), axis=1, keepdims=True)
        return (
            jnp.where(lane < SEG - 1, ahead_row, behind_row),
            jnp.where(lane == SEG - 1 + h * SEG, rest_sum, high_row))

    def fold_table(h, d_score):
        table_v2[h, 0], table_v2[h, 1] = fold_rows(h, d_score)

    def first_segment():
        key_number = lax.broadcasted_iota(jnp.int32, (ROWS + SEG, SEG), 0)
        hidden = jnp.logical_and(is_first, key_number < ROWS)

        def against(n, h, side):
            return jnp.concatenate([dot(first_kv[n, h], side, 1, 1), dot(kvx[n, h, :ROWS], side, 1, 1)], axis=0)

        scores = [against(0, h, qd0[0, h]) for h in heads]
        d_probs = [against(1, h, qd0[1, h]) for h in heads]
        d_scores = []
        for h in heads:
            bias = jnp.where(hidden, MASKED, bias_v[h, 0, :ROWS + SEG][:, :SEG])
            bias = bias - jnp.max(bias, axis=0, keepdims=True)
            e = jnp.exp2(scores[h] * (FACTOR * LOG2E) + bias)
            inv = 1.0 / jnp.sum(e, axis=0, keepdims=True)
            delta = jnp.sum(e * d_probs[h], axis=0, keepdims=True) * inv
            prob = e * inv
            d_scores.append(prob * (d_probs[h] - delta))
            first_prob[h] = prob.astype(BF16)
            first_d_low[h] = d_scores[h].astype(BF16)
        products = [dot(d_scores[h].astype(BF16), qd0[0, h], 1, 0) for h in heads]
        for h in heads:
            tile = jnp.concatenate([d_scores[h], jnp.zeros((ROWS + SEG, SEG), F32)], axis=1)
            rows = fold_rows(h, jnp.concatenate([tile, jnp.zeros((SEG, PAIR), F32)], axis=0))
            for j in range(2):
                table_v2[h, j] = table_v2[h, j] + rows[j]
        gain = jnp.zeros((1, HEAD_DIM), F32)
        for h in heads:
            dk = products[h]
            first_dk[h] = dk
            gain = gain + jnp.sum(dk[:SEG] * first_kv[0, h].astype(F32), axis=0, keepdims=True)
            gain = gain + jnp.sum(dk[SEG:] * kvx[0, h, :ROWS].astype(F32), axis=0, keepdims=True)
        extra_gain[...] = gain

    def first_results(h):
        d_low = first_d_low[h]
        dv = dot(first_prob[h], qd0[1, h], 1, 0)
        dq_from_before[h] = dot(d_low[:SEG], first_kv[0, h], 0, 0) + dot(d_low[SEG:], kvx[0, h, :ROWS], 0, 0)
        for n, part in enumerate((first_dk[h] * FACTOR, dv)):
            to_before_first[n, h] = part[:SEG].astype(BF16)
            from_before[n, h] = part[ROWS:].astype(BF16)
        dkx[h, :BEFORE] = dkx[h, :BEFORE] + first_dk[h, SEG:ROWS]
        dvx[h, :BEFORE] = dvx[h, :BEFORE] + dv[SEG:ROWS]

    heads = range(HEADS)
    work([(h, 0, 2) for h in heads])

    go_on(forth[2:], jnp.logical_and(tp == 1, place < total - 1))
    @pl.when(tp == 1)
    def _():
        pl.semaphore_wait(round1, len(close))
        for a, n in enumerate(sizes[:2]):
            if n > 5:
                for o in near(n, 2):
                    signal(round2, along(a, o))

    def wait_left(piece):
        @pl.when(place > 0)
        def _():
            if piece < HEADS:
                forth[piece].wait_recv()
            else:
                @pl.when(opens)
                def _():
                    wait_bytes(kvx.at[:, :, :PAIR], left_recv.at[piece - 1])

                @pl.when(takes_back)
                def _():
                    forth[piece].wait_recv()

    def wait_right():
        @pl.when(takes_next)
        def _():
            wait_bytes(kvx.at[:, :, :PAIR], right_recv)

    beside = sorted({*near(ny), *near(ny, 2)})

    def greet_far():
        @pl.when(tp == 1)
        def _():
            count = sum(len(near(n, 2)) for n in sizes[:2] if n > 5)
            if count:
                pl.semaphore_wait(round2, count)
            for o in beside:
                signal(plane_round, along(1, o))
            if nz > 9:
                for o in near(nz, 3):
                    signal(round3, along(0, o))

    def do_first():
        @pl.when(opens)
        def _():
            first_segment()

    @pl.when(x == nx - 1)
    def _():
        wait_left(0)
        work([(h, 0, 1) for h in heads])
        for h in heads:
            wait_left(1 + h)
            work([(h, 0, 0)], [(h, 0, False)])
            if not h:
                greet_far()
        wait_right()
        work([(h, 1, b) for b in range(3) for h in heads], [(h, 1, True) for h in heads])
        if nx == 1:
            do_first()

    if nx > 1:
        @pl.when(x == 0)
        def _():
            wait_right()
            work([(h, 1, b) for b in (1, 2) for h in heads])
            greet_far()
            wait_left(0)
            work([(h, p, 1 - p) for p in (1, 0) for h in heads], [(h, 1, False) for h in heads])
            for h in heads:
                wait_left(1 + h)
                work([(h, 0, 0)], [(h, 0, True)])
            do_first()

    if nx > 2:
        @pl.when(jnp.logical_and(x > 0, x < nx - 1))
        def _():
            wait_left(0)
            work([(h, 0, 1) for h in heads])
            wait_right()
            work([(h, 1, b) for b in range(3) for h in heads], [(h, 1, False) for h in heads])
            greet_far()
            for h in heads:
                wait_left(1 + h)
                work([(h, 0, 0)], [(h, 0, True)])

    gain = gain_v[0, 0] + gain_v[0, 1] + gain_v[1, 0] + gain_v[1, 1] + jnp.where(opens, extra_gain[...], 0.0)
    second = jnp.where(lane < SEG, table_v2[0, 1], table_v2[1, 1])
    vec = jnp.concatenate([table_v2[0, 0], table_v2[1, 0], second, gain * FACTOR], axis=0)
    chip = y * nx + x

    to_neighbours = [
        remote(to_before.at[:, h], from_after.at[:, h], more_sem, after_recv, before) for h in range(HEADS)]
    to_next = [
        remote(to_after, from_before, table_sem, before_recv, after),
        remote(dqx.at[:, BEFORE:], dq_from_before, table_sem, before_recv, after)]
    to_plane_before = remote(to_before_first, from_after_first, more_sem, after_recv, before)

    def stage_results():
        @pl.when(takes_next)
        def _():
            wait_bytes(kvx.at[:, :, :BEFORE], load_sem)

        @pl.when(closes_early)
        def _():
            wait_bytes(kvx.at[:, :, :ROWS], load_sem)

        @pl.when(takes_back)
        def _():
            wait_bytes(kvx.at[:, :, :PAIR], gains_sem)

        for h in range(HEADS):
            low, high_tile = (dot(prob_v[h, p], qdx[1, h, p * PAIR:(p + 1) * PAIR], 1, 0) for p in range(2))
            dvx[h, :PAIR] = low[:PAIR]
            dvx[h, PAIR:3 * PAIR] = low[PAIR:] + high_tile[:2 * PAIR]
            dvx[h, 3 * PAIR:] = high_tile[2 * PAIR:]

            @pl.when(opens)
            def _(h=h):
                first_results(h)

            lanes = slice(h * HEAD_DIM, (h + 1) * HEAD_DIM)
            to_before[0, h] = (dkx[h, :BEFORE] * FACTOR).astype(BF16)
            to_before[1, h] = dvx[h, :BEFORE].astype(BF16)
            to_after[0, h] = (dkx[h, BEFORE + ROWS:] * FACTOR).astype(BF16)
            to_after[1, h] = dvx[h, BEFORE + ROWS:].astype(BF16)
            for p in range(2):
                dqx[h, p * PAIR:(p + 1) * PAIR] = dot(d_low_v[h, p], kvx[0, h, p * PAIR:(p + 3) * PAIR], 0, 0)
            dq_v[SEG:, lanes] = query_rows(dqx[h, :BEFORE], qu[h, SEG:], qr[h, SEG:])

    def send_results(when):
        @pl.when(jnp.logical_and(when, place > 0))
        def _():
            for copy in to_neighbours:
                copy.start()

        @pl.when(jnp.logical_and(when, opens_later))
        def _():
            to_plane_before.start()

        @pl.when(jnp.logical_and(when, takes_next))
        def _():
            for copy in to_next:
                copy.start()

    def sum_of(ref, first, count):
        parts = [ref[n] for n in range(first, first + count)]
        while len(parts) > 1:
            parts = [sum(parts[n:n + 2]) for n in range(0, len(parts), 2)]
        return parts[0]

    has_across = ny > 3 and ny % 2 == 0
    across, column = nx * ny, nx * ny + nx

    @pl.when(tp == 1)
    def _():
        rows_x[x] = vec
        for o in far_first(nx):
            remote(rows_x.at[x], rows_x.at[x], sum_send, x_recv, along(2, o)).start()
        if beside:
            pl.semaphore_wait(plane_round, len(beside))
        signal(round1, (z, y, x, 0))
        if has_across:
            for o in far_first(nx) + [0]:
                remote(
                    rows_x.at[x], plane.at[across + x], sum_send, plane_recv,
                    (z, lax.rem(y + ny // 2, ny), lax.rem(x + o, nx), 1)).start()
        stage_results()
        send_results(jnp.logical_and(x > 0, x < nx - 1))
        if nx > 1:
            wait_bytes(rows_x.at[:nx - 1], x_recv)
        plane[column + y] = sum_of(rows_x, 0, nx)
        y_ways = [o for o in far_first(ny) if not has_across or o != ny // 2]
        for o in y_ways:
            remote(plane.at[column + y], plane.at[column + y], sum_send, plane_recv, along(1, o)).start()
        came = nx * ny + len(y_ways) + (nx if has_across else 0)
        wait_bytes(plane.at[:came], plane_recv)
        if has_across:
            plane[column + lax.rem(y + ny // 2, ny)] = sum_of(plane, across, nx)
        others, part = sum_of(plane, 0, nx * ny), sum_of(plane, column, ny)
        gain = part[3:] + others[3:]
        for core, rows in enumerate((others, part)):
            zout[core, :3] = rows[:3]
            zout[core, 3:] = gain
        zbuf[z] = zout[1]
        if nz > 9:
            pl.semaphore_wait(round3, len(near(nz, 3)))
        for o in [*far_first(nz), 0]:
            for core in range(2 if o else 1):
                remote(zout.at[core], zbuf.at[z], sum_send, z_recv, along(0, o, core)).start()
        send_results(jnp.logical_or(x == 0, x == nx - 1))
        signal(round2, (z, y, x, 0))

    @pl.when(tp == 0)
    def _():
        plane[chip] = vec
        pl.semaphore_wait(round1, 1)
        for oy, ox in sorted(
                ((oy, ox) for oy in range(ny) for ox in range(nx)),
                key=lambda o: -min(o[0], ny - o[0]) - min(o[1], nx - o[1])):
            remote(
                plane.at[chip], plane.at[chip], sum_send, plane_recv,
                (z, lax.rem(y + oy, ny), lax.rem(x + ox, nx), 1)).start()
        stage_results()
        send_results(jnp.logical_or(opens, jnp.logical_and(x > 0, x < nx - 1)))
        pl.semaphore_wait(round2, 1)
        send_results(jnp.logical_and(jnp.logical_not(opens), jnp.logical_or(x == 0, x == nx - 1)))

    @pl.when(takes_back)
    def _():
        wait_bytes(kvx.at[:, :, :PAIR], before_recv)

    @pl.when(takes_next)
    def _():
        wait_bytes(from_after, after_recv)

    @pl.when(closes_early)
    def _():
        wait_bytes(kvx.at[:, :, :ROWS], after_recv)

    for h in range(HEADS):
        dq_v[:SEG, h * HEAD_DIM:(h + 1) * HEAD_DIM] = query_rows(dq_from_before[h], qu[h, :SEG], qr[h, :SEG])

    for h in range(HEADS):
        lanes = slice(h * HEAD_DIM, (h + 1) * HEAD_DIM)
        sums_in = [
            jnp.concatenate([
                jnp.where(takes_next, 0.0, jnp.where(is_last, 0.0, from_after_first[n, h].astype(F32)))
                + from_before[n, h].astype(F32), from_after[n, h].astype(F32)], axis=0) for n in range(2)]
        g = (dkx[h, BEFORE:BEFORE + ROWS] * FACTOR + sums_in[0]) * gain_k
        u = ku[h]
        dk_v[:, lanes] = (kr[h] * (g - u * jnp.mean(g * u, axis=-1, keepdims=True))).astype(BF16)
        dv_v[:, lanes] = (dvx[h, BEFORE:BEFORE + ROWS] + sums_in[1]).astype(BF16)

    @pl.when(takes_next)
    def _():
        wait_bytes(kvx.at[:, :, :PAIR], table_sem)

    @pl.when(takes_back)
    def _():
        wait_bytes(from_after, more_sem)

    @pl.when(opens_later)
    def _():
        wait_bytes(kvx.at[:, :, :ROWS], more_sem)

    @pl.when(tp == 1)
    def _():
        wait_bytes(plane.at[:nx - 1 + 2 * nz - 1 + ny - 1 + (nx - 1 if has_across else 0)], sum_send)
        if nz > 1:
            wait_bytes(zbuf.at[:nz - 1], z_recv)

    @pl.when(tp == 0)
    def _():
        wait_bytes(plane.at[:nx * ny], sum_send)
        wait_bytes(zbuf.at[:nz], z_recv)

    result = zbuf[0]
    for n in range(1, nz):
        result = result + zbuf[n]
    for j in range(HEADS):
        dtab_v[j:j + 1, :PAIR] = result[j:j + 1]
        dtab_v[j:j + 1, PAIR:] = result[2:3, j * SEG:(j + 1) * SEG]
    dgain_v[0:1] = result[3:] / gain_q
    dgain_v[1:2] = result[3:] / gain_k


def write_out(*refs):
    count = len(refs) // 2
    copies = [pltpu.make_async_copy(refs[n], refs[count + n], refs[-1].at[n]) for n in range(count)]
    for copy in copies:
        copy.start()
    for copy in copies:
        copy.wait()


def local(sizes, queries, keys, values, gains, bias_table, d_out):
    nz, ny, nx = sizes
    width = HEADS * HEAD_DIM
    hbm_spec = pl.BlockSpec(memory_space=pltpu.HBM)
    vmem_spec = pl.BlockSpec(memory_space=pltpu.VMEM)
    first = (HEADS, SEG, HEAD_DIM)
    tile = (HEADS, ROWS, HEAD_DIM)
    wide = (HEADS, 2 * ROWS, HEAD_DIM)
    pairs = (HEADS, 2, 3 * PAIR, PAIR)
    dma, regular = pltpu.SemaphoreType.DMA, pltpu.SemaphoreType.REGULAR
    vmem = pltpu.VMEM
    outs = [((ROWS, width), BF16)] * 3 + [((HEADS, ENTRIES), F32), ((2, HEAD_DIM), F32)]
    out = pl.pallas_call(
        functools.partial(kernel, sizes),
        out_shape=tuple(vmem(*o) for o in outs),
        in_specs=[hbm_spec] * 6,
        out_specs=(vmem_spec,) * 5,
        scratch_shapes=[
            vmem(tile, BF16), vmem(tile, BF16), vmem((2, *tile), BF16), vmem((2, *first), BF16), vmem((2, *wide), BF16), vmem((2, *first), BF16),
            vmem((2, HEAD_DIM), F32), vmem((HEADS, ENTRIES), F32),
            vmem(tile, F32), vmem(tile, F32), vmem(tile, F32), vmem(tile, F32),
            vmem(pairs, F32), vmem(pairs, F32), vmem(pairs, F32),
            vmem(wide, F32), vmem(wide, F32), vmem(tile, F32), vmem((HEADS, 3 * PAIR, PAIR), F32),
            vmem(pairs, BF16), vmem(pairs, BF16), vmem((HEADS, 2, 6, 1, PAIR), F32), vmem((HEADS, 2, 1, PAIR), F32),
            vmem((HEADS, 2, 1, PAIR), F32), vmem((1, HEAD_DIM), F32),
            vmem((HEADS, ROWS + SEG, SEG), BF16), vmem((HEADS, ROWS + SEG, SEG), BF16), vmem((HEADS, ROWS + SEG, HEAD_DIM), F32),
            vmem((2, HEADS, BEFORE, HEAD_DIM), BF16), vmem((2, HEADS, BEFORE, HEAD_DIM), BF16),
            vmem((2, *first), BF16), vmem((2, *first), BF16), vmem(first, F32), vmem((2, *first), BF16), vmem((2, *first), BF16),
            vmem((nx, 4, HEAD_DIM), F32), vmem((nx * ny + nx + ny + 2 * nz, 4, HEAD_DIM), F32), vmem((2, 4, HEAD_DIM), F32), vmem((2 * nz, 4, HEAD_DIM), F32),
            dma, dma, dma, dma, dma((HEADS + 1,)), dma, dma, dma,
            dma, dma, dma, dma, regular, regular, regular, regular,
        ],
        compiler_params=pltpu.CompilerParams(
            collective_id=0, has_side_effects=True, vmem_limit_bytes=32 * 1024 * 1024),
        name="segment_attention_grad",
    )(*(pltpu.with_memory_space_constraint(a, pltpu.HBM) for a in (queries, keys, values, d_out, gains, bias_table.T)))
    d_queries, d_keys, d_values, d_table, d_gains = pl.pallas_call(
        write_out,
        out_shape=tuple(jax.ShapeDtypeStruct(*o) for o in outs),
        in_specs=[vmem_spec] * 5,
        out_specs=(hbm_spec,) * 5,
        scratch_shapes=[dma((5,))],
        name="write_out",
    )(*(pltpu.with_memory_space_constraint(o, pltpu.VMEM) for o in out))
    return d_queries, d_keys, d_values, d_table.T, d_gains


def solution(mesh):
    shape = (12, 8, 4)
    if mesh.shape["sp"] != int(np.prod(shape)):
        shape = mesh.small_shape
    split = Mesh(mesh.devices.reshape(*shape, mesh.shape["tp"]), AXES)
    placed = (P(SP, "tp"), P(SP, "tp"), P(SP, "tp"), P(), P(None, "tp"), P(SP, "tp"))
    return jax.shard_map(
        functools.partial(local, shape),
        mesh=split,
        in_specs=placed,
        out_specs=(P(SP, "tp"), P(SP, "tp"), P(SP, "tp"), P(None, "tp"), P()),
        check_vma=False,
    )
```

```python
import functools

import jax
import jax.numpy as jnp
import numpy as np
from jax import lax
from jax.experimental import pallas as pl
from jax.experimental.pallas import tpu as pltpu
from jax.sharding import Mesh
from jax.sharding import PartitionSpec as P

HEAD_DIM = 128
SEG = 64
LEFT = 4
MAX_REL = 128
ENTRIES = MAX_REL + SEG
ROWS = LEFT * SEG
HEADS = 2
PAIR = 2 * SEG
BEFORE = 3 * SEG
AXES = ("sp_0", "sp_1", "sp_2", "tp")
SP = AXES[:3]

EPSILON = 1e-06
FACTOR = HEAD_DIM ** (-0.5)
LOG2E = 1.4426950408889634
MASKED = -1e30
F32, BF16 = jnp.float32, jnp.bfloat16


def dot(a, b, a_dim, b_dim):
    return lax.dot_general(a, b, (((a_dim,), (b_dim,)), ((), ())), preferred_element_type=F32)


def near(size, step=1):
    return sorted({step % size, -step % size} - {0})


def far_first(size):
    return sorted(range(1, size), key=lambda d: -min(d, size - d))


def unit(raw):
    wide = raw.astype(F32)
    inv_rms = lax.rsqrt(jnp.mean(wide * wide, axis=-1, keepdims=True) + EPSILON)
    return wide * inv_rms, inv_rms


def kernel(sizes, q_hbm, k_hbm, v_hbm, do_hbm, gains_hbm, table_hbm,
           dq_v, dk_v, dv_v, dtab_v, dgain_v,
           q_raw, k_raw, qdx, qd0, kvx, first_kv, gains_v, table_v,
           qu, qr, ku, kr, bias_v, e_v, dp_v,
           dkx, dvx, dqx, d_v, prob_v, d_low_v, sum_v, gain_v, table_v2, extra_gain, first_prob, first_d_low, first_dk,
           to_before, from_after, to_after, from_before, dq_from_before, to_before_first, from_after_first,
           rows_x, plane, zout, zbuf,
           load_sem, more_sem, gains_sem, table_sem, left_recv, right_recv, after_recv, before_recv,
           sum_send, x_recv, plane_recv, z_recv, round1, round2, round3, plane_round):
    nz, ny, nx = sizes
    z, y, x, tp = (lax.axis_index(a) for a in AXES)
    place = (z * ny + y) * nx + x
    total = nz * ny * nx
    is_first, is_last = place == 0, place == total - 1
    opens, closes = jnp.logical_and(x == 0, y == 0), jnp.logical_and(x == nx - 1, y == ny - 1)
    opens_later, closes_early = jnp.logical_and(opens, place > 0), jnp.logical_and(closes, place < total - 1)
    takes_back, takes_next = jnp.logical_not(opens), jnp.logical_not(closes)

    def at(number, core):
        return (number // (ny * nx), (number // nx) % ny, number % nx, core)

    after = at(jnp.minimum(place + 1, total - 1), tp)
    before = at(jnp.maximum(place - 1, 0), tp)

    def along(axis, offset, core=1):
        if axis == 0:
            return (lax.rem(z + offset, nz), y, x, core)
        if axis == 1:
            return (z, lax.rem(y + offset, ny), x, core)
        return (z, y, lax.rem(x + offset, nx), core)

    def signal(sem, target):
        pl.semaphore_signal(sem, inc=1, device_id=target, device_id_type=pl.DeviceIdType.MESH)

    def remote(src, dst, send, recv, target):
        return pltpu.make_async_remote_copy(
            src_ref=src, dst_ref=dst, send_sem=send, recv_sem=recv,
            device_id=target, device_id_type=pl.DeviceIdType.MESH)

    def wait_bytes(ref, sem):
        pltpu.make_async_copy(ref, ref, sem).wait()

    barrier = pltpu.get_barrier_semaphore()

    @pl.when(place > 0)
    def _():
        signal(barrier, before)

    @pl.when(place < total - 1)
    def _():
        signal(barrier, after)

    sides = jnp.where(is_first, 0, 1) + jnp.where(is_last, 0, 1)
    small_loads = [pltpu.make_async_copy(gains_hbm, gains_v, gains_sem), pltpu.make_async_copy(table_hbm, table_v, table_sem)]
    for load in small_loads:
        load.start()
    for h in range(HEADS):
        lanes = slice(h * HEAD_DIM, (h + 1) * HEAD_DIM)
        pltpu.make_async_copy(k_hbm.at[:, lanes], k_raw.at[h], load_sem).start()
        pltpu.make_async_copy(q_hbm.at[:, lanes], q_raw.at[h], load_sem).start()
        pltpu.make_async_copy(v_hbm.at[:, lanes], kvx.at[1, h, BEFORE:BEFORE + ROWS], load_sem).start()
        pltpu.make_async_copy(do_hbm.at[:SEG, lanes], qd0.at[1, h], load_sem).start()
        pltpu.make_async_copy(do_hbm.at[SEG:, lanes], qdx.at[1, h, :BEFORE], more_sem).start()

    close = [(a, o) for a, n in enumerate(sizes) for o in near(n)]

    @pl.when(tp == 1)
    def _():
        for a, o in close:
            signal(barrier, along(a, o))
        signal(barrier, (z, y, x, 0))

    @pl.when(tp == 0)
    def _():
        signal(barrier, (z, y, x, 1))

    for load in small_loads:
        load.wait()
    gains = gains_v[...]
    gain_q, gain_k = gains[0:1, :], gains[1:2, :]
    wait_bytes(kvx.at[:, :, :ROWS + PAIR + SEG // 2], load_sem)
    def norm_keys(first, size):
        for h in range(HEADS):
            u, r = unit(k_raw[h, first:first + size])
            ku[h, first:first + size] = u
            kr[h, first:first + size] = jnp.broadcast_to(r, u.shape)
            kvx[0, h, BEFORE + first:BEFORE + first + size] = (u * gain_k).astype(BF16)

    def norm_queries(first, size, out):
        for h in range(HEADS):
            u, r = unit(q_raw[h, first:first + size])
            qu[h, first:first + size] = u
            qr[h, first:first + size] = jnp.broadcast_to(r, u.shape)
            out[h] = (u * gain_q).astype(BF16)

    forth = [remote(
        kvx.at[:, :, ROWS + PAIR:ROWS + BEFORE], kvx.at[:, :, PAIR:BEFORE], load_sem, left_recv.at[HEADS], after)]
    back = {}
    for h in range(HEADS):
        forth.append(remote(
            kvx.at[:, h, ROWS:ROWS + PAIR], kvx.at[:, h, :PAIR], load_sem, left_recv.at[h], after))
        back[h] = [
            remote(kvx.at[:, h, BEFORE:ROWS], kvx.at[:, h, BEFORE + ROWS:], gains_sem, right_recv, before),
            remote(qd0.at[:, h], qdx.at[:, h, BEFORE:], gains_sem, right_recv, before)]

    plane_piece = remote(kvx.at[:, :, BEFORE:ROWS], first_kv, load_sem, left_recv.at[HEADS - 1], after)

    def go_on(pieces, when=place < total - 1):
        @pl.when(when)
        def _():
            for copy in pieces:
                copy.start()

    norm_keys(BEFORE, SEG)
    pl.semaphore_wait(barrier, sides + jnp.where(tp == 1, 1 + len(close), 1))
    go_on(forth[:1])
    norm_keys(0, SEG)
    norm_queries(0, SEG, qd0.at[0])

    go_on([copy for h in range(HEADS) for copy in back[h]], takes_back)
    norm_keys(SEG, PAIR)
    go_on(forth[1:], jnp.logical_and(tp == 0, place < total - 1))
    go_on(forth[1:2], jnp.logical_and(tp == 1, place < total - 1))
    go_on([plane_piece], closes_early)
    norm_queries(SEG, BEFORE, qdx.at[0, :, :BEFORE])

    @pl.when(tp == 1)
    def _():
        for a, o in close:
            signal(round1, along(a, o))

    wait_bytes(qdx.at[1, :, :BEFORE], more_sem)

    @pl.when(is_first)
    def _():
        for h in range(HEADS):
            for n in range(2):
                kvx[n, h, :BEFORE] = kvx[n, h, BEFORE:2 * BEFORE]
                first_kv[n, h] = kvx[n, h, BEFORE:ROWS]

    @pl.when(closes)
    def _():
        for h in range(HEADS):
            for n in range(2):
                kvx[n, h, BEFORE + ROWS:] = kvx[n, h, BEFORE:ROWS]
            qdx[0, h, BEFORE:] = qd0[0, h]
            qdx[1, h, BEFORE:] = jnp.zeros((SEG, HEAD_DIM), BF16)

    @pl.when(is_last)
    def _():
        for h in range(HEADS):
            for n in range(2):
                from_after[n, h] = jnp.zeros((BEFORE, HEAD_DIM), BF16)

    key_at = lax.broadcasted_iota(jnp.int32, (PAIR, PAIR), 0)
    query_at = lax.broadcasted_iota(jnp.int32, (PAIR, PAIR), 1)
    past = query_at >= key_at
    early = query_at < SEG
    high = key_at >= SEG
    lane = lax.broadcasted_iota(jnp.int32, (1, PAIR), 1)
    table = table_v[...]
    low_part = table[:, :PAIR]
    high_part = jnp.concatenate([table[:, PAIR:], jnp.zeros((HEADS, 2 * PAIR - ENTRIES), F32)], axis=1)
    low_rolled = pltpu.roll(low_part, PAIR - SEG + 1, 1)
    high_rolled = pltpu.roll(high_part, PAIR - SEG + 1, 1)
    for h in range(HEADS):
        last = table[h:h + 1, ENTRIES - 1:ENTRIES]
        dist_low = low_rolled[h:h + 1]
        dist_row = jnp.where(lane <= SEG, dist_low, high_rolled[h:h + 1])
        ahead = pltpu.roll(jnp.broadcast_to(dist_low, (PAIR, PAIR)), 0, 1, stride=1, stride_axis=0)
        behind = pltpu.roll(jnp.broadcast_to(dist_row, (PAIR, PAIR)), 0, 1, stride=1, stride_axis=0)
        tile0 = jnp.where(jnp.logical_or(early, high), last, MASKED)
        tile1 = jnp.where(past, last, behind)
        tile2 = jnp.where(jnp.logical_and(early, high), MASKED, jnp.where(past, behind, ahead))
        none, low = (jnp.where(is_first, MASKED, t) for t in (tile0, tile1))
        for p, tiles in enumerate((
                (none, jnp.where(high, tile1, low), tile2),
                (jnp.where(high, tile0, none), tile1, tile2))):
            top = jnp.max(jnp.maximum(jnp.maximum(tiles[0], tiles[1]), tiles[2]), axis=0, keepdims=True)
            for b, tile in enumerate(tiles):
                bias_v[h, p, b * PAIR:(b + 1) * PAIR] = (tile - top) * LOG2E

    def work(blocks, tiles=()):
        at_keys = {(p, b): slice((p + b) * PAIR, (p + b + 1) * PAIR) for h, p, b in blocks}
        at_queries = [slice(p * PAIR, (p + 1) * PAIR) for p in range(2)]
        at_rows = [slice(b * PAIR, (b + 1) * PAIR) for b in range(3)]
        scores = [dot(kvx[0, h, at_keys[p, b]], qdx[0, h, at_queries[p]], 1, 1) for h, p, b in blocks]
        d_probs = [dot(kvx[1, h, at_keys[p, b]], qdx[1, h, at_queries[p]], 1, 1) for h, p, b in blocks]
        for (h, p, b), s, dp in zip(blocks, scores, d_probs):
            e = jnp.exp2(s * (FACTOR * LOG2E) + bias_v[h, p, at_rows[b]])
            e_v[h, p, at_rows[b]] = e
            dp_v[h, p, at_rows[b]] = dp
            sum_v[h, p, b] = jnp.sum(e, axis=0, keepdims=True)
            sum_v[h, p, 3 + b] = jnp.sum(e * dp, axis=0, keepdims=True)
        d_scores, products = [], []
        for h, p, _ in tiles:
            inv = 1.0 / (sum_v[h, p, 0] + sum_v[h, p, 1] + sum_v[h, p, 2])
            delta = (sum_v[h, p, 3] + sum_v[h, p, 4] + sum_v[h, p, 5]) * inv
            prob = e_v[h, p] * inv
            d_score = prob * (dp_v[h, p] - delta)
            d_low = d_score.astype(BF16)
            prob_v[h, p] = prob.astype(BF16)
            d_low_v[h, p] = d_low
            d_scores.append(d_score)
            products.append(dot(d_low, qdx[0, h, at_queries[p]], 1, 0))
        for (h, p, again), d_score in zip(tiles, d_scores):
            if again:
                fold_table(h, d_v[h] + d_score)
            else:
                d_v[h] = d_score
        for (h, p, again), dk in zip(tiles, products):
            keys = slice(p * PAIR, (p + 3) * PAIR)
            gain_v[h, p] = jnp.sum(dk * kvx[0, h, keys].astype(F32), axis=0, keepdims=True)
            if again:
                shared, alone = slice(PAIR, 3 * PAIR), slice(3 * p * PAIR, (3 * p + 1) * PAIR)
                dkx[h, alone] = dk[2 * p * PAIR:(2 * p + 1) * PAIR]
                dkx[h, shared] = dkx[h, shared] + dk[(1 - p) * PAIR:(3 - p) * PAIR]
            else:
                dkx[h, keys] = dk

    def query_rows(g, u, r):
        g = g * FACTOR * gain_q
        return (r * (g - u * jnp.mean(g * u, axis=-1, keepdims=True))).astype(BF16)

    sublane = lax.broadcasted_iota(jnp.int32, (8, PAIR), 0)

    def skewed_sum(tile, right):
        parts = [pltpu.roll(tile[first:first + 8], (right - first) % PAIR, 1) for first in range(0, PAIR, 8)]
        while len(parts) > 1:
            parts = [a + b for a, b in zip(parts[::2], parts[1::2])]
        total = parts[0]
        for bit in range(1, 8):
            total = jnp.where(sublane == bit, pltpu.roll(parts[0], PAIR - bit, 1), total)
        return jnp.sum(total, axis=0, keepdims=True)

    def fold_rows(h, d_score):
        d0, d1, d2 = (d_score[b * PAIR:(b + 1) * PAIR] for b in range(3))
        mixed = jnp.where(past, d2, d1)
        ahead = jnp.where(past, 0.0, d2)
        rest = d0 + jnp.where(past, d1, 0.0)
        behind_row, ahead_row = skewed_sum(mixed, SEG - 1), skewed_sum(ahead, SEG - 1)
        high_row = skewed_sum(mixed, SEG - 1 + SEG) if h else behind_row
        rest_sum = jnp.sum(jnp.sum(rest, axis=0, keepdims=True), axis=1, keepdims=True)
        return (
            jnp.where(lane < SEG - 1, ahead_row, behind_row),
            jnp.where(lane == SEG - 1 + h * SEG, rest_sum, high_row))

    def fold_table(h, d_score):
        table_v2[h, 0], table_v2[h, 1] = fold_rows(h, d_score)

    def first_segment():
        key_number = lax.broadcasted_iota(jnp.int32, (ROWS + SEG, SEG), 0)
        hidden = jnp.logical_and(is_first, key_number < ROWS)

        def against(n, h, side):
            return jnp.concatenate([dot(first_kv[n, h], side, 1, 1), dot(kvx[n, h, :ROWS], side, 1, 1)], axis=0)

        scores = [against(0, h, qd0[0, h]) for h in heads]
        d_probs = [against(1, h, qd0[1, h]) for h in heads]
        d_scores = []
        for h in heads:
            bias = jnp.where(hidden, MASKED, bias_v[h, 0, :ROWS + SEG][:, :SEG])
            bias = bias - jnp.max(bias, axis=0, keepdims=True)
            e = jnp.exp2(scores[h] * (FACTOR * LOG2E) + bias)
            inv = 1.0 / jnp.sum(e, axis=0, keepdims=True)
            delta = jnp.sum(e * d_probs[h], axis=0, keepdims=True) * inv
            prob = e * inv
            d_scores.append(prob * (d_probs[h] - delta))
            first_prob[h] = prob.astype(BF16)
            first_d_low[h] = d_scores[h].astype(BF16)
        products = [dot(d_scores[h].astype(BF16), qd0[0, h], 1, 0) for h in heads]
        for h in heads:
            tile = jnp.concatenate([d_scores[h], jnp.zeros((ROWS + SEG, SEG), F32)], axis=1)
            rows = fold_rows(h, jnp.concatenate([tile, jnp.zeros((SEG, PAIR), F32)], axis=0))
            for j in range(2):
                table_v2[h, j] = table_v2[h, j] + rows[j]
        gain = jnp.zeros((1, HEAD_DIM), F32)
        for h in heads:
            dk = products[h]
            first_dk[h] = dk
            gain = gain + jnp.sum(dk[:SEG] * first_kv[0, h].astype(F32), axis=0, keepdims=True)
            gain = gain + jnp.sum(dk[SEG:] * kvx[0, h, :ROWS].astype(F32), axis=0, keepdims=True)
        extra_gain[...] = gain

    def first_results(h):
        d_low = first_d_low[h]
        dv = dot(first_prob[h], qd0[1, h], 1, 0)
        dq_from_before[h] = dot(d_low[:SEG], first_kv[0, h], 0, 0) + dot(d_low[SEG:], kvx[0, h, :ROWS], 0, 0)
        for n, part in enumerate((first_dk[h] * FACTOR, dv)):
            to_before_first[n, h] = part[:SEG].astype(BF16)
            from_before[n, h] = part[ROWS:].astype(BF16)
        dkx[h, :BEFORE] = dkx[h, :BEFORE] + first_dk[h, SEG:ROWS]
        dvx[h, :BEFORE] = dvx[h, :BEFORE] + dv[SEG:ROWS]

    heads = range(HEADS)
    work([(h, 0, 2) for h in heads])

    go_on(forth[2:], jnp.logical_and(tp == 1, place < total - 1))
    @pl.when(tp == 1)
    def _():
        pl.semaphore_wait(round1, len(close))
        for a, n in enumerate(sizes[:2]):
            if n > 5:
                for o in near(n, 2):
                    signal(round2, along(a, o))

    def wait_left(piece):
        @pl.when(place > 0)
        def _():
            if piece < HEADS:
                forth[piece].wait_recv()
            else:
                @pl.when(opens)
                def _():
                    wait_bytes(kvx.at[:, :, :PAIR], left_recv.at[piece - 1])

                @pl.when(takes_back)
                def _():
                    forth[piece].wait_recv()

    def wait_right():
        @pl.when(takes_next)
        def _():
            wait_bytes(kvx.at[:, :, :PAIR], right_recv)

    beside = sorted({*near(ny), *near(ny, 2)})

    def greet_far():
        @pl.when(tp == 1)
        def _():
            count = sum(len(near(n, 2)) for n in sizes[:2] if n > 5)
            if count:
                pl.semaphore_wait(round2, count)
            for o in beside:
                signal(plane_round, along(1, o))
            if nz > 9:
                for o in near(nz, 3):
                    signal(round3, along(0, o))

    def do_first():
        @pl.when(opens)
        def _():
            first_segment()

    @pl.when(x == nx - 1)
    def _():
        wait_left(0)
        work([(h, 0, 1) for h in heads])
        for h in heads:
            wait_left(1 + h)
            work([(h, 0, 0)], [(h, 0, False)])
            if not h:
                greet_far()
        wait_right()
        work([(h, 1, b) for b in range(3) for h in heads], [(h, 1, True) for h in heads])
        if nx == 1:
            do_first()

    if nx > 1:
        @pl.when(x == 0)
        def _():
            wait_right()
            work([(h, 1, b) for b in (1, 2) for h in heads])
            greet_far()
            wait_left(0)
            work([(h, p, 1 - p) for p in (1, 0) for h in heads], [(h, 1, False) for h in heads])
            for h in heads:
                wait_left(1 + h)
                work([(h, 0, 0)], [(h, 0, True)])
            do_first()

    if nx > 2:
        @pl.when(jnp.logical_and(x > 0, x < nx - 1))
        def _():
            wait_left(0)
            work([(h, 0, 1) for h in heads])
            wait_right()
            work([(h, 1, b) for b in range(3) for h in heads], [(h, 1, False) for h in heads])
            greet_far()
            for h in heads:
                wait_left(1 + h)
                work([(h, 0, 0)], [(h, 0, True)])

    gain = gain_v[0, 0] + gain_v[0, 1] + gain_v[1, 0] + gain_v[1, 1] + jnp.where(opens, extra_gain[...], 0.0)
    second = jnp.where(lane < SEG, table_v2[0, 1], table_v2[1, 1])
    vec = jnp.concatenate([table_v2[0, 0], table_v2[1, 0], second, gain * FACTOR], axis=0)
    chip = y * nx + x

    to_neighbours = [
        remote(to_before.at[:, h], from_after.at[:, h], more_sem, after_recv, before) for h in range(HEADS)]
    to_next = [
        remote(to_after, from_before, table_sem, before_recv, after),
        remote(dqx.at[:, BEFORE:], dq_from_before, table_sem, before_recv, after)]
    to_plane_before = remote(to_before_first, from_after_first, more_sem, after_recv, before)

    def stage_results():
        @pl.when(takes_next)
        def _():
            wait_bytes(kvx.at[:, :, :BEFORE], load_sem)

        @pl.when(closes_early)
        def _():
            wait_bytes(kvx.at[:, :, :ROWS], load_sem)

        @pl.when(takes_back)
        def _():
            wait_bytes(kvx.at[:, :, :PAIR], gains_sem)

        for h in range(HEADS):
            low, high_tile = (dot(prob_v[h, p], qdx[1, h, p * PAIR:(p + 1) * PAIR], 1, 0) for p in range(2))
            dvx[h, :PAIR] = low[:PAIR]
            dvx[h, PAIR:3 * PAIR] = low[PAIR:] + high_tile[:2 * PAIR]
            dvx[h, 3 * PAIR:] = high_tile[2 * PAIR:]

            @pl.when(opens)
            def _(h=h):
                first_results(h)

            lanes = slice(h * HEAD_DIM, (h + 1) * HEAD_DIM)
            to_before[0, h] = (dkx[h, :BEFORE] * FACTOR).astype(BF16)
            to_before[1, h] = dvx[h, :BEFORE].astype(BF16)
            to_after[0, h] = (dkx[h, BEFORE + ROWS:] * FACTOR).astype(BF16)
            to_after[1, h] = dvx[h, BEFORE + ROWS:].astype(BF16)
            for p in range(2):
                dqx[h, p * PAIR:(p + 1) * PAIR] = dot(d_low_v[h, p], kvx[0, h, p * PAIR:(p + 3) * PAIR], 0, 0)
            dq_v[SEG:, lanes] = query_rows(dqx[h, :BEFORE], qu[h, SEG:], qr[h, SEG:])

    def send_results(when):
        @pl.when(jnp.logical_and(when, place > 0))
        def _():
            for copy in to_neighbours:
                copy.start()

        @pl.when(jnp.logical_and(when, opens_later))
        def _():
            to_plane_before.start()

        @pl.when(jnp.logical_and(when, takes_next))
        def _():
            for copy in to_next:
                copy.start()

    def sum_of(ref, first, count):
        parts = [ref[n] for n in range(first, first + count)]
        while len(parts) > 1:
            parts = [sum(parts[n:n + 2]) for n in range(0, len(parts), 2)]
        return parts[0]

    has_across = ny > 3 and ny % 2 == 0
    across, column = nx * ny, nx * ny + nx

    @pl.when(tp == 1)
    def _():
        rows_x[x] = vec
        for o in far_first(nx):
            remote(rows_x.at[x], rows_x.at[x], sum_send, x_recv, along(2, o)).start()
        if beside:
            pl.semaphore_wait(plane_round, len(beside))
        signal(round1, (z, y, x, 0))
        if has_across:
            for o in far_first(nx) + [0]:
                remote(
                    rows_x.at[x], plane.at[across + x], sum_send, plane_recv,
                    (z, lax.rem(y + ny // 2, ny), lax.rem(x + o, nx), 1)).start()
        stage_results()
        send_results(jnp.logical_and(x > 0, x < nx - 1))
        if nx > 1:
            wait_bytes(rows_x.at[:nx - 1], x_recv)
        plane[column + y] = sum_of(rows_x, 0, nx)
        y_ways = [o for o in far_first(ny) if not has_across or o != ny // 2]
        for o in y_ways:
            remote(plane.at[column + y], plane.at[column + y], sum_send, plane_recv, along(1, o)).start()
        came = nx * ny + len(y_ways) + (nx if has_across else 0)
        wait_bytes(plane.at[:came], plane_recv)
        if has_across:
            plane[column + lax.rem(y + ny // 2, ny)] = sum_of(plane, across, nx)
        others, part = sum_of(plane, 0, nx * ny), sum_of(plane, column, ny)
        gain = part[3:] + others[3:]
        for core, rows in enumerate((others, part)):
            zout[core, :3] = rows[:3]
            zout[core, 3:] = gain
        zbuf[z] = zout[1]
        if nz > 9:
            pl.semaphore_wait(round3, len(near(nz, 3)))
        for o in [*far_first(nz), 0]:
            for core in ((1, 0) if o else (0,)):
                remote(zout.at[core], zbuf.at[z], sum_send, z_recv, along(0, o, core)).start()
        send_results(jnp.logical_or(x == 0, x == nx - 1))
        signal(round2, (z, y, x, 0))

    @pl.when(tp == 0)
    def _():
        plane[chip] = vec
        pl.semaphore_wait(round1, 1)
        for oy, ox in sorted(
                ((oy, ox) for oy in range(ny) for ox in range(nx)),
                key=lambda o: -min(o[0], ny - o[0]) - min(o[1], nx - o[1])):
            remote(
                plane.at[chip], plane.at[chip], sum_send, plane_recv,
                (z, lax.rem(y + oy, ny), lax.rem(x + ox, nx), 1)).start()
        stage_results()
        send_results(jnp.logical_or(opens, jnp.logical_and(x > 0, x < nx - 1)))
        pl.semaphore_wait(round2, 1)
        send_results(jnp.logical_and(jnp.logical_not(opens), jnp.logical_or(x == 0, x == nx - 1)))

    @pl.when(takes_back)
    def _():
        wait_bytes(kvx.at[:, :, :PAIR], before_recv)

    @pl.when(takes_next)
    def _():
        wait_bytes(from_after, after_recv)

    @pl.when(closes_early)
    def _():
        wait_bytes(kvx.at[:, :, :ROWS], after_recv)

    for h in range(HEADS):
        dq_v[:SEG, h * HEAD_DIM:(h + 1) * HEAD_DIM] = query_rows(dq_from_before[h], qu[h, :SEG], qr[h, :SEG])

    for h in range(HEADS):
        lanes = slice(h * HEAD_DIM, (h + 1) * HEAD_DIM)
        sums_in = [
            jnp.concatenate([
                jnp.where(takes_next, 0.0, jnp.where(is_last, 0.0, from_after_first[n, h].astype(F32)))
                + from_before[n, h].astype(F32), from_after[n, h].astype(F32)], axis=0) for n in range(2)]
        g = (dkx[h, BEFORE:BEFORE + ROWS] * FACTOR + sums_in[0]) * gain_k
        u = ku[h]
        dk_v[:, lanes] = (kr[h] * (g - u * jnp.mean(g * u, axis=-1, keepdims=True))).astype(BF16)
        dv_v[:, lanes] = (dvx[h, BEFORE:BEFORE + ROWS] + sums_in[1]).astype(BF16)

    @pl.when(takes_next)
    def _():
        wait_bytes(kvx.at[:, :, :PAIR], table_sem)

    @pl.when(takes_back)
    def _():
        wait_bytes(from_after, more_sem)

    @pl.when(opens_later)
    def _():
        wait_bytes(kvx.at[:, :, :ROWS], more_sem)

    @pl.when(tp == 1)
    def _():
        wait_bytes(plane.at[:nx - 1 + 2 * nz - 1 + ny - 1 + (nx - 1 if has_across else 0)], sum_send)
        if nz > 1:
            wait_bytes(zbuf.at[:nz - 1], z_recv)

    @pl.when(tp == 0)
    def _():
        wait_bytes(plane.at[:nx * ny], sum_send)
        wait_bytes(zbuf.at[:nz], z_recv)

    result = zbuf[0]
    for n in range(1, nz):
        result = result + zbuf[n]
    for j in range(HEADS):
        dtab_v[j:j + 1, :PAIR] = result[j:j + 1]
        dtab_v[j:j + 1, PAIR:] = result[2:3, j * SEG:(j + 1) * SEG]
    dgain_v[0:1] = result[3:] / gain_q
    dgain_v[1:2] = result[3:] / gain_k


def write_out(*refs):
    count = len(refs) // 2
    copies = [pltpu.make_async_copy(refs[n], refs[count + n], refs[-1].at[n]) for n in range(count)]
    for copy in copies:
        copy.start()
    for copy in copies:
        copy.wait()


def local(sizes, queries, keys, values, gains, bias_table, d_out):
    nz, ny, nx = sizes
    width = HEADS * HEAD_DIM
    hbm_spec = pl.BlockSpec(memory_space=pltpu.HBM)
    vmem_spec = pl.BlockSpec(memory_space=pltpu.VMEM)
    first = (HEADS, SEG, HEAD_DIM)
    tile = (HEADS, ROWS, HEAD_DIM)
    wide = (HEADS, 2 * ROWS, HEAD_DIM)
    pairs = (HEADS, 2, 3 * PAIR, PAIR)
    dma, regular = pltpu.SemaphoreType.DMA, pltpu.SemaphoreType.REGULAR
    vmem = pltpu.VMEM
    outs = [((ROWS, width), BF16)] * 3 + [((HEADS, ENTRIES), F32), ((2, HEAD_DIM), F32)]
    out = pl.pallas_call(
        functools.partial(kernel, sizes),
        out_shape=tuple(vmem(*o) for o in outs),
        in_specs=[hbm_spec] * 6,
        out_specs=(vmem_spec,) * 5,
        scratch_shapes=[
            vmem(tile, BF16), vmem(tile, BF16), vmem((2, *tile), BF16), vmem((2, *first), BF16), vmem((2, *wide), BF16), vmem((2, *first), BF16),
            vmem((2, HEAD_DIM), F32), vmem((HEADS, ENTRIES), F32),
            vmem(tile, F32), vmem(tile, F32), vmem(tile, F32), vmem(tile, F32),
            vmem(pairs, F32), vmem(pairs, F32), vmem(pairs, F32),
            vmem(wide, F32), vmem(wide, F32), vmem(tile, F32), vmem((HEADS, 3 * PAIR, PAIR), F32),
            vmem(pairs, BF16), vmem(pairs, BF16), vmem((HEADS, 2, 6, 1, PAIR), F32), vmem((HEADS, 2, 1, PAIR), F32),
            vmem((HEADS, 2, 1, PAIR), F32), vmem((1, HEAD_DIM), F32),
            vmem((HEADS, ROWS + SEG, SEG), BF16), vmem((HEADS, ROWS + SEG, SEG), BF16), vmem((HEADS, ROWS + SEG, HEAD_DIM), F32),
            vmem((2, HEADS, BEFORE, HEAD_DIM), BF16), vmem((2, HEADS, BEFORE, HEAD_DIM), BF16),
            vmem((2, *first), BF16), vmem((2, *first), BF16), vmem(first, F32), vmem((2, *first), BF16), vmem((2, *first), BF16),
            vmem((nx, 4, HEAD_DIM), F32), vmem((nx * ny + nx + ny + 2 * nz, 4, HEAD_DIM), F32), vmem((2, 4, HEAD_DIM), F32), vmem((2 * nz, 4, HEAD_DIM), F32),
            dma, dma, dma, dma, dma((HEADS + 1,)), dma, dma, dma,
            dma, dma, dma, dma, regular, regular, regular, regular,
        ],
        compiler_params=pltpu.CompilerParams(
            collective_id=0, has_side_effects=True, vmem_limit_bytes=32 * 1024 * 1024),
        name="segment_attention_grad",
    )(*(pltpu.with_memory_space_constraint(a, pltpu.HBM) for a in (queries, keys, values, d_out, gains, bias_table.T)))
    d_queries, d_keys, d_values, d_table, d_gains = pl.pallas_call(
        write_out,
        out_shape=tuple(jax.ShapeDtypeStruct(*o) for o in outs),
        in_specs=[vmem_spec] * 5,
        out_specs=(hbm_spec,) * 5,
        scratch_shapes=[dma((5,))],
        name="write_out",
    )(*(pltpu.with_memory_space_constraint(o, pltpu.VMEM) for o in out))
    return d_queries, d_keys, d_values, d_table.T, d_gains


def solution(mesh):
    shape = (12, 8, 4)
    if mesh.shape["sp"] != int(np.prod(shape)):
        shape = mesh.small_shape
    split = Mesh(mesh.devices.reshape(*shape, mesh.shape["tp"]), AXES)
    placed = (P(SP, "tp"), P(SP, "tp"), P(SP, "tp"), P(), P(None, "tp"), P(SP, "tp"))
    return jax.shard_map(
        functools.partial(local, shape),
        mesh=split,
        in_specs=placed,
        out_specs=(P(SP, "tp"), P(SP, "tp"), P(SP, "tp"), P(None, "tp"), P()),
        check_vma=False,
    )
```

```python
import functools

import jax
import jax.numpy as jnp
import numpy as np
from jax import lax
from jax.experimental import pallas as pl
from jax.experimental.pallas import tpu as pltpu
from jax.sharding import Mesh
from jax.sharding import PartitionSpec as P

HEAD_DIM = 128
SEG = 64
LEFT = 4
MAX_REL = 128
ENTRIES = MAX_REL + SEG
ROWS = LEFT * SEG
HEADS = 2
PAIR = 2 * SEG
BEFORE = 3 * SEG
AXES = ("sp_0", "sp_1", "sp_2", "tp")
SP = AXES[:3]

EPSILON = 1e-06
FACTOR = HEAD_DIM ** (-0.5)
LOG2E = 1.4426950408889634
MASKED = -1e30
F32, BF16 = jnp.float32, jnp.bfloat16


def dot(a, b, a_dim, b_dim):
    return lax.dot_general(a, b, (((a_dim,), (b_dim,)), ((), ())), preferred_element_type=F32)


def near(size, step=1):
    return sorted({step % size, -step % size} - {0})


def far_first(size):
    return sorted(range(1, size), key=lambda d: -min(d, size - d))


def unit(raw):
    wide = raw.astype(F32)
    inv_rms = lax.rsqrt(jnp.mean(wide * wide, axis=-1, keepdims=True) + EPSILON)
    return wide * inv_rms, inv_rms


def kernel(sizes, q_hbm, k_hbm, v_hbm, do_hbm, gains_hbm, table_hbm,
           dq_v, dk_v, dv_v, dtab_v, dgain_v,
           qdx, qd0, kvx, first_kv, gains_v, table_v,
           qn, qn0, qu, qr, kn, ku, kr, first_kn, first_ku, bias_v, e_v, dp_v,
           dkx, dvx, dqx, d_v, prob_v, d_low_v, sum_v, gain_v, table_v2, extra_gain, first_prob, first_d_low, first_dk,
           to_before, from_after, to_after, from_before, dq_from_before, to_before_first, from_after_first,
           rows_x, plane, zout, zbuf,
           load_sem, more_sem, gains_sem, table_sem, left_recv, right_recv, after_recv, before_recv,
           sum_send, x_recv, plane_recv, z_recv, round1, round2, round3, plane_round):
    nz, ny, nx = sizes
    z, y, x, tp = (lax.axis_index(a) for a in AXES)
    place = (z * ny + y) * nx + x
    total = nz * ny * nx
    is_first, is_last = place == 0, place == total - 1
    opens, closes = jnp.logical_and(x == 0, y == 0), jnp.logical_and(x == nx - 1, y == ny - 1)
    opens_later, closes_early = jnp.logical_and(opens, place > 0), jnp.logical_and(closes, place < total - 1)
    takes_back, takes_next = jnp.logical_not(opens), jnp.logical_not(closes)

    def at(number, core):
        return (number // (ny * nx), (number // nx) % ny, number % nx, core)

    after = at(jnp.minimum(place + 1, total - 1), tp)
    before = at(jnp.maximum(place - 1, 0), tp)

    def along(axis, offset, core=1):
        if axis == 0:
            return (lax.rem(z + offset, nz), y, x, core)
        if axis == 1:
            return (z, lax.rem(y + offset, ny), x, core)
        return (z, y, lax.rem(x + offset, nx), core)

    def signal(sem, target):
        pl.semaphore_signal(sem, inc=1, device_id=target, device_id_type=pl.DeviceIdType.MESH)

    def remote(src, dst, send, recv, target):
        return pltpu.make_async_remote_copy(
            src_ref=src, dst_ref=dst, send_sem=send, recv_sem=recv,
            device_id=target, device_id_type=pl.DeviceIdType.MESH)

    def wait_bytes(ref, sem):
        pltpu.make_async_copy(ref, ref, sem).wait()

    barrier = pltpu.get_barrier_semaphore()

    @pl.when(place > 0)
    def _():
        signal(barrier, before)

    @pl.when(place < total - 1)
    def _():
        signal(barrier, after)

    sides = jnp.where(is_first, 0, 1) + jnp.where(is_last, 0, 1)
    small_loads = [pltpu.make_async_copy(gains_hbm, gains_v, gains_sem), pltpu.make_async_copy(table_hbm, table_v, table_sem)]
    for load in small_loads:
        load.start()
    for h in range(HEADS):
        lanes = slice(h * HEAD_DIM, (h + 1) * HEAD_DIM)
        for n, (keys_or_values, queries_or_cotangents) in enumerate(((k_hbm, q_hbm), (v_hbm, do_hbm))):
            pltpu.make_async_copy(keys_or_values.at[:, lanes], kvx.at[n, h, BEFORE:BEFORE + ROWS], load_sem).start()
            pltpu.make_async_copy(queries_or_cotangents.at[:SEG, lanes], qd0.at[n, h], load_sem).start()
            pltpu.make_async_copy(queries_or_cotangents.at[SEG:, lanes], qdx.at[n, h, :BEFORE], more_sem).start()

    close = [(a, o) for a, n in enumerate(sizes) for o in near(n)]

    @pl.when(tp == 1)
    def _():
        for a, o in close:
            signal(barrier, along(a, o))
        signal(barrier, (z, y, x, 0))

    @pl.when(tp == 0)
    def _():
        signal(barrier, (z, y, x, 1))

    forth = [remote(
        kvx.at[:, :, ROWS + PAIR:ROWS + BEFORE], kvx.at[:, :, PAIR:BEFORE], load_sem, left_recv.at[HEADS], after)]
    back = {}
    for h in range(HEADS):
        forth.append(remote(
            kvx.at[:, h, ROWS:ROWS + PAIR], kvx.at[:, h, :PAIR], load_sem, left_recv.at[h], after))
        back[h] = [
            remote(kvx.at[:, h, BEFORE:ROWS], kvx.at[:, h, BEFORE + ROWS:], gains_sem, right_recv, before),
            remote(qd0.at[:, h], qdx.at[:, h, BEFORE:], gains_sem, right_recv, before)]

    plane_piece = remote(kvx.at[:, :, BEFORE:ROWS], first_kv, load_sem, left_recv.at[HEADS - 1], after)

    def go_on(pieces, when=place < total - 1):
        @pl.when(when)
        def _():
            for copy in pieces:
                copy.start()

    wait_bytes(kvx.at[:, :, :ROWS + SEG], load_sem)
    small_loads[0].wait()
    pl.semaphore_wait(barrier, sides + jnp.where(tp == 1, 1 + len(close), 1))
    go_on(forth[:1])
    go_on([copy for h in range(HEADS) for copy in back[h]], takes_back)
    go_on(forth[1:], jnp.logical_and(tp == 0, place < total - 1))
    go_on(forth[1:2], jnp.logical_and(tp == 1, place < total - 1))
    go_on([plane_piece], closes_early)

    @pl.when(tp == 1)
    def _():
        for a, o in close:
            signal(round1, along(a, o))

    wait_bytes(qdx.at[:, :, :BEFORE], more_sem)
    small_loads[1].wait()
    gains = gains_v[...]
    gain_q, gain_k = gains[0:1, :], gains[1:2, :]

    def take_keys(h, first, size):
        u, r = unit(kvx[0, h, first:first + size])
        ku[h, first:first + size] = u
        kn[h, first:first + size] = (u * gain_k).astype(BF16)
        return r

    def take_queries(h):
        qn[h, BEFORE:] = (unit(qdx[0, h, BEFORE:])[0] * gain_q).astype(BF16)

    for h in range(HEADS):
        kr[h] = jnp.broadcast_to(take_keys(h, BEFORE, ROWS), (ROWS, HEAD_DIM))
        for raw, normed, rows in (
                (qd0[0, h], qn0.at[h], slice(0, SEG)),
                (qdx[0, h, :BEFORE], qn.at[h, :BEFORE], slice(SEG, ROWS))):
            u, r = unit(raw)
            qu[h, rows] = u
            qr[h, rows] = jnp.broadcast_to(r, u.shape)
            normed[...] = (u * gain_q).astype(BF16)

    @pl.when(is_first)
    def _():
        for h in range(HEADS):
            for n in range(2):
                kvx[n, h, :BEFORE] = kvx[n, h, BEFORE:2 * BEFORE]
                first_kv[n, h] = kvx[n, h, BEFORE:ROWS]

    @pl.when(closes)
    def _():
        for h in range(HEADS):
            for n in range(2):
                kvx[n, h, BEFORE + ROWS:] = kvx[n, h, BEFORE:ROWS]
            qdx[0, h, BEFORE:] = qd0[0, h]
            qdx[1, h, BEFORE:] = jnp.zeros((SEG, HEAD_DIM), BF16)

    @pl.when(is_last)
    def _():
        for h in range(HEADS):
            for n in range(2):
                from_after[n, h] = jnp.zeros((BEFORE, HEAD_DIM), BF16)

    key_at = lax.broadcasted_iota(jnp.int32, (PAIR, PAIR), 0)
    query_at = lax.broadcasted_iota(jnp.int32, (PAIR, PAIR), 1)
    past = query_at >= key_at
    early = query_at < SEG
    high = key_at >= SEG
    lane = lax.broadcasted_iota(jnp.int32, (1, PAIR), 1)
    table = table_v[...]
    low_part = table[:, :PAIR]
    high_part = jnp.concatenate([table[:, PAIR:], jnp.zeros((HEADS, 2 * PAIR - ENTRIES), F32)], axis=1)
    low_rolled = pltpu.roll(low_part, PAIR - SEG + 1, 1)
    high_rolled = pltpu.roll(high_part, PAIR - SEG + 1, 1)
    for h in range(HEADS):
        last = table[h:h + 1, ENTRIES - 1:ENTRIES]
        dist_low = low_rolled[h:h + 1]
        dist_row = jnp.where(lane <= SEG, dist_low, high_rolled[h:h + 1])
        ahead = pltpu.roll(jnp.broadcast_to(dist_low, (PAIR, PAIR)), 0, 1, stride=1, stride_axis=0)
        behind = pltpu.roll(jnp.broadcast_to(dist_row, (PAIR, PAIR)), 0, 1, stride=1, stride_axis=0)
        tile0 = jnp.where(jnp.logical_or(early, high), last, MASKED)
        tile1 = jnp.where(past, last, behind)
        tile2 = jnp.where(jnp.logical_and(early, high), MASKED, jnp.where(past, behind, ahead))
        none, low = (jnp.where(is_first, MASKED, t) for t in (tile0, tile1))
        for p, tiles in enumerate((
                (none, jnp.where(high, tile1, low), tile2),
                (jnp.where(high, tile0, none), tile1, tile2))):
            top = jnp.max(jnp.maximum(jnp.maximum(tiles[0], tiles[1]), tiles[2]), axis=0, keepdims=True)
            for b, tile in enumerate(tiles):
                bias_v[h, p, b * PAIR:(b + 1) * PAIR] = (tile - top) * LOG2E

    def work(blocks, tiles=()):
        at_keys = {(p, b): slice((p + b) * PAIR, (p + b + 1) * PAIR) for h, p, b in blocks}
        at_queries = [slice(p * PAIR, (p + 1) * PAIR) for p in range(2)]
        at_rows = [slice(b * PAIR, (b + 1) * PAIR) for b in range(3)]
        scores = [dot(kn[h, at_keys[p, b]], qn[h, at_queries[p]], 1, 1) for h, p, b in blocks]
        d_probs = [dot(kvx[1, h, at_keys[p, b]], qdx[1, h, at_queries[p]], 1, 1) for h, p, b in blocks]
        for (h, p, b), s, dp in zip(blocks, scores, d_probs):
            e = jnp.exp2(s * (FACTOR * LOG2E) + bias_v[h, p, at_rows[b]])
            e_v[h, p, at_rows[b]] = e
            dp_v[h, p, at_rows[b]] = dp
            sum_v[h, p, b] = jnp.sum(e, axis=0, keepdims=True)
            sum_v[h, p, 3 + b] = jnp.sum(e * dp, axis=0, keepdims=True)
        d_scores, products = [], []
        for h, p, _ in tiles:
            inv = 1.0 / (sum_v[h, p, 0] + sum_v[h, p, 1] + sum_v[h, p, 2])
            delta = (sum_v[h, p, 3] + sum_v[h, p, 4] + sum_v[h, p, 5]) * inv
            prob = e_v[h, p] * inv
            d_score = prob * (dp_v[h, p] - delta)
            d_low = d_score.astype(BF16)
            prob_v[h, p] = prob.astype(BF16)
            d_low_v[h, p] = d_low
            d_scores.append(d_score)
            products.append(dot(d_low, qn[h, at_queries[p]], 1, 0))
        for (h, p, again), d_score in zip(tiles, d_scores):
            if again:
                fold_table(h, d_v[h] + d_score)
            else:
                d_v[h] = d_score
        for (h, p, again), dk in zip(tiles, products):
            keys = slice(p * PAIR, (p + 3) * PAIR)
            gain_v[h, p, 0] = jnp.sum(dk * kn[h, keys].astype(F32), axis=0, keepdims=True)
            gain_v[h, p, 1] = jnp.sum(dk * ku[h, keys], axis=0, keepdims=True)
            if again:
                shared, alone = slice(PAIR, 3 * PAIR), slice(3 * p * PAIR, (3 * p + 1) * PAIR)
                dkx[h, alone] = dk[2 * p * PAIR:(2 * p + 1) * PAIR]
                dkx[h, shared] = dkx[h, shared] + dk[(1 - p) * PAIR:(3 - p) * PAIR]
            else:
                dkx[h, keys] = dk

    def query_rows(g, u, r):
        g = g * FACTOR * gain_q
        return (r * (g - u * jnp.mean(g * u, axis=-1, keepdims=True))).astype(BF16)

    sublane = lax.broadcasted_iota(jnp.int32, (8, PAIR), 0)

    def skewed_sum(tile, right):
        parts = [pltpu.roll(tile[first:first + 8], (right - first) % PAIR, 1) for first in range(0, PAIR, 8)]
        while len(parts) > 1:
            parts = [a + b for a, b in zip(parts[::2], parts[1::2])]
        total = parts[0]
        for bit in range(1, 8):
            total = jnp.where(sublane == bit, pltpu.roll(parts[0], PAIR - bit, 1), total)
        return jnp.sum(total, axis=0, keepdims=True)

    def fold_rows(h, d_score):
        d0, d1, d2 = (d_score[b * PAIR:(b + 1) * PAIR] for b in range(3))
        mixed = jnp.where(past, d2, d1)
        ahead = jnp.where(past, 0.0, d2)
        rest = d0 + jnp.where(past, d1, 0.0)
        behind_row, ahead_row = skewed_sum(mixed, SEG - 1), skewed_sum(ahead, SEG - 1)
        high_row = skewed_sum(mixed, SEG - 1 + SEG) if h else behind_row
        rest_sum = jnp.sum(jnp.sum(rest, axis=0, keepdims=True), axis=1, keepdims=True)
        return (
            jnp.where(lane < SEG - 1, ahead_row, behind_row),
            jnp.where(lane == SEG - 1 + h * SEG, rest_sum, high_row))

    def fold_table(h, d_score):
        table_v2[h, 0], table_v2[h, 1] = fold_rows(h, d_score)

    def first_segment():
        key_number = lax.broadcasted_iota(jnp.int32, (ROWS + SEG, SEG), 0)
        hidden = jnp.logical_and(is_first, key_number < ROWS)

        for h in heads:
            u, _ = unit(first_kv[0, h])
            first_ku[h] = u
            first_kn[h] = (u * gain_k).astype(BF16)

        def against(first, rest, side):
            return jnp.concatenate([dot(first, side, 1, 1), dot(rest, side, 1, 1)], axis=0)

        scores = [against(first_kn[h], kn[h, :ROWS], qn0[h]) for h in heads]
        d_probs = [against(first_kv[1, h], kvx[1, h, :ROWS], qd0[1, h]) for h in heads]
        d_scores = []
        for h in heads:
            bias = jnp.where(hidden, MASKED, bias_v[h, 0, :ROWS + SEG][:, :SEG])
            bias = bias - jnp.max(bias, axis=0, keepdims=True)
            e = jnp.exp2(scores[h] * (FACTOR * LOG2E) + bias)
            inv = 1.0 / jnp.sum(e, axis=0, keepdims=True)
            delta = jnp.sum(e * d_probs[h], axis=0, keepdims=True) * inv
            prob = e * inv
            d_scores.append(prob * (d_probs[h] - delta))
            first_prob[h] = prob.astype(BF16)
            first_d_low[h] = d_scores[h].astype(BF16)
        products = [dot(d_scores[h].astype(BF16), qn0[h], 1, 0) for h in heads]
        for h in heads:
            tile = jnp.concatenate([d_scores[h], jnp.zeros((ROWS + SEG, SEG), F32)], axis=1)
            rows = fold_rows(h, jnp.concatenate([tile, jnp.zeros((SEG, PAIR), F32)], axis=0))
            for j in range(2):
                table_v2[h, j] = table_v2[h, j] + rows[j]
        for h in heads:
            first_dk[h] = products[h]
        for n, (first, rest) in enumerate(((first_kn, kn), (first_ku, ku))):
            gain = jnp.zeros((1, HEAD_DIM), F32)
            for h in heads:
                gain = gain + jnp.sum(products[h][:SEG] * first[h].astype(F32), axis=0, keepdims=True)
                gain = gain + jnp.sum(products[h][SEG:] * rest[h, :ROWS].astype(F32), axis=0, keepdims=True)
            extra_gain[n:n + 1] = gain

    def first_results(h):
        d_low = first_d_low[h]
        dv = dot(first_prob[h], qd0[1, h], 1, 0)
        dq_from_before[h] = dot(d_low[:SEG], first_kn[h], 0, 0) + dot(d_low[SEG:], kn[h, :ROWS], 0, 0)
        for n, part in enumerate((first_dk[h] * FACTOR, dv)):
            to_before_first[n, h] = part[:SEG].astype(BF16)
            from_before[n, h] = part[ROWS:].astype(BF16)
        dkx[h, :BEFORE] = dkx[h, :BEFORE] + first_dk[h, SEG:ROWS]
        dvx[h, :BEFORE] = dvx[h, :BEFORE] + dv[SEG:ROWS]

    heads = range(HEADS)
    work([(h, 0, 2) for h in heads])

    go_on(forth[2:], jnp.logical_and(tp == 1, place < total - 1))
    @pl.when(tp == 1)
    def _():
        pl.semaphore_wait(round1, len(close))
        for a, n in enumerate(sizes[:2]):
            if n > 5:
                for o in near(n, 2):
                    signal(round2, along(a, o))

    def wait_left(piece):
        @pl.when(place > 0)
        def _():
            if piece < HEADS:
                forth[piece].wait_recv()
            else:
                @pl.when(opens)
                def _():
                    wait_bytes(kvx.at[:, :, :PAIR], left_recv.at[piece - 1])

                @pl.when(takes_back)
                def _():
                    forth[piece].wait_recv()

    def wait_right():
        @pl.when(takes_next)
        def _():
            wait_bytes(kvx.at[:, :, :PAIR], right_recv)

    beside = sorted({*near(ny), *near(ny, 2)})

    def greet_far():
        @pl.when(tp == 1)
        def _():
            count = sum(len(near(n, 2)) for n in sizes[:2] if n > 5)
            if count:
                pl.semaphore_wait(round2, count)
            for o in beside:
                signal(plane_round, along(1, o))
            if nz > 9:
                for o in near(nz, 3):
                    signal(round3, along(0, o))

    def do_first():
        @pl.when(opens)
        def _():
            first_segment()

    def near_keys():
        for h in heads:
            take_keys(h, PAIR, SEG)

    def next_rows():
        for h in heads:
            take_keys(h, BEFORE + ROWS, SEG)
            take_queries(h)

    @pl.when(x == nx - 1)
    def _():
        wait_left(0)
        near_keys()
        work([(h, 0, 1) for h in heads])
        for h in heads:
            wait_left(1 + h)
            take_keys(h, 0, PAIR)
            work([(h, 0, 0)], [(h, 0, False)])
            if not h:
                greet_far()
        wait_right()
        next_rows()
        work([(h, 1, b) for b in range(3) for h in heads], [(h, 1, True) for h in heads])
        if nx == 1:
            do_first()

    if nx > 1:
        @pl.when(x == 0)
        def _():
            wait_right()
            next_rows()
            work([(h, 1, b) for b in (1, 2) for h in heads])
            greet_far()
            wait_left(0)
            near_keys()
            work([(h, p, 1 - p) for p in (1, 0) for h in heads], [(h, 1, False) for h in heads])
            for h in heads:
                wait_left(1 + h)
                take_keys(h, 0, PAIR)
                work([(h, 0, 0)], [(h, 0, True)])
            do_first()

    if nx > 2:
        @pl.when(jnp.logical_and(x > 0, x < nx - 1))
        def _():
            wait_left(0)
            near_keys()
            work([(h, 0, 1) for h in heads])
            wait_right()
            next_rows()
            work([(h, 1, b) for b in range(3) for h in heads], [(h, 1, False) for h in heads])
            greet_far()
            for h in heads:
                wait_left(1 + h)
                take_keys(h, 0, PAIR)
                work([(h, 0, 0)], [(h, 0, True)])

    second = jnp.where(lane < SEG, table_v2[0, 1], table_v2[1, 1])
    gain_rows = [
        (gain_v[0, 0, j] + gain_v[0, 1, j] + gain_v[1, 0, j] + gain_v[1, 1, j]
         + jnp.where(opens, extra_gain[j:j + 1], 0.0)) * FACTOR for j in range(2)]
    vec = jnp.concatenate([table_v2[0, 0], table_v2[1, 0], second, *gain_rows], axis=0)
    chip = y * nx + x

    to_neighbours = [
        remote(to_before.at[:, h], from_after.at[:, h], more_sem, after_recv, before) for h in range(HEADS)]
    to_next = [
        remote(to_after, from_before, table_sem, before_recv, after),
        remote(dqx.at[:, BEFORE:], dq_from_before, table_sem, before_recv, after)]
    to_plane_before = remote(to_before_first, from_after_first, more_sem, after_recv, before)

    def stage_results():
        @pl.when(takes_next)
        def _():
            wait_bytes(kvx.at[:, :, :BEFORE], load_sem)

        @pl.when(closes_early)
        def _():
            wait_bytes(kvx.at[:, :, :ROWS], load_sem)

        @pl.when(takes_back)
        def _():
            wait_bytes(kvx.at[:, :, :PAIR], gains_sem)

        for h in range(HEADS):
            low, high_tile = (dot(prob_v[h, p], qdx[1, h, p * PAIR:(p + 1) * PAIR], 1, 0) for p in range(2))
            dvx[h, :PAIR] = low[:PAIR]
            dvx[h, PAIR:3 * PAIR] = low[PAIR:] + high_tile[:2 * PAIR]
            dvx[h, 3 * PAIR:] = high_tile[2 * PAIR:]

            @pl.when(opens)
            def _(h=h):
                first_results(h)

            lanes = slice(h * HEAD_DIM, (h + 1) * HEAD_DIM)
            to_before[0, h] = (dkx[h, :BEFORE] * FACTOR).astype(BF16)
            to_before[1, h] = dvx[h, :BEFORE].astype(BF16)
            to_after[0, h] = (dkx[h, BEFORE + ROWS:] * FACTOR).astype(BF16)
            to_after[1, h] = dvx[h, BEFORE + ROWS:].astype(BF16)
            for p in range(2):
                dqx[h, p * PAIR:(p + 1) * PAIR] = dot(d_low_v[h, p], kn[h, p * PAIR:(p + 3) * PAIR], 0, 0)
            dq_v[SEG:, lanes] = query_rows(dqx[h, :BEFORE], qu[h, SEG:], qr[h, SEG:])

    def send_results(when):
        @pl.when(jnp.logical_and(when, place > 0))
        def _():
            for copy in to_neighbours:
                copy.start()

        @pl.when(jnp.logical_and(when, opens_later))
        def _():
            to_plane_before.start()

        @pl.when(jnp.logical_and(when, takes_next))
        def _():
            for copy in to_next:
                copy.start()

    def sum_of(ref, first, count):
        parts = [ref[n] for n in range(first, first + count)]
        while len(parts) > 1:
            parts = [sum(parts[n:n + 2]) for n in range(0, len(parts), 2)]
        return parts[0]

    has_across = ny > 3 and ny % 2 == 0
    across, column = nx * ny, nx * ny + nx

    @pl.when(tp == 1)
    def _():
        rows_x[x] = vec
        for o in far_first(nx):
            remote(rows_x.at[x], rows_x.at[x], sum_send, x_recv, along(2, o)).start()
        if beside:
            pl.semaphore_wait(plane_round, len(beside))
        signal(round1, (z, y, x, 0))
        if has_across:
            for o in far_first(nx) + [0]:
                remote(
                    rows_x.at[x], plane.at[across + x], sum_send, plane_recv,
                    (z, lax.rem(y + ny // 2, ny), lax.rem(x + o, nx), 1)).start()
        stage_results()
        send_results(jnp.logical_and(x > 0, x < nx - 1))
        if nx > 1:
            wait_bytes(rows_x.at[:nx - 1], x_recv)
        plane[column + y] = sum_of(rows_x, 0, nx)
        y_ways = [o for o in far_first(ny) if not has_across or o != ny // 2]
        for o in y_ways:
            remote(plane.at[column + y], plane.at[column + y], sum_send, plane_recv, along(1, o)).start()
        came = nx * ny + len(y_ways) + (nx if has_across else 0)
        wait_bytes(plane.at[:came], plane_recv)
        if has_across:
            plane[column + lax.rem(y + ny // 2, ny)] = sum_of(plane, across, nx)
        others, part = sum_of(plane, 0, nx * ny), sum_of(plane, column, ny)
        gain = part[3:] + others[3:]
        for core, rows in enumerate((others, part)):
            zout[core, :3] = rows[:3]
            zout[core, 3:] = gain
        zbuf[z] = zout[1]
        if nz > 9:
            pl.semaphore_wait(round3, len(near(nz, 3)))
        for o in [*far_first(nz), 0]:
            for core in ((1, 0) if o else (0,)):
                remote(zout.at[core], zbuf.at[z], sum_send, z_recv, along(0, o, core)).start()
        send_results(jnp.logical_or(x == 0, x == nx - 1))
        signal(round2, (z, y, x, 0))

    @pl.when(tp == 0)
    def _():
        plane[chip] = vec
        pl.semaphore_wait(round1, 1)
        for oy, ox in sorted(
                ((oy, ox) for oy in range(ny) for ox in range(nx)),
                key=lambda o: -min(o[0], ny - o[0]) - min(o[1], nx - o[1])):
            remote(
                plane.at[chip], plane.at[chip], sum_send, plane_recv,
                (z, lax.rem(y + oy, ny), lax.rem(x + ox, nx), 1)).start()
        stage_results()
        send_results(jnp.logical_or(opens, jnp.logical_and(x > 0, x < nx - 1)))
        pl.semaphore_wait(round2, 1)
        send_results(jnp.logical_and(jnp.logical_not(opens), jnp.logical_or(x == 0, x == nx - 1)))

    @pl.when(takes_back)
    def _():
        wait_bytes(kvx.at[:, :, :PAIR], before_recv)

    @pl.when(takes_next)
    def _():
        wait_bytes(from_after, after_recv)

    @pl.when(closes_early)
    def _():
        wait_bytes(kvx.at[:, :, :ROWS], after_recv)

    for h in range(HEADS):
        dq_v[:SEG, h * HEAD_DIM:(h + 1) * HEAD_DIM] = query_rows(dq_from_before[h], qu[h, :SEG], qr[h, :SEG])

    for h in range(HEADS):
        lanes = slice(h * HEAD_DIM, (h + 1) * HEAD_DIM)
        sums_in = [
            jnp.concatenate([
                jnp.where(takes_next, 0.0, jnp.where(is_last, 0.0, from_after_first[n, h].astype(F32)))
                + from_before[n, h].astype(F32), from_after[n, h].astype(F32)], axis=0) for n in range(2)]
        g = (dkx[h, BEFORE:BEFORE + ROWS] * FACTOR + sums_in[0]) * gain_k
        u = ku[h, BEFORE:BEFORE + ROWS]
        dk_v[:, lanes] = (kr[h] * (g - u * jnp.mean(g * u, axis=-1, keepdims=True))).astype(BF16)
        dv_v[:, lanes] = (dvx[h, BEFORE:BEFORE + ROWS] + sums_in[1]).astype(BF16)

    @pl.when(takes_next)
    def _():
        wait_bytes(kvx.at[:, :, :PAIR], table_sem)

    @pl.when(takes_back)
    def _():
        wait_bytes(from_after, more_sem)

    @pl.when(opens_later)
    def _():
        wait_bytes(kvx.at[:, :, :ROWS], more_sem)

    @pl.when(tp == 1)
    def _():
        wait_bytes(plane.at[:nx - 1 + 2 * nz - 1 + ny - 1 + (nx - 1 if has_across else 0)], sum_send)
        if nz > 1:
            wait_bytes(zbuf.at[:nz - 1], z_recv)

    @pl.when(tp == 0)
    def _():
        wait_bytes(plane.at[:nx * ny], sum_send)
        wait_bytes(zbuf.at[:nz], z_recv)

    result = zbuf[0]
    for n in range(1, nz):
        result = result + zbuf[n]
    for j in range(HEADS):
        dtab_v[j:j + 1, :PAIR] = result[j:j + 1]
        dtab_v[j:j + 1, PAIR:] = result[2:3, j * SEG:(j + 1) * SEG]
    dgain_v[0:1] = result[3:4] / gain_q
    dgain_v[1:2] = result[4:5]


def write_out(*refs):
    count = len(refs) // 2
    copies = [pltpu.make_async_copy(refs[n], refs[count + n], refs[-1].at[n]) for n in range(count)]
    for copy in copies:
        copy.start()
    for copy in copies:
        copy.wait()


def local(sizes, queries, keys, values, gains, bias_table, d_out):
    nz, ny, nx = sizes
    width = HEADS * HEAD_DIM
    hbm_spec = pl.BlockSpec(memory_space=pltpu.HBM)
    vmem_spec = pl.BlockSpec(memory_space=pltpu.VMEM)
    first = (HEADS, SEG, HEAD_DIM)
    tile = (HEADS, ROWS, HEAD_DIM)
    wide = (HEADS, 2 * ROWS, HEAD_DIM)
    pairs = (HEADS, 2, 3 * PAIR, PAIR)
    dma, regular = pltpu.SemaphoreType.DMA, pltpu.SemaphoreType.REGULAR
    vmem = pltpu.VMEM
    outs = [((ROWS, width), BF16)] * 3 + [((HEADS, ENTRIES), F32), ((2, HEAD_DIM), F32)]
    out = pl.pallas_call(
        functools.partial(kernel, sizes),
        out_shape=tuple(vmem(*o) for o in outs),
        in_specs=[hbm_spec] * 6,
        out_specs=(vmem_spec,) * 5,
        scratch_shapes=[
            vmem((2, *tile), BF16), vmem((2, *first), BF16), vmem((2, *wide), BF16), vmem((2, *first), BF16),
            vmem((2, HEAD_DIM), F32), vmem((HEADS, ENTRIES), F32),
            vmem(tile, BF16), vmem(first, BF16), vmem(tile, F32), vmem(tile, F32),
            vmem(wide, BF16), vmem(wide, F32), vmem(tile, F32),
            vmem(first, BF16), vmem(first, F32),
            vmem(pairs, F32), vmem(pairs, F32), vmem(pairs, F32),
            vmem(wide, F32), vmem(wide, F32), vmem(tile, F32), vmem((HEADS, 3 * PAIR, PAIR), F32),
            vmem(pairs, BF16), vmem(pairs, BF16), vmem((HEADS, 2, 6, 1, PAIR), F32), vmem((HEADS, 2, 2, 1, PAIR), F32),
            vmem((HEADS, 2, 1, PAIR), F32), vmem((2, HEAD_DIM), F32),
            vmem((HEADS, ROWS + SEG, SEG), BF16), vmem((HEADS, ROWS + SEG, SEG), BF16), vmem((HEADS, ROWS + SEG, HEAD_DIM), F32),
            vmem((2, HEADS, BEFORE, HEAD_DIM), BF16), vmem((2, HEADS, BEFORE, HEAD_DIM), BF16),
            vmem((2, *first), BF16), vmem((2, *first), BF16), vmem(first, F32), vmem((2, *first), BF16), vmem((2, *first), BF16),
            vmem((nx, 5, HEAD_DIM), F32), vmem((nx * ny + nx + ny + 2 * nz, 5, HEAD_DIM), F32), vmem((2, 5, HEAD_DIM), F32), vmem((2 * nz, 5, HEAD_DIM), F32),
            dma, dma, dma, dma, dma((HEADS + 1,)), dma, dma, dma,
            dma, dma, dma, dma, regular, regular, regular, regular,
        ],
        compiler_params=pltpu.CompilerParams(
            collective_id=0, has_side_effects=True, vmem_limit_bytes=32 * 1024 * 1024),
        name="segment_attention_grad",
    )(*(pltpu.with_memory_space_constraint(a, pltpu.HBM) for a in (queries, keys, values, d_out, gains, bias_table.T)))
    d_queries, d_keys, d_values, d_table, d_gains = pl.pallas_call(
        write_out,
        out_shape=tuple(jax.ShapeDtypeStruct(*o) for o in outs),
        in_specs=[vmem_spec] * 5,
        out_specs=(hbm_spec,) * 5,
        scratch_shapes=[dma((5,))],
        name="write_out",
    )(*(pltpu.with_memory_space_constraint(o, pltpu.VMEM) for o in out))
    return d_queries, d_keys, d_values, d_table.T, d_gains


def solution(mesh):
    shape = (12, 8, 4)
    if mesh.shape["sp"] != int(np.prod(shape)):
        shape = mesh.small_shape
    split = Mesh(mesh.devices.reshape(*shape, mesh.shape["tp"]), AXES)
    placed = (P(SP, "tp"), P(SP, "tp"), P(SP, "tp"), P(), P(None, "tp"), P(SP, "tp"))
    return jax.shard_map(
        functools.partial(local, shape),
        mesh=split,
        in_specs=placed,
        out_specs=(P(SP, "tp"), P(SP, "tp"), P(SP, "tp"), P(None, "tp"), P()),
        check_vma=False,
    )
```

```python
import functools

import jax
import jax.numpy as jnp
import numpy as np
from jax import lax
from jax.experimental import pallas as pl
from jax.experimental.pallas import tpu as pltpu
from jax.sharding import Mesh
from jax.sharding import PartitionSpec as P

HEAD_DIM = 128
SEG = 64
LEFT = 4
MAX_REL = 128
ENTRIES = MAX_REL + SEG
ROWS = LEFT * SEG
HEADS = 2
PAIR = 2 * SEG
BEFORE = 3 * SEG
AXES = ("sp_0", "sp_1", "sp_2", "tp")
SP = AXES[:3]

EPSILON = 1e-06
FACTOR = HEAD_DIM ** (-0.5)
LOG2E = 1.4426950408889634
MASKED = -1e30
F32, BF16 = jnp.float32, jnp.bfloat16


def dot(a, b, a_dim, b_dim):
    return lax.dot_general(a, b, (((a_dim,), (b_dim,)), ((), ())), preferred_element_type=F32)


def near(size, step=1):
    return sorted({step % size, -step % size} - {0})


def far_first(size):
    return sorted(range(1, size), key=lambda d: -min(d, size - d))


def unit(raw):
    wide = raw.astype(F32)
    inv_rms = lax.rsqrt(jnp.mean(wide * wide, axis=-1, keepdims=True) + EPSILON)
    return wide * inv_rms, inv_rms


def kernel(sizes, q_hbm, k_hbm, v_hbm, do_hbm, gains_hbm, table_hbm,
           dq_v, dk_v, dv_v, dtab_v, dgain_v,
           qdx, qd0, kvx, first_kv, gains_v, table_v,
           qn, qn0, qu, qr, kn, ku, kr, first_kn, first_ku, bias_v, e_v, dp_v,
           dkx, dvx, dqx, d_v, prob_v, d_low_v, sum_v, gain_v, table_v2, extra_gain, first_prob, first_d_low, first_dk,
           to_before, from_after, to_after, from_before, dq_from_before, to_before_first, from_after_first,
           rows_x, plane, zout, zbuf,
           load_sem, more_sem, gains_sem, table_sem, left_recv, right_recv, after_recv, before_recv,
           sum_send, x_recv, plane_recv, z_recv, round1, round2, round3, plane_round):
    nz, ny, nx = sizes
    z, y, x, tp = (lax.axis_index(a) for a in AXES)
    place = (z * ny + y) * nx + x
    total = nz * ny * nx
    is_first, is_last = place == 0, place == total - 1
    opens, closes = jnp.logical_and(x == 0, y == 0), jnp.logical_and(x == nx - 1, y == ny - 1)
    opens_later, closes_early = jnp.logical_and(opens, place > 0), jnp.logical_and(closes, place < total - 1)
    takes_back, takes_next = jnp.logical_not(opens), jnp.logical_not(closes)

    def at(number, core):
        return (number // (ny * nx), (number // nx) % ny, number % nx, core)

    after = at(jnp.minimum(place + 1, total - 1), tp)
    before = at(jnp.maximum(place - 1, 0), tp)

    def along(axis, offset, core=1):
        if axis == 0:
            return (lax.rem(z + offset, nz), y, x, core)
        if axis == 1:
            return (z, lax.rem(y + offset, ny), x, core)
        return (z, y, lax.rem(x + offset, nx), core)

    def signal(sem, target):
        pl.semaphore_signal(sem, inc=1, device_id=target, device_id_type=pl.DeviceIdType.MESH)

    def remote(src, dst, send, recv, target):
        return pltpu.make_async_remote_copy(
            src_ref=src, dst_ref=dst, send_sem=send, recv_sem=recv,
            device_id=target, device_id_type=pl.DeviceIdType.MESH)

    def wait_bytes(ref, sem):
        pltpu.make_async_copy(ref, ref, sem).wait()

    barrier = pltpu.get_barrier_semaphore()

    @pl.when(place > 0)
    def _():
        signal(barrier, before)

    @pl.when(place < total - 1)
    def _():
        signal(barrier, after)

    sides = jnp.where(is_first, 0, 1) + jnp.where(is_last, 0, 1)
    small_loads = [pltpu.make_async_copy(gains_hbm, gains_v, gains_sem), pltpu.make_async_copy(table_hbm, table_v, table_sem)]
    for load in small_loads:
        load.start()
    for h in range(HEADS):
        lanes = slice(h * HEAD_DIM, (h + 1) * HEAD_DIM)
        for n, (keys_or_values, queries_or_cotangents) in enumerate(((k_hbm, q_hbm), (v_hbm, do_hbm))):
            pltpu.make_async_copy(keys_or_values.at[:, lanes], kvx.at[n, h, BEFORE:BEFORE + ROWS], load_sem).start()
            pltpu.make_async_copy(queries_or_cotangents.at[:SEG, lanes], qd0.at[n, h], load_sem).start()
            pltpu.make_async_copy(queries_or_cotangents.at[SEG:, lanes], qdx.at[n, h, :BEFORE], more_sem).start()

    close = [(a, o) for a, n in enumerate(sizes) for o in near(n)]

    @pl.when(tp == 1)
    def _():
        for a, o in close:
            signal(barrier, along(a, o))
        signal(barrier, (z, y, x, 0))

    @pl.when(tp == 0)
    def _():
        signal(barrier, (z, y, x, 1))

    forth = [remote(
        kvx.at[:, :, ROWS + PAIR:ROWS + BEFORE], kvx.at[:, :, PAIR:BEFORE], load_sem, left_recv.at[HEADS], after)]
    back = {}
    for h in range(HEADS):
        forth.append(remote(
            kvx.at[:, h, ROWS:ROWS + PAIR], kvx.at[:, h, :PAIR], load_sem, left_recv.at[h], after))
        back[h] = [
            remote(kvx.at[:, h, BEFORE:ROWS], kvx.at[:, h, BEFORE + ROWS:], gains_sem, right_recv, before),
            remote(qd0.at[:, h], qdx.at[:, h, BEFORE:], gains_sem, right_recv, before)]

    plane_piece = remote(kvx.at[:, :, BEFORE:ROWS], first_kv, load_sem, left_recv.at[HEADS - 1], after)

    def go_on(pieces, when=place < total - 1):
        @pl.when(when)
        def _():
            for copy in pieces:
                copy.start()

    wait_bytes(kvx.at[:, :, :ROWS + SEG], load_sem)
    small_loads[0].wait()
    gains = gains_v[...]
    gain_q, gain_k = gains[0:1, :], gains[1:2, :]

    def take_keys(h, first, size):
        u, r = unit(kvx[0, h, first:first + size])
        ku[h, first:first + size] = u
        kn[h, first:first + size] = (u * gain_k).astype(BF16)
        return r

    def take_queries(h):
        qn[h, BEFORE:] = (unit(qdx[0, h, BEFORE:])[0] * gain_q).astype(BF16)

    for h in range(HEADS):
        kr[h] = jnp.broadcast_to(take_keys(h, BEFORE, ROWS), (ROWS, HEAD_DIM))
    pl.semaphore_wait(barrier, sides + jnp.where(tp == 1, 1 + len(close), 1))
    go_on(forth[:1])
    go_on([copy for h in range(HEADS) for copy in back[h]], takes_back)
    go_on(forth[1:], jnp.logical_and(tp == 0, place < total - 1))
    go_on(forth[1:2], jnp.logical_and(tp == 1, place < total - 1))
    go_on([plane_piece], closes_early)

    @pl.when(tp == 1)
    def _():
        for a, o in close:
            signal(round1, along(a, o))

    wait_bytes(qdx.at[:, :, :BEFORE], more_sem)
    small_loads[1].wait()
    for h in range(HEADS):
        for raw, normed, rows in (
                (qd0[0, h], qn0.at[h], slice(0, SEG)),
                (qdx[0, h, :BEFORE], qn.at[h, :BEFORE], slice(SEG, ROWS))):
            u, r = unit(raw)
            qu[h, rows] = u
            qr[h, rows] = jnp.broadcast_to(r, u.shape)
            normed[...] = (u * gain_q).astype(BF16)

    @pl.when(is_first)
    def _():
        for h in range(HEADS):
            for n in range(2):
                kvx[n, h, :BEFORE] = kvx[n, h, BEFORE:2 * BEFORE]
                first_kv[n, h] = kvx[n, h, BEFORE:ROWS]

    @pl.when(closes)
    def _():
        for h in range(HEADS):
            for n in range(2):
                kvx[n, h, BEFORE + ROWS:] = kvx[n, h, BEFORE:ROWS]
            qdx[0, h, BEFORE:] = qd0[0, h]
            qdx[1, h, BEFORE:] = jnp.zeros((SEG, HEAD_DIM), BF16)

    @pl.when(is_last)
    def _():
        for h in range(HEADS):
            for n in range(2):
                from_after[n, h] = jnp.zeros((BEFORE, HEAD_DIM), BF16)

    key_at = lax.broadcasted_iota(jnp.int32, (PAIR, PAIR), 0)
    query_at = lax.broadcasted_iota(jnp.int32, (PAIR, PAIR), 1)
    past = query_at >= key_at
    early = query_at < SEG
    high = key_at >= SEG
    lane = lax.broadcasted_iota(jnp.int32, (1, PAIR), 1)
    table = table_v[...]
    low_part = table[:, :PAIR]
    high_part = jnp.concatenate([table[:, PAIR:], jnp.zeros((HEADS, 2 * PAIR - ENTRIES), F32)], axis=1)
    low_rolled = pltpu.roll(low_part, PAIR - SEG + 1, 1)
    high_rolled = pltpu.roll(high_part, PAIR - SEG + 1, 1)
    for h in range(HEADS):
        last = table[h:h + 1, ENTRIES - 1:ENTRIES]
        dist_low = low_rolled[h:h + 1]
        dist_row = jnp.where(lane <= SEG, dist_low, high_rolled[h:h + 1])
        ahead = pltpu.roll(jnp.broadcast_to(dist_low, (PAIR, PAIR)), 0, 1, stride=1, stride_axis=0)
        behind = pltpu.roll(jnp.broadcast_to(dist_row, (PAIR, PAIR)), 0, 1, stride=1, stride_axis=0)
        tile0 = jnp.where(jnp.logical_or(early, high), last, MASKED)
        tile1 = jnp.where(past, last, behind)
        tile2 = jnp.where(jnp.logical_and(early, high), MASKED, jnp.where(past, behind, ahead))
        none, low = (jnp.where(is_first, MASKED, t) for t in (tile0, tile1))
        for p, tiles in enumerate((
                (none, jnp.where(high, tile1, low), tile2),
                (jnp.where(high, tile0, none), tile1, tile2))):
            top = jnp.max(jnp.maximum(jnp.maximum(tiles[0], tiles[1]), tiles[2]), axis=0, keepdims=True)
            for b, tile in enumerate(tiles):
                bias_v[h, p, b * PAIR:(b + 1) * PAIR] = (tile - top) * LOG2E

    def work(blocks, tiles=()):
        at_keys = {(p, b): slice((p + b) * PAIR, (p + b + 1) * PAIR) for h, p, b in blocks}
        at_queries = [slice(p * PAIR, (p + 1) * PAIR) for p in range(2)]
        at_rows = [slice(b * PAIR, (b + 1) * PAIR) for b in range(3)]
        scores = [dot(kn[h, at_keys[p, b]], qn[h, at_queries[p]], 1, 1) for h, p, b in blocks]
        d_probs = [dot(kvx[1, h, at_keys[p, b]], qdx[1, h, at_queries[p]], 1, 1) for h, p, b in blocks]
        for (h, p, b), s, dp in zip(blocks, scores, d_probs):
            e = jnp.exp2(s * (FACTOR * LOG2E) + bias_v[h, p, at_rows[b]])
            e_v[h, p, at_rows[b]] = e
            dp_v[h, p, at_rows[b]] = dp
            sum_v[h, p, b] = jnp.sum(e, axis=0, keepdims=True)
            sum_v[h, p, 3 + b] = jnp.sum(e * dp, axis=0, keepdims=True)
        d_scores, products = [], []
        for h, p, _ in tiles:
            inv = 1.0 / (sum_v[h, p, 0] + sum_v[h, p, 1] + sum_v[h, p, 2])
            delta = (sum_v[h, p, 3] + sum_v[h, p, 4] + sum_v[h, p, 5]) * inv
            prob = e_v[h, p] * inv
            d_score = prob * (dp_v[h, p] - delta)
            d_low = d_score.astype(BF16)
            prob_v[h, p] = prob.astype(BF16)
            d_low_v[h, p] = d_low
            d_scores.append(d_score)
            products.append(dot(d_low, qn[h, at_queries[p]], 1, 0))
        for (h, p, again), d_score in zip(tiles, d_scores):
            if again:
                fold_table(h, d_v[h] + d_score)
            else:
                d_v[h] = d_score
        for (h, p, again), dk in zip(tiles, products):
            keys = slice(p * PAIR, (p + 3) * PAIR)
            gain_v[h, p, 0] = jnp.sum(dk * kn[h, keys].astype(F32), axis=0, keepdims=True)
            gain_v[h, p, 1] = jnp.sum(dk * ku[h, keys], axis=0, keepdims=True)
            if again:
                shared, alone = slice(PAIR, 3 * PAIR), slice(3 * p * PAIR, (3 * p + 1) * PAIR)
                dkx[h, alone] = dk[2 * p * PAIR:(2 * p + 1) * PAIR]
                dkx[h, shared] = dkx[h, shared] + dk[(1 - p) * PAIR:(3 - p) * PAIR]
            else:
                dkx[h, keys] = dk

    def query_rows(g, u, r):
        g = g * FACTOR * gain_q
        return (r * (g - u * jnp.mean(g * u, axis=-1, keepdims=True))).astype(BF16)

    sublane = lax.broadcasted_iota(jnp.int32, (8, PAIR), 0)

    def skewed_sum(tile, right):
        parts = [pltpu.roll(tile[first:first + 8], (right - first) % PAIR, 1) for first in range(0, PAIR, 8)]
        while len(parts) > 1:
            parts = [a + b for a, b in zip(parts[::2], parts[1::2])]
        total = parts[0]
        for bit in range(1, 8):
            total = jnp.where(sublane == bit, pltpu.roll(parts[0], PAIR - bit, 1), total)
        return jnp.sum(total, axis=0, keepdims=True)

    def fold_rows(h, d_score):
        d0, d1, d2 = (d_score[b * PAIR:(b + 1) * PAIR] for b in range(3))
        mixed = jnp.where(past, d2, d1)
        ahead = jnp.where(past, 0.0, d2)
        rest = d0 + jnp.where(past, d1, 0.0)
        behind_row, ahead_row = skewed_sum(mixed, SEG - 1), skewed_sum(ahead, SEG - 1)
        high_row = skewed_sum(mixed, SEG - 1 + SEG) if h else behind_row
        rest_sum = jnp.sum(jnp.sum(rest, axis=0, keepdims=True), axis=1, keepdims=True)
        return (
            jnp.where(lane < SEG - 1, ahead_row, behind_row),
            jnp.where(lane == SEG - 1 + h * SEG, rest_sum, high_row))

    def fold_table(h, d_score):
        table_v2[h, 0], table_v2[h, 1] = fold_rows(h, d_score)

    def first_segment():
        key_number = lax.broadcasted_iota(jnp.int32, (ROWS + SEG, SEG), 0)
        hidden = jnp.logical_and(is_first, key_number < ROWS)

        for h in heads:
            u, _ = unit(first_kv[0, h])
            first_ku[h] = u
            first_kn[h] = (u * gain_k).astype(BF16)

        def against(first, rest, side):
            return jnp.concatenate([dot(first, side, 1, 1), dot(rest, side, 1, 1)], axis=0)

        scores = [against(first_kn[h], kn[h, :ROWS], qn0[h]) for h in heads]
        d_probs = [against(first_kv[1, h], kvx[1, h, :ROWS], qd0[1, h]) for h in heads]
        d_scores = []
        for h in heads:
            bias = jnp.where(hidden, MASKED, bias_v[h, 0, :ROWS + SEG][:, :SEG])
            bias = bias - jnp.max(bias, axis=0, keepdims=True)
            e = jnp.exp2(scores[h] * (FACTOR * LOG2E) + bias)
            inv = 1.0 / jnp.sum(e, axis=0, keepdims=True)
            delta = jnp.sum(e * d_probs[h], axis=0, keepdims=True) * inv
            prob = e * inv
            d_scores.append(prob * (d_probs[h] - delta))
            first_prob[h] = prob.astype(BF16)
            first_d_low[h] = d_scores[h].astype(BF16)
        products = [dot(d_scores[h].astype(BF16), qn0[h], 1, 0) for h in heads]
        for h in heads:
            tile = jnp.concatenate([d_scores[h], jnp.zeros((ROWS + SEG, SEG), F32)], axis=1)
            rows = fold_rows(h, jnp.concatenate([tile, jnp.zeros((SEG, PAIR), F32)], axis=0))
            for j in range(2):
                table_v2[h, j] = table_v2[h, j] + rows[j]
        for h in heads:
            first_dk[h] = products[h]
        for n, (first, rest) in enumerate(((first_kn, kn), (first_ku, ku))):
            gain = jnp.zeros((1, HEAD_DIM), F32)
            for h in heads:
                gain = gain + jnp.sum(products[h][:SEG] * first[h].astype(F32), axis=0, keepdims=True)
                gain = gain + jnp.sum(products[h][SEG:] * rest[h, :ROWS].astype(F32), axis=0, keepdims=True)
            extra_gain[n:n + 1] = gain

    def first_results(h):
        d_low = first_d_low[h]
        dv = dot(first_prob[h], qd0[1, h], 1, 0)
        dq_from_before[h] = dot(d_low[:SEG], first_kn[h], 0, 0) + dot(d_low[SEG:], kn[h, :ROWS], 0, 0)
        for n, part in enumerate((first_dk[h] * FACTOR, dv)):
            to_before_first[n, h] = part[:SEG].astype(BF16)
            from_before[n, h] = part[ROWS:].astype(BF16)
        dkx[h, :BEFORE] = dkx[h, :BEFORE] + first_dk[h, SEG:ROWS]
        dvx[h, :BEFORE] = dvx[h, :BEFORE] + dv[SEG:ROWS]

    heads = range(HEADS)
    work([(h, 0, 2) for h in heads])

    go_on(forth[2:], jnp.logical_and(tp == 1, place < total - 1))
    @pl.when(tp == 1)
    def _():
        pl.semaphore_wait(round1, len(close))
        for a, n in enumerate(sizes[:2]):
            if n > 5:
                for o in near(n, 2):
                    signal(round2, along(a, o))

    def wait_left(piece):
        @pl.when(place > 0)
        def _():
            if piece < HEADS:
                forth[piece].wait_recv()
            else:
                @pl.when(opens)
                def _():
                    wait_bytes(kvx.at[:, :, :PAIR], left_recv.at[piece - 1])

                @pl.when(takes_back)
                def _():
                    forth[piece].wait_recv()

    def wait_right():
        @pl.when(takes_next)
        def _():
            wait_bytes(kvx.at[:, :, :PAIR], right_recv)

    beside = sorted({*near(ny), *near(ny, 2)})

    def greet_far():
        @pl.when(tp == 1)
        def _():
            count = sum(len(near(n, 2)) for n in sizes[:2] if n > 5)
            if count:
                pl.semaphore_wait(round2, count)
            for o in beside:
                signal(plane_round, along(1, o))
            if nz > 9:
                for o in near(nz, 3):
                    signal(round3, along(0, o))

    def do_first():
        @pl.when(opens)
        def _():
            first_segment()

    def near_keys():
        for h in heads:
            take_keys(h, PAIR, SEG)

    def next_rows():
        for h in heads:
            take_keys(h, BEFORE + ROWS, SEG)
            take_queries(h)

    @pl.when(x == nx - 1)
    def _():
        wait_left(0)
        near_keys()
        work([(h, 0, 1) for h in heads])
        for h in heads:
            wait_left(1 + h)
            take_keys(h, 0, PAIR)
            work([(h, 0, 0)], [(h, 0, False)])
            if not h:
                greet_far()
        wait_right()
        next_rows()
        work([(h, 1, b) for b in range(3) for h in heads], [(h, 1, True) for h in heads])
        if nx == 1:
            do_first()

    if nx > 1:
        @pl.when(x == 0)
        def _():
            wait_right()
            next_rows()
            work([(h, 1, b) for b in (1, 2) for h in heads])
            greet_far()
            wait_left(0)
            near_keys()
            work([(h, p, 1 - p) for p in (1, 0) for h in heads], [(h, 1, False) for h in heads])
            for h in heads:
                wait_left(1 + h)
                take_keys(h, 0, PAIR)
                work([(h, 0, 0)], [(h, 0, True)])
            do_first()

    if nx > 2:
        @pl.when(jnp.logical_and(x > 0, x < nx - 1))
        def _():
            wait_left(0)
            near_keys()
            work([(h, 0, 1) for h in heads])
            wait_right()
            next_rows()
            work([(h, 1, b) for b in range(3) for h in heads], [(h, 1, False) for h in heads])
            greet_far()
            for h in heads:
                wait_left(1 + h)
                take_keys(h, 0, PAIR)
                work([(h, 0, 0)], [(h, 0, True)])

    second = jnp.where(lane < SEG, table_v2[0, 1], table_v2[1, 1])
    gain_rows = [
        (gain_v[0, 0, j] + gain_v[0, 1, j] + gain_v[1, 0, j] + gain_v[1, 1, j]
         + jnp.where(opens, extra_gain[j:j + 1], 0.0)) * FACTOR for j in range(2)]
    vec = jnp.concatenate([table_v2[0, 0], table_v2[1, 0], second, *gain_rows], axis=0)
    chip = y * nx + x

    to_neighbours = [
        remote(to_before.at[:, h], from_after.at[:, h], more_sem, after_recv, before) for h in range(HEADS)]
    to_next = [
        remote(to_after, from_before, table_sem, before_recv, after),
        remote(dqx.at[:, BEFORE:], dq_from_before, table_sem, before_recv, after)]
    to_plane_before = remote(to_before_first, from_after_first, more_sem, after_recv, before)

    def stage_results():
        @pl.when(takes_next)
        def _():
            wait_bytes(kvx.at[:, :, :BEFORE], load_sem)

        @pl.when(closes_early)
        def _():
            wait_bytes(kvx.at[:, :, :ROWS], load_sem)

        @pl.when(takes_back)
        def _():
            wait_bytes(kvx.at[:, :, :PAIR], gains_sem)

        for h in range(HEADS):
            low, high_tile = (dot(prob_v[h, p], qdx[1, h, p * PAIR:(p + 1) * PAIR], 1, 0) for p in range(2))
            dvx[h, :PAIR] = low[:PAIR]
            dvx[h, PAIR:3 * PAIR] = low[PAIR:] + high_tile[:2 * PAIR]
            dvx[h, 3 * PAIR:] = high_tile[2 * PAIR:]

            @pl.when(opens)
            def _(h=h):
                first_results(h)

            lanes = slice(h * HEAD_DIM, (h + 1) * HEAD_DIM)
            to_before[0, h] = (dkx[h, :BEFORE] * FACTOR).astype(BF16)
            to_before[1, h] = dvx[h, :BEFORE].astype(BF16)
            to_after[0, h] = (dkx[h, BEFORE + ROWS:] * FACTOR).astype(BF16)
            to_after[1, h] = dvx[h, BEFORE + ROWS:].astype(BF16)
            for p in range(2):
                dqx[h, p * PAIR:(p + 1) * PAIR] = dot(d_low_v[h, p], kn[h, p * PAIR:(p + 3) * PAIR], 0, 0)
            dq_v[SEG:, lanes] = query_rows(dqx[h, :BEFORE], qu[h, SEG:], qr[h, SEG:])

    def send_results(when):
        @pl.when(jnp.logical_and(when, place > 0))
        def _():
            for copy in to_neighbours:
                copy.start()

        @pl.when(jnp.logical_and(when, opens_later))
        def _():
            to_plane_before.start()

        @pl.when(jnp.logical_and(when, takes_next))
        def _():
            for copy in to_next:
                copy.start()

    def sum_of(ref, first, count):
        parts = [ref[n] for n in range(first, first + count)]
        while len(parts) > 1:
            parts = [sum(parts[n:n + 2]) for n in range(0, len(parts), 2)]
        return parts[0]

    has_across = ny > 3 and ny % 2 == 0
    across, column = nx * ny, nx * ny + nx

    @pl.when(tp == 1)
    def _():
        rows_x[x] = vec
        for o in far_first(nx):
            remote(rows_x.at[x], rows_x.at[x], sum_send, x_recv, along(2, o)).start()
        if beside:
            pl.semaphore_wait(plane_round, len(beside))
        signal(round1, (z, y, x, 0))
        if has_across:
            for o in far_first(nx) + [0]:
                remote(
                    rows_x.at[x], plane.at[across + x], sum_send, plane_recv,
                    (z, lax.rem(y + ny // 2, ny), lax.rem(x + o, nx), 1)).start()
        stage_results()
        send_results(jnp.logical_and(x > 0, x < nx - 1))
        if nx > 1:
            wait_bytes(rows_x.at[:nx - 1], x_recv)
        plane[column + y] = sum_of(rows_x, 0, nx)
        y_ways = [o for o in far_first(ny) if not has_across or o != ny // 2]
        for o in y_ways:
            remote(plane.at[column + y], plane.at[column + y], sum_send, plane_recv, along(1, o)).start()
        came = nx * ny + len(y_ways) + (nx if has_across else 0)
        wait_bytes(plane.at[:came], plane_recv)
        if has_across:
            plane[column + lax.rem(y + ny // 2, ny)] = sum_of(plane, across, nx)
        others, part = sum_of(plane, 0, nx * ny), sum_of(plane, column, ny)
        gain = part[3:] + others[3:]
        for core, rows in enumerate((others, part)):
            zout[core, :3] = rows[:3]
            zout[core, 3:] = gain
        zbuf[z] = zout[1]
        if nz > 9:
            pl.semaphore_wait(round3, len(near(nz, 3)))
        for o in [*far_first(nz), 0]:
            for core in ((1, 0) if o else (0,)):
                remote(zout.at[core], zbuf.at[z], sum_send, z_recv, along(0, o, core)).start()
        send_results(jnp.logical_or(x == 0, x == nx - 1))
        signal(round2, (z, y, x, 0))

    @pl.when(tp == 0)
    def _():
        plane[chip] = vec
        pl.semaphore_wait(round1, 1)
        for oy, ox in sorted(
                ((oy, ox) for oy in range(ny) for ox in range(nx)),
                key=lambda o: -min(o[0], ny - o[0]) - min(o[1], nx - o[1])):
            remote(
                plane.at[chip], plane.at[chip], sum_send, plane_recv,
                (z, lax.rem(y + oy, ny), lax.rem(x + ox, nx), 1)).start()
        stage_results()
        send_results(jnp.logical_or(opens, jnp.logical_and(x > 0, x < nx - 1)))
        pl.semaphore_wait(round2, 1)
        send_results(jnp.logical_and(jnp.logical_not(opens), jnp.logical_or(x == 0, x == nx - 1)))

    @pl.when(takes_back)
    def _():
        wait_bytes(kvx.at[:, :, :PAIR], before_recv)

    @pl.when(takes_next)
    def _():
        wait_bytes(from_after, after_recv)

    @pl.when(closes_early)
    def _():
        wait_bytes(kvx.at[:, :, :ROWS], after_recv)

    for h in range(HEADS):
        dq_v[:SEG, h * HEAD_DIM:(h + 1) * HEAD_DIM] = query_rows(dq_from_before[h], qu[h, :SEG], qr[h, :SEG])

    for h in range(HEADS):
        lanes = slice(h * HEAD_DIM, (h + 1) * HEAD_DIM)
        sums_in = [
            jnp.concatenate([
                jnp.where(takes_next, 0.0, jnp.where(is_last, 0.0, from_after_first[n, h].astype(F32)))
                + from_before[n, h].astype(F32), from_after[n, h].astype(F32)], axis=0) for n in range(2)]
        g = (dkx[h, BEFORE:BEFORE + ROWS] * FACTOR + sums_in[0]) * gain_k
        u = ku[h, BEFORE:BEFORE + ROWS]
        dk_v[:, lanes] = (kr[h] * (g - u * jnp.mean(g * u, axis=-1, keepdims=True))).astype(BF16)
        dv_v[:, lanes] = (dvx[h, BEFORE:BEFORE + ROWS] + sums_in[1]).astype(BF16)

    @pl.when(takes_next)
    def _():
        wait_bytes(kvx.at[:, :, :PAIR], table_sem)

    @pl.when(takes_back)
    def _():
        wait_bytes(from_after, more_sem)

    @pl.when(opens_later)
    def _():
        wait_bytes(kvx.at[:, :, :ROWS], more_sem)

    @pl.when(tp == 1)
    def _():
        wait_bytes(plane.at[:nx - 1 + 2 * nz - 1 + ny - 1 + (nx - 1 if has_across else 0)], sum_send)
        if nz > 1:
            wait_bytes(zbuf.at[:nz - 1], z_recv)

    @pl.when(tp == 0)
    def _():
        wait_bytes(plane.at[:nx * ny], sum_send)
        wait_bytes(zbuf.at[:nz], z_recv)

    result = zbuf[0]
    for n in range(1, nz):
        result = result + zbuf[n]
    for j in range(HEADS):
        dtab_v[j:j + 1, :PAIR] = result[j:j + 1]
        dtab_v[j:j + 1, PAIR:] = result[2:3, j * SEG:(j + 1) * SEG]
    dgain_v[0:1] = result[3:4] / gain_q
    dgain_v[1:2] = result[4:5]


def write_out(*refs):
    count = len(refs) // 2
    copies = [pltpu.make_async_copy(refs[n], refs[count + n], refs[-1].at[n]) for n in range(count)]
    for copy in copies:
        copy.start()
    for copy in copies:
        copy.wait()


def local(sizes, queries, keys, values, gains, bias_table, d_out):
    nz, ny, nx = sizes
    width = HEADS * HEAD_DIM
    hbm_spec = pl.BlockSpec(memory_space=pltpu.HBM)
    vmem_spec = pl.BlockSpec(memory_space=pltpu.VMEM)
    first = (HEADS, SEG, HEAD_DIM)
    tile = (HEADS, ROWS, HEAD_DIM)
    wide = (HEADS, 2 * ROWS, HEAD_DIM)
    pairs = (HEADS, 2, 3 * PAIR, PAIR)
    dma, regular = pltpu.SemaphoreType.DMA, pltpu.SemaphoreType.REGULAR
    vmem = pltpu.VMEM
    outs = [((ROWS, width), BF16)] * 3 + [((HEADS, ENTRIES), F32), ((2, HEAD_DIM), F32)]
    out = pl.pallas_call(
        functools.partial(kernel, sizes),
        out_shape=tuple(vmem(*o) for o in outs),
        in_specs=[hbm_spec] * 6,
        out_specs=(vmem_spec,) * 5,
        scratch_shapes=[
            vmem((2, *tile), BF16), vmem((2, *first), BF16), vmem((2, *wide), BF16), vmem((2, *first), BF16),
            vmem((2, HEAD_DIM), F32), vmem((HEADS, ENTRIES), F32),
            vmem(tile, BF16), vmem(first, BF16), vmem(tile, F32), vmem(tile, F32),
            vmem(wide, BF16), vmem(wide, F32), vmem(tile, F32),
            vmem(first, BF16), vmem(first, F32),
            vmem(pairs, F32), vmem(pairs, F32), vmem(pairs, F32),
            vmem(wide, F32), vmem(wide, F32), vmem(tile, F32), vmem((HEADS, 3 * PAIR, PAIR), F32),
            vmem(pairs, BF16), vmem(pairs, BF16), vmem((HEADS, 2, 6, 1, PAIR), F32), vmem((HEADS, 2, 2, 1, PAIR), F32),
            vmem((HEADS, 2, 1, PAIR), F32), vmem((2, HEAD_DIM), F32),
            vmem((HEADS, ROWS + SEG, SEG), BF16), vmem((HEADS, ROWS + SEG, SEG), BF16), vmem((HEADS, ROWS + SEG, HEAD_DIM), F32),
            vmem((2, HEADS, BEFORE, HEAD_DIM), BF16), vmem((2, HEADS, BEFORE, HEAD_DIM), BF16),
            vmem((2, *first), BF16), vmem((2, *first), BF16), vmem(first, F32), vmem((2, *first), BF16), vmem((2, *first), BF16),
            vmem((nx, 5, HEAD_DIM), F32), vmem((nx * ny + nx + ny + 2 * nz, 5, HEAD_DIM), F32), vmem((2, 5, HEAD_DIM), F32), vmem((2 * nz, 5, HEAD_DIM), F32),
            dma, dma, dma, dma, dma((HEADS + 1,)), dma, dma, dma,
            dma, dma, dma, dma, regular, regular, regular, regular,
        ],
        compiler_params=pltpu.CompilerParams(
            collective_id=0, has_side_effects=True, vmem_limit_bytes=32 * 1024 * 1024),
        name="segment_attention_grad",
    )(*(pltpu.with_memory_space_constraint(a, pltpu.HBM) for a in (queries, keys, values, d_out, gains, bias_table.T)))
    d_queries, d_keys, d_values, d_table, d_gains = pl.pallas_call(
        write_out,
        out_shape=tuple(jax.ShapeDtypeStruct(*o) for o in outs),
        in_specs=[vmem_spec] * 5,
        out_specs=(hbm_spec,) * 5,
        scratch_shapes=[dma((5,))],
        name="write_out",
    )(*(pltpu.with_memory_space_constraint(o, pltpu.VMEM) for o in out))
    return d_queries, d_keys, d_values, d_table.T, d_gains


def solution(mesh):
    shape = (12, 8, 4)
    if mesh.shape["sp"] != int(np.prod(shape)):
        shape = mesh.small_shape
    split = Mesh(mesh.devices.reshape(*shape, mesh.shape["tp"]), AXES)
    placed = (P(SP, "tp"), P(SP, "tp"), P(SP, "tp"), P(), P(None, "tp"), P(SP, "tp"))
    return jax.shard_map(
        functools.partial(local, shape),
        mesh=split,
        in_specs=placed,
        out_specs=(P(SP, "tp"), P(SP, "tp"), P(SP, "tp"), P(None, "tp"), P()),
        check_vma=False,
    )
```

```python
import functools

import jax
import jax.numpy as jnp
import numpy as np
from jax import lax
from jax.experimental import pallas as pl
from jax.experimental.pallas import tpu as pltpu
from jax.sharding import Mesh
from jax.sharding import PartitionSpec as P

HEAD_DIM = 128
SEG = 64
LEFT = 4
MAX_REL = 128
ENTRIES = MAX_REL + SEG
ROWS = LEFT * SEG
HEADS = 2
PAIR = 2 * SEG
BEFORE = 3 * SEG
AXES = ("sp_0", "sp_1", "sp_2", "tp")
SP = AXES[:3]

EPSILON = 1e-06
FACTOR = HEAD_DIM ** (-0.5)
LOG2E = 1.4426950408889634
MASKED = -1e30
F32, BF16 = jnp.float32, jnp.bfloat16


def dot(a, b, a_dim, b_dim):
    return lax.dot_general(a, b, (((a_dim,), (b_dim,)), ((), ())), preferred_element_type=F32)


def near(size, step=1):
    return sorted({step % size, -step % size} - {0})


def far_first(size):
    return sorted(range(1, size), key=lambda d: -min(d, size - d))


def unit(raw):
    wide = raw.astype(F32)
    inv_rms = lax.rsqrt(jnp.mean(wide * wide, axis=-1, keepdims=True) + EPSILON)
    return wide * inv_rms, inv_rms


def kernel(sizes, q_hbm, k_hbm, v_hbm, do_hbm, gains_hbm, table_hbm,
           dq_v, dk_v, dv_v, dtab_v, dgain_v,
           qdx, qd0, kvx, first_kv, gains_v, table_v,
           qn, qn0, qu, qr, kn, ku, kr, first_kn, first_ku, bias_v, e_v, dp_v,
           dkx, dvx, dqx, d_v, prob_v, d_low_v, sum_v, gain_v, table_v2, extra_gain, first_prob, first_d_low, first_dk,
           to_before, from_after, to_after, from_before, dq_from_before, to_before_first, from_after_first,
           rows_x, plane, zout, zbuf,
           load_sem, more_sem, gains_sem, table_sem, left_recv, right_recv, after_recv, before_recv,
           sum_send, x_recv, plane_recv, z_recv, round1, round2, round3, plane_round):
    nz, ny, nx = sizes
    z, y, x, tp = (lax.axis_index(a) for a in AXES)
    place = (z * ny + y) * nx + x
    total = nz * ny * nx
    is_first, is_last = place == 0, place == total - 1
    opens, closes = jnp.logical_and(x == 0, y == 0), jnp.logical_and(x == nx - 1, y == ny - 1)
    opens_later, closes_early = jnp.logical_and(opens, place > 0), jnp.logical_and(closes, place < total - 1)
    takes_back, takes_next = jnp.logical_not(opens), jnp.logical_not(closes)

    def at(number, core):
        return (number // (ny * nx), (number // nx) % ny, number % nx, core)

    after = at(jnp.minimum(place + 1, total - 1), tp)
    before = at(jnp.maximum(place - 1, 0), tp)

    def along(axis, offset, core=1):
        if axis == 0:
            return (lax.rem(z + offset, nz), y, x, core)
        if axis == 1:
            return (z, lax.rem(y + offset, ny), x, core)
        return (z, y, lax.rem(x + offset, nx), core)

    def signal(sem, target):
        pl.semaphore_signal(sem, inc=1, device_id=target, device_id_type=pl.DeviceIdType.MESH)

    def remote(src, dst, send, recv, target):
        return pltpu.make_async_remote_copy(
            src_ref=src, dst_ref=dst, send_sem=send, recv_sem=recv,
            device_id=target, device_id_type=pl.DeviceIdType.MESH)

    def wait_bytes(ref, sem):
        pltpu.make_async_copy(ref, ref, sem).wait()

    barrier = pltpu.get_barrier_semaphore()

    @pl.when(place > 0)
    def _():
        signal(barrier, before)

    @pl.when(place < total - 1)
    def _():
        signal(barrier, after)

    sides = jnp.where(is_first, 0, 1) + jnp.where(is_last, 0, 1)
    small_loads = [pltpu.make_async_copy(gains_hbm, gains_v, gains_sem), pltpu.make_async_copy(table_hbm, table_v, table_sem)]
    for load in small_loads:
        load.start()
    for h in range(HEADS):
        lanes = slice(h * HEAD_DIM, (h + 1) * HEAD_DIM)
        for n, (keys_or_values, queries_or_cotangents) in enumerate(((k_hbm, q_hbm), (v_hbm, do_hbm))):
            pltpu.make_async_copy(keys_or_values.at[:, lanes], kvx.at[n, h, BEFORE:BEFORE + ROWS], load_sem).start()
            pltpu.make_async_copy(queries_or_cotangents.at[:SEG, lanes], qd0.at[n, h], load_sem).start()
            pltpu.make_async_copy(queries_or_cotangents.at[SEG:, lanes], qdx.at[n, h, :BEFORE], more_sem).start()

    close = [(a, o) for a, n in enumerate(sizes) for o in near(n)]

    @pl.when(tp == 1)
    def _():
        for a, o in close:
            signal(barrier, along(a, o))
        signal(barrier, (z, y, x, 0))

    @pl.when(tp == 0)
    def _():
        signal(barrier, (z, y, x, 1))

    forth = [remote(
        kvx.at[:, :, ROWS + PAIR:ROWS + BEFORE], kvx.at[:, :, PAIR:BEFORE], load_sem, left_recv.at[HEADS], after)]
    back = {}
    for h in range(HEADS):
        forth.append(remote(
            kvx.at[:, h, ROWS:ROWS + PAIR], kvx.at[:, h, :PAIR], load_sem, left_recv.at[h], after))
        back[h] = [
            remote(kvx.at[:, h, BEFORE:ROWS], kvx.at[:, h, BEFORE + ROWS:], gains_sem, right_recv, before),
            remote(qd0.at[:, h], qdx.at[:, h, BEFORE:], gains_sem, right_recv, before)]

    plane_piece = remote(kvx.at[:, :, BEFORE:ROWS], first_kv, load_sem, left_recv.at[HEADS - 1], after)

    def go_on(pieces, when=place < total - 1):
        @pl.when(when)
        def _():
            for copy in pieces:
                copy.start()

    wait_bytes(kvx.at[:, :, :ROWS + SEG], load_sem)
    small_loads[0].wait()
    gains = gains_v[...]
    gain_q, gain_k = gains[0:1, :], gains[1:2, :]

    def take_keys(h, first, size):
        u, _ = unit(kvx[0, h, first:first + size])
        ku[h, first:first + size] = u
        kn[h, first:first + size] = (u * gain_k).astype(BF16)

    def take_queries(h):
        qn[h, BEFORE:] = (unit(qdx[0, h, BEFORE:])[0] * gain_q).astype(BF16)

    for h in range(HEADS):
        take_keys(h, BEFORE, ROWS)
    pl.semaphore_wait(barrier, sides + jnp.where(tp == 1, 1 + len(close), 1))
    go_on(forth[:1])
    go_on([copy for h in range(HEADS) for copy in back[h]], takes_back)
    go_on(forth[1:], jnp.logical_and(tp == 0, place < total - 1))
    go_on(forth[1:2], jnp.logical_and(tp == 1, place < total - 1))
    go_on([plane_piece], closes_early)

    @pl.when(tp == 1)
    def _():
        for a, o in close:
            signal(round1, along(a, o))

    wait_bytes(qdx.at[:, :, :BEFORE], more_sem)
    small_loads[1].wait()
    for h in range(HEADS):
        for raw, normed in ((qd0[0, h], qn0.at[h]), (qdx[0, h, :BEFORE], qn.at[h, :BEFORE])):
            normed[...] = (unit(raw)[0] * gain_q).astype(BF16)

    @pl.when(is_first)
    def _():
        for h in range(HEADS):
            for n in range(2):
                kvx[n, h, :BEFORE] = kvx[n, h, BEFORE:2 * BEFORE]
                first_kv[n, h] = kvx[n, h, BEFORE:ROWS]

    @pl.when(closes)
    def _():
        for h in range(HEADS):
            for n in range(2):
                kvx[n, h, BEFORE + ROWS:] = kvx[n, h, BEFORE:ROWS]
            qdx[0, h, BEFORE:] = qd0[0, h]
            qdx[1, h, BEFORE:] = jnp.zeros((SEG, HEAD_DIM), BF16)

    @pl.when(is_last)
    def _():
        for h in range(HEADS):
            for n in range(2):
                from_after[n, h] = jnp.zeros((BEFORE, HEAD_DIM), BF16)

    key_at = lax.broadcasted_iota(jnp.int32, (PAIR, PAIR), 0)
    query_at = lax.broadcasted_iota(jnp.int32, (PAIR, PAIR), 1)
    past = query_at >= key_at
    early = query_at < SEG
    high = key_at >= SEG
    lane = lax.broadcasted_iota(jnp.int32, (1, PAIR), 1)
    table = table_v[...]
    low_part = table[:, :PAIR]
    high_part = jnp.concatenate([table[:, PAIR:], jnp.zeros((HEADS, 2 * PAIR - ENTRIES), F32)], axis=1)
    low_rolled = pltpu.roll(low_part, PAIR - SEG + 1, 1)
    high_rolled = pltpu.roll(high_part, PAIR - SEG + 1, 1)
    for h in range(HEADS):
        last = table[h:h + 1, ENTRIES - 1:ENTRIES]
        dist_low = low_rolled[h:h + 1]
        dist_row = jnp.where(lane <= SEG, dist_low, high_rolled[h:h + 1])
        ahead = pltpu.roll(jnp.broadcast_to(dist_low, (PAIR, PAIR)), 0, 1, stride=1, stride_axis=0)
        behind = pltpu.roll(jnp.broadcast_to(dist_row, (PAIR, PAIR)), 0, 1, stride=1, stride_axis=0)
        tile0 = jnp.where(jnp.logical_or(early, high), last, MASKED)
        tile1 = jnp.where(past, last, behind)
        tile2 = jnp.where(jnp.logical_and(early, high), MASKED, jnp.where(past, behind, ahead))
        none, low = (jnp.where(is_first, MASKED, t) for t in (tile0, tile1))
        for p, tiles in enumerate((
                (none, jnp.where(high, tile1, low), tile2),
                (jnp.where(high, tile0, none), tile1, tile2))):
            top = jnp.max(jnp.maximum(jnp.maximum(tiles[0], tiles[1]), tiles[2]), axis=0, keepdims=True)
            for b, tile in enumerate(tiles):
                bias_v[h, p, b * PAIR:(b + 1) * PAIR] = (tile - top) * LOG2E

    def work(blocks, tiles=()):
        at_keys = {(p, b): slice((p + b) * PAIR, (p + b + 1) * PAIR) for h, p, b in blocks}
        at_queries = [slice(p * PAIR, (p + 1) * PAIR) for p in range(2)]
        at_rows = [slice(b * PAIR, (b + 1) * PAIR) for b in range(3)]
        scores = [dot(kn[h, at_keys[p, b]], qn[h, at_queries[p]], 1, 1) for h, p, b in blocks]
        d_probs = [dot(kvx[1, h, at_keys[p, b]], qdx[1, h, at_queries[p]], 1, 1) for h, p, b in blocks]
        for (h, p, b), s, dp in zip(blocks, scores, d_probs):
            e = jnp.exp2(s * (FACTOR * LOG2E) + bias_v[h, p, at_rows[b]])
            e_v[h, p, at_rows[b]] = e
            dp_v[h, p, at_rows[b]] = dp
            sum_v[h, p, b] = jnp.sum(e, axis=0, keepdims=True)
            sum_v[h, p, 3 + b] = jnp.sum(e * dp, axis=0, keepdims=True)
        d_scores, products = [], []
        for h, p, _ in tiles:
            inv = 1.0 / (sum_v[h, p, 0] + sum_v[h, p, 1] + sum_v[h, p, 2])
            delta = (sum_v[h, p, 3] + sum_v[h, p, 4] + sum_v[h, p, 5]) * inv
            prob = e_v[h, p] * inv
            d_score = prob * (dp_v[h, p] - delta)
            d_low = d_score.astype(BF16)
            prob_v[h, p] = prob.astype(BF16)
            d_low_v[h, p] = d_low
            d_scores.append(d_score)
            products.append(dot(d_low, qn[h, at_queries[p]], 1, 0))
        for (h, p, again), d_score in zip(tiles, d_scores):
            if again:
                fold_table(h, d_v[h] + d_score)
            else:
                d_v[h] = d_score
        for (h, p, again), dk in zip(tiles, products):
            keys = slice(p * PAIR, (p + 3) * PAIR)
            gain_v[h, p, 0] = jnp.sum(dk * kn[h, keys].astype(F32), axis=0, keepdims=True)
            gain_v[h, p, 1] = jnp.sum(dk * ku[h, keys], axis=0, keepdims=True)
            if again:
                shared, alone = slice(PAIR, 3 * PAIR), slice(3 * p * PAIR, (3 * p + 1) * PAIR)
                dkx[h, alone] = dk[2 * p * PAIR:(2 * p + 1) * PAIR]
                dkx[h, shared] = dkx[h, shared] + dk[(1 - p) * PAIR:(3 - p) * PAIR]
            else:
                dkx[h, keys] = dk

    def query_rows(g, u, r):
        g = g * FACTOR * gain_q
        return (r * (g - u * jnp.mean(g * u, axis=-1, keepdims=True))).astype(BF16)

    sublane = lax.broadcasted_iota(jnp.int32, (8, PAIR), 0)

    def skewed_sum(tile, right):
        parts = [pltpu.roll(tile[first:first + 8], (right - first) % PAIR, 1) for first in range(0, PAIR, 8)]
        while len(parts) > 1:
            parts = [a + b for a, b in zip(parts[::2], parts[1::2])]
        total = parts[0]
        for bit in range(1, 8):
            total = jnp.where(sublane == bit, pltpu.roll(parts[0], PAIR - bit, 1), total)
        return jnp.sum(total, axis=0, keepdims=True)

    def fold_rows(h, d_score):
        d0, d1, d2 = (d_score[b * PAIR:(b + 1) * PAIR] for b in range(3))
        mixed = jnp.where(past, d2, d1)
        ahead = jnp.where(past, 0.0, d2)
        rest = d0 + jnp.where(past, d1, 0.0)
        behind_row, ahead_row = skewed_sum(mixed, SEG - 1), skewed_sum(ahead, SEG - 1)
        high_row = skewed_sum(mixed, SEG - 1 + SEG) if h else behind_row
        rest_sum = jnp.sum(jnp.sum(rest, axis=0, keepdims=True), axis=1, keepdims=True)
        return (
            jnp.where(lane < SEG - 1, ahead_row, behind_row),
            jnp.where(lane == SEG - 1 + h * SEG, rest_sum, high_row))

    def fold_table(h, d_score):
        table_v2[h, 0], table_v2[h, 1] = fold_rows(h, d_score)

    def first_segment():
        key_number = lax.broadcasted_iota(jnp.int32, (ROWS + SEG, SEG), 0)
        hidden = jnp.logical_and(is_first, key_number < ROWS)

        for h in heads:
            u, _ = unit(first_kv[0, h])
            first_ku[h] = u
            first_kn[h] = (u * gain_k).astype(BF16)

        def against(first, rest, side):
            return jnp.concatenate([dot(first, side, 1, 1), dot(rest, side, 1, 1)], axis=0)

        scores = [against(first_kn[h], kn[h, :ROWS], qn0[h]) for h in heads]
        d_probs = [against(first_kv[1, h], kvx[1, h, :ROWS], qd0[1, h]) for h in heads]
        d_scores = []
        for h in heads:
            bias = jnp.where(hidden, MASKED, bias_v[h, 0, :ROWS + SEG][:, :SEG])
            bias = bias - jnp.max(bias, axis=0, keepdims=True)
            e = jnp.exp2(scores[h] * (FACTOR * LOG2E) + bias)
            inv = 1.0 / jnp.sum(e, axis=0, keepdims=True)
            delta = jnp.sum(e * d_probs[h], axis=0, keepdims=True) * inv
            prob = e * inv
            d_scores.append(prob * (d_probs[h] - delta))
            first_prob[h] = prob.astype(BF16)
            first_d_low[h] = d_scores[h].astype(BF16)
        products = [dot(d_scores[h].astype(BF16), qn0[h], 1, 0) for h in heads]
        for h in heads:
            tile = jnp.concatenate([d_scores[h], jnp.zeros((ROWS + SEG, SEG), F32)], axis=1)
            rows = fold_rows(h, jnp.concatenate([tile, jnp.zeros((SEG, PAIR), F32)], axis=0))
            for j in range(2):
                table_v2[h, j] = table_v2[h, j] + rows[j]
        for h in heads:
            first_dk[h] = products[h]
        for n, (first, rest) in enumerate(((first_kn, kn), (first_ku, ku))):
            gain = jnp.zeros((1, HEAD_DIM), F32)
            for h in heads:
                gain = gain + jnp.sum(products[h][:SEG] * first[h].astype(F32), axis=0, keepdims=True)
                gain = gain + jnp.sum(products[h][SEG:] * rest[h, :ROWS].astype(F32), axis=0, keepdims=True)
            extra_gain[n:n + 1] = gain

    def first_results(h):
        d_low = first_d_low[h]
        dv = dot(first_prob[h], qd0[1, h], 1, 0)
        dq_from_before[h] = dot(d_low[:SEG], first_kn[h], 0, 0) + dot(d_low[SEG:], kn[h, :ROWS], 0, 0)
        for n, part in enumerate((first_dk[h] * FACTOR, dv)):
            to_before_first[n, h] = part[:SEG].astype(BF16)
            from_before[n, h] = part[ROWS:].astype(BF16)
        dkx[h, :BEFORE] = dkx[h, :BEFORE] + first_dk[h, SEG:ROWS]
        dvx[h, :BEFORE] = dvx[h, :BEFORE] + dv[SEG:ROWS]

    heads = range(HEADS)
    work([(h, 0, 2) for h in heads])

    go_on(forth[2:], jnp.logical_and(tp == 1, place < total - 1))
    @pl.when(tp == 1)
    def _():
        pl.semaphore_wait(round1, len(close))
        for a, n in enumerate(sizes[:2]):
            if n > 5:
                for o in near(n, 2):
                    signal(round2, along(a, o))

    def wait_left(piece):
        @pl.when(place > 0)
        def _():
            if piece < HEADS:
                forth[piece].wait_recv()
            else:
                @pl.when(opens)
                def _():
                    wait_bytes(kvx.at[:, :, :PAIR], left_recv.at[piece - 1])

                @pl.when(takes_back)
                def _():
                    forth[piece].wait_recv()

    def wait_right():
        @pl.when(takes_next)
        def _():
            wait_bytes(kvx.at[:, :, :PAIR], right_recv)

    beside = sorted({*near(ny), *near(ny, 2)})

    def greet_far():
        @pl.when(tp == 1)
        def _():
            count = sum(len(near(n, 2)) for n in sizes[:2] if n > 5)
            if count:
                pl.semaphore_wait(round2, count)
            for o in beside:
                signal(plane_round, along(1, o))
            if nz > 9:
                for o in near(nz, 3):
                    signal(round3, along(0, o))

    def do_first():
        @pl.when(opens)
        def _():
            first_segment()

    def near_keys():
        for h in heads:
            take_keys(h, PAIR, SEG)

    def next_rows():
        for h in heads:
            take_keys(h, BEFORE + ROWS, SEG)
            take_queries(h)

    @pl.when(x == nx - 1)
    def _():
        wait_left(0)
        near_keys()
        work([(h, 0, 1) for h in heads])
        for h in heads:
            wait_left(1 + h)
            take_keys(h, 0, PAIR)
            work([(h, 0, 0)], [(h, 0, False)])
            if not h:
                greet_far()
        wait_right()
        next_rows()
        work([(h, 1, b) for b in range(3) for h in heads], [(h, 1, True) for h in heads])
        if nx == 1:
            do_first()

    if nx > 1:
        @pl.when(x == 0)
        def _():
            wait_right()
            next_rows()
            work([(h, 1, b) for b in (1, 2) for h in heads])
            greet_far()
            wait_left(0)
            near_keys()
            work([(h, p, 1 - p) for p in (1, 0) for h in heads], [(h, 1, False) for h in heads])
            for h in heads:
                wait_left(1 + h)
                take_keys(h, 0, PAIR)
                work([(h, 0, 0)], [(h, 0, True)])
            do_first()

    if nx > 2:
        @pl.when(jnp.logical_and(x > 0, x < nx - 1))
        def _():
            wait_left(0)
            near_keys()
            work([(h, 0, 1) for h in heads])
            wait_right()
            next_rows()
            work([(h, 1, b) for b in range(3) for h in heads], [(h, 1, False) for h in heads])
            greet_far()
            for h in heads:
                wait_left(1 + h)
                take_keys(h, 0, PAIR)
                work([(h, 0, 0)], [(h, 0, True)])

    second = jnp.where(lane < SEG, table_v2[0, 1], table_v2[1, 1])
    gain_rows = [
        (gain_v[0, 0, j] + gain_v[0, 1, j] + gain_v[1, 0, j] + gain_v[1, 1, j]
         + jnp.where(opens, extra_gain[j:j + 1], 0.0)) * FACTOR for j in range(2)]
    vec = jnp.concatenate([table_v2[0, 0], table_v2[1, 0], second, *gain_rows], axis=0)
    chip = y * nx + x

    to_neighbours = [
        remote(to_before.at[:, h], from_after.at[:, h], more_sem, after_recv, before) for h in range(HEADS)]
    to_next = [
        remote(to_after, from_before, table_sem, before_recv, after),
        remote(dqx.at[:, BEFORE:], dq_from_before, table_sem, before_recv, after)]
    to_plane_before = remote(to_before_first, from_after_first, more_sem, after_recv, before)

    def stage_results():
        @pl.when(takes_next)
        def _():
            wait_bytes(kvx.at[:, :, :BEFORE], load_sem)

        @pl.when(closes_early)
        def _():
            wait_bytes(kvx.at[:, :, :ROWS], load_sem)

        @pl.when(takes_back)
        def _():
            wait_bytes(kvx.at[:, :, :PAIR], gains_sem)

        for h in range(HEADS):
            low, high_tile = (dot(prob_v[h, p], qdx[1, h, p * PAIR:(p + 1) * PAIR], 1, 0) for p in range(2))
            dvx[h, :PAIR] = low[:PAIR]
            dvx[h, PAIR:3 * PAIR] = low[PAIR:] + high_tile[:2 * PAIR]
            dvx[h, 3 * PAIR:] = high_tile[2 * PAIR:]

            @pl.when(opens)
            def _(h=h):
                first_results(h)

            lanes = slice(h * HEAD_DIM, (h + 1) * HEAD_DIM)
            to_before[0, h] = (dkx[h, :BEFORE] * FACTOR).astype(BF16)
            to_before[1, h] = dvx[h, :BEFORE].astype(BF16)
            to_after[0, h] = (dkx[h, BEFORE + ROWS:] * FACTOR).astype(BF16)
            to_after[1, h] = dvx[h, BEFORE + ROWS:].astype(BF16)
            for p in range(2):
                dqx[h, p * PAIR:(p + 1) * PAIR] = dot(d_low_v[h, p], kn[h, p * PAIR:(p + 3) * PAIR], 0, 0)
            qu[h], r = unit(qd0[0, h])
            qr[h] = jnp.broadcast_to(r, (SEG, HEAD_DIM))
            kr[h] = jnp.broadcast_to(unit(kvx[0, h, BEFORE:BEFORE + ROWS])[1], (ROWS, HEAD_DIM))
            dq_v[SEG:, lanes] = query_rows(dqx[h, :BEFORE], *unit(qdx[0, h, :BEFORE]))

    def send_results(when):
        @pl.when(jnp.logical_and(when, place > 0))
        def _():
            for copy in to_neighbours:
                copy.start()

        @pl.when(jnp.logical_and(when, opens_later))
        def _():
            to_plane_before.start()

        @pl.when(jnp.logical_and(when, takes_next))
        def _():
            for copy in to_next:
                copy.start()

    def sum_of(ref, first, count):
        parts = [ref[n] for n in range(first, first + count)]
        while len(parts) > 1:
            parts = [sum(parts[n:n + 2]) for n in range(0, len(parts), 2)]
        return parts[0]

    has_across = ny > 3 and ny % 2 == 0
    across, column = nx * ny, nx * ny + nx

    @pl.when(tp == 1)
    def _():
        rows_x[x] = vec
        for o in far_first(nx):
            remote(rows_x.at[x], rows_x.at[x], sum_send, x_recv, along(2, o)).start()
        if beside:
            pl.semaphore_wait(plane_round, len(beside))
        signal(round1, (z, y, x, 0))
        if has_across:
            for o in far_first(nx) + [0]:
                remote(
                    rows_x.at[x], plane.at[across + x], sum_send, plane_recv,
                    (z, lax.rem(y + ny // 2, ny), lax.rem(x + o, nx), 1)).start()
        stage_results()
        send_results(jnp.logical_and(x > 0, x < nx - 1))
        if nx > 1:
            wait_bytes(rows_x.at[:nx - 1], x_recv)
        plane[column + y] = sum_of(rows_x, 0, nx)
        y_ways = [o for o in far_first(ny) if not has_across or o != ny // 2]
        for o in y_ways:
            remote(plane.at[column + y], plane.at[column + y], sum_send, plane_recv, along(1, o)).start()
        came = nx * ny + len(y_ways) + (nx if has_across else 0)
        wait_bytes(plane.at[:came], plane_recv)
        if has_across:
            plane[column + lax.rem(y + ny // 2, ny)] = sum_of(plane, across, nx)
        others, part = sum_of(plane, 0, nx * ny), sum_of(plane, column, ny)
        gain = part[3:] + others[3:]
        for core, rows in enumerate((others, part)):
            zout[core, :3] = rows[:3]
            zout[core, 3:] = gain
        zbuf[z] = zout[1]
        if nz > 9:
            pl.semaphore_wait(round3, len(near(nz, 3)))
        for o in [*far_first(nz), 0]:
            for core in ((1, 0) if o else (0,)):
                remote(zout.at[core], zbuf.at[z], sum_send, z_recv, along(0, o, core)).start()
        send_results(jnp.logical_or(x == 0, x == nx - 1))
        signal(round2, (z, y, x, 0))

    @pl.when(tp == 0)
    def _():
        plane[chip] = vec
        pl.semaphore_wait(round1, 1)
        for oy, ox in sorted(
                ((oy, ox) for oy in range(ny) for ox in range(nx)),
                key=lambda o: -min(o[0], ny - o[0]) - min(o[1], nx - o[1])):
            remote(
                plane.at[chip], plane.at[chip], sum_send, plane_recv,
                (z, lax.rem(y + oy, ny), lax.rem(x + ox, nx), 1)).start()
        stage_results()
        send_results(jnp.logical_or(opens, jnp.logical_and(x > 0, x < nx - 1)))
        pl.semaphore_wait(round2, 1)
        send_results(jnp.logical_and(jnp.logical_not(opens), jnp.logical_or(x == 0, x == nx - 1)))

    @pl.when(takes_back)
    def _():
        wait_bytes(kvx.at[:, :, :PAIR], before_recv)

    @pl.when(takes_next)
    def _():
        wait_bytes(from_after, after_recv)

    @pl.when(closes_early)
    def _():
        wait_bytes(kvx.at[:, :, :ROWS], after_recv)

    for h in range(HEADS):
        dq_v[:SEG, h * HEAD_DIM:(h + 1) * HEAD_DIM] = query_rows(dq_from_before[h], qu[h], qr[h])

    for h in range(HEADS):
        lanes = slice(h * HEAD_DIM, (h + 1) * HEAD_DIM)
        sums_in = [
            jnp.concatenate([
                jnp.where(takes_next, 0.0, jnp.where(is_last, 0.0, from_after_first[n, h].astype(F32)))
                + from_before[n, h].astype(F32), from_after[n, h].astype(F32)], axis=0) for n in range(2)]
        g = (dkx[h, BEFORE:BEFORE + ROWS] * FACTOR + sums_in[0]) * gain_k
        u = ku[h, BEFORE:BEFORE + ROWS]
        dk_v[:, lanes] = (kr[h] * (g - u * jnp.mean(g * u, axis=-1, keepdims=True))).astype(BF16)
        dv_v[:, lanes] = (dvx[h, BEFORE:BEFORE + ROWS] + sums_in[1]).astype(BF16)

    @pl.when(takes_next)
    def _():
        wait_bytes(kvx.at[:, :, :PAIR], table_sem)

    @pl.when(takes_back)
    def _():
        wait_bytes(from_after, more_sem)

    @pl.when(opens_later)
    def _():
        wait_bytes(kvx.at[:, :, :ROWS], more_sem)

    @pl.when(tp == 1)
    def _():
        wait_bytes(plane.at[:nx - 1 + 2 * nz - 1 + ny - 1 + (nx - 1 if has_across else 0)], sum_send)
        if nz > 1:
            wait_bytes(zbuf.at[:nz - 1], z_recv)

    @pl.when(tp == 0)
    def _():
        wait_bytes(plane.at[:nx * ny], sum_send)
        wait_bytes(zbuf.at[:nz], z_recv)

    result = zbuf[0]
    for n in range(1, nz):
        result = result + zbuf[n]
    for j in range(HEADS):
        dtab_v[j:j + 1, :PAIR] = result[j:j + 1]
        dtab_v[j:j + 1, PAIR:] = result[2:3, j * SEG:(j + 1) * SEG]
    dgain_v[0:1] = result[3:4] / gain_q
    dgain_v[1:2] = result[4:5]


def write_out(*refs):
    count = len(refs) // 2
    copies = [pltpu.make_async_copy(refs[n], refs[count + n], refs[-1].at[n]) for n in range(count)]
    for copy in copies:
        copy.start()
    for copy in copies:
        copy.wait()


def local(sizes, queries, keys, values, gains, bias_table, d_out):
    nz, ny, nx = sizes
    width = HEADS * HEAD_DIM
    hbm_spec = pl.BlockSpec(memory_space=pltpu.HBM)
    vmem_spec = pl.BlockSpec(memory_space=pltpu.VMEM)
    first = (HEADS, SEG, HEAD_DIM)
    tile = (HEADS, ROWS, HEAD_DIM)
    wide = (HEADS, 2 * ROWS, HEAD_DIM)
    pairs = (HEADS, 2, 3 * PAIR, PAIR)
    dma, regular = pltpu.SemaphoreType.DMA, pltpu.SemaphoreType.REGULAR
    vmem = pltpu.VMEM
    outs = [((ROWS, width), BF16)] * 3 + [((HEADS, ENTRIES), F32), ((2, HEAD_DIM), F32)]
    out = pl.pallas_call(
        functools.partial(kernel, sizes),
        out_shape=tuple(vmem(*o) for o in outs),
        in_specs=[hbm_spec] * 6,
        out_specs=(vmem_spec,) * 5,
        scratch_shapes=[
            vmem((2, *tile), BF16), vmem((2, *first), BF16), vmem((2, *wide), BF16), vmem((2, *first), BF16),
            vmem((2, HEAD_DIM), F32), vmem((HEADS, ENTRIES), F32),
            vmem(tile, BF16), vmem(first, BF16), vmem(first, F32), vmem(first, F32),
            vmem(wide, BF16), vmem(wide, F32), vmem(tile, F32),
            vmem(first, BF16), vmem(first, F32),
            vmem(pairs, F32), vmem(pairs, F32), vmem(pairs, F32),
            vmem(wide, F32), vmem(wide, F32), vmem(tile, F32), vmem((HEADS, 3 * PAIR, PAIR), F32),
            vmem(pairs, BF16), vmem(pairs, BF16), vmem((HEADS, 2, 6, 1, PAIR), F32), vmem((HEADS, 2, 2, 1, PAIR), F32),
            vmem((HEADS, 2, 1, PAIR), F32), vmem((2, HEAD_DIM), F32),
            vmem((HEADS, ROWS + SEG, SEG), BF16), vmem((HEADS, ROWS + SEG, SEG), BF16), vmem((HEADS, ROWS + SEG, HEAD_DIM), F32),
            vmem((2, HEADS, BEFORE, HEAD_DIM), BF16), vmem((2, HEADS, BEFORE, HEAD_DIM), BF16),
            vmem((2, *first), BF16), vmem((2, *first), BF16), vmem(first, F32), vmem((2, *first), BF16), vmem((2, *first), BF16),
            vmem((nx, 5, HEAD_DIM), F32), vmem((nx * ny + nx + ny + 2 * nz, 5, HEAD_DIM), F32), vmem((2, 5, HEAD_DIM), F32), vmem((2 * nz, 5, HEAD_DIM), F32),
            dma, dma, dma, dma, dma((HEADS + 1,)), dma, dma, dma,
            dma, dma, dma, dma, regular, regular, regular, regular,
        ],
        compiler_params=pltpu.CompilerParams(
            collective_id=0, has_side_effects=True, vmem_limit_bytes=32 * 1024 * 1024),
        name="segment_attention_grad",
    )(*(pltpu.with_memory_space_constraint(a, pltpu.HBM) for a in (queries, keys, values, d_out, gains, bias_table.T)))
    d_queries, d_keys, d_values, d_table, d_gains = pl.pallas_call(
        write_out,
        out_shape=tuple(jax.ShapeDtypeStruct(*o) for o in outs),
        in_specs=[vmem_spec] * 5,
        out_specs=(hbm_spec,) * 5,
        scratch_shapes=[dma((5,))],
        name="write_out",
    )(*(pltpu.with_memory_space_constraint(o, pltpu.VMEM) for o in out))
    return d_queries, d_keys, d_values, d_table.T, d_gains


def solution(mesh):
    shape = (12, 8, 4)
    if mesh.shape["sp"] != int(np.prod(shape)):
        shape = mesh.small_shape
    split = Mesh(mesh.devices.reshape(*shape, mesh.shape["tp"]), AXES)
    placed = (P(SP, "tp"), P(SP, "tp"), P(SP, "tp"), P(), P(None, "tp"), P(SP, "tp"))
    return jax.shard_map(
        functools.partial(local, shape),
        mesh=split,
        in_specs=placed,
        out_specs=(P(SP, "tp"), P(SP, "tp"), P(SP, "tp"), P(None, "tp"), P()),
        check_vma=False,
    )
```

```python
import functools

import jax
import jax.numpy as jnp
import numpy as np
from jax import lax
from jax.experimental import pallas as pl
from jax.experimental.pallas import tpu as pltpu
from jax.sharding import Mesh
from jax.sharding import PartitionSpec as P

HEAD_DIM = 128
SEG = 64
LEFT = 4
MAX_REL = 128
ENTRIES = MAX_REL + SEG
ROWS = LEFT * SEG
HEADS = 2
PAIR = 2 * SEG
BEFORE = 3 * SEG
AXES = ("sp_0", "sp_1", "sp_2", "tp")
SP = AXES[:3]

EPSILON = 1e-06
FACTOR = HEAD_DIM ** (-0.5)
LOG2E = 1.4426950408889634
MASKED = -1e30
F32, BF16 = jnp.float32, jnp.bfloat16


def dot(a, b, a_dim, b_dim):
    return lax.dot_general(a, b, (((a_dim,), (b_dim,)), ((), ())), preferred_element_type=F32)


def near(size, step=1):
    return sorted({step % size, -step % size} - {0})


def far_first(size):
    return sorted(range(1, size), key=lambda d: -min(d, size - d))


def unit(raw):
    wide = raw.astype(F32)
    inv_rms = lax.rsqrt(jnp.mean(wide * wide, axis=-1, keepdims=True) + EPSILON)
    return wide * inv_rms, inv_rms


def kernel(sizes, q_hbm, k_hbm, v_hbm, do_hbm, gains_hbm, table_hbm,
           dq_v, dk_v, dv_v, dtab_v, dgain_v,
           qdx, qd0, kvx, first_kv, gains_v, table_v,
           qn, qn0, qu, qr, kn, ku, kr, first_kn, first_ku, bias_v, e_v, dp_v,
           dkx, dvx, dqx, d_v, prob_v, d_low_v, sum_v, gain_v, table_v2, extra_gain, first_prob, first_d_low, first_dk,
           to_before, from_after, to_after, from_before, dq_from_before, to_before_first, from_after_first,
           rows_x, plane, zout, zbuf,
           load_sem, more_sem, gains_sem, table_sem, left_recv, right_recv, after_recv, before_recv,
           sum_send, x_recv, plane_recv, z_recv, round1, round2, round3, plane_round):
    nz, ny, nx = sizes
    z, y, x, tp = (lax.axis_index(a) for a in AXES)
    place = (z * ny + y) * nx + x
    total = nz * ny * nx
    is_first, is_last = place == 0, place == total - 1
    opens, closes = jnp.logical_and(x == 0, y == 0), jnp.logical_and(x == nx - 1, y == ny - 1)
    opens_later, closes_early = jnp.logical_and(opens, place > 0), jnp.logical_and(closes, place < total - 1)
    takes_back, takes_next = jnp.logical_not(opens), jnp.logical_not(closes)

    def at(number, core):
        return (number // (ny * nx), (number // nx) % ny, number % nx, core)

    after = at(jnp.minimum(place + 1, total - 1), tp)
    before = at(jnp.maximum(place - 1, 0), tp)

    def along(axis, offset, core=1):
        if axis == 0:
            return (lax.rem(z + offset, nz), y, x, core)
        if axis == 1:
            return (z, lax.rem(y + offset, ny), x, core)
        return (z, y, lax.rem(x + offset, nx), core)

    def signal(sem, target):
        pl.semaphore_signal(sem, inc=1, device_id=target, device_id_type=pl.DeviceIdType.MESH)

    def remote(src, dst, send, recv, target):
        return pltpu.make_async_remote_copy(
            src_ref=src, dst_ref=dst, send_sem=send, recv_sem=recv,
            device_id=target, device_id_type=pl.DeviceIdType.MESH)

    def wait_bytes(ref, sem):
        pltpu.make_async_copy(ref, ref, sem).wait()

    barrier = pltpu.get_barrier_semaphore()

    @pl.when(place > 0)
    def _():
        signal(barrier, before)

    @pl.when(place < total - 1)
    def _():
        signal(barrier, after)

    sides = jnp.where(is_first, 0, 1) + jnp.where(is_last, 0, 1)
    small_loads = [pltpu.make_async_copy(gains_hbm, gains_v, gains_sem), pltpu.make_async_copy(table_hbm, table_v, table_sem)]
    for load in small_loads:
        load.start()
    for h in range(HEADS):
        lanes = slice(h * HEAD_DIM, (h + 1) * HEAD_DIM)
        for n, (keys_or_values, queries_or_cotangents) in enumerate(((k_hbm, q_hbm), (v_hbm, do_hbm))):
            pltpu.make_async_copy(keys_or_values.at[:, lanes], kvx.at[n, h, BEFORE:BEFORE + ROWS], load_sem).start()
            pltpu.make_async_copy(queries_or_cotangents.at[:SEG, lanes], qd0.at[n, h], load_sem).start()
            pltpu.make_async_copy(queries_or_cotangents.at[SEG:, lanes], qdx.at[n, h, :BEFORE], more_sem).start()

    close = [(a, o) for a, n in enumerate(sizes) for o in near(n)]

    @pl.when(tp == 1)
    def _():
        for a, o in close:
            signal(barrier, along(a, o))
        signal(barrier, (z, y, x, 0))

    @pl.when(tp == 0)
    def _():
        signal(barrier, (z, y, x, 1))

    forth = [remote(
        kvx.at[:, :, ROWS + PAIR:ROWS + BEFORE], kvx.at[:, :, PAIR:BEFORE], load_sem, left_recv.at[HEADS], after)]
    back = {}
    for h in range(HEADS):
        forth.append(remote(
            kvx.at[:, h, ROWS:ROWS + PAIR], kvx.at[:, h, :PAIR], load_sem, left_recv.at[h], after))
        back[h] = [
            remote(kvx.at[:, h, BEFORE:ROWS], kvx.at[:, h, BEFORE + ROWS:], gains_sem, right_recv, before),
            remote(qd0.at[:, h], qdx.at[:, h, BEFORE:], gains_sem, right_recv, before)]

    plane_piece = remote(kvx.at[:, :, BEFORE:ROWS], first_kv, load_sem, left_recv.at[HEADS - 1], after)

    def go_on(pieces, when=place < total - 1):
        @pl.when(when)
        def _():
            for copy in pieces:
                copy.start()

    wait_bytes(kvx.at[:, :, :ROWS + SEG], load_sem)
    small_loads[0].wait()
    gains = gains_v[...]
    gain_q, gain_k = gains[0:1, :], gains[1:2, :]

    def take_keys(h, first, size):
        u, r = unit(kvx[0, h, first:first + size])
        ku[h, first:first + size] = u
        kn[h, first:first + size] = (u * gain_k).astype(BF16)
        return r

    def take_queries(h):
        qn[h, BEFORE:] = (unit(qdx[0, h, BEFORE:])[0] * gain_q).astype(BF16)

    for h in range(HEADS):
        kr[h] = jnp.broadcast_to(take_keys(h, BEFORE, ROWS), (ROWS, HEAD_DIM))
    pl.semaphore_wait(barrier, sides + jnp.where(tp == 1, 1 + len(close), 1))
    go_on([plane_piece], closes_early)
    go_on(forth[:1])
    go_on([copy for h in range(HEADS) for copy in back[h]], takes_back)
    go_on(forth[1:], jnp.logical_and(tp == 0, place < total - 1))
    go_on(forth[1:2], jnp.logical_and(tp == 1, place < total - 1))

    @pl.when(tp == 1)
    def _():
        for a, o in close:
            signal(round1, along(a, o))

    wait_bytes(qdx.at[:, :, :BEFORE], more_sem)
    small_loads[1].wait()
    for h in range(HEADS):
        for raw, normed, rows in (
                (qd0[0, h], qn0.at[h], slice(0, SEG)),
                (qdx[0, h, :BEFORE], qn.at[h, :BEFORE], slice(SEG, ROWS))):
            u, r = unit(raw)
            qu[h, rows] = u
            qr[h, rows] = jnp.broadcast_to(r, u.shape)
            normed[...] = (u * gain_q).astype(BF16)

    @pl.when(is_first)
    def _():
        for h in range(HEADS):
            for n in range(2):
                kvx[n, h, :BEFORE] = kvx[n, h, BEFORE:2 * BEFORE]
                first_kv[n, h] = kvx[n, h, BEFORE:ROWS]

    @pl.when(closes)
    def _():
        for h in range(HEADS):
            for n in range(2):
                kvx[n, h, BEFORE + ROWS:] = kvx[n, h, BEFORE:ROWS]
            qdx[0, h, BEFORE:] = qd0[0, h]
            qdx[1, h, BEFORE:] = jnp.zeros((SEG, HEAD_DIM), BF16)

    @pl.when(is_last)
    def _():
        for h in range(HEADS):
            for n in range(2):
                from_after[n, h] = jnp.zeros((BEFORE, HEAD_DIM), BF16)

    key_at = lax.broadcasted_iota(jnp.int32, (PAIR, PAIR), 0)
    query_at = lax.broadcasted_iota(jnp.int32, (PAIR, PAIR), 1)
    past = query_at >= key_at
    early = query_at < SEG
    high = key_at >= SEG
    lane = lax.broadcasted_iota(jnp.int32, (1, PAIR), 1)
    table = table_v[...]
    low_part = table[:, :PAIR]
    high_part = jnp.concatenate([table[:, PAIR:], jnp.zeros((HEADS, 2 * PAIR - ENTRIES), F32)], axis=1)
    low_rolled = pltpu.roll(low_part, PAIR - SEG + 1, 1)
    high_rolled = pltpu.roll(high_part, PAIR - SEG + 1, 1)
    for h in range(HEADS):
        last = table[h:h + 1, ENTRIES - 1:ENTRIES]
        dist_low = low_rolled[h:h + 1]
        dist_row = jnp.where(lane <= SEG, dist_low, high_rolled[h:h + 1])
        ahead = pltpu.roll(jnp.broadcast_to(dist_low, (PAIR, PAIR)), 0, 1, stride=1, stride_axis=0)
        behind = pltpu.roll(jnp.broadcast_to(dist_row, (PAIR, PAIR)), 0, 1, stride=1, stride_axis=0)
        tile0 = jnp.where(jnp.logical_or(early, high), last, MASKED)
        tile1 = jnp.where(past, last, behind)
        tile2 = jnp.where(jnp.logical_and(early, high), MASKED, jnp.where(past, behind, ahead))
        none, low = (jnp.where(is_first, MASKED, t) for t in (tile0, tile1))
        for p, tiles in enumerate((
                (none, jnp.where(high, tile1, low), tile2),
                (jnp.where(high, tile0, none), tile1, tile2))):
            top = jnp.max(jnp.maximum(jnp.maximum(tiles[0], tiles[1]), tiles[2]), axis=0, keepdims=True)
            for b, tile in enumerate(tiles):
                bias_v[h, p, b * PAIR:(b + 1) * PAIR] = (tile - top) * LOG2E

    def work(blocks, tiles=()):
        at_keys = {(p, b): slice((p + b) * PAIR, (p + b + 1) * PAIR) for h, p, b in blocks}
        at_queries = [slice(p * PAIR, (p + 1) * PAIR) for p in range(2)]
        at_rows = [slice(b * PAIR, (b + 1) * PAIR) for b in range(3)]
        scores = [dot(kn[h, at_keys[p, b]], qn[h, at_queries[p]], 1, 1) for h, p, b in blocks]
        d_probs = [dot(kvx[1, h, at_keys[p, b]], qdx[1, h, at_queries[p]], 1, 1) for h, p, b in blocks]
        for (h, p, b), s, dp in zip(blocks, scores, d_probs):
            e = jnp.exp2(s * (FACTOR * LOG2E) + bias_v[h, p, at_rows[b]])
            e_v[h, p, at_rows[b]] = e
            dp_v[h, p, at_rows[b]] = dp
            sum_v[h, p, b] = jnp.sum(e, axis=0, keepdims=True)
            sum_v[h, p, 3 + b] = jnp.sum(e * dp, axis=0, keepdims=True)
        d_scores, products = [], []
        for h, p, _ in tiles:
            inv = 1.0 / (sum_v[h, p, 0] + sum_v[h, p, 1] + sum_v[h, p, 2])
            delta = (sum_v[h, p, 3] + sum_v[h, p, 4] + sum_v[h, p, 5]) * inv
            prob = e_v[h, p] * inv
            d_score = prob * (dp_v[h, p] - delta)
            d_low = d_score.astype(BF16)
            prob_v[h, p] = prob.astype(BF16)
            d_low_v[h, p] = d_low
            d_scores.append(d_score)
            products.append(dot(d_low, qn[h, at_queries[p]], 1, 0))
        for (h, p, again), d_score in zip(tiles, d_scores):
            if again:
                fold_table(h, d_v[h] + d_score)
            else:
                d_v[h] = d_score
        for (h, p, again), dk in zip(tiles, products):
            keys = slice(p * PAIR, (p + 3) * PAIR)
            gain_v[h, p, 0] = jnp.sum(dk * kn[h, keys].astype(F32), axis=0, keepdims=True)
            gain_v[h, p, 1] = jnp.sum(dk * ku[h, keys], axis=0, keepdims=True)
            if again:
                shared, alone = slice(PAIR, 3 * PAIR), slice(3 * p * PAIR, (3 * p + 1) * PAIR)
                dkx[h, alone] = dk[2 * p * PAIR:(2 * p + 1) * PAIR]
                dkx[h, shared] = dkx[h, shared] + dk[(1 - p) * PAIR:(3 - p) * PAIR]
            else:
                dkx[h, keys] = dk

    def query_rows(g, u, r):
        g = g * FACTOR * gain_q
        return (r * (g - u * jnp.mean(g * u, axis=-1, keepdims=True))).astype(BF16)

    sublane = lax.broadcasted_iota(jnp.int32, (8, PAIR), 0)

    def skewed_sum(tile, right):
        parts = [pltpu.roll(tile[first:first + 8], (right - first) % PAIR, 1) for first in range(0, PAIR, 8)]
        while len(parts) > 1:
            parts = [a + b for a, b in zip(parts[::2], parts[1::2])]
        total = parts[0]
        for bit in range(1, 8):
            total = jnp.where(sublane == bit, pltpu.roll(parts[0], PAIR - bit, 1), total)
        return jnp.sum(total, axis=0, keepdims=True)

    def fold_rows(h, d_score):
        d0, d1, d2 = (d_score[b * PAIR:(b + 1) * PAIR] for b in range(3))
        mixed = jnp.where(past, d2, d1)
        ahead = jnp.where(past, 0.0, d2)
        rest = d0 + jnp.where(past, d1, 0.0)
        behind_row, ahead_row = skewed_sum(mixed, SEG - 1), skewed_sum(ahead, SEG - 1)
        high_row = skewed_sum(mixed, SEG - 1 + SEG) if h else behind_row
        rest_sum = jnp.sum(jnp.sum(rest, axis=0, keepdims=True), axis=1, keepdims=True)
        return (
            jnp.where(lane < SEG - 1, ahead_row, behind_row),
            jnp.where(lane == SEG - 1 + h * SEG, rest_sum, high_row))

    def fold_table(h, d_score):
        table_v2[h, 0], table_v2[h, 1] = fold_rows(h, d_score)

    def first_segment():
        key_number = lax.broadcasted_iota(jnp.int32, (ROWS + SEG, SEG), 0)
        hidden = jnp.logical_and(is_first, key_number < ROWS)

        for h in heads:
            u, _ = unit(first_kv[0, h])
            first_ku[h] = u
            first_kn[h] = (u * gain_k).astype(BF16)

        def against(first, rest, side):
            return jnp.concatenate([dot(first, side, 1, 1), dot(rest, side, 1, 1)], axis=0)

        scores = [against(first_kn[h], kn[h, :ROWS], qn0[h]) for h in heads]
        d_probs = [against(first_kv[1, h], kvx[1, h, :ROWS], qd0[1, h]) for h in heads]
        d_scores = []
        for h in heads:
            bias = jnp.where(hidden, MASKED, bias_v[h, 0, :ROWS + SEG][:, :SEG])
            bias = bias - jnp.max(bias, axis=0, keepdims=True)
            e = jnp.exp2(scores[h] * (FACTOR * LOG2E) + bias)
            inv = 1.0 / jnp.sum(e, axis=0, keepdims=True)
            delta = jnp.sum(e * d_probs[h], axis=0, keepdims=True) * inv
            prob = e * inv
            d_scores.append(prob * (d_probs[h] - delta))
            first_prob[h] = prob.astype(BF16)
            first_d_low[h] = d_scores[h].astype(BF16)
        products = [dot(d_scores[h].astype(BF16), qn0[h], 1, 0) for h in heads]
        for h in heads:
            tile = jnp.concatenate([d_scores[h], jnp.zeros((ROWS + SEG, SEG), F32)], axis=1)
            rows = fold_rows(h, jnp.concatenate([tile, jnp.zeros((SEG, PAIR), F32)], axis=0))
            for j in range(2):
                table_v2[h, j] = table_v2[h, j] + rows[j]
        for h in heads:
            first_dk[h] = products[h]
        for n, (first, rest) in enumerate(((first_kn, kn), (first_ku, ku))):
            gain = jnp.zeros((1, HEAD_DIM), F32)
            for h in heads:
                gain = gain + jnp.sum(products[h][:SEG] * first[h].astype(F32), axis=0, keepdims=True)
                gain = gain + jnp.sum(products[h][SEG:] * rest[h, :ROWS].astype(F32), axis=0, keepdims=True)
            extra_gain[n:n + 1] = gain

    def first_results(h):
        d_low = first_d_low[h]
        dv = dot(first_prob[h], qd0[1, h], 1, 0)
        dq_from_before[h] = dot(d_low[:SEG], first_kn[h], 0, 0) + dot(d_low[SEG:], kn[h, :ROWS], 0, 0)
        for n, part in enumerate((first_dk[h] * FACTOR, dv)):
            to_before_first[n, h] = part[:SEG].astype(BF16)
            from_before[n, h] = part[ROWS:].astype(BF16)
        dkx[h, :BEFORE] = dkx[h, :BEFORE] + first_dk[h, SEG:ROWS]
        dvx[h, :BEFORE] = dvx[h, :BEFORE] + dv[SEG:ROWS]

    heads = range(HEADS)
    work([(h, 0, 2) for h in heads])

    go_on(forth[2:], jnp.logical_and(tp == 1, place < total - 1))
    @pl.when(tp == 1)
    def _():
        pl.semaphore_wait(round1, len(close))
        for a, n in enumerate(sizes[:2]):
            if n > 5:
                for o in near(n, 2):
                    signal(round2, along(a, o))

    def wait_left(piece):
        @pl.when(place > 0)
        def _():
            if piece < HEADS:
                forth[piece].wait_recv()
            else:
                @pl.when(opens)
                def _():
                    wait_bytes(kvx.at[:, :, :PAIR], left_recv.at[piece - 1])

                @pl.when(takes_back)
                def _():
                    forth[piece].wait_recv()

    def wait_right():
        @pl.when(takes_next)
        def _():
            wait_bytes(kvx.at[:, :, :PAIR], right_recv)

    beside = sorted({*near(ny), *near(ny, 2)})

    def greet_far():
        @pl.when(tp == 1)
        def _():
            count = sum(len(near(n, 2)) for n in sizes[:2] if n > 5)
            if count:
                pl.semaphore_wait(round2, count)
            for o in beside:
                signal(plane_round, along(1, o))
            if nz > 9:
                for o in near(nz, 3):
                    signal(round3, along(0, o))

    def do_first():
        @pl.when(opens)
        def _():
            first_segment()

    def near_keys():
        for h in heads:
            take_keys(h, PAIR, SEG)

    def next_rows():
        for h in heads:
            take_keys(h, BEFORE + ROWS, SEG)
            take_queries(h)

    @pl.when(x == nx - 1)
    def _():
        wait_left(0)
        near_keys()
        work([(h, 0, 1) for h in heads])
        for h in heads:
            wait_left(1 + h)
            take_keys(h, 0, PAIR)
            work([(h, 0, 0)], [(h, 0, False)])
            if not h:
                greet_far()
        wait_right()
        next_rows()
        work([(h, 1, b) for b in range(3) for h in heads], [(h, 1, True) for h in heads])
        if nx == 1:
            do_first()

    if nx > 1:
        @pl.when(x == 0)
        def _():
            wait_right()
            next_rows()
            work([(h, 1, b) for b in (1, 2) for h in heads])
            greet_far()
            wait_left(0)
            near_keys()
            work([(h, p, 1 - p) for p in (1, 0) for h in heads], [(h, 1, False) for h in heads])
            for h in heads:
                wait_left(1 + h)
                take_keys(h, 0, PAIR)
                work([(h, 0, 0)], [(h, 0, True)])
            do_first()

    if nx > 2:
        @pl.when(jnp.logical_and(x > 0, x < nx - 1))
        def _():
            wait_left(0)
            near_keys()
            work([(h, 0, 1) for h in heads])
            wait_right()
            next_rows()
            work([(h, 1, b) for b in range(3) for h in heads], [(h, 1, False) for h in heads])
            greet_far()
            for h in heads:
                wait_left(1 + h)
                take_keys(h, 0, PAIR)
                work([(h, 0, 0)], [(h, 0, True)])

    second = jnp.where(lane < SEG, table_v2[0, 1], table_v2[1, 1])
    gain_rows = [
        (gain_v[0, 0, j] + gain_v[0, 1, j] + gain_v[1, 0, j] + gain_v[1, 1, j]
         + jnp.where(opens, extra_gain[j:j + 1], 0.0)) * FACTOR for j in range(2)]
    vec = jnp.concatenate([table_v2[0, 0], table_v2[1, 0], second, *gain_rows], axis=0)
    chip = y * nx + x

    to_neighbours = [
        remote(to_before.at[:, h], from_after.at[:, h], more_sem, after_recv, before) for h in range(HEADS)]
    to_next = [
        remote(to_after, from_before, table_sem, before_recv, after),
        remote(dqx.at[:, BEFORE:], dq_from_before, table_sem, before_recv, after)]
    to_plane_before = remote(to_before_first, from_after_first, more_sem, after_recv, before)

    def stage_results():
        @pl.when(takes_next)
        def _():
            wait_bytes(kvx.at[:, :, :BEFORE], load_sem)

        @pl.when(closes_early)
        def _():
            wait_bytes(kvx.at[:, :, :ROWS], load_sem)

        @pl.when(takes_back)
        def _():
            wait_bytes(kvx.at[:, :, :PAIR], gains_sem)

        for h in range(HEADS):
            low, high_tile = (dot(prob_v[h, p], qdx[1, h, p * PAIR:(p + 1) * PAIR], 1, 0) for p in range(2))
            dvx[h, :PAIR] = low[:PAIR]
            dvx[h, PAIR:3 * PAIR] = low[PAIR:] + high_tile[:2 * PAIR]
            dvx[h, 3 * PAIR:] = high_tile[2 * PAIR:]

            @pl.when(opens)
            def _(h=h):
                first_results(h)

            lanes = slice(h * HEAD_DIM, (h + 1) * HEAD_DIM)
            to_before[0, h] = (dkx[h, :BEFORE] * FACTOR).astype(BF16)
            to_before[1, h] = dvx[h, :BEFORE].astype(BF16)
            to_after[0, h] = (dkx[h, BEFORE + ROWS:] * FACTOR).astype(BF16)
            to_after[1, h] = dvx[h, BEFORE + ROWS:].astype(BF16)
            for p in range(2):
                dqx[h, p * PAIR:(p + 1) * PAIR] = dot(d_low_v[h, p], kn[h, p * PAIR:(p + 3) * PAIR], 0, 0)
            dq_v[SEG:, lanes] = query_rows(dqx[h, :BEFORE], qu[h, SEG:], qr[h, SEG:])

    def send_results(when):
        @pl.when(jnp.logical_and(when, place > 0))
        def _():
            for copy in to_neighbours:
                copy.start()

        @pl.when(jnp.logical_and(when, opens_later))
        def _():
            to_plane_before.start()

        @pl.when(jnp.logical_and(when, takes_next))
        def _():
            for copy in to_next:
                copy.start()

    def sum_of(ref, first, count):
        parts = [ref[n] for n in range(first, first + count)]
        while len(parts) > 1:
            parts = [sum(parts[n:n + 2]) for n in range(0, len(parts), 2)]
        return parts[0]

    has_across = ny > 3 and ny % 2 == 0
    across, column = nx * ny, nx * ny + nx

    @pl.when(tp == 1)
    def _():
        rows_x[x] = vec
        for o in far_first(nx):
            remote(rows_x.at[x], rows_x.at[x], sum_send, x_recv, along(2, o)).start()
        if beside:
            pl.semaphore_wait(plane_round, len(beside))
        signal(round1, (z, y, x, 0))
        if has_across:
            for o in far_first(nx) + [0]:
                remote(
                    rows_x.at[x], plane.at[across + x], sum_send, plane_recv,
                    (z, lax.rem(y + ny // 2, ny), lax.rem(x + o, nx), 1)).start()
        stage_results()
        send_results(jnp.logical_and(x > 0, x < nx - 1))
        if nx > 1:
            wait_bytes(rows_x.at[:nx - 1], x_recv)
        plane[column + y] = sum_of(rows_x, 0, nx)
        y_ways = [o for o in far_first(ny) if not has_across or o != ny // 2]
        for o in y_ways:
            remote(plane.at[column + y], plane.at[column + y], sum_send, plane_recv, along(1, o)).start()
        came = nx * ny + len(y_ways) + (nx if has_across else 0)
        wait_bytes(plane.at[:came], plane_recv)
        if has_across:
            plane[column + lax.rem(y + ny // 2, ny)] = sum_of(plane, across, nx)
        others, part = sum_of(plane, 0, nx * ny), sum_of(plane, column, ny)
        gain = part[3:] + others[3:]
        for core, rows in enumerate((others, part)):
            zout[core, :3] = rows[:3]
            zout[core, 3:] = gain
        zbuf[z] = zout[1]
        if nz > 9:
            pl.semaphore_wait(round3, len(near(nz, 3)))
        for o in [*far_first(nz), 0]:
            for core in ((1, 0) if o else (0,)):
                remote(zout.at[core], zbuf.at[z], sum_send, z_recv, along(0, o, core)).start()
        send_results(jnp.logical_or(x == 0, x == nx - 1))
        signal(round2, (z, y, x, 0))

    @pl.when(tp == 0)
    def _():
        plane[chip] = vec
        pl.semaphore_wait(round1, 1)
        for oy, ox in sorted(
                ((oy, ox) for oy in range(ny) for ox in range(nx)),
                key=lambda o: -min(o[0], ny - o[0]) - min(o[1], nx - o[1])):
            remote(
                plane.at[chip], plane.at[chip], sum_send, plane_recv,
                (z, lax.rem(y + oy, ny), lax.rem(x + ox, nx), 1)).start()
        stage_results()
        send_results(jnp.logical_or(opens, jnp.logical_and(x > 0, x < nx - 1)))
        pl.semaphore_wait(round2, 1)
        send_results(jnp.logical_and(jnp.logical_not(opens), jnp.logical_or(x == 0, x == nx - 1)))

    @pl.when(takes_back)
    def _():
        wait_bytes(kvx.at[:, :, :PAIR], before_recv)

    @pl.when(takes_next)
    def _():
        wait_bytes(from_after, after_recv)

    @pl.when(closes_early)
    def _():
        wait_bytes(kvx.at[:, :, :ROWS], after_recv)

    for h in range(HEADS):
        dq_v[:SEG, h * HEAD_DIM:(h + 1) * HEAD_DIM] = query_rows(dq_from_before[h], qu[h, :SEG], qr[h, :SEG])

    for h in range(HEADS):
        lanes = slice(h * HEAD_DIM, (h + 1) * HEAD_DIM)
        sums_in = [
            jnp.concatenate([
                jnp.where(takes_next, 0.0, jnp.where(is_last, 0.0, from_after_first[n, h].astype(F32)))
                + from_before[n, h].astype(F32), from_after[n, h].astype(F32)], axis=0) for n in range(2)]
        g = (dkx[h, BEFORE:BEFORE + ROWS] * FACTOR + sums_in[0]) * gain_k
        u = ku[h, BEFORE:BEFORE + ROWS]
        dk_v[:, lanes] = (kr[h] * (g - u * jnp.mean(g * u, axis=-1, keepdims=True))).astype(BF16)
        dv_v[:, lanes] = (dvx[h, BEFORE:BEFORE + ROWS] + sums_in[1]).astype(BF16)

    @pl.when(takes_next)
    def _():
        wait_bytes(kvx.at[:, :, :PAIR], table_sem)

    @pl.when(takes_back)
    def _():
        wait_bytes(from_after, more_sem)

    @pl.when(opens_later)
    def _():
        wait_bytes(kvx.at[:, :, :ROWS], more_sem)

    @pl.when(tp == 1)
    def _():
        wait_bytes(plane.at[:nx - 1 + 2 * nz - 1 + ny - 1 + (nx - 1 if has_across else 0)], sum_send)
        if nz > 1:
            wait_bytes(zbuf.at[:nz - 1], z_recv)

    @pl.when(tp == 0)
    def _():
        wait_bytes(plane.at[:nx * ny], sum_send)
        wait_bytes(zbuf.at[:nz], z_recv)

    result = zbuf[0]
    for n in range(1, nz):
        result = result + zbuf[n]
    for j in range(HEADS):
        dtab_v[j:j + 1, :PAIR] = result[j:j + 1]
        dtab_v[j:j + 1, PAIR:] = result[2:3, j * SEG:(j + 1) * SEG]
    dgain_v[0:1] = result[3:4] / gain_q
    dgain_v[1:2] = result[4:5]


def write_out(*refs):
    count = len(refs) // 2
    copies = [pltpu.make_async_copy(refs[n], refs[count + n], refs[-1].at[n]) for n in range(count)]
    for copy in copies:
        copy.start()
    for copy in copies:
        copy.wait()


def local(sizes, queries, keys, values, gains, bias_table, d_out):
    nz, ny, nx = sizes
    width = HEADS * HEAD_DIM
    hbm_spec = pl.BlockSpec(memory_space=pltpu.HBM)
    vmem_spec = pl.BlockSpec(memory_space=pltpu.VMEM)
    first = (HEADS, SEG, HEAD_DIM)
    tile = (HEADS, ROWS, HEAD_DIM)
    wide = (HEADS, 2 * ROWS, HEAD_DIM)
    pairs = (HEADS, 2, 3 * PAIR, PAIR)
    dma, regular = pltpu.SemaphoreType.DMA, pltpu.SemaphoreType.REGULAR
    vmem = pltpu.VMEM
    outs = [((ROWS, width), BF16)] * 3 + [((HEADS, ENTRIES), F32), ((2, HEAD_DIM), F32)]
    out = pl.pallas_call(
        functools.partial(kernel, sizes),
        out_shape=tuple(vmem(*o) for o in outs),
        in_specs=[hbm_spec] * 6,
        out_specs=(vmem_spec,) * 5,
        scratch_shapes=[
            vmem((2, *tile), BF16), vmem((2, *first), BF16), vmem((2, *wide), BF16), vmem((2, *first), BF16),
            vmem((2, HEAD_DIM), F32), vmem((HEADS, ENTRIES), F32),
            vmem(tile, BF16), vmem(first, BF16), vmem(tile, F32), vmem(tile, F32),
            vmem(wide, BF16), vmem(wide, F32), vmem(tile, F32),
            vmem(first, BF16), vmem(first, F32),
            vmem(pairs, F32), vmem(pairs, F32), vmem(pairs, F32),
            vmem(wide, F32), vmem(wide, F32), vmem(tile, F32), vmem((HEADS, 3 * PAIR, PAIR), F32),
            vmem(pairs, BF16), vmem(pairs, BF16), vmem((HEADS, 2, 6, 1, PAIR), F32), vmem((HEADS, 2, 2, 1, PAIR), F32),
            vmem((HEADS, 2, 1, PAIR), F32), vmem((2, HEAD_DIM), F32),
            vmem((HEADS, ROWS + SEG, SEG), BF16), vmem((HEADS, ROWS + SEG, SEG), BF16), vmem((HEADS, ROWS + SEG, HEAD_DIM), F32),
            vmem((2, HEADS, BEFORE, HEAD_DIM), BF16), vmem((2, HEADS, BEFORE, HEAD_DIM), BF16),
            vmem((2, *first), BF16), vmem((2, *first), BF16), vmem(first, F32), vmem((2, *first), BF16), vmem((2, *first), BF16),
            vmem((nx, 5, HEAD_DIM), F32), vmem((nx * ny + nx + ny + 2 * nz, 5, HEAD_DIM), F32), vmem((2, 5, HEAD_DIM), F32), vmem((2 * nz, 5, HEAD_DIM), F32),
            dma, dma, dma, dma, dma((HEADS + 1,)), dma, dma, dma,
            dma, dma, dma, dma, regular, regular, regular, regular,
        ],
        compiler_params=pltpu.CompilerParams(
            collective_id=0, has_side_effects=True, vmem_limit_bytes=32 * 1024 * 1024),
        name="segment_attention_grad",
    )(*(pltpu.with_memory_space_constraint(a, pltpu.HBM) for a in (queries, keys, values, d_out, gains, bias_table.T)))
    d_queries, d_keys, d_values, d_table, d_gains = pl.pallas_call(
        write_out,
        out_shape=tuple(jax.ShapeDtypeStruct(*o) for o in outs),
        in_specs=[vmem_spec] * 5,
        out_specs=(hbm_spec,) * 5,
        scratch_shapes=[dma((5,))],
        name="write_out",
    )(*(pltpu.with_memory_space_constraint(o, pltpu.VMEM) for o in out))
    return d_queries, d_keys, d_values, d_table.T, d_gains


def solution(mesh):
    shape = (12, 8, 4)
    if mesh.shape["sp"] != int(np.prod(shape)):
        shape = mesh.small_shape
    split = Mesh(mesh.devices.reshape(*shape, mesh.shape["tp"]), AXES)
    placed = (P(SP, "tp"), P(SP, "tp"), P(SP, "tp"), P(), P(None, "tp"), P(SP, "tp"))
    return jax.shard_map(
        functools.partial(local, shape),
        mesh=split,
        in_specs=placed,
        out_specs=(P(SP, "tp"), P(SP, "tp"), P(SP, "tp"), P(None, "tp"), P()),
        check_vma=False,
    )
```
